32 devices in a mesh: grp: 2 (over y), st: 4 (over z), tp: 4 (over x, core).
Axes of the slice: x: 2, y: 2, z: 4, core: 2. Of those that a mesh axis runs over, the one named last changes fastest.
Arguments:
- pass_ids: int32 [64, 4], P(('grp', 'st')), parts along dimension 0, may hold values from 0 to 63, as said below
- store: bfloat16 [64, 64, 2048], P('st', None, 'tp'), may hold values from -6 to 6
- queries: bfloat16 [8192, 1024], P(('grp', 'st'), 'tp'), parts along dimension 0, may hold values from -40 to 40
- gate_pre: bfloat16 [8192, 1024], P(('grp', 'st'), 'tp'), parts along dimension 0, may hold values from -6 to 6
- w_query: bfloat16 [2048, 1024], P(None, 'tp'), may hold values from -0.125 to 0.125
- w_gate: bfloat16 [2048, 1024], P(None, 'tp'), may hold values from -0.125 to 0.125
- w_key: bfloat16 [2048, 1024], P(None, 'tp'), may hold values from -0.125 to 0.125
- w_value: bfloat16 [2048, 1024], P(None, 'tp'), may hold values from -0.125 to 0.125
- d_mem: bfloat16 [8192, 1024], P(('grp', 'st'), 'tp'), parts along dimension 0, may hold values from -6 to 6
Outputs:
- d_tokens: bfloat16 [8192, 2048], P(('grp', 'st', 'tp')), parts along dimension 0
- d_store: bfloat16 [128, 64, 2048], P(('grp', 'st', 'tp')), parts along dimension 0
- d_wkey: float32 [4096, 1024], P(('grp', 'st'), 'tp'), parts along dimension 0
The draws below stay inside these ranges and needn't reach their ends.
There are 2 independent parts, one for each index of `grp`. The reference program is written for one: setup_inputs(seed, part) draws one part's arguments, and reference() takes and returns one part's arrays. A program takes and returns all parts, laid end to end along the dimension named above; an argument that names none is the same for every part. Nothing has to cross between parts.
Inputs may be any that keep to these rules, and one draw needn't show every extreme that they name: `pass_ids`: the 8 blocks of one index of st name at most 8 passages (counted with repetition) held by any one index of st o, that is passages o * 16 to o * 16 + 15. Every index of st takes exactly 8 passages from each of 4 indices of st and none from the others, so the bound 8 is reached by every index.
All inputs are finite; a program needn't handle non-finite values.
Results may differ from the reference program's by a relative error of at most 0.02.
Values may be sent and summed in bfloat16 or wider, within the bound.
A program may use at most 128 MiB of HBM per device.

```python
import jax
import jax.numpy as jnp
from jax import lax

D = 2048
HD = 256
MH = 4
BLK = 128
PB = 4
PL = 64
PASS_DEV = 16
MW = 1024
NBLK_DEV = 8
NBLK = 32
TOKENS = 4096
NPASS = 64
MOST = 8
N_ST = 4
N_TP = 4


def draw_pass_ids(key, part):
    folded = jax.random.fold_in(key, 17)
    key_hot, key_rank, key_order, key_pick, key_shift = jax.random.split(folded, 5)
    total_req = NBLK_DEV * PB
    used_owners = total_req // MOST
    device = jnp.arange(N_ST, dtype=jnp.int32)[:, None]
    owner_row = jnp.arange(N_ST, dtype=jnp.int32)[None, :]
    hottest = jax.random.randint(key_hot, (), 0, N_ST)
    levels = jnp.where(owner_row == hottest, 3, jnp.where(owner_row == (device - 1) % N_ST, 2, jnp.where(owner_row == (device + N_ST // 2) % N_ST, 1, 0)))
    jitter = jax.random.randint(key_rank, (N_ST, N_ST), 0, 1000)
    scores = levels * (1000 * N_ST) + jitter * N_ST + owner_row
    chosen = lax.top_k(scores, used_owners)[1].astype(jnp.int32)
    owners = jnp.repeat(chosen, MOST, axis=1)
    order_keys = jax.random.randint(key_order, (N_ST, total_req), 0, 1000) * total_req + jnp.arange(total_req, dtype=jnp.int32)[None, :]
    ordering = jnp.argsort(order_keys, axis=1)
    owners = jnp.take_along_axis(owners, ordering, axis=1)
    samples = jax.random.randint(key_pick, (3, N_ST, total_req), 0, PASS_DEV)
    popular = jnp.min(samples, axis=0)
    offsets = jax.random.randint(key_shift, (N_ST,), 0, PASS_DEV)
    within = (popular + offsets[owners]) % PASS_DEV
    passage_ids = owners * PASS_DEV + within
    return passage_ids.reshape(N_ST * NBLK_DEV, PB).astype(jnp.int32)


def draw_queries(key, part):
    folded = jax.random.fold_in(key, 23)
    key_base = jax.random.fold_in(folded, 0)
    base = jnp.clip(jax.random.normal(key_base, (TOKENS, MW), jnp.float32), -6.0, 6.0)
    return base.astype(jnp.bfloat16)


def level_of(own_key, dims, cuts, least, high):
    def one(dim, shards_of):
        steps = jax.random.uniform(jax.random.fold_in(jax.random.fold_in(own_key, 6), dim), (shards_of,), jnp.float32, least / len(cuts), high / len(cuts))
        return jnp.repeat(jnp.exp(steps), dims[dim] // shards_of).reshape((-1,) + (1,) * (len(dims) - dim - 1))

    loudness = one(*cuts[0])
    for cut in cuts[1:]:
        loudness = loudness * one(*cut)
    return loudness


def bell_draw(key, shape, deviation, reach, cuts=(), kind=jnp.bfloat16):
    array = jax.random.normal(key, shape, jnp.float32) * deviation
    if len(cuts) > 0:
        array = level_of(key, shape, cuts, -0.22, 0.18) * array
    return jnp.clip(array, min=-reach, max=reach).astype(kind)


def setup_inputs(seed: int = 0, part: int = 0) -> dict:
    keys = jax.random.split(jax.random.key(seed), 10)
    part_keys = jax.random.split(jax.random.fold_in(keys[9], part), 10)
    return {
        "pass_ids": draw_pass_ids(jax.random.fold_in(jax.random.fold_in(keys[9], part), 71), part),
        "store": bell_draw(keys[1], (NPASS, PL, D), 1.0, 6.0, ((0, 4), (2, 4))),
        "queries": draw_queries(jax.random.fold_in(jax.random.fold_in(keys[9], part), 71), part),
        "gate_pre": bell_draw(part_keys[3], (TOKENS, MW), 1.5, 6.0, ((0, 4), (1, 4))),
        "w_query": bell_draw(keys[4], (D, MW), D ** -0.5, 0.125, ((1, 4),)),
        "w_gate": bell_draw(keys[5], (D, MW), D ** -0.5, 0.125, ((1, 4),)),
        "w_key": bell_draw(keys[6], (D, MW), D ** -0.5, 0.125, ((1, 4),)),
        "w_value": bell_draw(keys[7], (D, MW), D ** -0.5, 0.125, ((1, 4),)),
        "d_mem": bell_draw(part_keys[8], (TOKENS, MW), 1.0, 6.0, ((0, 4), (1, 4))),
    }


def rounded_copy(values):
    return lax.optimization_barrier(values.astype(jnp.bfloat16)).astype(jnp.float32)


def reference(pass_ids, store, queries, gate_pre, w_query, w_gate, w_key, w_value, d_mem):
    flat_rows = store.reshape(NPASS * PL, D)
    keys_all = jnp.dot(flat_rows, w_key, preferred_element_type=jnp.float32).astype(jnp.bfloat16).reshape(NPASS, PL, MW)
    values_all = jnp.dot(flat_rows, w_value, preferred_element_type=jnp.float32).astype(jnp.bfloat16).reshape(NPASS, PL, MW)
    request_ids = pass_ids.reshape(-1).astype(jnp.int32)
    key_rows = keys_all[request_ids].reshape(NBLK, PB * PL, MH, HD).astype(jnp.float32)
    value_rows = values_all[request_ids].reshape(NBLK, PB * PL, MH, HD).astype(jnp.float32)
    query_rows = queries.reshape(NBLK, BLK, MH, HD).astype(jnp.float32)
    score_scale = HD ** -0.5
    scores = jnp.einsum('nqhd,nkhd->nhqk', query_rows, key_rows) * score_scale
    shifted = jnp.exp(scores - jnp.max(scores, axis=-1, keepdims=True))
    prob_rows = shifted / jnp.sum(shifted, axis=-1, keepdims=True)
    probs_low = rounded_copy(prob_rows)
    attended = jnp.einsum('nhqk,nkhd->nqhd', probs_low, value_rows).reshape(TOKENS, MW)
    gate_vals = gate_pre.astype(jnp.float32)
    sigmoid_vals = jax.nn.sigmoid(gate_vals)
    mem_grad = d_mem.astype(jnp.float32)
    attended_grad = rounded_copy(gate_vals * sigmoid_vals * mem_grad)
    gate_grad = rounded_copy(mem_grad * attended * sigmoid_vals * (1.0 + gate_vals * (1.0 - sigmoid_vals)))
    attended_four = attended_grad.reshape(NBLK, BLK, MH, HD)
    prob_grad = jnp.einsum('nqhd,nkhd->nhqk', attended_four, value_rows)
    score_grad = rounded_copy(score_scale * prob_rows * (prob_grad - jnp.sum(prob_rows * prob_grad, axis=-1, keepdims=True)))
    query_grad = rounded_copy(jnp.einsum('nhqk,nkhd->nqhd', score_grad, key_rows).reshape(TOKENS, MW))
    key_grad = rounded_copy(jnp.einsum('nhqk,nqhd->nkhd', score_grad, query_rows)).reshape(NBLK * PB, PL, MW)
    value_grad = rounded_copy(jnp.einsum('nhqk,nqhd->nkhd', probs_low, attended_four)).reshape(NBLK * PB, PL, MW)
    key_sums = jax.ops.segment_sum(key_grad, request_ids, NPASS).astype(jnp.bfloat16).reshape(NPASS * PL, MW)
    value_sums = jax.ops.segment_sum(value_grad, request_ids, NPASS).astype(jnp.bfloat16).reshape(NPASS * PL, MW)
    d_wkey = jnp.dot(flat_rows.T, key_sums, preferred_element_type=jnp.float32)
    group_width = MW // N_TP
    query_low = query_grad.astype(jnp.bfloat16)
    gate_low = gate_grad.astype(jnp.bfloat16)
    store_total = jnp.zeros((NPASS * PL, D), jnp.float32)
    token_total = jnp.zeros((TOKENS, D), jnp.float32)
    for group_index in range(N_TP):
        col_low = group_index * group_width
        col_high = col_low + group_width
        store_part = jnp.dot(key_sums[:, col_low:col_high], w_key[:, col_low:col_high].T, preferred_element_type=jnp.float32)
        store_part = store_part + jnp.dot(value_sums[:, col_low:col_high], w_value[:, col_low:col_high].T, preferred_element_type=jnp.float32)
        store_total = store_total + rounded_copy(store_part)
        token_part = jnp.dot(query_low[:, col_low:col_high], w_query[:, col_low:col_high].T, preferred_element_type=jnp.float32)
        token_part = token_part + jnp.dot(gate_low[:, col_low:col_high], w_gate[:, col_low:col_high].T, preferred_element_type=jnp.float32)
        token_total = token_total + rounded_copy(token_part)
    d_store = store_total.astype(jnp.bfloat16).reshape(NPASS, PL, D)
    d_tokens = token_total.astype(jnp.bfloat16)
    return (d_tokens, d_store, d_wkey)
```

```python
import functools

import jax
import jax.numpy as jnp
from jax import lax
from jax.experimental import pallas as pl
from jax.experimental.pallas import tpu as pltpu
from jax.sharding import PartitionSpec as P

HD = 256
BLK = 128
PB = 4
BF = jnp.bfloat16
F32 = jnp.float32
MESH = pl.DeviceIdType.MESH
NT = (((1,), (1,)), ((), ()))
TN = (((0,), (0,)), ((), ()))


def dot(a, b, dims=(((1,), (0,)), ((), ()))):
    return lax.dot_general(a, b, dims, preferred_element_type=F32)


def remote(src, dst, send, recv, device):
    return pltpu.make_async_remote_copy(
        src_ref=src,
        dst_ref=dst,
        send_sem=send,
        recv_sem=recv,
        device_id=device,
        device_id_type=MESH,
    )


def tile_of(size, most):
    while size % most:
        most //= 2
    return most


def kernel(
    st_n, tp_n, depth, pass_len,
    slot_ref, req_ref, ask_ref, store_ref, q_hbm, g_hbm, wq_hbm, wg_hbm, wk_hbm, wv_hbm, m_hbm,
    tok_out, store_out, wkey_out,
    rows, wkv, wqg, q_v, g_v, m_v, acc, kv, ask_in, ask_s, out, inc_k, inc_v, ret, prob_v, kvb, reqg, gboth, arr,
    hot, plow, dwp, dwr, tp_part, tp_pair, tp_recv, sp_part, sp_pair, sp_recv,
    lsem, gs, gr, zs, zr, ps, pr, xs, xr,
):
    st = lax.axis_index("st")
    tp = lax.axis_index("tp")
    hi_n = tp_n // 2
    hi, lo = tp // 2, tp % 2
    mate = {"tp": hi * 2 + 1 - lo}
    pass_rows, chunk = rows.shape[1], rows.shape[2]
    model = wqg.shape[0]
    cols = q_v.shape[1]
    heads = cols // HD
    tok_rows = q_v.shape[0]
    blocks = tok_rows // BLK
    blk_keys = PB * pass_len

    def local(i, src, dst):
        copy = pltpu.make_async_copy(src, dst, lsem.at[i])
        copy.start()
        return copy

    own_rows = local(0, store_ref, rows.at[tp])
    loads_kv = [
        local(1, wk_hbm, wkv.at[:, pl.ds(0, cols)]),
        local(2, wv_hbm, wkv.at[:, pl.ds(cols, cols)]),
    ]
    loads_q = [local(3, q_hbm, q_v), local(4, g_hbm, g_v), local(5, m_hbm, m_v)]
    loads_qg = [
        local(6, wq_hbm, wqg.at[:, pl.ds(0, cols)]),
        local(7, wg_hbm, wqg.at[:, pl.ds(cols, cols)]),
    ]

    barrier = pltpu.get_barrier_semaphore()

    def greet_st(d, c):
        pl.semaphore_signal(
            barrier, inc=1, device_id={"st": (st + d) % st_n}, device_id_type=MESH
        )
        return c

    lax.fori_loop(1, st_n, greet_st, 0)
    for d in range(1, tp_n):
        pl.semaphore_signal(
            barrier, inc=1, device_id={"tp": (tp + d) % tp_n}, device_id_type=MESH
        )
    pl.semaphore_wait(barrier, st_n - 1 + tp_n - 1)

    across = []
    for d in range(1, hi_n):
        h = (hi + d) % hi_n
        across.append(
            remote(store_ref, rows.at[tp], gs.at[0, h], gr.at[tp], {"tp": h * 2 + lo})
        )
        across[-1].start()
    beside = remote(store_ref, rows.at[tp], gs.at[1, hi], gr.at[tp], mate)
    beside.start()

    upper = st >= st_n // 2
    mark = jnp.where(upper, st, st_n - 1 - st)

    def far_peer(d):
        i = d - 1
        i = i + jnp.where(i >= mark, 1, 0)
        return jnp.where(upper, i, st_n - 1 - i)

    def z_copy(phase, src, dst, peer):
        return remote(src, dst, zs.at[phase, peer], zr.at[phase, st], {"st": peer})

    def z_wait(phase, src, dst, peer):
        remote(src, dst, zs.at[phase, peer], zr.at[phase, peer], {"st": peer}).wait_recv()

    def ask_send(d, c):
        peer = (st + d) % st_n
        z_copy(0, ask_ref.at[peer], ask_in.at[st], peer).start()
        return c

    lax.fori_loop(1, st_n, ask_send, 0)
    ask_in[st] = ask_ref[st]

    m_tile = tile_of(pass_rows, 256)

    def project(t, first):
        def step(i, c):
            r = pl.ds(pl.multiple_of(i * m_tile, m_tile), m_tile)
            part = dot(rows[t, r], wkv[pl.ds(pl.multiple_of(t * chunk, chunk), chunk), :])
            acc[r] = part if first else acc[r] + part
            return c

        lax.fori_loop(0, pass_rows // m_tile, step, 0)

    def g_wait(t):
        remote(store_ref, rows.at[t], gs.at[1, hi], gr.at[t], mate).wait_recv()

    own_rows.wait()
    for copy in loads_kv:
        copy.wait()
    project(tp, True)
    g_wait(hi * 2 + 1 - lo)
    project(hi * 2 + 1 - lo, False)

    def ask_wait(d, c):
        peer = (st + d) % st_n
        z_wait(0, ask_ref.at[peer], ask_in.at[peer], peer)
        return c

    lax.fori_loop(1, st_n, ask_wait, 0)
    ask_copy = local(8, ask_in, ask_s)
    ask_copy.wait()

    hot_cols = depth * pass_len

    def hot_step(o, c):
        target = ask_in[o][0:1, :hot_cols]
        for i in range(pass_rows // m_tile):
            line = lax.broadcasted_iota(jnp.int32, (m_tile, hot_cols), 0) + i * m_tile
            hot[o, i * m_tile : (i + 1) * m_tile, :] = jnp.where(line == target, 1.0, 0.0).astype(BF)
        return c

    lax.fori_loop(0, st_n, hot_step, 0)
    onward = []
    for d in range(1, hi_n):
        h = (hi + d) % hi_n
        t = h * 2 + lo
        g_wait(t)
        onward.append(remote(rows.at[t], rows.at[t], gs.at[2, h], gr.at[t], mate))
        onward[-1].start()
        project(t, False)
    for d in range(1, hi_n):
        t = ((hi + d) % hi_n) * 2 + 1 - lo
        g_wait(t)
        project(t, False)

    def low_step(i, c):
        kv[i] = acc[pl.ds(pl.multiple_of(i * pass_len, pass_len), pass_len), :].astype(BF)
        return c

    lax.fori_loop(0, pass_rows // pass_len, low_step, 0)

    ks, vs_all = pl.ds(0, cols), pl.ds(cols, cols)

    def half(ref, peer, part):
        return ref.at[peer, :, :, part]

    def key_copy(peer):
        return z_copy(1, half(out, peer, ks), inc_k.at[st], peer)

    def value_copy(peer):
        return z_copy(4, half(out, peer, vs_all), inc_v.at[st], peer)

    def kv_send(d, c):
        peer = far_peer(d)
        for k in range(depth):
            out[peer, k] = kv[ask_s[peer, 1, k]]
        key_copy(peer).start()
        return c

    def value_send(d, c):
        value_copy(far_peer(d)).start()
        return c

    lax.fori_loop(1, st_n, kv_send, 0)
    lax.fori_loop(1, st_n, value_send, 0)
    for k in range(depth):
        picked = kv[ask_s[st, 1, k]]
        inc_k[st, k] = picked[:, :cols]
        inc_v[st, k] = picked[:, cols:]
    for copy in loads_q + loads_qg:
        copy.wait()

    def key_wait(d, c):
        peer = (st + d) % st_n
        z_wait(1, half(out, peer, ks), inc_k.at[peer], peer)
        return c

    lax.fori_loop(1, st_n, key_wait, 0)
    scale = HD ** (-0.5)

    def probs_step(b, c):
        r = pl.ds(pl.multiple_of(b * BLK, BLK), BLK)
        for j in range(PB):
            kvb[j * pass_len : (j + 1) * pass_len, :cols] = inc_k[
                slot_ref[0, b * PB + j], slot_ref[1, b * PB + j]
            ]
        for head in range(heads):
            hs = slice(head * HD, (head + 1) * HD)
            vs = slice(cols + head * HD, cols + (head + 1) * HD)
            gate = g_v[r, hs].astype(F32)
            scores = dot(q_v[r, hs], kvb[:, hs], NT) * scale
            shifted = jnp.exp(scores - jnp.max(scores, axis=-1, keepdims=True))
            prob = shifted / jnp.sum(shifted, axis=-1, keepdims=True)
            prob_v[head, r, :] = prob
            sig = 1.0 / (1.0 + jnp.exp(-gate))
            att_grad = (gate * sig * m_v[r, hs].astype(F32)).astype(BF)
            value_grad = dot(prob.astype(BF), att_grad, TN).astype(BF)
            for j in range(PB):
                reqg[b * PB + j, :, vs] = value_grad[j * pass_len : (j + 1) * pass_len]
        return c

    lax.fori_loop(0, blocks, probs_step, 0)

    def back_copy(phase, part, peer):
        return z_copy(phase, half(ret, peer, part), half(arr, st, part), peer)

    def give_back(phase, part, span):
        def send(d, c):
            peer = far_peer(d)
            for k in range(depth):
                ret[peer, k, :, span] = reqg[req_ref[peer, k]][:, span]
            back_copy(phase, part, peer).start()
            return c

        lax.fori_loop(1, st_n, send, 0)
        for k in range(depth):
            arr[st, k, :, span] = reqg[req_ref[st, k]][:, span]

    give_back(2, vs_all, slice(cols, 2 * cols))

    def value_wait(d, c):
        peer = (st + d) % st_n
        z_wait(4, half(out, peer, vs_all), inc_v.at[peer], peer)
        return c

    lax.fori_loop(1, st_n, value_wait, 0)

    def block_step(b, c):
        r = pl.ds(pl.multiple_of(b * BLK, BLK), BLK)
        for j in range(PB):
            o, k = slot_ref[0, b * PB + j], slot_ref[1, b * PB + j]
            kvb[j * pass_len : (j + 1) * pass_len, :cols] = inc_k[o, k]
            kvb[j * pass_len : (j + 1) * pass_len, cols:] = inc_v[o, k]
        for head in range(heads):
            hs = slice(head * HD, (head + 1) * HD)
            vs = slice(cols + head * HD, cols + (head + 1) * HD)
            q = q_v[r, hs]
            key = kvb[:, hs]
            value = kvb[:, vs]
            gate = g_v[r, hs].astype(F32)
            grad = m_v[r, hs].astype(F32)
            prob = prob_v[head, r, :]
            attended = dot(prob.astype(BF), value)
            sig = 1.0 / (1.0 + jnp.exp(-gate))
            att_grad = (gate * sig * grad).astype(BF)
            gboth[r, vs] = (grad * attended * sig * (1.0 + gate * (1.0 - sig))).astype(BF)
            prob_grad = dot(att_grad, value, NT)
            inner = jnp.sum(prob * prob_grad, axis=-1, keepdims=True)
            score_grad = (scale * prob * (prob_grad - inner)).astype(BF)
            gboth[r, hs] = dot(score_grad, key).astype(BF)
            key_grad = dot(score_grad, q, TN).astype(BF)
            for j in range(PB):
                reqg[b * PB + j, :, hs] = key_grad[j * pass_len : (j + 1) * pass_len]
        return c

    lax.fori_loop(0, blocks, block_step, 0)
    give_back(5, ks, slice(0, cols))

    n_tile = tile_of(model, 512)

    def expand(src, weight, part, pair_rows, t):
        base = pl.multiple_of(t * pair_rows, pair_rows)
        a = src[pl.ds(base, pair_rows), :]

        def step(i, c):
            n = pl.ds(pl.multiple_of(i * n_tile, n_tile), n_tile)
            part[t, :, n] = dot(a, weight[n, :], NT).astype(BF)
            return c

        lax.fori_loop(0, model // n_tile, step, 0)

    def pair_copy(which, part, pair, h):
        return remote(part.at[h * 2 + 1 - lo], pair.at[h], ps.at[which, h], pr.at[which, h], mate)

    def scatter_first(which, src, weight, part, pair, pair_rows):
        for d in range(1, hi_n + 1):
            h = (hi + d) % hi_n
            expand(src, weight, part, pair_rows, h * 2 + 1 - lo)
            pair_copy(which, part, pair, h).start()

    def cross(which, send, recv, h):
        return remote(
            send.at[h * 2 + lo], recv.at[hi], xs.at[which, h], xr.at[which, hi], {"tp": h * 2 + lo}
        )

    def scatter_second(which, src, weight, part, pair, send, recv, pair_rows):
        for d in range(1, hi_n + 1):
            h = (hi + d) % hi_n
            expand(src, weight, part, pair_rows, h * 2 + lo)
            pair_copy(which, part, pair, h).wait_recv()
            if d < hi_n:
                part[h * 2 + lo] = (part[h * 2 + lo].astype(F32) + pair[h].astype(F32)).astype(BF)
                cross(which, part, recv, h).start()

    def scatter_last(which, part, pair, send, recv, result):
        for d in range(1, hi_n):
            h = (hi + d) % hi_n
            remote(
                send.at[h * 2 + lo], recv.at[h], xs.at[which, h], xr.at[which, h], {"tp": h * 2 + lo}
            ).wait_recv()
        total = part[tp].astype(F32) + pair[hi].astype(F32)
        for d in range(1, hi_n):
            total = total + recv[(hi + d) % hi_n].astype(F32)
        result[...] = total.astype(BF)

    tok_pair = tok_rows // tp_n
    sto_pair = pass_rows // tp_n
    scatter_first(0, gboth, wqg, tp_part, tp_pair, tok_pair)
    scatter_second(0, gboth, wqg, tp_part, tp_pair, tp_part, tp_recv, tok_pair)

    def gather_sums(o, span, first):
        def step(i, c):
            r = pl.ds(pl.multiple_of(i * m_tile, m_tile), m_tile)
            part = dot(hot[o, r, :], arr[o, :, :, span].reshape(hot_cols, cols))
            acc[r, span] = part if first else acc[r, span] + part
            return c

        lax.fori_loop(0, pass_rows // m_tile, step, 0)

    for phase, part, span in ((2, vs_all, slice(cols, 2 * cols)), (5, ks, slice(0, cols))):
        gather_sums(st, span, True)

        def grad_wait(d, c):
            peer = (st + d) % st_n
            z_wait(phase, half(ret, peer, part), half(arr, peer, part), peer)
            gather_sums(peer, span, False)
            return c

        lax.fori_loop(1, st_n, grad_wait, 0)
        plow[:, span] = acc[:, span].astype(BF)

    scatter_first(1, plow, wkv, sp_part, sp_pair, sto_pair)

    def wkey_step(t, c):
        dwp[pl.ds(pl.multiple_of(t * chunk, chunk), chunk), :] = dot(
            rows[t], plow[:, :cols], TN
        ).astype(BF)
        return c

    lax.fori_loop(0, tp_n, wkey_step, 0)
    share = model // st_n

    def part_of(s):
        return dwp.at[pl.ds(pl.multiple_of(s * share, share), share), :]

    def wkey_send(d, c):
        peer = far_peer(d)
        z_copy(3, part_of(peer), dwr.at[st], peer).start()
        return c

    lax.fori_loop(1, st_n, wkey_send, 0)
    scatter_second(1, plow, wkv, sp_part, sp_pair, sp_part, sp_recv, sto_pair)
    scatter_last(0, tp_part, tp_pair, tp_part, tp_recv, tok_out)
    wkey_out[...] = part_of(st)[...].astype(F32)

    def wkey_wait(d, c):
        peer = (st + d) % st_n
        z_wait(3, part_of(peer), dwr.at[peer], peer)
        wkey_out[...] += dwr[peer].astype(F32)
        return c

    lax.fori_loop(1, st_n, wkey_wait, 0)
    scatter_last(1, sp_part, sp_pair, sp_part, sp_recv, store_out)

    for copy in across + [beside] + onward:
        copy.wait_send()

    def drain(d, c):
        peer = (st + d) % st_n
        z_copy(0, ask_ref.at[peer], ask_in.at[st], peer).wait_send()
        key_copy(peer).wait_send()
        value_copy(peer).wait_send()
        back_copy(2, vs_all, peer).wait_send()
        back_copy(5, ks, peer).wait_send()
        z_copy(3, part_of(peer), dwr.at[st], peer).wait_send()
        return c

    lax.fori_loop(1, st_n, drain, 0)
    for d in range(1, hi_n + 1):
        h = (hi + d) % hi_n
        pair_copy(0, tp_part, tp_pair, h).wait_send()
        pair_copy(1, sp_part, sp_pair, h).wait_send()
        if d < hi_n:
            cross(0, tp_part, tp_recv, h).wait_send()
            cross(1, sp_part, sp_recv, h).wait_send()


def gathered_kernel(
    st_n, tp_n, depth, pass_len,
    ids_ref, req_ref, ask_ref, store_ref, q_hbm, g_hbm, wq_hbm, wg_hbm, wk_hbm, wv_hbm, m_hbm,
    tok_out, store_out, wkey_out,
    rows, wall, wqg, q_v, g_v, m_v, acc, vterm, k_all, v_all, ask_in, ret, prob_v, kvb, reqg, gboth, arr,
    hot, plow, sums, dwp, dwu, dwd, tp_part, tp_pair, tp_recv,
    lsem, gs, gr, fs, fr, zs, zr, ps, pr, xs, xr, ws, wr, ss, sr, us, ur,
):
    grp = lax.axis_index("grp")
    st = lax.axis_index("st")
    tp = lax.axis_index("tp")
    hi_n = tp_n // 2
    hi, lo = tp // 2, tp % 2
    mate_t = hi * 2 + 1 - lo
    mate = {"tp": mate_t}
    twin = {"grp": 1 - grp}
    pass_rows, chunk = rows.shape[1], rows.shape[2]
    passages = pass_rows // pass_len
    model = wqg.shape[0]
    cols = q_v.shape[1]
    heads = cols // HD
    tok_rows = q_v.shape[0]
    blocks = tok_rows // BLK
    half_pass = passages // 2
    some = tile_of(half_pass, 2)
    some_rows = some * pass_len
    n_some = half_pass // some
    key_cols, value_cols = slice(0, cols), slice(cols, 2 * cols)

    def local(i, src, dst):
        copy = pltpu.make_async_copy(src, dst, lsem.at[i])
        copy.start()
        return copy

    loads_kv = [
        local(0, store_ref, rows.at[tp]),
        local(1, wk_hbm, wall.at[tp, :, pl.ds(0, cols)]),
        local(2, wv_hbm, wall.at[tp, :, pl.ds(cols, cols)]),
    ]
    loads_q = [
        local(3, q_hbm, q_v),
        local(4, g_hbm, g_v),
        local(5, m_hbm, m_v),
        local(6, wq_hbm, wqg.at[:, pl.ds(0, cols)]),
        local(7, wg_hbm, wqg.at[:, pl.ds(cols, cols)]),
    ]

    barrier = pltpu.get_barrier_semaphore()

    def greet_st(d, c):
        pl.semaphore_signal(
            barrier, inc=1, device_id={"st": (st + d) % st_n}, device_id_type=MESH
        )
        return c

    lax.fori_loop(1, st_n, greet_st, 0)
    for d in range(1, tp_n):
        pl.semaphore_signal(
            barrier, inc=1, device_id={"tp": (tp + d) % tp_n}, device_id_type=MESH
        )
    pl.semaphore_signal(barrier, inc=1, device_id=twin, device_id_type=MESH)
    pl.semaphore_wait(barrier, st_n + tp_n - 1)

    def first_row(i):
        part = (grp + i // n_some) % 2
        return pl.multiple_of((part * n_some + i % n_some) * some_rows, some_rows)

    def g_copy(way, i, t, source, peer, slot):
        r = pl.ds(first_row(i), some_rows)
        src = store_ref.at[r] if source is None else rows.at[source, r]
        return remote(src, rows.at[t, r], gs.at[way, slot, i], gr.at[t, i], peer)

    def across(d, i):
        h = (hi + d) % hi_n
        return g_copy(0, i, tp, None, {"tp": h * 2 + lo}, h)

    def beside(i):
        return g_copy(1, i, tp, None, mate, hi)

    def onward(d, i):
        h = (hi + d) % hi_n
        return g_copy(2, i, h * 2 + lo, h * 2 + lo, mate, h)

    def g_wait(t, i):
        g_copy(1, i, t, None, mate, hi).wait_recv()

    def rows_send(i, c):
        for d in range(1, hi_n):
            across(d, i).start()
        beside(i).start()
        return c

    lax.fori_loop(0, 2 * n_some, rows_send, 0)

    upper = st >= st_n // 2
    mark = jnp.where(upper, st, st_n - 1 - st)

    def far_peer(d):
        i = d - 1
        i = i + jnp.where(i >= mark, 1, 0)
        return jnp.where(upper, i, st_n - 1 - i)

    def z_copy(phase, src, dst, peer):
        return remote(src, dst, zs.at[phase, peer], zr.at[phase, st], {"st": peer})

    def z_wait(phase, src, dst, peer):
        remote(src, dst, zs.at[phase, peer], zr.at[phase, peer], {"st": peer}).wait_recv()

    def ask_send(d, c):
        peer = (st + d) % st_n
        z_copy(0, ask_ref.at[peer], ask_in.at[st], peer).start()
        return c

    lax.fori_loop(1, st_n, ask_send, 0)
    ask_in[st] = ask_ref[st]

    def project(i):
        r = pl.ds(first_row(i), some_rows)

        def term(t):
            w = wall[tp, pl.ds(pl.multiple_of(t * chunk, chunk), chunk), :]
            return dot(rows[t, r], w)

        for d in range(1, hi_n):
            g_wait(((hi + d) % hi_n) * 2 + lo, i)
            onward(d, i).start()
        g_wait(mate_t, i)
        total = term(tp) + term(mate_t)
        for d in range(1, hi_n):
            total = total + term(((hi + d) % hi_n) * 2 + lo)
        for d in range(1, hi_n):
            t = ((hi + d) % hi_n) * 2 + 1 - lo
            g_wait(t, i)
            total = total + term(t)
        low = total.astype(BF)
        first = st * passages + first_row(i) // pass_len
        for p in range(some):
            k_all[first + p] = low[p * pass_len : (p + 1) * pass_len, key_cols]
            v_all[first + p] = low[p * pass_len : (p + 1) * pass_len, value_cols]

    def part_of_all(kind, o, c, side):
        ref = k_all if kind == 0 else v_all
        return ref.at[pl.ds(o * passages + side * half_pass + c * some, some)]

    def chain_copy(kind, o, c, way, peer):
        part = part_of_all(kind, o, c, grp)
        return remote(part, part, fs.at[kind, o, c, way], fr.at[kind, o, c, 0], {"st": peer})

    def twin_copy(kind, o, c):
        part = part_of_all(kind, o, c, grp)
        return remote(part, part, fs.at[kind, o, c, 2], fr.at[kind, o, c, 1], twin)

    def own_copies(kind, c, act):
        @pl.when(st + 1 < st_n)
        def _():
            act(chain_copy(kind, st, c, 0, st + 1))

        @pl.when(st > 0)
        def _():
            act(chain_copy(kind, st, c, 1, st - 1))

    def relay_copies(kind, d, c, act, ready):
        for way, sign in ((0, -1), (1, 1)):
            o = st + sign * d
            onto = st - sign

            @pl.when((o >= 0) & (o < st_n))
            def _():
                if ready:
                    chain_copy(kind, o, c, way, st).wait_recv()

                @pl.when((onto >= 0) & (onto < st_n))
                def _():
                    act(chain_copy(kind, o, c, way, onto))

                act(twin_copy(kind, o, c))

    def start(copy):
        copy.start()

    def own_send(kind, c):
        own_copies(kind, c, start)

    def relay(kind, d, c):
        relay_copies(kind, d, c, start, True)

    def twin_wait(kind):
        def step(i, c):
            o = (st + 1 + i // n_some) % st_n
            k = i % n_some
            part = part_of_all(kind, o, k, 1 - grp)
            remote(part, part, fs.at[kind, o, k, 2], fr.at[kind, o, k, 1], twin).wait_recv()
            return c

        lax.fori_loop(0, (st_n - 1) * n_some, step, 0)

    for copy in loads_kv:
        copy.wait()

    def early_step(i, c):
        project(i)
        own_send(0, i)

        @pl.when(i > 0)
        def _():
            relay(0, 1, i - 1)

        return c

    lax.fori_loop(0, n_some, early_step, 0)
    relay(0, 1, n_some - 1)

    def value_send(i, c):
        own_send(1, i)
        return c

    lax.fori_loop(0, n_some, value_send, 0)

    def late_step(i, c):
        project(n_some + i)
        relay(0, 2, i)
        return c

    lax.fori_loop(0, n_some, late_step, 0)

    w_half = model // 2
    w_mine = pl.ds(pl.multiple_of(grp * w_half, w_half), w_half)
    w_other = pl.ds(pl.multiple_of((1 - grp) * w_half, w_half), w_half)

    def w_across(d):
        h = (hi + d) % hi_n
        part = wall.at[tp, w_mine]
        return remote(part, part, ws.at[0, h], wr.at[0, tp], {"tp": h * 2 + lo})

    def w_twin(d):
        t = ((hi + d) % hi_n) * 2 + lo
        part = wall.at[t, w_mine]
        return remote(part, part, ws.at[1, (hi + d) % hi_n], wr.at[1, t], twin)

    def w_onward(d, k):
        t = ((hi + d) % hi_n) * 2 + lo
        part = wall.at[t, w_other if k else w_mine]
        return remote(part, part, ws.at[2 + k, (hi + d) % hi_n], wr.at[2 + k, t], mate)

    w_beside = remote(wall.at[tp], wall.at[tp], ws.at[4, 0], wr.at[4, tp], mate)

    def w_wait(kind, t, part):
        remote(wall.at[t, part], wall.at[t, part], ws.at[kind, 0], wr.at[kind, t], mate).wait_recv()

    for d in range(1, hi_n):
        w_across(d).start()
    w_beside.start()

    def relay_rest(kind, first, last):
        def step(i, c):
            relay(kind, 1 + i // n_some, i % n_some)
            return c

        lax.fori_loop(first, last, step, 0)

    relays = (st_n - 1) * n_some
    relay_rest(0, 2 * n_some, relays)
    for copy in loads_q:
        copy.wait()
    twin_wait(0)
    scale = HD ** (-0.5)

    def fill(ref, span, b):
        for j in range(PB):
            kvb[j * pass_len : (j + 1) * pass_len, span] = ref[ids_ref[b * PB + j]]

    def probs_step(b, c):
        r = pl.ds(pl.multiple_of(b * BLK, BLK), BLK)
        fill(k_all, key_cols, b)
        for head in range(heads):
            hs = slice(head * HD, (head + 1) * HD)
            vs = slice(cols + head * HD, cols + (head + 1) * HD)
            gate = g_v[r, hs].astype(F32)
            scores = dot(q_v[r, hs], kvb[:, hs], NT) * scale
            shifted = jnp.exp(scores - jnp.max(scores, axis=-1, keepdims=True))
            prob = shifted / jnp.sum(shifted, axis=-1, keepdims=True)
            prob_v[head, r, :] = prob
            sig = 1.0 / (1.0 + jnp.exp(-gate))
            att_grad = (gate * sig * m_v[r, hs].astype(F32)).astype(BF)
            value_grad = dot(prob.astype(BF), att_grad, TN).astype(BF)
            for j in range(PB):
                reqg[b * PB + j, :, vs] = value_grad[j * pass_len : (j + 1) * pass_len]

        @pl.when(b < relays)
        def _():
            relay(1, 1 + b // n_some, b % n_some)

        return c

    lax.fori_loop(0, blocks, probs_step, 0)

    def half(ref, peer, part):
        return ref.at[peer, :, :, part]

    def back_copy(phase, part, peer):
        return z_copy(phase, half(ret, peer, part), half(arr, st, part), peer)

    def give_back(phase, part, span):
        def send(d, c):
            peer = far_peer(d)
            for k in range(depth):
                ret[peer, k, :, span] = reqg[req_ref[peer, k]][:, span]
            back_copy(phase, part, peer).start()
            return c

        lax.fori_loop(1, st_n, send, 0)
        for k in range(depth):
            arr[st, k, :, span] = reqg[req_ref[st, k]][:, span]

    ks, vs_all = pl.ds(0, cols), pl.ds(cols, cols)
    give_back(1, vs_all, value_cols)
    relay_rest(1, min(blocks, relays), relays)
    twin_wait(1)

    def block_step(b, c):
        r = pl.ds(pl.multiple_of(b * BLK, BLK), BLK)
        fill(k_all, key_cols, b)
        fill(v_all, value_cols, b)
        for head in range(heads):
            hs = slice(head * HD, (head + 1) * HD)
            vs = slice(cols + head * HD, cols + (head + 1) * HD)
            q = q_v[r, hs]
            key = kvb[:, hs]
            value = kvb[:, vs]
            gate = g_v[r, hs].astype(F32)
            grad = m_v[r, hs].astype(F32)
            prob = prob_v[head, r, :]
            attended = dot(prob.astype(BF), value)
            sig = 1.0 / (1.0 + jnp.exp(-gate))
            att_grad = (gate * sig * grad).astype(BF)
            gboth[r, vs] = (grad * attended * sig * (1.0 + gate * (1.0 - sig))).astype(BF)
            prob_grad = dot(att_grad, value, NT)
            inner = jnp.sum(prob * prob_grad, axis=-1, keepdims=True)
            score_grad = (scale * prob * (prob_grad - inner)).astype(BF)
            gboth[r, hs] = dot(score_grad, key).astype(BF)
            key_grad = dot(score_grad, q, TN).astype(BF)
            for j in range(PB):
                reqg[b * PB + j, :, hs] = key_grad[j * pass_len : (j + 1) * pass_len]
        return c

    lax.fori_loop(0, blocks, block_step, 0)
    give_back(2, ks, key_cols)

    for d in range(1, hi_n):
        w_wait(0, ((hi + d) % hi_n) * 2 + lo, w_mine)
        w_twin(d).start()
        w_onward(d, 0).start()

    n_tile = tile_of(model, 512)

    def expand(t):
        a = gboth[pl.ds(pl.multiple_of(t * tok_pair, tok_pair), tok_pair), :]

        def step(i, c):
            n = pl.ds(pl.multiple_of(i * n_tile, n_tile), n_tile)
            tp_part[t, :, n] = dot(a, wqg[n, :], NT).astype(BF)
            return c

        lax.fori_loop(0, model // n_tile, step, 0)

    def pair_copy(h):
        return remote(tp_part.at[h * 2 + 1 - lo], tp_pair.at[h], ps.at[h], pr.at[h], mate)

    def cross(h):
        return remote(
            tp_part.at[h * 2 + lo], tp_recv.at[hi], xs.at[h], xr.at[hi], {"tp": h * 2 + lo}
        )

    tok_pair = tok_rows // tp_n
    for d in range(1, hi_n + 1):
        h = (hi + d) % hi_n
        expand(h * 2 + 1 - lo)
        pair_copy(h).start()
    for d in range(1, hi_n + 1):
        h = (hi + d) % hi_n
        expand(h * 2 + lo)
        pair_copy(h).wait_recv()
        if d < hi_n:
            tp_part[h * 2 + lo] = (tp_part[h * 2 + lo].astype(F32) + tp_pair[h].astype(F32)).astype(BF)
            cross(h).start()

    def ask_wait(d, c):
        peer = (st + d) % st_n
        z_wait(0, ask_ref.at[peer], ask_in.at[peer], peer)
        return c

    lax.fori_loop(1, st_n, ask_wait, 0)
    hot_cols = depth * pass_len
    m_tile = tile_of(pass_rows, 256)

    def hot_step(o, c):
        target = ask_in[o][0:1, :hot_cols]
        for i in range(pass_rows // m_tile):
            line = lax.broadcasted_iota(jnp.int32, (m_tile, hot_cols), 0) + i * m_tile
            hot[o, i * m_tile : (i + 1) * m_tile, :] = jnp.where(line == target, 1.0, 0.0).astype(BF)
        return c

    lax.fori_loop(0, st_n, hot_step, 0)

    def gather_sums(o, span, first):
        def step(i, c):
            r = pl.ds(pl.multiple_of(i * m_tile, m_tile), m_tile)
            part = dot(hot[o, r, :], arr[o, :, :, span].reshape(hot_cols, cols))
            acc[r, :] = part if first else acc[r, :] + part
            return c

        lax.fori_loop(0, pass_rows // m_tile, step, 0)

    sto_pair = pass_rows // tp_n

    def sums_copy(kind, part, d):
        t = (tp + d) % tp_n
        src = plow.at[pl.ds(pl.multiple_of(t * sto_pair, sto_pair), sto_pair), part]
        return remote(src, sums.at[tp, :, part], ss.at[kind, t], sr.at[kind, tp], {"tp": t})

    def sums_wait(kind, part, t):
        dst = sums.at[t, :, part]
        remote(dst, dst, ss.at[kind, t], sr.at[kind, t], mate).wait_recv()

    def collect(phase, kind, part, span):
        gather_sums(st, span, True)

        def grad_wait(d, c):
            peer = (st + d) % st_n
            z_wait(phase, half(ret, peer, part), half(arr, peer, part), peer)
            gather_sums(peer, span, False)
            return c

        lax.fori_loop(1, st_n, grad_wait, 0)
        plow[:, span] = acc[...].astype(BF)
        for d in range(1, tp_n):
            sums_copy(kind, part, d).start()
        sums[tp, :, span] = plow[pl.ds(pl.multiple_of(tp * sto_pair, sto_pair), sto_pair), span]

    collect(1, 1, vs_all, value_cols)

    for d in range(1, hi_n):
        w_wait(1, ((hi + d) % hi_n) * 2 + lo, w_other)
        w_onward(d, 1).start()
    w_wait(4, mate_t, pl.ds(0, model))
    for d in range(1, hi_n):
        t = ((hi + d) % hi_n) * 2 + 1 - lo
        w_wait(2, t, w_mine)
        w_wait(3, t, w_other)

    for d in range(1, hi_n):
        h = (hi + d) % hi_n
        remote(
            tp_part.at[h * 2 + lo], tp_recv.at[h], xs.at[h], xr.at[h], {"tp": h * 2 + lo}
        ).wait_recv()
    total = tp_part[tp].astype(F32) + tp_pair[hi].astype(F32)
    for d in range(1, hi_n):
        total = total + tp_recv[(hi + d) % hi_n].astype(F32)
    tok_out[...] = total.astype(BF)

    def store_terms(span, done):
        def step(i, c):
            n = pl.ds(pl.multiple_of(i * n_tile, n_tile), n_tile)
            part = dot(sums[0, :, span], wall[0, n, span], NT)
            for t in range(1, tp_n):
                part = part + dot(sums[t, :, span], wall[t, n, span], NT)
            done(n, part)
            return c

        lax.fori_loop(0, model // n_tile, step, 0)

    def keep_values(n, part):
        vterm[:, n] = part

    def keep_store(n, part):
        store_out[:, n] = (vterm[:, n] + part).astype(BF)

    for d in range(1, tp_n):
        sums_wait(1, vs_all, (tp + d) % tp_n)
    store_terms(value_cols, keep_values)

    collect(2, 0, ks, key_cols)

    def wkey_step(t, c):
        dwp[pl.ds(pl.multiple_of(t * chunk, chunk), chunk), :] = dot(
            rows[t], plow[:, key_cols], TN
        ).astype(BF)
        return c

    lax.fori_loop(0, tp_n, wkey_step, 0)
    share = model // st_n
    bits = 2
    bit = share // bits

    def dw_copy(way, s, b, whole):
        ref = dwu if way == 0 else dwd
        line = pl.ds(b * bit, bit)
        src = dwp.at[pl.ds(pl.multiple_of(s * share + b * bit, bit), bit), :] if whole else ref.at[s, line]
        peer = st + 1 if way == 0 else st - 1
        return remote(src, ref.at[s, line], us.at[way, s, b], ur.at[way, s, b], {"st": peer})

    def dw_wait(way, s, b):
        dw_copy(way, s, b, False).wait_recv()

    def dw_own(s, b):
        return dwp[pl.ds(pl.multiple_of(s * share + b * bit, bit), bit), :].astype(F32)

    def dw_each(edge, act):
        for j in range(st_n - 1):
            for b in range(bits):
                for way, s in ((0, st_n - 1 - j), (1, j)):
                    at_edge = st == (0 if way == 0 else st_n - 1)
                    goes = (s > st) if way == 0 else (s < st)

                    @pl.when(goes & (at_edge if edge else jnp.logical_not(at_edge)))
                    def _():
                        act(way, s, b)

    def dw_first(way, s, b):
        dw_copy(way, s, b, True).start()

    def dw_relay(way, s, b):
        dw_wait(way, s, b)
        ref = dwu if way == 0 else dwd
        line = slice(b * bit, (b + 1) * bit)
        ref[s, line, :] = (ref[s, line, :].astype(F32) + dw_own(s, b)).astype(BF)
        dw_copy(way, s, b, False).start()

    dw_each(True, dw_first)

    for d in range(1, tp_n):
        sums_wait(0, ks, (tp + d) % tp_n)
    store_terms(key_cols, keep_store)

    dw_each(False, dw_relay)
    for b in range(bits):
        line = slice(b * bit, (b + 1) * bit)
        wkey_out[line, :] = dw_own(st, b)
        for way, there in ((0, st > 0), (1, st + 1 < st_n)):
            @pl.when(there)
            def _():
                dw_wait(way, st, b)
                ref = dwu if way == 0 else dwd
                wkey_out[line, :] += ref[st, line, :].astype(F32)

    def wait_send(copy):
        copy.wait_send()

    def rows_drain(i, c):
        for d in range(1, hi_n):
            across(d, i).wait_send()
            onward(d, i).wait_send()
        beside(i).wait_send()
        return c

    lax.fori_loop(0, 2 * n_some, rows_drain, 0)

    def all_drain(i, c):
        for kind in (0, 1):
            own_copies(kind, i, wait_send)
            for d in range(1, st_n):
                relay_copies(kind, d, i, wait_send, False)
        return c

    lax.fori_loop(0, n_some, all_drain, 0)
    for d in range(1, hi_n):
        w_across(d).wait_send()
        w_twin(d).wait_send()
        w_onward(d, 0).wait_send()
        w_onward(d, 1).wait_send()
    w_beside.wait_send()

    def drain(d, c):
        peer = (st + d) % st_n
        z_copy(0, ask_ref.at[peer], ask_in.at[st], peer).wait_send()
        back_copy(1, vs_all, peer).wait_send()
        back_copy(2, ks, peer).wait_send()
        return c

    lax.fori_loop(1, st_n, drain, 0)
    for d in range(1, tp_n):
        sums_copy(0, ks, d).wait_send()
        sums_copy(1, vs_all, d).wait_send()
    for d in range(1, hi_n + 1):
        h = (hi + d) % hi_n
        pair_copy(h).wait_send()
        if d < hi_n:
            cross(h).wait_send()
    dw_each(True, lambda way, s, b: dw_copy(way, s, b, True).wait_send())
    dw_each(False, lambda way, s, b: dw_copy(way, s, b, False).wait_send())


def local(pass_ids, store, queries, gate_pre, w_query, w_gate, w_key, w_value, d_mem):
    st_n = lax.axis_size("st")
    tp_n = lax.axis_size("tp")
    hi_n = tp_n // 2
    tok_rows, cols = queries.shape
    blocks = tok_rows // BLK
    passages, pass_len, chunk = store.shape
    model = w_key.shape[0]
    requests = blocks * PB
    depth = max(2, requests // st_n)
    pass_rows = passages * pass_len
    share = model // st_n

    ids = pass_ids.reshape(-1)
    owners = ids // passages
    within = ids % passages
    order = jnp.arange(requests, dtype=jnp.int32)
    earlier = (owners[None, :] == owners[:, None]) & (order[None, :] < order[:, None])
    rank = jnp.sum(earlier.astype(jnp.int32), axis=1)
    slots = jnp.stack([owners, rank])
    o_i = jnp.arange(st_n, dtype=jnp.int32)[:, None, None]
    k_i = jnp.arange(depth, dtype=jnp.int32)[None, :, None]
    match = (owners[None, None, :] == o_i) & (rank[None, None, :] == k_i)
    asked = jnp.max(jnp.where(match, within[None, None, :], -1), axis=2)
    req_of = jnp.max(jnp.where(match, order[None, None, :], 0), axis=2)
    hot_cols = depth * pass_len
    width = -(-hot_cols // 128) * 128
    lane = jnp.arange(width, dtype=jnp.int32)
    spread = jnp.repeat(asked, pass_len, axis=1)
    spread = jnp.pad(spread, ((0, 0), (0, width - hot_cols)), constant_values=-1)
    target = jnp.where(spread < 0, -1, spread * pass_len + lane[None, :] % pass_len)
    flat = jnp.pad(jnp.maximum(asked, 0), ((0, 0), (0, width - depth)))
    ask = jnp.concatenate(
        [target[:, None], flat[:, None], jnp.zeros((st_n, 6, width), jnp.int32)], axis=1
    )

    vmem = pl.BlockSpec(memory_space=pltpu.VMEM)
    smem = pl.BlockSpec(memory_space=pltpu.SMEM)
    hbm = pl.BlockSpec(memory_space=pl.ANY)
    V = pltpu.VMEM
    DMA = pltpu.SemaphoreType.DMA
    pair = 2 * cols
    tok_pair = tok_rows // tp_n
    sto_pair = pass_rows // tp_n
    gathered_bytes = 2 * 2 * st_n * pass_rows * cols
    if lax.axis_size("grp") == 2 and hi_n == 2 and passages % 2 == 0 and gathered_bytes <= 8 << 20:
        half_pass = passages // 2
        n_some = half_pass // tile_of(half_pass, 2)
        d_tokens, d_store, d_wkey = pl.pallas_call(
            functools.partial(gathered_kernel, st_n, tp_n, depth, pass_len),
            out_shape=(
                jax.ShapeDtypeStruct((tok_pair, model), BF),
                jax.ShapeDtypeStruct((sto_pair, model), BF),
                jax.ShapeDtypeStruct((share, cols), F32),
            ),
            in_specs=[smem, smem, vmem] + [hbm] * 8,
            out_specs=(vmem, vmem, vmem),
            scratch_shapes=[
                V((tp_n, pass_rows, chunk), BF),
                V((tp_n, model, pair), BF),
                V((model, pair), BF),
                V((tok_rows, cols), BF),
                V((tok_rows, cols), BF),
                V((tok_rows, cols), BF),
                V((pass_rows, cols), F32),
                V((sto_pair, model), F32),
                V((st_n * passages, pass_len, cols), BF),
                V((st_n * passages, pass_len, cols), BF),
                V((st_n, 8, width), jnp.int32),
                V((st_n, depth, pass_len, pair), BF),
                V((cols // HD, tok_rows, PB * pass_len), F32),
                V((PB * pass_len, pair), BF),
                V((requests, pass_len, pair), BF),
                V((tok_rows, pair), BF),
                V((st_n, depth, pass_len, pair), BF),
                V((st_n, pass_rows, hot_cols), BF),
                V((pass_rows, pair), BF),
                V((tp_n, sto_pair, pair), BF),
                V((model, cols), BF),
                V((st_n, share, cols), BF),
                V((st_n, share, cols), BF),
                V((tp_n, tok_pair, model), BF),
                V((hi_n, tok_pair, model), BF),
                V((hi_n, tok_pair, model), BF),
                DMA((8,)),
                DMA((3, hi_n, 2 * n_some)),
                DMA((tp_n, 2 * n_some)),
                DMA((2, st_n, n_some, 3)),
                DMA((2, st_n, n_some, 2)),
                DMA((3, st_n)),
                DMA((3, st_n)),
                DMA((hi_n,)),
                DMA((hi_n,)),
                DMA((hi_n,)),
                DMA((hi_n,)),
                DMA((5, hi_n)),
                DMA((5, tp_n)),
                DMA((2, tp_n)),
                DMA((2, tp_n)),
                DMA((2, st_n, 2)),
                DMA((2, st_n, 2)),
            ],
            compiler_params=pltpu.CompilerParams(
                collective_id=0, has_side_effects=True, vmem_limit_bytes=67043328
            ),
        )(
            ids, req_of, ask, store.reshape(pass_rows, chunk),
            queries, gate_pre, w_query, w_gate, w_key, w_value, d_mem,
        )
        return d_tokens, d_store.reshape(passages // tp_n, pass_len, model), d_wkey
    d_tokens, d_store, d_wkey = pl.pallas_call(
        functools.partial(kernel, st_n, tp_n, depth, pass_len),
        out_shape=(
            jax.ShapeDtypeStruct((tok_pair, model), BF),
            jax.ShapeDtypeStruct((sto_pair, model), BF),
            jax.ShapeDtypeStruct((share, cols), F32),
        ),
        in_specs=[smem, smem, vmem] + [hbm] * 8,
        out_specs=(vmem, vmem, vmem),
        scratch_shapes=[
            V((tp_n, pass_rows, chunk), BF),
            V((model, pair), BF),
            V((model, pair), BF),
            V((tok_rows, cols), BF),
            V((tok_rows, cols), BF),
            V((tok_rows, cols), BF),
            V((pass_rows, pair), F32),
            V((passages, pass_len, pair), BF),
            V((st_n, 8, width), jnp.int32),
            pltpu.SMEM((st_n, 8, width), jnp.int32),
            V((st_n, depth, pass_len, pair), BF),
            V((st_n, depth, pass_len, cols), BF),
            V((st_n, depth, pass_len, cols), BF),
            V((st_n, depth, pass_len, pair), BF),
            V((cols // HD, tok_rows, PB * pass_len), F32),
            V((PB * pass_len, pair), BF),
            V((requests, pass_len, pair), BF),
            V((tok_rows, pair), BF),
            V((st_n, depth, pass_len, pair), BF),
            V((st_n, pass_rows, hot_cols), BF),
            V((pass_rows, pair), BF),
            V((model, cols), BF),
            V((st_n, share, cols), BF),
            V((tp_n, tok_pair, model), BF),
            V((hi_n, tok_pair, model), BF),
            V((hi_n, tok_pair, model), BF),
            V((tp_n, sto_pair, model), BF),
            V((hi_n, sto_pair, model), BF),
            V((hi_n, sto_pair, model), BF),
            DMA((9,)),
            DMA((3, hi_n)),
            DMA((tp_n,)),
            DMA((6, st_n)),
            DMA((6, st_n)),
            DMA((2, hi_n)),
            DMA((2, hi_n)),
            DMA((2, hi_n)),
            DMA((2, hi_n)),
        ],
        compiler_params=pltpu.CompilerParams(
            collective_id=0, has_side_effects=True, vmem_limit_bytes=67043328
        ),
    )(
        slots, req_of, ask, store.reshape(pass_rows, chunk),
        queries, gate_pre, w_query, w_gate, w_key, w_value, d_mem,
    )
    return d_tokens, d_store.reshape(passages // tp_n, pass_len, model), d_wkey


def solution(mesh):
    return jax.shard_map(
        local,
        mesh=mesh,
        in_specs=(
            P(("grp", "st"), None),
            P("st", None, "tp"),
            P(("grp", "st"), "tp"),
            P(("grp", "st"), "tp"),
            P(None, "tp"),
            P(None, "tp"),
            P(None, "tp"),
            P(None, "tp"),
            P(("grp", "st"), "tp"),
        ),
        out_specs=(
            P(("grp", "st", "tp"), None),
            P(("grp", "st", "tp"), None, None),
            P(("grp", "st"), "tp"),
        ),
        check_vma=False,
    )
```

```python
import functools

import jax
import jax.numpy as jnp
from jax import lax
from jax.experimental import pallas as pl
from jax.experimental.pallas import tpu as pltpu
from jax.sharding import PartitionSpec as P

HD = 256
BLK = 128
PB = 4
BF = jnp.bfloat16
F32 = jnp.float32
MESH = pl.DeviceIdType.MESH
NT = (((1,), (1,)), ((), ()))
TN = (((0,), (0,)), ((), ()))


def dot(a, b, dims=(((1,), (0,)), ((), ()))):
    return lax.dot_general(a, b, dims, preferred_element_type=F32)


def remote(src, dst, send, recv, device):
    return pltpu.make_async_remote_copy(
        src_ref=src,
        dst_ref=dst,
        send_sem=send,
        recv_sem=recv,
        device_id=device,
        device_id_type=MESH,
    )


def tile_of(size, most):
    while size % most:
        most //= 2
    return most


def kernel(
    st_n, tp_n, depth, pass_len,
    slot_ref, req_ref, ask_ref, store_ref, q_hbm, g_hbm, wq_hbm, wg_hbm, wk_hbm, wv_hbm, m_hbm,
    tok_out, store_out, wkey_out,
    rows, wkv, wqg, q_v, g_v, m_v, acc, kv, ask_in, ask_s, out, inc_k, inc_v, ret, prob_v, kvb, reqg, gboth, arr,
    hot, plow, dwp, dwr, tp_part, tp_pair, tp_recv, sp_part, sp_pair, sp_recv,
    lsem, gs, gr, zs, zr, ps, pr, xs, xr,
):
    st = lax.axis_index("st")
    tp = lax.axis_index("tp")
    hi_n = tp_n // 2
    hi, lo = tp // 2, tp % 2
    mate = {"tp": hi * 2 + 1 - lo}
    pass_rows, chunk = rows.shape[1], rows.shape[2]
    model = wqg.shape[0]
    cols = q_v.shape[1]
    heads = cols // HD
    tok_rows = q_v.shape[0]
    blocks = tok_rows // BLK
    blk_keys = PB * pass_len

    def local(i, src, dst):
        copy = pltpu.make_async_copy(src, dst, lsem.at[i])
        copy.start()
        return copy

    own_rows = local(0, store_ref, rows.at[tp])
    loads_kv = [
        local(1, wk_hbm, wkv.at[:, pl.ds(0, cols)]),
        local(2, wv_hbm, wkv.at[:, pl.ds(cols, cols)]),
    ]
    loads_q = [local(3, q_hbm, q_v), local(4, g_hbm, g_v), local(5, m_hbm, m_v)]
    loads_qg = [
        local(6, wq_hbm, wqg.at[:, pl.ds(0, cols)]),
        local(7, wg_hbm, wqg.at[:, pl.ds(cols, cols)]),
    ]

    barrier = pltpu.get_barrier_semaphore()

    def greet_st(d, c):
        pl.semaphore_signal(
            barrier, inc=1, device_id={"st": (st + d) % st_n}, device_id_type=MESH
        )
        return c

    lax.fori_loop(1, st_n, greet_st, 0)
    for d in range(1, tp_n):
        pl.semaphore_signal(
            barrier, inc=1, device_id={"tp": (tp + d) % tp_n}, device_id_type=MESH
        )
    pl.semaphore_wait(barrier, st_n - 1 + tp_n - 1)

    across = []
    for d in range(1, hi_n):
        h = (hi + d) % hi_n
        across.append(
            remote(store_ref, rows.at[tp], gs.at[0, h], gr.at[tp], {"tp": h * 2 + lo})
        )
        across[-1].start()
    beside = remote(store_ref, rows.at[tp], gs.at[1, hi], gr.at[tp], mate)
    beside.start()

    upper = st >= st_n // 2
    mark = jnp.where(upper, st, st_n - 1 - st)

    def far_peer(d):
        i = d - 1
        i = i + jnp.where(i >= mark, 1, 0)
        return jnp.where(upper, i, st_n - 1 - i)

    def z_copy(phase, src, dst, peer):
        return remote(src, dst, zs.at[phase, peer], zr.at[phase, st], {"st": peer})

    def z_wait(phase, src, dst, peer):
        remote(src, dst, zs.at[phase, peer], zr.at[phase, peer], {"st": peer}).wait_recv()

    def ask_send(d, c):
        peer = (st + d) % st_n
        z_copy(0, ask_ref.at[peer], ask_in.at[st], peer).start()
        return c

    lax.fori_loop(1, st_n, ask_send, 0)
    ask_in[st] = ask_ref[st]

    m_tile = tile_of(pass_rows, 256)

    def project(t, first):
        def step(i, c):
            r = pl.ds(pl.multiple_of(i * m_tile, m_tile), m_tile)
            part = dot(rows[t, r], wkv[pl.ds(pl.multiple_of(t * chunk, chunk), chunk), :])
            acc[r] = part if first else acc[r] + part
            return c

        lax.fori_loop(0, pass_rows // m_tile, step, 0)

    def g_wait(t):
        remote(store_ref, rows.at[t], gs.at[1, hi], gr.at[t], mate).wait_recv()

    own_rows.wait()
    for copy in loads_kv:
        copy.wait()
    project(tp, True)
    g_wait(hi * 2 + 1 - lo)
    project(hi * 2 + 1 - lo, False)

    def ask_wait(d, c):
        peer = (st + d) % st_n
        z_wait(0, ask_ref.at[peer], ask_in.at[peer], peer)
        return c

    lax.fori_loop(1, st_n, ask_wait, 0)
    ask_copy = local(8, ask_in, ask_s)
    ask_copy.wait()

    hot_cols = depth * pass_len

    def hot_step(o, c):
        target = ask_in[o][0:1, :hot_cols]
        for i in range(pass_rows // m_tile):
            line = lax.broadcasted_iota(jnp.int32, (m_tile, hot_cols), 0) + i * m_tile
            hot[o, i * m_tile : (i + 1) * m_tile, :] = jnp.where(line == target, 1.0, 0.0).astype(BF)
        return c

    lax.fori_loop(0, st_n, hot_step, 0)
    onward = []
    for d in range(1, hi_n):
        h = (hi + d) % hi_n
        t = h * 2 + lo
        g_wait(t)
        onward.append(remote(rows.at[t], rows.at[t], gs.at[2, h], gr.at[t], mate))
        onward[-1].start()
        project(t, False)
    for d in range(1, hi_n):
        t = ((hi + d) % hi_n) * 2 + 1 - lo
        g_wait(t)
        project(t, False)

    def low_step(i, c):
        kv[i] = acc[pl.ds(pl.multiple_of(i * pass_len, pass_len), pass_len), :].astype(BF)
        return c

    lax.fori_loop(0, pass_rows // pass_len, low_step, 0)

    ks, vs_all = pl.ds(0, cols), pl.ds(cols, cols)

    def half(ref, peer, part):
        return ref.at[peer, :, :, part]

    def key_copy(peer):
        return z_copy(1, half(out, peer, ks), inc_k.at[st], peer)

    def value_copy(peer):
        return z_copy(4, half(out, peer, vs_all), inc_v.at[st], peer)

    def kv_send(d, c):
        peer = far_peer(d)
        for k in range(depth):
            out[peer, k] = kv[ask_s[peer, 1, k]]
        key_copy(peer).start()
        return c

    def value_send(d, c):
        value_copy(far_peer(d)).start()
        return c

    lax.fori_loop(1, st_n, kv_send, 0)
    lax.fori_loop(1, st_n, value_send, 0)
    for k in range(depth):
        picked = kv[ask_s[st, 1, k]]
        inc_k[st, k] = picked[:, :cols]
        inc_v[st, k] = picked[:, cols:]
    for copy in loads_q + loads_qg:
        copy.wait()

    def key_wait(d, c):
        peer = (st + d) % st_n
        z_wait(1, half(out, peer, ks), inc_k.at[peer], peer)
        return c

    lax.fori_loop(1, st_n, key_wait, 0)
    scale = HD ** (-0.5)

    def probs_step(b, c):
        r = pl.ds(pl.multiple_of(b * BLK, BLK), BLK)
        for j in range(PB):
            kvb[j * pass_len : (j + 1) * pass_len, :cols] = inc_k[
                slot_ref[0, b * PB + j], slot_ref[1, b * PB + j]
            ]
        for head in range(heads):
            hs = slice(head * HD, (head + 1) * HD)
            vs = slice(cols + head * HD, cols + (head + 1) * HD)
            gate = g_v[r, hs].astype(F32)
            scores = dot(q_v[r, hs], kvb[:, hs], NT) * scale
            shifted = jnp.exp(scores - jnp.max(scores, axis=-1, keepdims=True))
            prob = shifted / jnp.sum(shifted, axis=-1, keepdims=True)
            prob_v[head, r, :] = prob
            sig = 1.0 / (1.0 + jnp.exp(-gate))
            att_grad = (gate * sig * m_v[r, hs].astype(F32)).astype(BF)
            value_grad = dot(prob.astype(BF), att_grad, TN).astype(BF)
            for j in range(PB):
                reqg[b * PB + j, :, vs] = value_grad[j * pass_len : (j + 1) * pass_len]
        return c

    lax.fori_loop(0, blocks, probs_step, 0)

    def back_copy(phase, part, peer):
        return z_copy(phase, half(ret, peer, part), half(arr, st, part), peer)

    def give_back(phase, part, span):
        def send(d, c):
            peer = far_peer(d)
            for k in range(depth):
                ret[peer, k, :, span] = reqg[req_ref[peer, k]][:, span]
            back_copy(phase, part, peer).start()
            return c

        lax.fori_loop(1, st_n, send, 0)
        for k in range(depth):
            arr[st, k, :, span] = reqg[req_ref[st, k]][:, span]

    give_back(2, vs_all, slice(cols, 2 * cols))

    def value_wait(d, c):
        peer = (st + d) % st_n
        z_wait(4, half(out, peer, vs_all), inc_v.at[peer], peer)
        return c

    lax.fori_loop(1, st_n, value_wait, 0)

    def block_step(b, c):
        r = pl.ds(pl.multiple_of(b * BLK, BLK), BLK)
        for j in range(PB):
            o, k = slot_ref[0, b * PB + j], slot_ref[1, b * PB + j]
            kvb[j * pass_len : (j + 1) * pass_len, :cols] = inc_k[o, k]
            kvb[j * pass_len : (j + 1) * pass_len, cols:] = inc_v[o, k]
        for head in range(heads):
            hs = slice(head * HD, (head + 1) * HD)
            vs = slice(cols + head * HD, cols + (head + 1) * HD)
            q = q_v[r, hs]
            key = kvb[:, hs]
            value = kvb[:, vs]
            gate = g_v[r, hs].astype(F32)
            grad = m_v[r, hs].astype(F32)
            prob = prob_v[head, r, :]
            attended = dot(prob.astype(BF), value)
            sig = 1.0 / (1.0 + jnp.exp(-gate))
            att_grad = (gate * sig * grad).astype(BF)
            gboth[r, vs] = (grad * attended * sig * (1.0 + gate * (1.0 - sig))).astype(BF)
            prob_grad = dot(att_grad, value, NT)
            inner = jnp.sum(prob * prob_grad, axis=-1, keepdims=True)
            score_grad = (scale * prob * (prob_grad - inner)).astype(BF)
            gboth[r, hs] = dot(score_grad, key).astype(BF)
            key_grad = dot(score_grad, q, TN).astype(BF)
            for j in range(PB):
                reqg[b * PB + j, :, hs] = key_grad[j * pass_len : (j + 1) * pass_len]
        return c

    lax.fori_loop(0, blocks, block_step, 0)
    give_back(5, ks, slice(0, cols))

    n_tile = tile_of(model, 512)

    def expand(src, weight, part, pair_rows, t):
        base = pl.multiple_of(t * pair_rows, pair_rows)
        a = src[pl.ds(base, pair_rows), :]

        def step(i, c):
            n = pl.ds(pl.multiple_of(i * n_tile, n_tile), n_tile)
            part[t, :, n] = dot(a, weight[n, :], NT).astype(BF)
            return c

        lax.fori_loop(0, model // n_tile, step, 0)

    def pair_copy(which, part, pair, h):
        return remote(part.at[h * 2 + 1 - lo], pair.at[h], ps.at[which, h], pr.at[which, h], mate)

    def scatter_first(which, src, weight, part, pair, pair_rows):
        for d in range(1, hi_n + 1):
            h = (hi + d) % hi_n
            expand(src, weight, part, pair_rows, h * 2 + 1 - lo)
            pair_copy(which, part, pair, h).start()

    def cross(which, send, recv, h):
        return remote(
            send.at[h * 2 + lo], recv.at[hi], xs.at[which, h], xr.at[which, hi], {"tp": h * 2 + lo}
        )

    def scatter_second(which, src, weight, part, pair, send, recv, pair_rows):
        for d in range(1, hi_n + 1):
            h = (hi + d) % hi_n
            expand(src, weight, part, pair_rows, h * 2 + lo)
            pair_copy(which, part, pair, h).wait_recv()
            if d < hi_n:
                part[h * 2 + lo] = (part[h * 2 + lo].astype(F32) + pair[h].astype(F32)).astype(BF)
                cross(which, part, recv, h).start()

    def scatter_last(which, part, pair, send, recv, result):
        for d in range(1, hi_n):
            h = (hi + d) % hi_n
            remote(
                send.at[h * 2 + lo], recv.at[h], xs.at[which, h], xr.at[which, h], {"tp": h * 2 + lo}
            ).wait_recv()
        total = part[tp].astype(F32) + pair[hi].astype(F32)
        for d in range(1, hi_n):
            total = total + recv[(hi + d) % hi_n].astype(F32)
        result[...] = total.astype(BF)

    tok_pair = tok_rows // tp_n
    sto_pair = pass_rows // tp_n
    scatter_first(0, gboth, wqg, tp_part, tp_pair, tok_pair)
    scatter_second(0, gboth, wqg, tp_part, tp_pair, tp_part, tp_recv, tok_pair)

    def gather_sums(o, span, first):
        def step(i, c):
            r = pl.ds(pl.multiple_of(i * m_tile, m_tile), m_tile)
            part = dot(hot[o, r, :], arr[o, :, :, span].reshape(hot_cols, cols))
            acc[r, span] = part if first else acc[r, span] + part
            return c

        lax.fori_loop(0, pass_rows // m_tile, step, 0)

    for phase, part, span in ((2, vs_all, slice(cols, 2 * cols)), (5, ks, slice(0, cols))):
        gather_sums(st, span, True)

        def grad_wait(d, c):
            peer = (st + d) % st_n
            z_wait(phase, half(ret, peer, part), half(arr, peer, part), peer)
            gather_sums(peer, span, False)
            return c

        lax.fori_loop(1, st_n, grad_wait, 0)
        plow[:, span] = acc[:, span].astype(BF)

    scatter_first(1, plow, wkv, sp_part, sp_pair, sto_pair)

    def wkey_step(t, c):
        dwp[pl.ds(pl.multiple_of(t * chunk, chunk), chunk), :] = dot(
            rows[t], plow[:, :cols], TN
        ).astype(BF)
        return c

    lax.fori_loop(0, tp_n, wkey_step, 0)
    share = model // st_n

    def part_of(s):
        return dwp.at[pl.ds(pl.multiple_of(s * share, share), share), :]

    def wkey_send(d, c):
        peer = far_peer(d)
        z_copy(3, part_of(peer), dwr.at[st], peer).start()
        return c

    lax.fori_loop(1, st_n, wkey_send, 0)
    scatter_second(1, plow, wkv, sp_part, sp_pair, sp_part, sp_recv, sto_pair)
    scatter_last(0, tp_part, tp_pair, tp_part, tp_recv, tok_out)
    wkey_out[...] = part_of(st)[...].astype(F32)

    def wkey_wait(d, c):
        peer = (st + d) % st_n
        z_wait(3, part_of(peer), dwr.at[peer], peer)
        wkey_out[...] += dwr[peer].astype(F32)
        return c

    lax.fori_loop(1, st_n, wkey_wait, 0)
    scatter_last(1, sp_part, sp_pair, sp_part, sp_recv, store_out)

    for copy in across + [beside] + onward:
        copy.wait_send()

    def drain(d, c):
        peer = (st + d) % st_n
        z_copy(0, ask_ref.at[peer], ask_in.at[st], peer).wait_send()
        key_copy(peer).wait_send()
        value_copy(peer).wait_send()
        back_copy(2, vs_all, peer).wait_send()
        back_copy(5, ks, peer).wait_send()
        z_copy(3, part_of(peer), dwr.at[st], peer).wait_send()
        return c

    lax.fori_loop(1, st_n, drain, 0)
    for d in range(1, hi_n + 1):
        h = (hi + d) % hi_n
        pair_copy(0, tp_part, tp_pair, h).wait_send()
        pair_copy(1, sp_part, sp_pair, h).wait_send()
        if d < hi_n:
            cross(0, tp_part, tp_recv, h).wait_send()
            cross(1, sp_part, sp_recv, h).wait_send()


def gathered_kernel(
    st_n, tp_n, depth, pass_len,
    ids_ref, req_ref, ask_ref, store_ref, q_hbm, g_hbm, wq_hbm, wg_hbm, wk_hbm, wv_hbm, m_hbm,
    tok_out, store_out, wkey_out,
    rows, wall, wqg, q_v, g_v, m_v, acc, vterm, k_all, v_all, ask_in, ret, prob_v, kvb, reqg, gboth, arr,
    hot, plow, sums, dwp, dwc, dwf, tp_part, tp_pair, tp_recv,
    lsem, gs, gr, fs, fr, zs, zr, ps, pr, xs, xr, ws, wr, ss, sr, us, ur,
):
    grp = lax.axis_index("grp")
    st = lax.axis_index("st")
    tp = lax.axis_index("tp")
    hi_n = tp_n // 2
    hi, lo = tp // 2, tp % 2
    mate_t = hi * 2 + 1 - lo
    mate = {"tp": mate_t}
    twin = {"grp": 1 - grp}
    pass_rows, chunk = rows.shape[1], rows.shape[2]
    passages = pass_rows // pass_len
    model = wqg.shape[0]
    cols = q_v.shape[1]
    heads = cols // HD
    tok_rows = q_v.shape[0]
    blocks = tok_rows // BLK
    half_pass = passages // 2
    some = tile_of(half_pass, 2)
    some_rows = some * pass_len
    n_some = half_pass // some
    key_cols, value_cols = slice(0, cols), slice(cols, 2 * cols)

    def local(i, src, dst):
        copy = pltpu.make_async_copy(src, dst, lsem.at[i])
        copy.start()
        return copy

    loads_kv = [
        local(0, store_ref, rows.at[tp]),
        local(1, wk_hbm, wall.at[tp, :, pl.ds(0, cols)]),
        local(2, wv_hbm, wall.at[tp, :, pl.ds(cols, cols)]),
    ]
    loads_q = [
        local(3, q_hbm, q_v),
        local(4, g_hbm, g_v),
        local(5, m_hbm, m_v),
        local(6, wq_hbm, wqg.at[:, pl.ds(0, cols)]),
        local(7, wg_hbm, wqg.at[:, pl.ds(cols, cols)]),
    ]

    barrier = pltpu.get_barrier_semaphore()

    def greet_st(d, c):
        pl.semaphore_signal(
            barrier, inc=1, device_id={"st": (st + d) % st_n}, device_id_type=MESH
        )
        return c

    lax.fori_loop(1, st_n, greet_st, 0)
    for d in range(1, tp_n):
        pl.semaphore_signal(
            barrier, inc=1, device_id={"tp": (tp + d) % tp_n}, device_id_type=MESH
        )
    pl.semaphore_signal(barrier, inc=1, device_id=twin, device_id_type=MESH)
    pl.semaphore_wait(barrier, st_n + tp_n - 1)

    def first_row(i):
        part = (grp + i // n_some) % 2
        return pl.multiple_of((part * n_some + i % n_some) * some_rows, some_rows)

    def g_copy(way, i, t, source, peer, slot):
        r = pl.ds(first_row(i), some_rows)
        src = store_ref.at[r] if source is None else rows.at[source, r]
        return remote(src, rows.at[t, r], gs.at[way, slot, i], gr.at[t, i], peer)

    def across(d, i):
        h = (hi + d) % hi_n
        return g_copy(0, i, tp, None, {"tp": h * 2 + lo}, h)

    def beside(i):
        return g_copy(1, i, tp, None, mate, hi)

    def onward(d, i):
        h = (hi + d) % hi_n
        return g_copy(2, i, h * 2 + lo, h * 2 + lo, mate, h)

    def g_wait(t, i):
        g_copy(1, i, t, None, mate, hi).wait_recv()

    def rows_send(i, c):
        for d in range(1, hi_n):
            across(d, i).start()
        beside(i).start()
        return c

    lax.fori_loop(0, 2 * n_some, rows_send, 0)

    upper = st >= st_n // 2
    mark = jnp.where(upper, st, st_n - 1 - st)

    def far_peer(d):
        i = d - 1
        i = i + jnp.where(i >= mark, 1, 0)
        return jnp.where(upper, i, st_n - 1 - i)

    def z_copy(phase, src, dst, peer):
        return remote(src, dst, zs.at[phase, peer], zr.at[phase, st], {"st": peer})

    def z_wait(phase, src, dst, peer):
        remote(src, dst, zs.at[phase, peer], zr.at[phase, peer], {"st": peer}).wait_recv()

    def ask_send(d, c):
        peer = (st + d) % st_n
        z_copy(0, ask_ref.at[peer], ask_in.at[st], peer).start()
        return c

    lax.fori_loop(1, st_n, ask_send, 0)
    ask_in[st] = ask_ref[st]

    def project(i):
        r = pl.ds(first_row(i), some_rows)

        def term(t):
            w = wall[tp, pl.ds(pl.multiple_of(t * chunk, chunk), chunk), :]
            return dot(rows[t, r], w)

        for d in range(1, hi_n):
            g_wait(((hi + d) % hi_n) * 2 + lo, i)
            onward(d, i).start()
        g_wait(mate_t, i)
        total = term(tp) + term(mate_t)
        for d in range(1, hi_n):
            total = total + term(((hi + d) % hi_n) * 2 + lo)
        for d in range(1, hi_n):
            t = ((hi + d) % hi_n) * 2 + 1 - lo
            g_wait(t, i)
            total = total + term(t)
        low = total.astype(BF)
        first = st * passages + first_row(i) // pass_len
        for p in range(some):
            k_all[first + p] = low[p * pass_len : (p + 1) * pass_len, key_cols]
            v_all[first + p] = low[p * pass_len : (p + 1) * pass_len, value_cols]

    def part_of_all(kind, o, c, side):
        ref = k_all if kind == 0 else v_all
        return ref.at[pl.ds(o * passages + side * half_pass + c * some, some)]

    def chain_copy(kind, o, c, way, peer):
        part = part_of_all(kind, o, c, grp)
        return remote(part, part, fs.at[kind, o, c, way], fr.at[kind, o, c, 0], {"st": peer})

    def twin_copy(kind, o, c):
        part = part_of_all(kind, o, c, grp)
        return remote(part, part, fs.at[kind, o, c, 2], fr.at[kind, o, c, 1], twin)

    lower = st < st_n // 2

    def own_copies(kind, c, act, inward=True, outward=True):
        ways = ((0, st + 1, lower), (1, st - 1, jnp.logical_not(lower)))
        for way, onto, toward in ways:
            there = (onto >= 0) & (onto < st_n)
            if not outward:
                there = there & toward
            if not inward:
                there = there & jnp.logical_not(toward)

            @pl.when(there)
            def _():
                act(chain_copy(kind, st, c, way, onto))

    def relay_copies(kind, d, c, act, ready):
        for way, sign in ((0, -1), (1, 1)):
            o = st + sign * d
            onto = st - sign

            @pl.when((o >= 0) & (o < st_n))
            def _():
                if ready:
                    chain_copy(kind, o, c, way, st).wait_recv()

                @pl.when((onto >= 0) & (onto < st_n))
                def _():
                    act(chain_copy(kind, o, c, way, onto))

                act(twin_copy(kind, o, c))

    def start(copy):
        copy.start()

    def own_send(kind, c, **which):
        own_copies(kind, c, start, **which)

    def relay(kind, d, c):
        relay_copies(kind, d, c, start, True)

    def twin_wait(kind):
        def step(i, c):
            o = (st + 1 + i // n_some) % st_n
            k = i % n_some
            part = part_of_all(kind, o, k, 1 - grp)
            remote(part, part, fs.at[kind, o, k, 2], fr.at[kind, o, k, 1], twin).wait_recv()
            return c

        lax.fori_loop(0, (st_n - 1) * n_some, step, 0)

    for copy in loads_kv:
        copy.wait()

    def early_step(i, c):
        project(i)
        own_send(0, i)

        @pl.when(i > 0)
        def _():
            relay(0, 1, i - 1)

        return c

    lax.fori_loop(0, n_some, early_step, 0)
    relay(0, 1, n_some - 1)

    def inward_send(i, c):
        own_send(1, i, outward=False)
        return c

    def outward_send(i, c):
        own_send(1, i, inward=False)
        return c

    lax.fori_loop(0, n_some, inward_send, 0)

    def late_step(i, c):
        project(n_some + i)
        relay(0, 2, i)
        return c

    lax.fori_loop(0, n_some, late_step, 0)
    lax.fori_loop(0, n_some, outward_send, 0)

    w_half = model // 2
    w_mine = pl.ds(pl.multiple_of(grp * w_half, w_half), w_half)
    w_other = pl.ds(pl.multiple_of((1 - grp) * w_half, w_half), w_half)

    def w_across(d):
        h = (hi + d) % hi_n
        part = wall.at[tp, w_mine]
        return remote(part, part, ws.at[0, h], wr.at[0, tp], {"tp": h * 2 + lo})

    def w_twin(d):
        t = ((hi + d) % hi_n) * 2 + lo
        part = wall.at[t, w_mine]
        return remote(part, part, ws.at[1, (hi + d) % hi_n], wr.at[1, t], twin)

    def w_onward(d, k):
        t = ((hi + d) % hi_n) * 2 + lo
        part = wall.at[t, w_other if k else w_mine]
        return remote(part, part, ws.at[2 + k, (hi + d) % hi_n], wr.at[2 + k, t], mate)

    w_beside = remote(wall.at[tp], wall.at[tp], ws.at[4, 0], wr.at[4, tp], mate)

    def w_wait(kind, t, part):
        remote(wall.at[t, part], wall.at[t, part], ws.at[kind, 0], wr.at[kind, t], mate).wait_recv()

    for d in range(1, hi_n):
        w_across(d).start()
    w_beside.start()

    def relay_rest(kind, first, last):
        def step(i, c):
            relay(kind, 1 + i // n_some, i % n_some)
            return c

        lax.fori_loop(first, last, step, 0)

    relays = (st_n - 1) * n_some
    ahead = jnp.where((st > 0) & (st < st_n - 1), n_some, 0)
    relay_rest(1, 0, ahead)
    relay_rest(0, 2 * n_some, relays)
    for copy in loads_q:
        copy.wait()
    twin_wait(0)
    scale = HD ** (-0.5)

    def fill(ref, span, b):
        for j in range(PB):
            kvb[j * pass_len : (j + 1) * pass_len, span] = ref[ids_ref[b * PB + j]]

    def probs_step(b, c):
        r = pl.ds(pl.multiple_of(b * BLK, BLK), BLK)
        fill(k_all, key_cols, b)
        for head in range(heads):
            hs = slice(head * HD, (head + 1) * HD)
            vs = slice(cols + head * HD, cols + (head + 1) * HD)
            gate = g_v[r, hs].astype(F32)
            scores = dot(q_v[r, hs], kvb[:, hs], NT) * scale
            shifted = jnp.exp(scores - jnp.max(scores, axis=-1, keepdims=True))
            prob = shifted / jnp.sum(shifted, axis=-1, keepdims=True)
            prob_v[head, r, :] = prob
            sig = 1.0 / (1.0 + jnp.exp(-gate))
            att_grad = (gate * sig * m_v[r, hs].astype(F32)).astype(BF)
            value_grad = dot(prob.astype(BF), att_grad, TN).astype(BF)
            for j in range(PB):
                reqg[b * PB + j, :, vs] = value_grad[j * pass_len : (j + 1) * pass_len]

        i = ahead + b

        @pl.when(i < relays)
        def _():
            relay(1, 1 + i // n_some, i % n_some)

        return c

    lax.fori_loop(0, blocks, probs_step, 0)

    def half(ref, peer, part):
        return ref.at[peer, :, :, part]

    def back_copy(phase, part, peer):
        return z_copy(phase, half(ret, peer, part), half(arr, st, part), peer)

    def give_back(phase, part, span):
        def send(d, c):
            peer = far_peer(d)
            for k in range(depth):
                ret[peer, k, :, span] = reqg[req_ref[peer, k]][:, span]
            back_copy(phase, part, peer).start()
            return c

        lax.fori_loop(1, st_n, send, 0)
        for k in range(depth):
            arr[st, k, :, span] = reqg[req_ref[st, k]][:, span]

    ks, vs_all = pl.ds(0, cols), pl.ds(cols, cols)
    give_back(1, vs_all, value_cols)
    relay_rest(1, jnp.minimum(ahead + blocks, relays), relays)
    twin_wait(1)

    def block_step(b, c):
        r = pl.ds(pl.multiple_of(b * BLK, BLK), BLK)
        fill(k_all, key_cols, b)
        fill(v_all, value_cols, b)
        for head in range(heads):
            hs = slice(head * HD, (head + 1) * HD)
            vs = slice(cols + head * HD, cols + (head + 1) * HD)
            q = q_v[r, hs]
            key = kvb[:, hs]
            value = kvb[:, vs]
            gate = g_v[r, hs].astype(F32)
            grad = m_v[r, hs].astype(F32)
            prob = prob_v[head, r, :]
            attended = dot(prob.astype(BF), value)
            sig = 1.0 / (1.0 + jnp.exp(-gate))
            att_grad = (gate * sig * grad).astype(BF)
            gboth[r, vs] = (grad * attended * sig * (1.0 + gate * (1.0 - sig))).astype(BF)
            prob_grad = dot(att_grad, value, NT)
            inner = jnp.sum(prob * prob_grad, axis=-1, keepdims=True)
            score_grad = (scale * prob * (prob_grad - inner)).astype(BF)
            gboth[r, hs] = dot(score_grad, key).astype(BF)
            key_grad = dot(score_grad, q, TN).astype(BF)
            for j in range(PB):
                reqg[b * PB + j, :, hs] = key_grad[j * pass_len : (j + 1) * pass_len]
        return c

    lax.fori_loop(0, blocks, block_step, 0)
    give_back(2, ks, key_cols)

    for d in range(1, hi_n):
        w_wait(0, ((hi + d) % hi_n) * 2 + lo, w_mine)
        w_twin(d).start()
        w_onward(d, 0).start()

    n_tile = tile_of(model, 512)

    def expand(t):
        a = gboth[pl.ds(pl.multiple_of(t * tok_pair, tok_pair), tok_pair), :]

        def step(i, c):
            n = pl.ds(pl.multiple_of(i * n_tile, n_tile), n_tile)
            tp_part[t, :, n] = dot(a, wqg[n, :], NT).astype(BF)
            return c

        lax.fori_loop(0, model // n_tile, step, 0)

    def pair_copy(h):
        return remote(tp_part.at[h * 2 + 1 - lo], tp_pair.at[h], ps.at[h], pr.at[h], mate)

    def cross(h):
        return remote(
            tp_part.at[h * 2 + lo], tp_recv.at[hi], xs.at[h], xr.at[hi], {"tp": h * 2 + lo}
        )

    tok_pair = tok_rows // tp_n
    for d in range(1, hi_n + 1):
        h = (hi + d) % hi_n
        expand(h * 2 + 1 - lo)
        pair_copy(h).start()
    for d in range(1, hi_n + 1):
        h = (hi + d) % hi_n
        expand(h * 2 + lo)
        pair_copy(h).wait_recv()
        if d < hi_n:
            tp_part[h * 2 + lo] = (tp_part[h * 2 + lo].astype(F32) + tp_pair[h].astype(F32)).astype(BF)
            cross(h).start()

    def ask_wait(d, c):
        peer = (st + d) % st_n
        z_wait(0, ask_ref.at[peer], ask_in.at[peer], peer)
        return c

    lax.fori_loop(1, st_n, ask_wait, 0)
    hot_cols = depth * pass_len
    m_tile = tile_of(pass_rows, 256)

    def hot_step(o, c):
        target = ask_in[o][0:1, :hot_cols]
        for i in range(pass_rows // m_tile):
            line = lax.broadcasted_iota(jnp.int32, (m_tile, hot_cols), 0) + i * m_tile
            hot[o, i * m_tile : (i + 1) * m_tile, :] = jnp.where(line == target, 1.0, 0.0).astype(BF)
        return c

    lax.fori_loop(0, st_n, hot_step, 0)

    def gather_sums(o, span, first):
        def step(i, c):
            r = pl.ds(pl.multiple_of(i * m_tile, m_tile), m_tile)
            part = dot(hot[o, r, :], arr[o, :, :, span].reshape(hot_cols, cols))
            acc[r, :] = part if first else acc[r, :] + part
            return c

        lax.fori_loop(0, pass_rows // m_tile, step, 0)

    sto_pair = pass_rows // tp_n

    def sums_copy(kind, part, d):
        t = (tp + d) % tp_n
        src = plow.at[pl.ds(pl.multiple_of(t * sto_pair, sto_pair), sto_pair), part]
        return remote(src, sums.at[tp, :, part], ss.at[kind, t], sr.at[kind, tp], {"tp": t})

    def sums_wait(kind, part, t):
        dst = sums.at[t, :, part]
        remote(dst, dst, ss.at[kind, t], sr.at[kind, t], mate).wait_recv()

    def collect(phase, kind, part, span):
        gather_sums(st, span, True)

        def grad_wait(d, c):
            peer = (st + d) % st_n
            z_wait(phase, half(ret, peer, part), half(arr, peer, part), peer)
            gather_sums(peer, span, False)
            return c

        lax.fori_loop(1, st_n, grad_wait, 0)
        plow[:, span] = acc[...].astype(BF)
        for d in range(1, tp_n):
            sums_copy(kind, part, d).start()
        sums[tp, :, span] = plow[pl.ds(pl.multiple_of(tp * sto_pair, sto_pair), sto_pair), span]

    collect(1, 1, vs_all, value_cols)

    collect(2, 0, ks, key_cols)

    share = model // st_n
    bits = 2
    bit = share // bits
    beyond = jnp.where(lower, st_n - 1, 0)
    middle = jnp.where(lower, st_n // 2, st_n // 2 - 1)
    beside_st = st + 1 - 2 * (st % 2)
    outer = (st == 0) | (st == st_n - 1)
    inner = jnp.logical_not(outer)

    def dw_line(s, b):
        return pl.ds(pl.multiple_of(s * share + b * bit, bit), bit)

    def dw_copy(kind, b):
        line = pl.ds(b * bit, bit)
        if kind < 2:
            src, dst = dwp.at[dw_line(middle if kind else beyond, b)], dwc.at[kind, line]
            peer = beside_st
        elif kind == 2:
            src, dst, peer = dwp.at[dw_line(beside_st, b)], dwf.at[0, line], beside_st
        else:
            src, dst = dwc.at[kind - 3, line], dwf.at[1, line]
            peer = middle if kind == 4 else beyond
        return remote(src, dst, us.at[kind, b], ur.at[kind, b], {"st": peer})

    def dw_send(kind):
        for b in range(bits):
            dw_copy(kind, b).start()

    def dw_relay(q):
        for b in range(bits):
            line = slice(b * bit, (b + 1) * bit)
            dw_copy(q, b).wait_recv()
            own = dwp[dw_line(middle if q else beyond, b), :].astype(F32)
            dwc[q, line, :] = (dwc[q, line, :].astype(F32) + own).astype(BF)
            dw_copy(3 + q, b).start()

    def wkey_step(s):
        dwp[pl.ds(pl.multiple_of(s * chunk, chunk), chunk), :] = dot(
            rows[s], plow[:, key_cols], TN
        ).astype(BF)

    def wkey_turn(j, c):
        far = jnp.where(j == 0, beyond, middle)
        near = jnp.where(j == 2, beside_st, st)
        near_first = jnp.where(j == 0, beside_st, st)
        far_after = jnp.where(j == 1, beyond, middle)
        s = jnp.where(
            outer, jnp.where(j < 2, far, near), jnp.where((j == 0) | (j == 3), near_first, far_after)
        )
        wkey_step(s)
        for kind in range(3):
            @pl.when(outer & (j == kind))
            def _():
                dw_send(kind)

        @pl.when(inner & (j == 0))
        def _():
            dw_send(2)

        return c

    lax.fori_loop(0, st_n, wkey_turn, 0)

    for d in range(1, hi_n):
        w_wait(1, ((hi + d) % hi_n) * 2 + lo, w_other)
        w_onward(d, 1).start()
    w_wait(4, mate_t, pl.ds(0, model))
    for d in range(1, hi_n):
        t = ((hi + d) % hi_n) * 2 + 1 - lo
        w_wait(2, t, w_mine)
        w_wait(3, t, w_other)

    def store_terms(span, done):
        def step(i, c):
            n = pl.ds(pl.multiple_of(i * n_tile, n_tile), n_tile)
            part = dot(sums[0, :, span], wall[0, n, span], NT)
            for t in range(1, tp_n):
                part = part + dot(sums[t, :, span], wall[t, n, span], NT)
            done(n, part)
            return c

        lax.fori_loop(0, model // n_tile, step, 0)

    def keep_values(n, part):
        vterm[:, n] = part

    def keep_store(n, part):
        store_out[:, n] = (vterm[:, n] + part).astype(BF)

    for d in range(1, tp_n):
        sums_wait(1, vs_all, (tp + d) % tp_n)
    store_terms(value_cols, keep_values)

    @pl.when(inner)
    def _():
        dw_relay(0)

    for d in range(1, tp_n):
        sums_wait(0, ks, (tp + d) % tp_n)
    store_terms(key_cols, keep_store)

    for d in range(1, hi_n):
        h = (hi + d) % hi_n
        remote(
            tp_part.at[h * 2 + lo], tp_recv.at[h], xs.at[h], xr.at[h], {"tp": h * 2 + lo}
        ).wait_recv()
    total = tp_part[tp].astype(F32) + tp_pair[hi].astype(F32)
    for d in range(1, hi_n):
        total = total + tp_recv[(hi + d) % hi_n].astype(F32)
    tok_out[...] = total.astype(BF)

    @pl.when(inner)
    def _():
        dw_relay(1)

    for b in range(bits):
        line = slice(b * bit, (b + 1) * bit)
        dw_copy(2, b).wait_recv()
        wkey_out[line, :] = dwp[dw_line(st, b), :].astype(F32) + dwf[0, line, :].astype(F32)
    for b in range(bits):
        line = slice(b * bit, (b + 1) * bit)
        for kind, edge in ((3, outer), (4, inner)):
            @pl.when(edge)
            def _():
                dw_copy(kind, b).wait_recv()

        wkey_out[line, :] += dwf[1, line, :].astype(F32)

    def wait_send(copy):
        copy.wait_send()

    def rows_drain(i, c):
        for d in range(1, hi_n):
            across(d, i).wait_send()
            onward(d, i).wait_send()
        beside(i).wait_send()
        return c

    lax.fori_loop(0, 2 * n_some, rows_drain, 0)

    def all_drain(i, c):
        for kind in (0, 1):
            own_copies(kind, i, wait_send)
            for d in range(1, st_n):
                relay_copies(kind, d, i, wait_send, False)
        return c

    lax.fori_loop(0, n_some, all_drain, 0)
    for d in range(1, hi_n):
        w_across(d).wait_send()
        w_twin(d).wait_send()
        w_onward(d, 0).wait_send()
        w_onward(d, 1).wait_send()
    w_beside.wait_send()

    def drain(d, c):
        peer = (st + d) % st_n
        z_copy(0, ask_ref.at[peer], ask_in.at[st], peer).wait_send()
        back_copy(1, vs_all, peer).wait_send()
        back_copy(2, ks, peer).wait_send()
        return c

    lax.fori_loop(1, st_n, drain, 0)
    for d in range(1, tp_n):
        sums_copy(0, ks, d).wait_send()
        sums_copy(1, vs_all, d).wait_send()
    for d in range(1, hi_n + 1):
        h = (hi + d) % hi_n
        pair_copy(h).wait_send()
        if d < hi_n:
            cross(h).wait_send()
    for b in range(bits):
        dw_copy(2, b).wait_send()
        for q in (0, 1):
            @pl.when(outer)
            def _():
                dw_copy(q, b).wait_send()

            @pl.when(inner)
            def _():
                dw_copy(3 + q, b).wait_send()


def local(pass_ids, store, queries, gate_pre, w_query, w_gate, w_key, w_value, d_mem):
    st_n = lax.axis_size("st")
    tp_n = lax.axis_size("tp")
    hi_n = tp_n // 2
    tok_rows, cols = queries.shape
    blocks = tok_rows // BLK
    passages, pass_len, chunk = store.shape
    model = w_key.shape[0]
    requests = blocks * PB
    depth = max(2, requests // st_n)
    pass_rows = passages * pass_len
    share = model // st_n

    ids = pass_ids.reshape(-1)
    owners = ids // passages
    within = ids % passages
    order = jnp.arange(requests, dtype=jnp.int32)
    earlier = (owners[None, :] == owners[:, None]) & (order[None, :] < order[:, None])
    rank = jnp.sum(earlier.astype(jnp.int32), axis=1)
    slots = jnp.stack([owners, rank])
    o_i = jnp.arange(st_n, dtype=jnp.int32)[:, None, None]
    k_i = jnp.arange(depth, dtype=jnp.int32)[None, :, None]
    match = (owners[None, None, :] == o_i) & (rank[None, None, :] == k_i)
    asked = jnp.max(jnp.where(match, within[None, None, :], -1), axis=2)
    req_of = jnp.max(jnp.where(match, order[None, None, :], 0), axis=2)
    hot_cols = depth * pass_len
    width = -(-hot_cols // 128) * 128
    lane = jnp.arange(width, dtype=jnp.int32)
    spread = jnp.repeat(asked, pass_len, axis=1)
    spread = jnp.pad(spread, ((0, 0), (0, width - hot_cols)), constant_values=-1)
    target = jnp.where(spread < 0, -1, spread * pass_len + lane[None, :] % pass_len)
    flat = jnp.pad(jnp.maximum(asked, 0), ((0, 0), (0, width - depth)))
    ask = jnp.concatenate(
        [target[:, None], flat[:, None], jnp.zeros((st_n, 6, width), jnp.int32)], axis=1
    )

    vmem = pl.BlockSpec(memory_space=pltpu.VMEM)
    smem = pl.BlockSpec(memory_space=pltpu.SMEM)
    hbm = pl.BlockSpec(memory_space=pl.ANY)
    V = pltpu.VMEM
    DMA = pltpu.SemaphoreType.DMA
    pair = 2 * cols
    tok_pair = tok_rows // tp_n
    sto_pair = pass_rows // tp_n
    gathered_bytes = 2 * 2 * st_n * pass_rows * cols
    if lax.axis_size("grp") == 2 and hi_n == 2 and st_n == 4 and passages % 2 == 0 and gathered_bytes <= 8 << 20:
        half_pass = passages // 2
        n_some = half_pass // tile_of(half_pass, 2)
        d_tokens, d_store, d_wkey = pl.pallas_call(
            functools.partial(gathered_kernel, st_n, tp_n, depth, pass_len),
            out_shape=(
                jax.ShapeDtypeStruct((tok_pair, model), BF),
                jax.ShapeDtypeStruct((sto_pair, model), BF),
                jax.ShapeDtypeStruct((share, cols), F32),
            ),
            in_specs=[smem, smem, vmem] + [hbm] * 8,
            out_specs=(vmem, vmem, vmem),
            scratch_shapes=[
                V((tp_n, pass_rows, chunk), BF),
                V((tp_n, model, pair), BF),
                V((model, pair), BF),
                V((tok_rows, cols), BF),
                V((tok_rows, cols), BF),
                V((tok_rows, cols), BF),
                V((pass_rows, cols), F32),
                V((sto_pair, model), F32),
                V((st_n * passages, pass_len, cols), BF),
                V((st_n * passages, pass_len, cols), BF),
                V((st_n, 8, width), jnp.int32),
                V((st_n, depth, pass_len, pair), BF),
                V((cols // HD, tok_rows, PB * pass_len), F32),
                V((PB * pass_len, pair), BF),
                V((requests, pass_len, pair), BF),
                V((tok_rows, pair), BF),
                V((st_n, depth, pass_len, pair), BF),
                V((st_n, pass_rows, hot_cols), BF),
                V((pass_rows, pair), BF),
                V((tp_n, sto_pair, pair), BF),
                V((model, cols), BF),
                V((2, share, cols), BF),
                V((2, share, cols), BF),
                V((tp_n, tok_pair, model), BF),
                V((hi_n, tok_pair, model), BF),
                V((hi_n, tok_pair, model), BF),
                DMA((8,)),
                DMA((3, hi_n, 2 * n_some)),
                DMA((tp_n, 2 * n_some)),
                DMA((2, st_n, n_some, 3)),
                DMA((2, st_n, n_some, 2)),
                DMA((3, st_n)),
                DMA((3, st_n)),
                DMA((hi_n,)),
                DMA((hi_n,)),
                DMA((hi_n,)),
                DMA((hi_n,)),
                DMA((5, hi_n)),
                DMA((5, tp_n)),
                DMA((2, tp_n)),
                DMA((2, tp_n)),
                DMA((5, 2)),
                DMA((5, 2)),
            ],
            compiler_params=pltpu.CompilerParams(
                collective_id=0, has_side_effects=True, vmem_limit_bytes=67043328
            ),
        )(
            ids, req_of, ask, store.reshape(pass_rows, chunk),
            queries, gate_pre, w_query, w_gate, w_key, w_value, d_mem,
        )
        return d_tokens, d_store.reshape(passages // tp_n, pass_len, model), d_wkey
    d_tokens, d_store, d_wkey = pl.pallas_call(
        functools.partial(kernel, st_n, tp_n, depth, pass_len),
        out_shape=(
            jax.ShapeDtypeStruct((tok_pair, model), BF),
            jax.ShapeDtypeStruct((sto_pair, model), BF),
            jax.ShapeDtypeStruct((share, cols), F32),
        ),
        in_specs=[smem, smem, vmem] + [hbm] * 8,
        out_specs=(vmem, vmem, vmem),
        scratch_shapes=[
            V((tp_n, pass_rows, chunk), BF),
            V((model, pair), BF),
            V((model, pair), BF),
            V((tok_rows, cols), BF),
            V((tok_rows, cols), BF),
            V((tok_rows, cols), BF),
            V((pass_rows, pair), F32),
            V((passages, pass_len, pair), BF),
            V((st_n, 8, width), jnp.int32),
            pltpu.SMEM((st_n, 8, width), jnp.int32),
            V((st_n, depth, pass_len, pair), BF),
            V((st_n, depth, pass_len, cols), BF),
            V((st_n, depth, pass_len, cols), BF),
            V((st_n, depth, pass_len, pair), BF),
            V((cols // HD, tok_rows, PB * pass_len), F32),
            V((PB * pass_len, pair), BF),
            V((requests, pass_len, pair), BF),
            V((tok_rows, pair), BF),
            V((st_n, depth, pass_len, pair), BF),
            V((st_n, pass_rows, hot_cols), BF),
            V((pass_rows, pair), BF),
            V((model, cols), BF),
            V((st_n, share, cols), BF),
            V((tp_n, tok_pair, model), BF),
            V((hi_n, tok_pair, model), BF),
            V((hi_n, tok_pair, model), BF),
            V((tp_n, sto_pair, model), BF),
            V((hi_n, sto_pair, model), BF),
            V((hi_n, sto_pair, model), BF),
            DMA((9,)),
            DMA((3, hi_n)),
            DMA((tp_n,)),
            DMA((6, st_n)),
            DMA((6, st_n)),
            DMA((2, hi_n)),
            DMA((2, hi_n)),
            DMA((2, hi_n)),
            DMA((2, hi_n)),
        ],
        compiler_params=pltpu.CompilerParams(
            collective_id=0, has_side_effects=True, vmem_limit_bytes=67043328
        ),
    )(
        slots, req_of, ask, store.reshape(pass_rows, chunk),
        queries, gate_pre, w_query, w_gate, w_key, w_value, d_mem,
    )
    return d_tokens, d_store.reshape(passages // tp_n, pass_len, model), d_wkey


def solution(mesh):
    return jax.shard_map(
        local,
        mesh=mesh,
        in_specs=(
            P(("grp", "st"), None),
            P("st", None, "tp"),
            P(("grp", "st"), "tp"),
            P(("grp", "st"), "tp"),
            P(None, "tp"),
            P(None, "tp"),
            P(None, "tp"),
            P(None, "tp"),
            P(("grp", "st"), "tp"),
        ),
        out_specs=(
            P(("grp", "st", "tp"), None),
            P(("grp", "st", "tp"), None, None),
            P(("grp", "st"), "tp"),
        ),
        check_vma=False,
    )
```

```python
import functools

import jax
import jax.numpy as jnp
from jax import lax
from jax.experimental import pallas as pl
from jax.experimental.pallas import tpu as pltpu
from jax.sharding import PartitionSpec as P

HD = 256
BLK = 128
PB = 4
BF = jnp.bfloat16
F32 = jnp.float32
MESH = pl.DeviceIdType.MESH
NT = (((1,), (1,)), ((), ()))
TN = (((0,), (0,)), ((), ()))


def dot(a, b, dims=(((1,), (0,)), ((), ()))):
    return lax.dot_general(a, b, dims, preferred_element_type=F32)


def remote(src, dst, send, recv, device):
    return pltpu.make_async_remote_copy(
        src_ref=src,
        dst_ref=dst,
        send_sem=send,
        recv_sem=recv,
        device_id=device,
        device_id_type=MESH,
    )


def tile_of(size, most):
    while size % most:
        most //= 2
    return most


def kernel(
    st_n, tp_n, depth, pass_len,
    slot_ref, req_ref, ask_ref, store_ref, q_hbm, g_hbm, wq_hbm, wg_hbm, wk_hbm, wv_hbm, m_hbm,
    tok_out, store_out, wkey_out,
    rows, wkv, wqg, q_v, g_v, m_v, acc, kv, ask_in, ask_s, out, inc_k, inc_v, ret, prob_v, kvb, reqg, gboth, arr,
    hot, plow, dwp, dwr, tp_part, tp_pair, tp_recv, sp_part, sp_pair, sp_recv,
    lsem, gs, gr, zs, zr, ps, pr, xs, xr,
):
    st = lax.axis_index("st")
    tp = lax.axis_index("tp")
    hi_n = tp_n // 2
    hi, lo = tp // 2, tp % 2
    mate = {"tp": hi * 2 + 1 - lo}
    pass_rows, chunk = rows.shape[1], rows.shape[2]
    model = wqg.shape[0]
    cols = q_v.shape[1]
    heads = cols // HD
    tok_rows = q_v.shape[0]
    blocks = tok_rows // BLK
    blk_keys = PB * pass_len

    def local(i, src, dst):
        copy = pltpu.make_async_copy(src, dst, lsem.at[i])
        copy.start()
        return copy

    own_rows = local(0, store_ref, rows.at[tp])
    loads_kv = [
        local(1, wk_hbm, wkv.at[:, pl.ds(0, cols)]),
        local(2, wv_hbm, wkv.at[:, pl.ds(cols, cols)]),
    ]
    loads_q = [local(3, q_hbm, q_v), local(4, g_hbm, g_v), local(5, m_hbm, m_v)]
    loads_qg = [
        local(6, wq_hbm, wqg.at[:, pl.ds(0, cols)]),
        local(7, wg_hbm, wqg.at[:, pl.ds(cols, cols)]),
    ]

    barrier = pltpu.get_barrier_semaphore()

    def greet_st(d, c):
        pl.semaphore_signal(
            barrier, inc=1, device_id={"st": (st + d) % st_n}, device_id_type=MESH
        )
        return c

    lax.fori_loop(1, st_n, greet_st, 0)
    for d in range(1, tp_n):
        pl.semaphore_signal(
            barrier, inc=1, device_id={"tp": (tp + d) % tp_n}, device_id_type=MESH
        )
    pl.semaphore_wait(barrier, st_n - 1 + tp_n - 1)

    across = []
    for d in range(1, hi_n):
        h = (hi + d) % hi_n
        across.append(
            remote(store_ref, rows.at[tp], gs.at[0, h], gr.at[tp], {"tp": h * 2 + lo})
        )
        across[-1].start()
    beside = remote(store_ref, rows.at[tp], gs.at[1, hi], gr.at[tp], mate)
    beside.start()

    upper = st >= st_n // 2
    mark = jnp.where(upper, st, st_n - 1 - st)

    def far_peer(d):
        i = d - 1
        i = i + jnp.where(i >= mark, 1, 0)
        return jnp.where(upper, i, st_n - 1 - i)

    def z_copy(phase, src, dst, peer):
        return remote(src, dst, zs.at[phase, peer], zr.at[phase, st], {"st": peer})

    def z_wait(phase, src, dst, peer):
        remote(src, dst, zs.at[phase, peer], zr.at[phase, peer], {"st": peer}).wait_recv()

    def ask_send(d, c):
        peer = (st + d) % st_n
        z_copy(0, ask_ref.at[peer], ask_in.at[st], peer).start()
        return c

    lax.fori_loop(1, st_n, ask_send, 0)
    ask_in[st] = ask_ref[st]

    m_tile = tile_of(pass_rows, 256)

    def project(t, first):
        def step(i, c):
            r = pl.ds(pl.multiple_of(i * m_tile, m_tile), m_tile)
            part = dot(rows[t, r], wkv[pl.ds(pl.multiple_of(t * chunk, chunk), chunk), :])
            acc[r] = part if first else acc[r] + part
            return c

        lax.fori_loop(0, pass_rows // m_tile, step, 0)

    def g_wait(t):
        remote(store_ref, rows.at[t], gs.at[1, hi], gr.at[t], mate).wait_recv()

    own_rows.wait()
    for copy in loads_kv:
        copy.wait()
    project(tp, True)
    g_wait(hi * 2 + 1 - lo)
    project(hi * 2 + 1 - lo, False)

    def ask_wait(d, c):
        peer = (st + d) % st_n
        z_wait(0, ask_ref.at[peer], ask_in.at[peer], peer)
        return c

    lax.fori_loop(1, st_n, ask_wait, 0)
    ask_copy = local(8, ask_in, ask_s)
    ask_copy.wait()

    hot_cols = depth * pass_len

    def hot_step(o, c):
        target = ask_in[o][0:1, :hot_cols]
        for i in range(pass_rows // m_tile):
            line = lax.broadcasted_iota(jnp.int32, (m_tile, hot_cols), 0) + i * m_tile
            hot[o, i * m_tile : (i + 1) * m_tile, :] = jnp.where(line == target, 1.0, 0.0).astype(BF)
        return c

    lax.fori_loop(0, st_n, hot_step, 0)
    onward = []
    for d in range(1, hi_n):
        h = (hi + d) % hi_n
        t = h * 2 + lo
        g_wait(t)
        onward.append(remote(rows.at[t], rows.at[t], gs.at[2, h], gr.at[t], mate))
        onward[-1].start()
        project(t, False)
    for d in range(1, hi_n):
        t = ((hi + d) % hi_n) * 2 + 1 - lo
        g_wait(t)
        project(t, False)

    def low_step(i, c):
        kv[i] = acc[pl.ds(pl.multiple_of(i * pass_len, pass_len), pass_len), :].astype(BF)
        return c

    lax.fori_loop(0, pass_rows // pass_len, low_step, 0)

    ks, vs_all = pl.ds(0, cols), pl.ds(cols, cols)

    def half(ref, peer, part):
        return ref.at[peer, :, :, part]

    def key_copy(peer):
        return z_copy(1, half(out, peer, ks), inc_k.at[st], peer)

    def value_copy(peer):
        return z_copy(4, half(out, peer, vs_all), inc_v.at[st], peer)

    def kv_send(d, c):
        peer = far_peer(d)
        for k in range(depth):
            out[peer, k] = kv[ask_s[peer, 1, k]]
        key_copy(peer).start()
        return c

    def value_send(d, c):
        value_copy(far_peer(d)).start()
        return c

    lax.fori_loop(1, st_n, kv_send, 0)
    lax.fori_loop(1, st_n, value_send, 0)
    for k in range(depth):
        picked = kv[ask_s[st, 1, k]]
        inc_k[st, k] = picked[:, :cols]
        inc_v[st, k] = picked[:, cols:]
    for copy in loads_q + loads_qg:
        copy.wait()

    def key_wait(d, c):
        peer = (st + d) % st_n
        z_wait(1, half(out, peer, ks), inc_k.at[peer], peer)
        return c

    lax.fori_loop(1, st_n, key_wait, 0)
    scale = HD ** (-0.5)

    def probs_step(b, c):
        r = pl.ds(pl.multiple_of(b * BLK, BLK), BLK)
        for j in range(PB):
            kvb[j * pass_len : (j + 1) * pass_len, :cols] = inc_k[
                slot_ref[0, b * PB + j], slot_ref[1, b * PB + j]
            ]
        for head in range(heads):
            hs = slice(head * HD, (head + 1) * HD)
            vs = slice(cols + head * HD, cols + (head + 1) * HD)
            gate = g_v[r, hs].astype(F32)
            scores = dot(q_v[r, hs], kvb[:, hs], NT) * scale
            shifted = jnp.exp(scores - jnp.max(scores, axis=-1, keepdims=True))
            prob = shifted / jnp.sum(shifted, axis=-1, keepdims=True)
            prob_v[head, r, :] = prob
            sig = 1.0 / (1.0 + jnp.exp(-gate))
            att_grad = (gate * sig * m_v[r, hs].astype(F32)).astype(BF)
            value_grad = dot(prob.astype(BF), att_grad, TN).astype(BF)
            for j in range(PB):
                reqg[b * PB + j, :, vs] = value_grad[j * pass_len : (j + 1) * pass_len]
        return c

    lax.fori_loop(0, blocks, probs_step, 0)

    def back_copy(phase, part, peer):
        return z_copy(phase, half(ret, peer, part), half(arr, st, part), peer)

    def give_back(phase, part, span):
        def send(d, c):
            peer = far_peer(d)
            for k in range(depth):
                ret[peer, k, :, span] = reqg[req_ref[peer, k]][:, span]
            back_copy(phase, part, peer).start()
            return c

        lax.fori_loop(1, st_n, send, 0)
        for k in range(depth):
            arr[st, k, :, span] = reqg[req_ref[st, k]][:, span]

    give_back(2, vs_all, slice(cols, 2 * cols))

    def value_wait(d, c):
        peer = (st + d) % st_n
        z_wait(4, half(out, peer, vs_all), inc_v.at[peer], peer)
        return c

    lax.fori_loop(1, st_n, value_wait, 0)

    def block_step(b, c):
        r = pl.ds(pl.multiple_of(b * BLK, BLK), BLK)
        for j in range(PB):
            o, k = slot_ref[0, b * PB + j], slot_ref[1, b * PB + j]
            kvb[j * pass_len : (j + 1) * pass_len, :cols] = inc_k[o, k]
            kvb[j * pass_len : (j + 1) * pass_len, cols:] = inc_v[o, k]
        for head in range(heads):
            hs = slice(head * HD, (head + 1) * HD)
            vs = slice(cols + head * HD, cols + (head + 1) * HD)
            q = q_v[r, hs]
            key = kvb[:, hs]
            value = kvb[:, vs]
            gate = g_v[r, hs].astype(F32)
            grad = m_v[r, hs].astype(F32)
            prob = prob_v[head, r, :]
            attended = dot(prob.astype(BF), value)
            sig = 1.0 / (1.0 + jnp.exp(-gate))
            att_grad = (gate * sig * grad).astype(BF)
            gboth[r, vs] = (grad * attended * sig * (1.0 + gate * (1.0 - sig))).astype(BF)
            prob_grad = dot(att_grad, value, NT)
            inner = jnp.sum(prob * prob_grad, axis=-1, keepdims=True)
            score_grad = (scale * prob * (prob_grad - inner)).astype(BF)
            gboth[r, hs] = dot(score_grad, key).astype(BF)
            key_grad = dot(score_grad, q, TN).astype(BF)
            for j in range(PB):
                reqg[b * PB + j, :, hs] = key_grad[j * pass_len : (j + 1) * pass_len]
        return c

    lax.fori_loop(0, blocks, block_step, 0)
    give_back(5, ks, slice(0, cols))

    n_tile = tile_of(model, 512)

    def expand(src, weight, part, pair_rows, t):
        base = pl.multiple_of(t * pair_rows, pair_rows)
        a = src[pl.ds(base, pair_rows), :]

        def step(i, c):
            n = pl.ds(pl.multiple_of(i * n_tile, n_tile), n_tile)
            part[t, :, n] = dot(a, weight[n, :], NT).astype(BF)
            return c

        lax.fori_loop(0, model // n_tile, step, 0)

    def pair_copy(which, part, pair, h):
        return remote(part.at[h * 2 + 1 - lo], pair.at[h], ps.at[which, h], pr.at[which, h], mate)

    def scatter_first(which, src, weight, part, pair, pair_rows):
        for d in range(1, hi_n + 1):
            h = (hi + d) % hi_n
            expand(src, weight, part, pair_rows, h * 2 + 1 - lo)
            pair_copy(which, part, pair, h).start()

    def cross(which, send, recv, h):
        return remote(
            send.at[h * 2 + lo], recv.at[hi], xs.at[which, h], xr.at[which, hi], {"tp": h * 2 + lo}
        )

    def scatter_second(which, src, weight, part, pair, send, recv, pair_rows):
        for d in range(1, hi_n + 1):
            h = (hi + d) % hi_n
            expand(src, weight, part, pair_rows, h * 2 + lo)
            pair_copy(which, part, pair, h).wait_recv()
            if d < hi_n:
                part[h * 2 + lo] = (part[h * 2 + lo].astype(F32) + pair[h].astype(F32)).astype(BF)
                cross(which, part, recv, h).start()

    def scatter_last(which, part, pair, send, recv, result):
        for d in range(1, hi_n):
            h = (hi + d) % hi_n
            remote(
                send.at[h * 2 + lo], recv.at[h], xs.at[which, h], xr.at[which, h], {"tp": h * 2 + lo}
            ).wait_recv()
        total = part[tp].astype(F32) + pair[hi].astype(F32)
        for d in range(1, hi_n):
            total = total + recv[(hi + d) % hi_n].astype(F32)
        result[...] = total.astype(BF)

    tok_pair = tok_rows // tp_n
    sto_pair = pass_rows // tp_n
    scatter_first(0, gboth, wqg, tp_part, tp_pair, tok_pair)
    scatter_second(0, gboth, wqg, tp_part, tp_pair, tp_part, tp_recv, tok_pair)

    def gather_sums(o, span, first):
        def step(i, c):
            r = pl.ds(pl.multiple_of(i * m_tile, m_tile), m_tile)
            part = dot(hot[o, r, :], arr[o, :, :, span].reshape(hot_cols, cols))
            acc[r, span] = part if first else acc[r, span] + part
            return c

        lax.fori_loop(0, pass_rows // m_tile, step, 0)

    for phase, part, span in ((2, vs_all, slice(cols, 2 * cols)), (5, ks, slice(0, cols))):
        gather_sums(st, span, True)

        def grad_wait(d, c):
            peer = (st + d) % st_n
            z_wait(phase, half(ret, peer, part), half(arr, peer, part), peer)
            gather_sums(peer, span, False)
            return c

        lax.fori_loop(1, st_n, grad_wait, 0)
        plow[:, span] = acc[:, span].astype(BF)

    scatter_first(1, plow, wkv, sp_part, sp_pair, sto_pair)

    def wkey_step(t, c):
        dwp[pl.ds(pl.multiple_of(t * chunk, chunk), chunk), :] = dot(
            rows[t], plow[:, :cols], TN
        ).astype(BF)
        return c

    lax.fori_loop(0, tp_n, wkey_step, 0)
    share = model // st_n

    def part_of(s):
        return dwp.at[pl.ds(pl.multiple_of(s * share, share), share), :]

    def wkey_send(d, c):
        peer = far_peer(d)
        z_copy(3, part_of(peer), dwr.at[st], peer).start()
        return c

    lax.fori_loop(1, st_n, wkey_send, 0)
    scatter_second(1, plow, wkv, sp_part, sp_pair, sp_part, sp_recv, sto_pair)
    scatter_last(0, tp_part, tp_pair, tp_part, tp_recv, tok_out)
    wkey_out[...] = part_of(st)[...].astype(F32)

    def wkey_wait(d, c):
        peer = (st + d) % st_n
        z_wait(3, part_of(peer), dwr.at[peer], peer)
        wkey_out[...] += dwr[peer].astype(F32)
        return c

    lax.fori_loop(1, st_n, wkey_wait, 0)
    scatter_last(1, sp_part, sp_pair, sp_part, sp_recv, store_out)

    for copy in across + [beside] + onward:
        copy.wait_send()

    def drain(d, c):
        peer = (st + d) % st_n
        z_copy(0, ask_ref.at[peer], ask_in.at[st], peer).wait_send()
        key_copy(peer).wait_send()
        value_copy(peer).wait_send()
        back_copy(2, vs_all, peer).wait_send()
        back_copy(5, ks, peer).wait_send()
        z_copy(3, part_of(peer), dwr.at[st], peer).wait_send()
        return c

    lax.fori_loop(1, st_n, drain, 0)
    for d in range(1, hi_n + 1):
        h = (hi + d) % hi_n
        pair_copy(0, tp_part, tp_pair, h).wait_send()
        pair_copy(1, sp_part, sp_pair, h).wait_send()
        if d < hi_n:
            cross(0, tp_part, tp_recv, h).wait_send()
            cross(1, sp_part, sp_recv, h).wait_send()


def gathered_kernel(
    st_n, tp_n, depth, pass_len,
    ids_ref, req_ref, ask_ref, store_ref, q_hbm, g_hbm, wq_hbm, wg_hbm, wk_hbm, wv_hbm, m_hbm,
    tok_out, store_out, wkey_out,
    rows, wall, wqg, q_v, g_v, m_v, acc, terms, k_all, v_all, ask_in, ret, prob_v, kvb, reqg, gboth, arr,
    hot, plow, sums, dwp, dwc, dwf, tp_part, tp_pair, tp_recv,
    lsem, gs, gr, fs, fr, zs, zr, ps, pr, xs, xr, ws, wr, ss, sr, us, ur,
):
    grp = lax.axis_index("grp")
    st = lax.axis_index("st")
    tp = lax.axis_index("tp")
    hi_n = tp_n // 2
    hi, lo = tp // 2, tp % 2
    mate_t = hi * 2 + 1 - lo
    mate = {"tp": mate_t}
    twin = {"grp": 1 - grp}
    pass_rows, chunk = rows.shape[1], rows.shape[2]
    passages = pass_rows // pass_len
    model = wqg.shape[0]
    cols = q_v.shape[1]
    heads = cols // HD
    tok_rows = q_v.shape[0]
    blocks = tok_rows // BLK
    half_pass = passages // 2
    some = tile_of(half_pass, 2)
    some_rows = some * pass_len
    n_some = half_pass // some
    key_cols, value_cols = slice(0, cols), slice(cols, 2 * cols)

    def local(i, src, dst):
        copy = pltpu.make_async_copy(src, dst, lsem.at[i])
        copy.start()
        return copy

    own_rows = local(0, store_ref, rows.at[tp])
    loads_kv = [
        local(1, wk_hbm, wall.at[tp, :, pl.ds(0, cols)]),
        local(2, wv_hbm, wall.at[tp, :, pl.ds(cols, cols)]),
    ]
    loads_q = [
        local(3, q_hbm, q_v),
        local(4, g_hbm, g_v),
        local(5, m_hbm, m_v),
        local(6, wq_hbm, wqg.at[:, pl.ds(0, cols)]),
        local(7, wg_hbm, wqg.at[:, pl.ds(cols, cols)]),
    ]

    barrier = pltpu.get_barrier_semaphore()

    def greet_st(d, c):
        pl.semaphore_signal(
            barrier, inc=1, device_id={"st": (st + d) % st_n}, device_id_type=MESH
        )
        return c

    lax.fori_loop(1, st_n, greet_st, 0)
    for d in range(1, tp_n):
        pl.semaphore_signal(
            barrier, inc=1, device_id={"tp": (tp + d) % tp_n}, device_id_type=MESH
        )
    pl.semaphore_signal(barrier, inc=1, device_id=twin, device_id_type=MESH)
    pl.semaphore_wait(barrier, st_n + tp_n - 1)

    def first_row(i):
        part = (grp + i // n_some) % 2
        return pl.multiple_of((part * n_some + i % n_some) * some_rows, some_rows)

    def g_copy(way, i, t, source, peer, slot):
        r = pl.ds(first_row(i), some_rows)
        return remote(rows.at[source, r], rows.at[t, r], gs.at[way, slot, i], gr.at[t, i], peer)

    def across(d, i):
        h = (hi + d) % hi_n
        return g_copy(0, i, tp, tp, {"tp": h * 2 + lo}, h)

    def beside(i):
        return g_copy(1, i, tp, tp, mate, hi)

    def onward(d, i):
        h = (hi + d) % hi_n
        return g_copy(2, i, h * 2 + lo, h * 2 + lo, mate, h)

    def g_wait(t, i):
        g_copy(1, i, t, t, mate, hi).wait_recv()

    def rows_send(i, c):
        for d in range(1, hi_n):
            across(d, i).start()
        beside(i).start()
        return c

    own_rows.wait()
    lax.fori_loop(0, 2 * n_some, rows_send, 0)

    upper = st >= st_n // 2
    mark = jnp.where(upper, st, st_n - 1 - st)

    def far_peer(d):
        i = d - 1
        i = i + jnp.where(i >= mark, 1, 0)
        return jnp.where(upper, i, st_n - 1 - i)

    def z_copy(phase, src, dst, peer):
        return remote(src, dst, zs.at[phase, peer], zr.at[phase, st], {"st": peer})

    def z_wait(phase, src, dst, peer):
        remote(src, dst, zs.at[phase, peer], zr.at[phase, peer], {"st": peer}).wait_recv()

    def ask_send(d, c):
        peer = (st + d) % st_n
        z_copy(0, ask_ref.at[peer], ask_in.at[st], peer).start()
        return c

    lax.fori_loop(1, st_n, ask_send, 0)
    ask_in[st] = ask_ref[st]

    def project(i, send):
        r = pl.ds(first_row(i), some_rows)

        def term(t, span):
            return dot(rows[t, r], wall[tp, pl.ds(pl.multiple_of(t * chunk, chunk), chunk), span])

        for d in range(1, hi_n):
            g_wait(((hi + d) % hi_n) * 2 + lo, i)
            onward(d, i).start()
        g_wait(mate_t, i)
        near = [tp, mate_t] + [((hi + d) % hi_n) * 2 + lo for d in range(1, hi_n)]
        late = [((hi + d) % hi_n) * 2 + 1 - lo for d in range(1, hi_n)]
        total = sum(term(t, key_cols) for t in near[1:]) + term(near[0], key_cols)
        for t in late:
            g_wait(t, i)
            total = total + term(t, key_cols)
        low = total.astype(BF)
        first = st * passages + first_row(i) // pass_len
        for p in range(some):
            k_all[first + p] = low[p * pass_len : (p + 1) * pass_len]
        send()
        total = sum(term(t, value_cols) for t in near + late)
        low = total.astype(BF)
        for p in range(some):
            v_all[first + p] = low[p * pass_len : (p + 1) * pass_len]

    def part_of_all(kind, o, c, side):
        ref = k_all if kind == 0 else v_all
        return ref.at[pl.ds(o * passages + side * half_pass + c * some, some)]

    def chain_copy(kind, o, c, way, peer):
        part = part_of_all(kind, o, c, grp)
        return remote(part, part, fs.at[kind, o, c, way], fr.at[kind, o, c, 0], {"st": peer})

    def twin_copy(kind, o, c):
        part = part_of_all(kind, o, c, grp)
        return remote(part, part, fs.at[kind, o, c, 2], fr.at[kind, o, c, 1], twin)

    lower = st < st_n // 2

    def own_copies(kind, c, act, inward=True, outward=True):
        ways = ((0, st + 1, lower), (1, st - 1, jnp.logical_not(lower)))
        for way, onto, toward in ways:
            there = (onto >= 0) & (onto < st_n)
            if not outward:
                there = there & toward
            if not inward:
                there = there & jnp.logical_not(toward)

            @pl.when(there)
            def _():
                act(chain_copy(kind, st, c, way, onto))

    def relay_copies(kind, d, c, act, ready):
        for way, sign in ((0, -1), (1, 1)):
            o = st + sign * d
            onto = st - sign

            @pl.when((o >= 0) & (o < st_n))
            def _():
                if ready:
                    chain_copy(kind, o, c, way, st).wait_recv()

                @pl.when((onto >= 0) & (onto < st_n))
                def _():
                    act(chain_copy(kind, o, c, way, onto))

                act(twin_copy(kind, o, c))

    def start(copy):
        copy.start()

    def own_send(kind, c, **which):
        own_copies(kind, c, start, **which)

    def relay(kind, d, c):
        relay_copies(kind, d, c, start, True)

    def twin_wait(kind):
        def step(i, c):
            o = (st + 1 + i // n_some) % st_n
            k = i % n_some
            part = part_of_all(kind, o, k, 1 - grp)
            remote(part, part, fs.at[kind, o, k, 2], fr.at[kind, o, k, 1], twin).wait_recv()
            return c

        lax.fori_loop(0, (st_n - 1) * n_some, step, 0)

    for copy in loads_kv:
        copy.wait()

    def early_step(i, c):
        project(i, lambda: own_send(0, i))

        @pl.when(i > 0)
        def _():
            relay(0, 1, i - 1)

        return c

    lax.fori_loop(0, n_some, early_step, 0)
    relay(0, 1, n_some - 1)

    def inward_send(i, c):
        own_send(1, i, outward=False)
        return c

    lax.fori_loop(0, n_some, inward_send, 0)

    def second_step(i, c):
        relay(0, 2, i)
        return c

    def outward_send(i, c):
        own_send(1, i, inward=False)
        return c

    lax.fori_loop(0, n_some, second_step, 0)
    lax.fori_loop(0, n_some, outward_send, 0)

    def late_step(i, c):
        project(n_some + i, lambda: None)

        @pl.when(edge)
        def _():
            relay(0, 3, i)

        @pl.when(jnp.logical_not(edge))
        def _():
            relay(1, 1, i)

        return c

    w_part = model // 2
    w_mine = pl.ds(pl.multiple_of(grp * w_part, w_part), w_part)
    w_other = pl.ds(pl.multiple_of((1 - grp) * w_part, w_part), w_part)

    def w_across(d):
        h = (hi + d) % hi_n
        part = wall.at[tp, w_mine]
        return remote(part, part, ws.at[0, h], wr.at[0, tp], {"tp": h * 2 + lo})

    def w_twin(d):
        t = ((hi + d) % hi_n) * 2 + lo
        part = wall.at[t, w_mine]
        return remote(part, part, ws.at[1, (hi + d) % hi_n], wr.at[1, t], twin)

    def w_onward(d, k):
        t = ((hi + d) % hi_n) * 2 + lo
        part = wall.at[t, w_other if k else w_mine]
        return remote(part, part, ws.at[2 + k, (hi + d) % hi_n], wr.at[2 + k, t], mate)

    w_beside = remote(wall.at[tp], wall.at[tp], ws.at[4, 0], wr.at[4, tp], mate)

    def w_wait(kind, t, part):
        remote(wall.at[t, part], wall.at[t, part], ws.at[kind, 0], wr.at[kind, t], mate).wait_recv()

    for d in range(1, hi_n):
        w_across(d).start()

    def relay_rest(kind, first, last):
        def step(i, c):
            relay(kind, 1 + i // n_some, i % n_some)
            return c

        lax.fori_loop(first, last, step, 0)

    relays = (st_n - 1) * n_some
    edge = (st == 0) | (st == st_n - 1)
    lax.fori_loop(0, n_some, late_step, 0)
    w_beside.start()
    relay_rest(1, 0, jnp.where(edge, n_some // 2, 0))
    for copy in loads_q:
        copy.wait()
    twin_wait(0)
    scale = HD ** (-0.5)

    def fill(ref, span, b):
        for j in range(PB):
            kvb[j * pass_len : (j + 1) * pass_len, span] = ref[ids_ref[b * PB + j]]

    def probs_step(b, c):
        r = pl.ds(pl.multiple_of(b * BLK, BLK), BLK)
        fill(k_all, key_cols, b)
        for head in range(heads):
            hs = slice(head * HD, (head + 1) * HD)
            vs = slice(cols + head * HD, cols + (head + 1) * HD)
            gate = g_v[r, hs].astype(F32)
            scores = dot(q_v[r, hs], kvb[:, hs], NT) * scale
            shifted = jnp.exp(scores - jnp.max(scores, axis=-1, keepdims=True))
            prob = shifted / jnp.sum(shifted, axis=-1, keepdims=True)
            prob_v[head, r, :] = prob
            sig = 1.0 / (1.0 + jnp.exp(-gate))
            att_grad = (gate * sig * m_v[r, hs].astype(F32)).astype(BF)
            value_grad = dot(prob.astype(BF), att_grad, TN).astype(BF)
            for j in range(PB):
                reqg[b * PB + j, :, vs] = value_grad[j * pass_len : (j + 1) * pass_len]

        @pl.when((b < n_some) & jnp.logical_not(edge))
        def _():
            relay(1, 2, b)

        @pl.when((b < n_some) & edge & (b % 2 == 1))
        def _():
            relay(1, 1, n_some // 2 + b // 2)

        return c

    lax.fori_loop(0, blocks, probs_step, 0)

    def half(ref, peer, part):
        return ref.at[peer, :, :, part]

    def back_copy(phase, part, peer):
        return z_copy(phase, half(ret, peer, part), half(arr, st, part), peer)

    def give_back(phase, part, span, order, first, last):
        def send(d, c):
            peer = order(d)
            for k in range(depth):
                ret[peer, k, :, span] = reqg[req_ref[peer, k]][:, span]
            back_copy(phase, part, peer).start()
            return c

        lax.fori_loop(first, last, send, 0)

    def keep_own(span):
        for k in range(depth):
            arr[st, k, :, span] = reqg[req_ref[st, k]][:, span]

    def near_peer(d):
        return far_peer(st_n - d)

    ks, vs_all = pl.ds(0, cols), pl.ds(cols, cols)
    give_back(1, vs_all, value_cols, near_peer, 1, jnp.where(edge, st_n, st_n - 1))
    keep_own(value_cols)
    relay_rest(1, jnp.where(edge, n_some, 2 * n_some), relays)
    twin_wait(1)

    def block_step(b, c):
        r = pl.ds(pl.multiple_of(b * BLK, BLK), BLK)
        fill(k_all, key_cols, b)
        fill(v_all, value_cols, b)
        for head in range(heads):
            hs = slice(head * HD, (head + 1) * HD)
            vs = slice(cols + head * HD, cols + (head + 1) * HD)
            q = q_v[r, hs]
            key = kvb[:, hs]
            value = kvb[:, vs]
            gate = g_v[r, hs].astype(F32)
            grad = m_v[r, hs].astype(F32)
            prob = prob_v[head, r, :]
            attended = dot(prob.astype(BF), value)
            sig = 1.0 / (1.0 + jnp.exp(-gate))
            att_grad = (gate * sig * grad).astype(BF)
            gboth[r, vs] = (grad * attended * sig * (1.0 + gate * (1.0 - sig))).astype(BF)
            prob_grad = dot(att_grad, value, NT)
            inner = jnp.sum(prob * prob_grad, axis=-1, keepdims=True)
            score_grad = (scale * prob * (prob_grad - inner)).astype(BF)
            gboth[r, hs] = dot(score_grad, key).astype(BF)
            key_grad = dot(score_grad, q, TN).astype(BF)
            for j in range(PB):
                reqg[b * PB + j, :, hs] = key_grad[j * pass_len : (j + 1) * pass_len]
        return c

    lax.fori_loop(0, blocks, block_step, 0)
    give_back(2, ks, key_cols, far_peer, 1, st_n)
    keep_own(key_cols)

    n_tile = tile_of(model, 512)

    def expand(t):
        a = gboth[pl.ds(pl.multiple_of(t * tok_pair, tok_pair), tok_pair), :]

        def step(i, c):
            n = pl.ds(pl.multiple_of(i * n_tile, n_tile), n_tile)
            tp_part[t, :, n] = dot(a, wqg[n, :], NT).astype(BF)
            return c

        lax.fori_loop(0, model // n_tile, step, 0)

    def pair_copy(h):
        return remote(tp_part.at[h * 2 + 1 - lo], tp_pair.at[h], ps.at[h], pr.at[h], mate)

    def cross(h):
        return remote(
            tp_part.at[h * 2 + lo], tp_recv.at[hi], xs.at[h], xr.at[hi], {"tp": h * 2 + lo}
        )

    for d in range(1, hi_n):
        w_wait(0, ((hi + d) % hi_n) * 2 + lo, w_mine)
        w_twin(d).start()
        w_onward(d, 0).start()

    tok_pair = tok_rows // tp_n
    for d in range(1, hi_n + 1):
        h = (hi + d) % hi_n
        expand(h * 2 + 1 - lo)
        pair_copy(h).start()
        expand(h * 2 + lo)
        pair_copy(h).wait_recv()
        if d < hi_n:
            tp_part[h * 2 + lo] = (tp_part[h * 2 + lo].astype(F32) + tp_pair[h].astype(F32)).astype(BF)
            cross(h).start()

    def ask_wait(d, c):
        peer = (st + d) % st_n
        z_wait(0, ask_ref.at[peer], ask_in.at[peer], peer)
        return c

    lax.fori_loop(1, st_n, ask_wait, 0)
    hot_cols = depth * pass_len
    m_tile = tile_of(pass_rows, 256)

    def hot_step(o, c):
        target = ask_in[o][0:1, :hot_cols]
        for i in range(pass_rows // m_tile):
            line = lax.broadcasted_iota(jnp.int32, (m_tile, hot_cols), 0) + i * m_tile
            hot[o, i * m_tile : (i + 1) * m_tile, :] = jnp.where(line == target, 1.0, 0.0).astype(BF)
        return c

    lax.fori_loop(0, st_n, hot_step, 0)

    def gather_sums(kind, o, span, first):
        def step(i, c):
            r = pl.ds(pl.multiple_of(i * m_tile, m_tile), m_tile)
            part = dot(hot[o, r, :], arr[o, :, :, span].reshape(hot_cols, cols))
            acc[kind, r, :] = part if first else acc[kind, r, :] + part
            return c

        lax.fori_loop(0, pass_rows // m_tile, step, 0)

    sto_pair = pass_rows // tp_n

    def sums_copy(kind, part, d):
        t = (tp + d) % tp_n
        src = plow.at[pl.ds(pl.multiple_of(t * sto_pair, sto_pair), sto_pair), part]
        return remote(src, sums.at[tp, :, part], ss.at[kind, t], sr.at[kind, tp], {"tp": t})

    def sums_wait(kind, part, t):
        dst = sums.at[t, :, part]
        remote(dst, dst, ss.at[kind, t], sr.at[kind, t], mate).wait_recv()

    def grads_of(kind, peer):
        phase, part, span = (2, ks, key_cols) if kind == 0 else (1, vs_all, value_cols)
        z_wait(phase, half(ret, peer, part), half(arr, peer, part), peer)
        gather_sums(kind, peer, span, False)

    def sums_send(kind):
        part, span = (ks, key_cols) if kind == 0 else (vs_all, value_cols)
        plow[:, span] = acc[kind].astype(BF)
        for d in range(1, tp_n):
            sums_copy(kind, part, d).start()
        sums[tp, :, span] = plow[pl.ds(pl.multiple_of(tp * sto_pair, sto_pair), sto_pair), span]

    beyond = jnp.where(lower, st_n - 1, 0)
    middle = jnp.where(lower, st_n // 2, st_n // 2 - 1)
    beside_st = st + 1 - 2 * (st % 2)
    outer = edge
    inner = jnp.logical_not(outer)
    gather_sums(1, st, value_cols, True)
    gather_sums(0, st, key_cols, True)
    grads_of(1, beside_st)
    grads_of(1, jnp.where(outer, beyond, middle))

    grads_of(0, middle)

    @pl.when(inner)
    def _():
        give_back(1, vs_all, value_cols, near_peer, st_n - 1, st_n)

    grads_of(0, beyond)
    grads_of(0, beside_st)
    sums_send(0)

    share = model // st_n
    bits = 2
    bit = share // bits

    def dw_line(s, b):
        return pl.ds(pl.multiple_of(s * share + b * bit, bit), bit)

    def dw_copy(kind, b):
        line = pl.ds(b * bit, bit)
        if kind < 2:
            src, dst = dwp.at[dw_line(middle if kind else beyond, b)], dwc.at[kind, line]
            peer = beside_st
        elif kind == 2:
            src, dst, peer = dwp.at[dw_line(beside_st, b)], dwf.at[0, line], beside_st
        else:
            src, dst = dwc.at[kind - 3, line], dwf.at[1, line]
            peer = middle if kind == 4 else beyond
        return remote(src, dst, us.at[kind, b], ur.at[kind, b], {"st": peer})

    def dw_send(kind):
        for b in range(bits):
            dw_copy(kind, b).start()

    def dw_relay(q):
        for b in range(bits):
            line = slice(b * bit, (b + 1) * bit)
            dw_copy(q, b).wait_recv()
            own = dwp[dw_line(middle if q else beyond, b), :].astype(F32)
            dwc[q, line, :] = (dwc[q, line, :].astype(F32) + own).astype(BF)
            dw_copy(3 + q, b).start()

    def wkey_step(s):
        dwp[pl.ds(pl.multiple_of(s * chunk, chunk), chunk), :] = dot(
            rows[s], plow[:, key_cols], TN
        ).astype(BF)

    def wkey_turn(j, c):
        far = jnp.where(j == 0, beyond, middle)
        near = jnp.where(j == 2, beside_st, st)
        near_first = jnp.where(j == 0, beside_st, st)
        far_after = jnp.where(j == 1, beyond, middle)
        s = jnp.where(
            outer, jnp.where(j < 2, far, near), jnp.where((j == 0) | (j == 3), near_first, far_after)
        )
        wkey_step(s)
        for kind in range(3):
            @pl.when(outer & (j == kind))
            def _():
                dw_send(kind)

        @pl.when(inner & (j == 0))
        def _():
            dw_send(2)

        return c

    lax.fori_loop(0, st_n, wkey_turn, 0)

    for d in range(1, hi_n):
        t = ((hi + d) % hi_n) * 2 + lo
        w_wait(1, t, w_other)
        w_onward(d, 1).start()
    w_wait(4, mate_t, pl.ds(0, model))
    for d in range(1, hi_n):
        t = ((hi + d) % hi_n) * 2 + 1 - lo
        w_wait(2, t, w_mine)
        w_wait(3, t, w_other)

    def store_terms(span, done):
        def step(i, c):
            n = pl.ds(pl.multiple_of(i * n_tile, n_tile), n_tile)
            part = dot(sums[0, :, span], wall[0, n, span], NT)
            for t in range(1, tp_n):
                part = part + dot(sums[t, :, span], wall[t, n, span], NT)
            done(n, part)
            return c

        lax.fori_loop(0, model // n_tile, step, 0)

    def keep_terms(n, part):
        terms[:, n] = part

    def keep_store(n, part):
        store_out[:, n] = (terms[:, n] + part).astype(BF)

    @pl.when(inner)
    def _():
        dw_relay(0)

    grads_of(1, jnp.where(outer, middle, beyond))
    sums_send(1)

    for d in range(1, tp_n):
        sums_wait(0, ks, (tp + d) % tp_n)
    store_terms(key_cols, keep_terms)

    for d in range(1, hi_n):
        h = (hi + d) % hi_n
        remote(
            tp_part.at[h * 2 + lo], tp_recv.at[h], xs.at[h], xr.at[h], {"tp": h * 2 + lo}
        ).wait_recv()
    total = tp_part[tp].astype(F32) + tp_pair[hi].astype(F32)
    for d in range(1, hi_n):
        total = total + tp_recv[(hi + d) % hi_n].astype(F32)
    tok_out[...] = total.astype(BF)

    @pl.when(inner)
    def _():
        dw_relay(1)

    for d in range(1, tp_n):
        sums_wait(1, vs_all, (tp + d) % tp_n)
    store_terms(value_cols, keep_store)

    for b in range(bits):
        line = slice(b * bit, (b + 1) * bit)
        dw_copy(2, b).wait_recv()
        wkey_out[line, :] = dwp[dw_line(st, b), :].astype(F32) + dwf[0, line, :].astype(F32)
    for b in range(bits):
        line = slice(b * bit, (b + 1) * bit)
        for kind, edge in ((3, outer), (4, inner)):
            @pl.when(edge)
            def _():
                dw_copy(kind, b).wait_recv()

        wkey_out[line, :] += dwf[1, line, :].astype(F32)

    def wait_send(copy):
        copy.wait_send()

    def rows_drain(i, c):
        for d in range(1, hi_n):
            across(d, i).wait_send()
            onward(d, i).wait_send()
        beside(i).wait_send()
        return c

    lax.fori_loop(0, 2 * n_some, rows_drain, 0)

    def all_drain(i, c):
        for kind in (0, 1):
            own_copies(kind, i, wait_send)
            for d in range(1, st_n):
                relay_copies(kind, d, i, wait_send, False)
        return c

    lax.fori_loop(0, n_some, all_drain, 0)
    for d in range(1, hi_n):
        w_across(d).wait_send()
        w_twin(d).wait_send()
        w_onward(d, 0).wait_send()
        w_onward(d, 1).wait_send()
    w_beside.wait_send()

    def drain(d, c):
        peer = (st + d) % st_n
        z_copy(0, ask_ref.at[peer], ask_in.at[st], peer).wait_send()
        back_copy(1, vs_all, peer).wait_send()
        back_copy(2, ks, peer).wait_send()
        return c

    lax.fori_loop(1, st_n, drain, 0)
    for d in range(1, tp_n):
        sums_copy(0, ks, d).wait_send()
        sums_copy(1, vs_all, d).wait_send()
    for d in range(1, hi_n + 1):
        h = (hi + d) % hi_n
        pair_copy(h).wait_send()
        if d < hi_n:
            cross(h).wait_send()
    for b in range(bits):
        dw_copy(2, b).wait_send()
        for q in (0, 1):
            @pl.when(outer)
            def _():
                dw_copy(q, b).wait_send()

            @pl.when(inner)
            def _():
                dw_copy(3 + q, b).wait_send()


def local(pass_ids, store, queries, gate_pre, w_query, w_gate, w_key, w_value, d_mem):
    st_n = lax.axis_size("st")
    tp_n = lax.axis_size("tp")
    hi_n = tp_n // 2
    tok_rows, cols = queries.shape
    blocks = tok_rows // BLK
    passages, pass_len, chunk = store.shape
    model = w_key.shape[0]
    requests = blocks * PB
    depth = max(2, requests // st_n)
    pass_rows = passages * pass_len
    share = model // st_n

    ids = pass_ids.reshape(-1)
    owners = ids // passages
    within = ids % passages
    order = jnp.arange(requests, dtype=jnp.int32)
    earlier = (owners[None, :] == owners[:, None]) & (order[None, :] < order[:, None])
    rank = jnp.sum(earlier.astype(jnp.int32), axis=1)
    slots = jnp.stack([owners, rank])
    o_i = jnp.arange(st_n, dtype=jnp.int32)[:, None, None]
    k_i = jnp.arange(depth, dtype=jnp.int32)[None, :, None]
    match = (owners[None, None, :] == o_i) & (rank[None, None, :] == k_i)
    asked = jnp.max(jnp.where(match, within[None, None, :], -1), axis=2)
    req_of = jnp.max(jnp.where(match, order[None, None, :], 0), axis=2)
    hot_cols = depth * pass_len
    width = -(-hot_cols // 128) * 128
    lane = jnp.arange(width, dtype=jnp.int32)
    spread = jnp.repeat(asked, pass_len, axis=1)
    spread = jnp.pad(spread, ((0, 0), (0, width - hot_cols)), constant_values=-1)
    target = jnp.where(spread < 0, -1, spread * pass_len + lane[None, :] % pass_len)
    flat = jnp.pad(jnp.maximum(asked, 0), ((0, 0), (0, width - depth)))
    ask = jnp.concatenate(
        [target[:, None], flat[:, None], jnp.zeros((st_n, 6, width), jnp.int32)], axis=1
    )

    vmem = pl.BlockSpec(memory_space=pltpu.VMEM)
    smem = pl.BlockSpec(memory_space=pltpu.SMEM)
    hbm = pl.BlockSpec(memory_space=pl.ANY)
    V = pltpu.VMEM
    DMA = pltpu.SemaphoreType.DMA
    pair = 2 * cols
    tok_pair = tok_rows // tp_n
    sto_pair = pass_rows // tp_n
    gathered_bytes = 2 * 2 * st_n * pass_rows * cols
    if lax.axis_size("grp") == 2 and hi_n == 2 and st_n == 4 and passages % 2 == 0 and gathered_bytes <= 8 << 20:
        half_pass = passages // 2
        n_some = half_pass // tile_of(half_pass, 2)
        d_tokens, d_store, d_wkey = pl.pallas_call(
            functools.partial(gathered_kernel, st_n, tp_n, depth, pass_len),
            out_shape=(
                jax.ShapeDtypeStruct((tok_pair, model), BF),
                jax.ShapeDtypeStruct((sto_pair, model), BF),
                jax.ShapeDtypeStruct((share, cols), F32),
            ),
            in_specs=[smem, smem, vmem] + [hbm] * 8,
            out_specs=(vmem, vmem, vmem),
            scratch_shapes=[
                V((tp_n, pass_rows, chunk), BF),
                V((tp_n, model, pair), BF),
                V((model, pair), BF),
                V((tok_rows, cols), BF),
                V((tok_rows, cols), BF),
                V((tok_rows, cols), BF),
                V((2, pass_rows, cols), F32),
                V((sto_pair, model), F32),
                V((st_n * passages, pass_len, cols), BF),
                V((st_n * passages, pass_len, cols), BF),
                V((st_n, 8, width), jnp.int32),
                V((st_n, depth, pass_len, pair), BF),
                V((cols // HD, tok_rows, PB * pass_len), F32),
                V((PB * pass_len, pair), BF),
                V((requests, pass_len, pair), BF),
                V((tok_rows, pair), BF),
                V((st_n, depth, pass_len, pair), BF),
                V((st_n, pass_rows, hot_cols), BF),
                V((pass_rows, pair), BF),
                V((tp_n, sto_pair, pair), BF),
                V((model, cols), BF),
                V((2, share, cols), BF),
                V((2, share, cols), BF),
                V((tp_n, tok_pair, model), BF),
                V((hi_n, tok_pair, model), BF),
                V((hi_n, tok_pair, model), BF),
                DMA((8,)),
                DMA((3, hi_n, 2 * n_some)),
                DMA((tp_n, 2 * n_some)),
                DMA((2, st_n, n_some, 3)),
                DMA((2, st_n, n_some, 2)),
                DMA((3, st_n)),
                DMA((3, st_n)),
                DMA((hi_n,)),
                DMA((hi_n,)),
                DMA((hi_n,)),
                DMA((hi_n,)),
                DMA((5, hi_n)),
                DMA((5, tp_n)),
                DMA((2, tp_n)),
                DMA((2, tp_n)),
                DMA((5, 2)),
                DMA((5, 2)),
            ],
            compiler_params=pltpu.CompilerParams(
                collective_id=0, has_side_effects=True, vmem_limit_bytes=67043328
            ),
        )(
            ids, req_of, ask, store.reshape(pass_rows, chunk),
            queries, gate_pre, w_query, w_gate, w_key, w_value, d_mem,
        )
        return d_tokens, d_store.reshape(passages // tp_n, pass_len, model), d_wkey
    d_tokens, d_store, d_wkey = pl.pallas_call(
        functools.partial(kernel, st_n, tp_n, depth, pass_len),
        out_shape=(
            jax.ShapeDtypeStruct((tok_pair, model), BF),
            jax.ShapeDtypeStruct((sto_pair, model), BF),
            jax.ShapeDtypeStruct((share, cols), F32),
        ),
        in_specs=[smem, smem, vmem] + [hbm] * 8,
        out_specs=(vmem, vmem, vmem),
        scratch_shapes=[
            V((tp_n, pass_rows, chunk), BF),
            V((model, pair), BF),
            V((model, pair), BF),
            V((tok_rows, cols), BF),
            V((tok_rows, cols), BF),
            V((tok_rows, cols), BF),
            V((pass_rows, pair), F32),
            V((passages, pass_len, pair), BF),
            V((st_n, 8, width), jnp.int32),
            pltpu.SMEM((st_n, 8, width), jnp.int32),
            V((st_n, depth, pass_len, pair), BF),
            V((st_n, depth, pass_len, cols), BF),
            V((st_n, depth, pass_len, cols), BF),
            V((st_n, depth, pass_len, pair), BF),
            V((cols // HD, tok_rows, PB * pass_len), F32),
            V((PB * pass_len, pair), BF),
            V((requests, pass_len, pair), BF),
            V((tok_rows, pair), BF),
            V((st_n, depth, pass_len, pair), BF),
            V((st_n, pass_rows, hot_cols), BF),
            V((pass_rows, pair), BF),
            V((model, cols), BF),
            V((st_n, share, cols), BF),
            V((tp_n, tok_pair, model), BF),
            V((hi_n, tok_pair, model), BF),
            V((hi_n, tok_pair, model), BF),
            V((tp_n, sto_pair, model), BF),
            V((hi_n, sto_pair, model), BF),
            V((hi_n, sto_pair, model), BF),
            DMA((9,)),
            DMA((3, hi_n)),
            DMA((tp_n,)),
            DMA((6, st_n)),
            DMA((6, st_n)),
            DMA((2, hi_n)),
            DMA((2, hi_n)),
            DMA((2, hi_n)),
            DMA((2, hi_n)),
        ],
        compiler_params=pltpu.CompilerParams(
            collective_id=0, has_side_effects=True, vmem_limit_bytes=67043328
        ),
    )(
        slots, req_of, ask, store.reshape(pass_rows, chunk),
        queries, gate_pre, w_query, w_gate, w_key, w_value, d_mem,
    )
    return d_tokens, d_store.reshape(passages // tp_n, pass_len, model), d_wkey


def solution(mesh):
    return jax.shard_map(
        local,
        mesh=mesh,
        in_specs=(
            P(("grp", "st"), None),
            P("st", None, "tp"),
            P(("grp", "st"), "tp"),
            P(("grp", "st"), "tp"),
            P(None, "tp"),
            P(None, "tp"),
            P(None, "tp"),
            P(None, "tp"),
            P(("grp", "st"), "tp"),
        ),
        out_specs=(
            P(("grp", "st", "tp"), None),
            P(("grp", "st", "tp"), None, None),
            P(("grp", "st"), "tp"),
        ),
        check_vma=False,
    )
```

```python
import functools

import jax
import jax.numpy as jnp
from jax import lax
from jax.experimental import pallas as pl
from jax.experimental.pallas import tpu as pltpu
from jax.sharding import PartitionSpec as P

HD = 256
BLK = 128
PB = 4
BF = jnp.bfloat16
F32 = jnp.float32
MESH = pl.DeviceIdType.MESH
NT = (((1,), (1,)), ((), ()))
TN = (((0,), (0,)), ((), ()))


def dot(a, b, dims=(((1,), (0,)), ((), ()))):
    return lax.dot_general(a, b, dims, preferred_element_type=F32)


def remote(src, dst, send, recv, device):
    return pltpu.make_async_remote_copy(
        src_ref=src,
        dst_ref=dst,
        send_sem=send,
        recv_sem=recv,
        device_id=device,
        device_id_type=MESH,
    )


def tile_of(size, most):
    while size % most:
        most //= 2
    return most


def kernel(
    st_n, tp_n, depth, pass_len,
    slot_ref, req_ref, ask_ref, store_ref, q_hbm, g_hbm, wq_hbm, wg_hbm, wk_hbm, wv_hbm, m_hbm,
    tok_out, store_out, wkey_out,
    rows, wkv, wqg, q_v, g_v, m_v, acc, kv, ask_in, ask_s, out, inc_k, inc_v, ret, prob_v, kvb, reqg, gboth, arr,
    hot, plow, dwp, dwr, tp_part, tp_pair, tp_recv, sp_part, sp_pair, sp_recv,
    lsem, gs, gr, zs, zr, ps, pr, xs, xr,
):
    st = lax.axis_index("st")
    tp = lax.axis_index("tp")
    hi_n = tp_n // 2
    hi, lo = tp // 2, tp % 2
    mate = {"tp": hi * 2 + 1 - lo}
    pass_rows, chunk = rows.shape[1], rows.shape[2]
    model = wqg.shape[0]
    cols = q_v.shape[1]
    heads = cols // HD
    tok_rows = q_v.shape[0]
    blocks = tok_rows // BLK
    blk_keys = PB * pass_len

    def local(i, src, dst):
        copy = pltpu.make_async_copy(src, dst, lsem.at[i])
        copy.start()
        return copy

    own_rows = local(0, store_ref, rows.at[tp])
    loads_kv = [
        local(1, wk_hbm, wkv.at[:, pl.ds(0, cols)]),
        local(2, wv_hbm, wkv.at[:, pl.ds(cols, cols)]),
    ]
    loads_q = [local(3, q_hbm, q_v), local(4, g_hbm, g_v), local(5, m_hbm, m_v)]
    loads_qg = [
        local(6, wq_hbm, wqg.at[:, pl.ds(0, cols)]),
        local(7, wg_hbm, wqg.at[:, pl.ds(cols, cols)]),
    ]

    barrier = pltpu.get_barrier_semaphore()

    def greet_st(d, c):
        pl.semaphore_signal(
            barrier, inc=1, device_id={"st": (st + d) % st_n}, device_id_type=MESH
        )
        return c

    lax.fori_loop(1, st_n, greet_st, 0)
    for d in range(1, tp_n):
        pl.semaphore_signal(
            barrier, inc=1, device_id={"tp": (tp + d) % tp_n}, device_id_type=MESH
        )
    pl.semaphore_wait(barrier, st_n - 1 + tp_n - 1)

    across = []
    for d in range(1, hi_n):
        h = (hi + d) % hi_n
        across.append(
            remote(store_ref, rows.at[tp], gs.at[0, h], gr.at[tp], {"tp": h * 2 + lo})
        )
        across[-1].start()
    beside = remote(store_ref, rows.at[tp], gs.at[1, hi], gr.at[tp], mate)
    beside.start()

    upper = st >= st_n // 2
    mark = jnp.where(upper, st, st_n - 1 - st)

    def far_peer(d):
        i = d - 1
        i = i + jnp.where(i >= mark, 1, 0)
        return jnp.where(upper, i, st_n - 1 - i)

    def z_copy(phase, src, dst, peer):
        return remote(src, dst, zs.at[phase, peer], zr.at[phase, st], {"st": peer})

    def z_wait(phase, src, dst, peer):
        remote(src, dst, zs.at[phase, peer], zr.at[phase, peer], {"st": peer}).wait_recv()

    def ask_send(d, c):
        peer = (st + d) % st_n
        z_copy(0, ask_ref.at[peer], ask_in.at[st], peer).start()
        return c

    lax.fori_loop(1, st_n, ask_send, 0)
    ask_in[st] = ask_ref[st]

    m_tile = tile_of(pass_rows, 256)

    def project(t, first):
        def step(i, c):
            r = pl.ds(pl.multiple_of(i * m_tile, m_tile), m_tile)
            part = dot(rows[t, r], wkv[pl.ds(pl.multiple_of(t * chunk, chunk), chunk), :])
            acc[r] = part if first else acc[r] + part
            return c

        lax.fori_loop(0, pass_rows // m_tile, step, 0)

    def g_wait(t):
        remote(store_ref, rows.at[t], gs.at[1, hi], gr.at[t], mate).wait_recv()

    own_rows.wait()
    for copy in loads_kv:
        copy.wait()
    project(tp, True)
    g_wait(hi * 2 + 1 - lo)
    project(hi * 2 + 1 - lo, False)

    def ask_wait(d, c):
        peer = (st + d) % st_n
        z_wait(0, ask_ref.at[peer], ask_in.at[peer], peer)
        return c

    lax.fori_loop(1, st_n, ask_wait, 0)
    ask_copy = local(8, ask_in, ask_s)
    ask_copy.wait()

    hot_cols = depth * pass_len

    def hot_step(o, c):
        target = ask_in[o][0:1, :hot_cols]
        for i in range(pass_rows // m_tile):
            line = lax.broadcasted_iota(jnp.int32, (m_tile, hot_cols), 0) + i * m_tile
            hot[o, i * m_tile : (i + 1) * m_tile, :] = jnp.where(line == target, 1.0, 0.0).astype(BF)
        return c

    lax.fori_loop(0, st_n, hot_step, 0)
    onward = []
    for d in range(1, hi_n):
        h = (hi + d) % hi_n
        t = h * 2 + lo
        g_wait(t)
        onward.append(remote(rows.at[t], rows.at[t], gs.at[2, h], gr.at[t], mate))
        onward[-1].start()
        project(t, False)
    for d in range(1, hi_n):
        t = ((hi + d) % hi_n) * 2 + 1 - lo
        g_wait(t)
        project(t, False)

    def low_step(i, c):
        kv[i] = acc[pl.ds(pl.multiple_of(i * pass_len, pass_len), pass_len), :].astype(BF)
        return c

    lax.fori_loop(0, pass_rows // pass_len, low_step, 0)

    ks, vs_all = pl.ds(0, cols), pl.ds(cols, cols)

    def half(ref, peer, part):
        return ref.at[peer, :, :, part]

    def key_copy(peer):
        return z_copy(1, half(out, peer, ks), inc_k.at[st], peer)

    def value_copy(peer):
        return z_copy(4, half(out, peer, vs_all), inc_v.at[st], peer)

    def kv_send(d, c):
        peer = far_peer(d)
        for k in range(depth):
            out[peer, k] = kv[ask_s[peer, 1, k]]
        key_copy(peer).start()
        return c

    def value_send(d, c):
        value_copy(far_peer(d)).start()
        return c

    lax.fori_loop(1, st_n, kv_send, 0)
    lax.fori_loop(1, st_n, value_send, 0)
    for k in range(depth):
        picked = kv[ask_s[st, 1, k]]
        inc_k[st, k] = picked[:, :cols]
        inc_v[st, k] = picked[:, cols:]
    for copy in loads_q + loads_qg:
        copy.wait()

    def key_wait(d, c):
        peer = (st + d) % st_n
        z_wait(1, half(out, peer, ks), inc_k.at[peer], peer)
        return c

    lax.fori_loop(1, st_n, key_wait, 0)
    scale = HD ** (-0.5)

    def probs_step(b, c):
        r = pl.ds(pl.multiple_of(b * BLK, BLK), BLK)
        for j in range(PB):
            kvb[j * pass_len : (j + 1) * pass_len, :cols] = inc_k[
                slot_ref[0, b * PB + j], slot_ref[1, b * PB + j]
            ]
        for head in range(heads):
            hs = slice(head * HD, (head + 1) * HD)
            vs = slice(cols + head * HD, cols + (head + 1) * HD)
            gate = g_v[r, hs].astype(F32)
            scores = dot(q_v[r, hs], kvb[:, hs], NT) * scale
            shifted = jnp.exp(scores - jnp.max(scores, axis=-1, keepdims=True))
            prob = shifted / jnp.sum(shifted, axis=-1, keepdims=True)
            prob_v[head, r, :] = prob
            sig = 1.0 / (1.0 + jnp.exp(-gate))
            att_grad = (gate * sig * m_v[r, hs].astype(F32)).astype(BF)
            value_grad = dot(prob.astype(BF), att_grad, TN).astype(BF)
            for j in range(PB):
                reqg[b * PB + j, :, vs] = value_grad[j * pass_len : (j + 1) * pass_len]
        return c

    lax.fori_loop(0, blocks, probs_step, 0)

    def back_copy(phase, part, peer):
        return z_copy(phase, half(ret, peer, part), half(arr, st, part), peer)

    def give_back(phase, part, span):
        def send(d, c):
            peer = far_peer(d)
            for k in range(depth):
                ret[peer, k, :, span] = reqg[req_ref[peer, k]][:, span]
            back_copy(phase, part, peer).start()
            return c

        lax.fori_loop(1, st_n, send, 0)
        for k in range(depth):
            arr[st, k, :, span] = reqg[req_ref[st, k]][:, span]

    give_back(2, vs_all, slice(cols, 2 * cols))

    def value_wait(d, c):
        peer = (st + d) % st_n
        z_wait(4, half(out, peer, vs_all), inc_v.at[peer], peer)
        return c

    lax.fori_loop(1, st_n, value_wait, 0)

    def block_step(b, c):
        r = pl.ds(pl.multiple_of(b * BLK, BLK), BLK)
        for j in range(PB):
            o, k = slot_ref[0, b * PB + j], slot_ref[1, b * PB + j]
            kvb[j * pass_len : (j + 1) * pass_len, :cols] = inc_k[o, k]
            kvb[j * pass_len : (j + 1) * pass_len, cols:] = inc_v[o, k]
        for head in range(heads):
            hs = slice(head * HD, (head + 1) * HD)
            vs = slice(cols + head * HD, cols + (head + 1) * HD)
            q = q_v[r, hs]
            key = kvb[:, hs]
            value = kvb[:, vs]
            gate = g_v[r, hs].astype(F32)
            grad = m_v[r, hs].astype(F32)
            prob = prob_v[head, r, :]
            attended = dot(prob.astype(BF), value)
            sig = 1.0 / (1.0 + jnp.exp(-gate))
            att_grad = (gate * sig * grad).astype(BF)
            gboth[r, vs] = (grad * attended * sig * (1.0 + gate * (1.0 - sig))).astype(BF)
            prob_grad = dot(att_grad, value, NT)
            inner = jnp.sum(prob * prob_grad, axis=-1, keepdims=True)
            score_grad = (scale * prob * (prob_grad - inner)).astype(BF)
            gboth[r, hs] = dot(score_grad, key).astype(BF)
            key_grad = dot(score_grad, q, TN).astype(BF)
            for j in range(PB):
                reqg[b * PB + j, :, hs] = key_grad[j * pass_len : (j + 1) * pass_len]
        return c

    lax.fori_loop(0, blocks, block_step, 0)
    give_back(5, ks, slice(0, cols))

    n_tile = tile_of(model, 512)

    def expand(src, weight, part, pair_rows, t):
        base = pl.multiple_of(t * pair_rows, pair_rows)
        a = src[pl.ds(base, pair_rows), :]

        def step(i, c):
            n = pl.ds(pl.multiple_of(i * n_tile, n_tile), n_tile)
            part[t, :, n] = dot(a, weight[n, :], NT).astype(BF)
            return c

        lax.fori_loop(0, model // n_tile, step, 0)

    def pair_copy(which, part, pair, h):
        return remote(part.at[h * 2 + 1 - lo], pair.at[h], ps.at[which, h], pr.at[which, h], mate)

    def scatter_first(which, src, weight, part, pair, pair_rows):
        for d in range(1, hi_n + 1):
            h = (hi + d) % hi_n
            expand(src, weight, part, pair_rows, h * 2 + 1 - lo)
            pair_copy(which, part, pair, h).start()

    def cross(which, send, recv, h):
        return remote(
            send.at[h * 2 + lo], recv.at[hi], xs.at[which, h], xr.at[which, hi], {"tp": h * 2 + lo}
        )

    def scatter_second(which, src, weight, part, pair, send, recv, pair_rows):
        for d in range(1, hi_n + 1):
            h = (hi + d) % hi_n
            expand(src, weight, part, pair_rows, h * 2 + lo)
            pair_copy(which, part, pair, h).wait_recv()
            if d < hi_n:
                part[h * 2 + lo] = (part[h * 2 + lo].astype(F32) + pair[h].astype(F32)).astype(BF)
                cross(which, part, recv, h).start()

    def scatter_last(which, part, pair, send, recv, result):
        for d in range(1, hi_n):
            h = (hi + d) % hi_n
            remote(
                send.at[h * 2 + lo], recv.at[h], xs.at[which, h], xr.at[which, h], {"tp": h * 2 + lo}
            ).wait_recv()
        total = part[tp].astype(F32) + pair[hi].astype(F32)
        for d in range(1, hi_n):
            total = total + recv[(hi + d) % hi_n].astype(F32)
        result[...] = total.astype(BF)

    tok_pair = tok_rows // tp_n
    sto_pair = pass_rows // tp_n
    scatter_first(0, gboth, wqg, tp_part, tp_pair, tok_pair)
    scatter_second(0, gboth, wqg, tp_part, tp_pair, tp_part, tp_recv, tok_pair)

    def gather_sums(o, span, first):
        def step(i, c):
            r = pl.ds(pl.multiple_of(i * m_tile, m_tile), m_tile)
            part = dot(hot[o, r, :], arr[o, :, :, span].reshape(hot_cols, cols))
            acc[r, span] = part if first else acc[r, span] + part
            return c

        lax.fori_loop(0, pass_rows // m_tile, step, 0)

    for phase, part, span in ((2, vs_all, slice(cols, 2 * cols)), (5, ks, slice(0, cols))):
        gather_sums(st, span, True)

        def grad_wait(d, c):
            peer = (st + d) % st_n
            z_wait(phase, half(ret, peer, part), half(arr, peer, part), peer)
            gather_sums(peer, span, False)
            return c

        lax.fori_loop(1, st_n, grad_wait, 0)
        plow[:, span] = acc[:, span].astype(BF)

    scatter_first(1, plow, wkv, sp_part, sp_pair, sto_pair)

    def wkey_step(t, c):
        dwp[pl.ds(pl.multiple_of(t * chunk, chunk), chunk), :] = dot(
            rows[t], plow[:, :cols], TN
        ).astype(BF)
        return c

    lax.fori_loop(0, tp_n, wkey_step, 0)
    share = model // st_n

    def part_of(s):
        return dwp.at[pl.ds(pl.multiple_of(s * share, share), share), :]

    def wkey_send(d, c):
        peer = far_peer(d)
        z_copy(3, part_of(peer), dwr.at[st], peer).start()
        return c

    lax.fori_loop(1, st_n, wkey_send, 0)
    scatter_second(1, plow, wkv, sp_part, sp_pair, sp_part, sp_recv, sto_pair)
    scatter_last(0, tp_part, tp_pair, tp_part, tp_recv, tok_out)
    wkey_out[...] = part_of(st)[...].astype(F32)

    def wkey_wait(d, c):
        peer = (st + d) % st_n
        z_wait(3, part_of(peer), dwr.at[peer], peer)
        wkey_out[...] += dwr[peer].astype(F32)
        return c

    lax.fori_loop(1, st_n, wkey_wait, 0)
    scatter_last(1, sp_part, sp_pair, sp_part, sp_recv, store_out)

    for copy in across + [beside] + onward:
        copy.wait_send()

    def drain(d, c):
        peer = (st + d) % st_n
        z_copy(0, ask_ref.at[peer], ask_in.at[st], peer).wait_send()
        key_copy(peer).wait_send()
        value_copy(peer).wait_send()
        back_copy(2, vs_all, peer).wait_send()
        back_copy(5, ks, peer).wait_send()
        z_copy(3, part_of(peer), dwr.at[st], peer).wait_send()
        return c

    lax.fori_loop(1, st_n, drain, 0)
    for d in range(1, hi_n + 1):
        h = (hi + d) % hi_n
        pair_copy(0, tp_part, tp_pair, h).wait_send()
        pair_copy(1, sp_part, sp_pair, h).wait_send()
        if d < hi_n:
            cross(0, tp_part, tp_recv, h).wait_send()
            cross(1, sp_part, sp_recv, h).wait_send()


def gathered_kernel(
    st_n, tp_n, depth, pass_len,
    ids_ref, store_ref, q_hbm, g_hbm, wq_hbm, wg_hbm, wk_hbm, wv_hbm, m_hbm,
    tok_out, store_out, wkey_out,
    rows, wall, wqg, q_v, g_v, m_v, acc, terms, k_all, v_all, ask_v, ask_in, order_v, req_ref, gated, slope, ret, prob_v, kvb, reqg, gboth, arr,
    hot, plow, sums, dwp, dwc, dwf, tp_part, tp_pair, tp_recv,
    lsem, gs, gr, fs, fr, zs, zr, ps, pr, xs, xr, ws, wr, ss, sr, us, ur,
):
    grp = lax.axis_index("grp")
    st = lax.axis_index("st")
    tp = lax.axis_index("tp")
    hi_n = tp_n // 2
    hi, lo = tp // 2, tp % 2
    mate_t = hi * 2 + 1 - lo
    mate = {"tp": mate_t}
    twin = {"grp": 1 - grp}
    pass_rows, chunk = rows.shape[1], rows.shape[2]
    passages = pass_rows // pass_len
    model = wqg.shape[0]
    cols = q_v.shape[1]
    heads = cols // HD
    tok_rows = q_v.shape[0]
    blocks = tok_rows // BLK
    half_pass = passages // 2
    some = tile_of(half_pass, 2)
    some_rows = some * pass_len
    n_some = half_pass // some
    key_cols, value_cols = slice(0, cols), slice(cols, 2 * cols)

    def local(i, src, dst):
        copy = pltpu.make_async_copy(src, dst, lsem.at[i])
        copy.start()
        return copy

    own_rows = local(0, store_ref, rows.at[tp])
    loads_kv = [
        local(1, wk_hbm, wall.at[tp, :, pl.ds(0, cols)]),
        local(2, wv_hbm, wall.at[tp, :, pl.ds(cols, cols)]),
    ]
    loads_q = [
        local(3, q_hbm, q_v),
        local(4, g_hbm, g_v),
        local(5, m_hbm, m_v),
        local(6, wq_hbm, wqg.at[:, pl.ds(0, cols)]),
        local(7, wg_hbm, wqg.at[:, pl.ds(cols, cols)]),
    ]

    barrier = pltpu.get_barrier_semaphore()

    def greet_st(d, c):
        pl.semaphore_signal(
            barrier, inc=1, device_id={"st": (st + d) % st_n}, device_id_type=MESH
        )
        return c

    lax.fori_loop(1, st_n, greet_st, 0)
    for d in range(1, tp_n):
        pl.semaphore_signal(
            barrier, inc=1, device_id={"tp": (tp + d) % tp_n}, device_id_type=MESH
        )
    pl.semaphore_signal(barrier, inc=1, device_id=twin, device_id_type=MESH)

    def plan(wide):
        line = lax.broadcasted_iota(jnp.int32, (8, wide), 0)
        return line, lax.broadcasted_iota(jnp.int32, (8, wide), 1)

    width = ask_v.shape[2]
    line, lane = plan(width)
    slot, place = lane // pass_len, lane % pass_len
    short_line, short_lane = plan(order_v.shape[1])
    target = jnp.full((8, width), -1, jnp.int32)
    order = jnp.zeros(order_v.shape, jnp.int32)
    taken = [jnp.int32(0)] * st_n
    for j in range(PB):
        for n in range(blocks):
            i = ids_ref[j, n]
            owner = lax.div(i, jnp.int32(passages))
            within = i - owner * passages
            rank = sum(jnp.where(owner == o, taken[o], 0) for o in range(st_n))
            taken = [taken[o] + jnp.where(owner == o, 1, 0) for o in range(st_n)]
            target = jnp.where(
                (line == owner) & (slot == rank), within * pass_len + place, target
            )
            order = jnp.where(
                (short_line == owner) & (short_lane == rank), j * blocks + n, order
            )
    order_v[...] = order
    for o in range(st_n):
        ask_v[o] = jnp.broadcast_to(target[o : o + 1], (8, width))
    pl.semaphore_wait(barrier, st_n + tp_n - 1)

    def first_row(i):
        part = (grp + i // n_some) % 2
        return pl.multiple_of((part * n_some + i % n_some) * some_rows, some_rows)

    def g_copy(way, i, t, source, peer, slot):
        r = pl.ds(first_row(i), some_rows)
        return remote(rows.at[source, r], rows.at[t, r], gs.at[way, slot, i], gr.at[t, i], peer)

    def across(d, i):
        h = (hi + d) % hi_n
        return g_copy(0, i, tp, tp, {"tp": h * 2 + lo}, h)

    def beside(i):
        return g_copy(1, i, tp, tp, mate, hi)

    def onward(d, i):
        h = (hi + d) % hi_n
        return g_copy(2, i, h * 2 + lo, h * 2 + lo, mate, h)

    def g_wait(t, i):
        g_copy(1, i, t, t, mate, hi).wait_recv()

    def rows_send(i, c):
        for d in range(1, hi_n):
            across(d, i).start()
        beside(i).start()
        return c

    own_rows.wait()
    lax.fori_loop(0, 2 * n_some, rows_send, 0)

    upper = st >= st_n // 2
    mark = jnp.where(upper, st, st_n - 1 - st)

    def far_peer(d):
        i = d - 1
        i = i + jnp.where(i >= mark, 1, 0)
        return jnp.where(upper, i, st_n - 1 - i)

    def z_copy(phase, src, dst, peer):
        return remote(src, dst, zs.at[phase, peer], zr.at[phase, st], {"st": peer})

    def z_wait(phase, src, dst, peer):
        remote(src, dst, zs.at[phase, peer], zr.at[phase, peer], {"st": peer}).wait_recv()

    def ask_send(d, c):
        peer = (st + d) % st_n
        z_copy(0, ask_v.at[peer], ask_in.at[st], peer).start()
        return c

    lax.fori_loop(1, st_n, ask_send, 0)
    ask_in[st] = ask_v[st]
    order_copy = local(8, order_v, req_ref)

    def project(i, send):
        r = pl.ds(first_row(i), some_rows)

        def term(t, span):
            return dot(rows[t, r], wall[tp, pl.ds(pl.multiple_of(t * chunk, chunk), chunk), span])

        for d in range(1, hi_n):
            g_wait(((hi + d) % hi_n) * 2 + lo, i)
            onward(d, i).start()
        g_wait(mate_t, i)
        near = [tp, mate_t] + [((hi + d) % hi_n) * 2 + lo for d in range(1, hi_n)]
        late = [((hi + d) % hi_n) * 2 + 1 - lo for d in range(1, hi_n)]
        total = sum(term(t, key_cols) for t in near[1:]) + term(near[0], key_cols)
        for t in late:
            g_wait(t, i)
            total = total + term(t, key_cols)
        low = total.astype(BF)
        first = st * passages + first_row(i) // pass_len
        for p in range(some):
            k_all[first + p] = low[p * pass_len : (p + 1) * pass_len]
        send()
        total = sum(term(t, value_cols) for t in near + late)
        low = total.astype(BF)
        for p in range(some):
            v_all[first + p] = low[p * pass_len : (p + 1) * pass_len]

    def part_of_all(kind, o, c, side):
        ref = k_all if kind == 0 else v_all
        return ref.at[pl.ds(o * passages + side * half_pass + c * some, some)]

    def chain_copy(kind, o, c, way, peer):
        part = part_of_all(kind, o, c, grp)
        return remote(part, part, fs.at[kind, o, c, way], fr.at[kind, o, c, 0], {"st": peer})

    def twin_copy(kind, o, c):
        part = part_of_all(kind, o, c, grp)
        return remote(part, part, fs.at[kind, o, c, 2], fr.at[kind, o, c, 1], twin)

    lower = st < st_n // 2
    edge = (st == 0) | (st == st_n - 1)

    def own_copies(kind, c, act, inward=True, outward=True):
        ways = ((0, st + 1, lower), (1, st - 1, jnp.logical_not(lower)))
        for way, onto, toward in ways:
            there = (onto >= 0) & (onto < st_n)
            if not outward:
                there = there & toward
            if not inward:
                there = there & jnp.logical_not(toward)

            @pl.when(there)
            def _():
                act(chain_copy(kind, st, c, way, onto))

    def relay_copies(kind, d, c, act, ready):
        for way, sign in ((0, -1), (1, 1)):
            o = st + sign * d
            onto = st - sign

            @pl.when((o >= 0) & (o < st_n))
            def _():
                if ready:
                    chain_copy(kind, o, c, way, st).wait_recv()

                @pl.when((onto >= 0) & (onto < st_n))
                def _():
                    act(chain_copy(kind, o, c, way, onto))

                act(twin_copy(kind, o, c))

    def start(copy):
        copy.start()

    def own_send(kind, c, **which):
        own_copies(kind, c, start, **which)

    def relay(kind, d, c):
        relay_copies(kind, d, c, start, True)

    def twin_wait(kind):
        def step(i, c):
            o = (st + 1 + i // n_some) % st_n
            k = i % n_some
            part = part_of_all(kind, o, k, 1 - grp)
            remote(part, part, fs.at[kind, o, k, 2], fr.at[kind, o, k, 1], twin).wait_recv()
            return c

        lax.fori_loop(0, (st_n - 1) * n_some, step, 0)

    for copy in loads_kv + loads_q[:3]:
        copy.wait()

    gate_rows = tok_rows // n_some

    def gates(i):
        r = pl.ds(pl.multiple_of(i * gate_rows, gate_rows), gate_rows)
        gate = g_v[r, :].astype(F32)
        grad = m_v[r, :].astype(F32)
        sig = 1.0 / (1.0 + jnp.exp(-gate))
        gated[r, :] = (gate * sig * grad).astype(BF)
        slope[r, :] = grad * (sig * (1.0 + gate * (1.0 - sig)))

    def early_step(i, c):
        project(i, lambda: own_send(0, i))

        @pl.when(i > 0)
        def _():
            relay(0, 1, i - 1)

        @pl.when(edge | (i == 0))
        def _():
            own_send(1, i, outward=False)

        gates(i)
        return c

    lax.fori_loop(0, n_some, early_step, 0)
    relay(0, 1, n_some - 1)

    def inward_send(i, c):
        own_send(1, i, outward=False)
        return c

    lax.fori_loop(jnp.where(edge, n_some, 1), n_some, inward_send, 0)

    def second_step(i, c):
        relay(0, 2, i)
        return c

    def outward_send(i, c):
        own_send(1, i, inward=False)
        return c

    lax.fori_loop(0, n_some, second_step, 0)
    lax.fori_loop(0, n_some, outward_send, 0)

    def late_step(i, c):
        project(n_some + i, lambda: None)

        @pl.when(edge)
        def _():
            relay(0, 3, i)

        @pl.when(jnp.logical_not(edge))
        def _():
            relay(1, 1, i)

        return c

    w_part = model // 2
    w_mine = pl.ds(pl.multiple_of(grp * w_part, w_part), w_part)
    w_other = pl.ds(pl.multiple_of((1 - grp) * w_part, w_part), w_part)

    def w_across(d):
        h = (hi + d) % hi_n
        part = wall.at[tp, w_mine]
        return remote(part, part, ws.at[0, h], wr.at[0, tp], {"tp": h * 2 + lo})

    def w_twin(d):
        t = ((hi + d) % hi_n) * 2 + lo
        part = wall.at[t, w_mine]
        return remote(part, part, ws.at[1, (hi + d) % hi_n], wr.at[1, t], twin)

    def w_onward(d, k):
        t = ((hi + d) % hi_n) * 2 + lo
        part = wall.at[t, w_other if k else w_mine]
        return remote(part, part, ws.at[2 + k, (hi + d) % hi_n], wr.at[2 + k, t], mate)

    w_beside = remote(wall.at[tp], wall.at[tp], ws.at[4, 0], wr.at[4, tp], mate)

    def w_wait(kind, t, part):
        remote(wall.at[t, part], wall.at[t, part], ws.at[kind, 0], wr.at[kind, t], mate).wait_recv()

    for d in range(1, hi_n):
        w_across(d).start()

    def relay_rest(kind, first, last):
        def step(i, c):
            relay(kind, 1 + i // n_some, i % n_some)
            return c

        lax.fori_loop(first, last, step, 0)

    relays = (st_n - 1) * n_some
    lax.fori_loop(0, n_some, late_step, 0)
    w_beside.start()
    relay_rest(1, 0, jnp.where(edge, n_some, 0))
    for copy in loads_q[3:]:
        copy.wait()
    order_copy.wait()
    twin_wait(0)
    scale = HD ** (-0.5)

    def fill(n, ref, span, b):
        for j in range(PB):
            kvb[n, j * pass_len : (j + 1) * pass_len, span] = ref[ids_ref[j, b]]

    pairs = range(2)

    def block_rows(b):
        return pl.ds(pl.multiple_of(b * BLK, BLK), BLK)

    def probs_step(i, c):
        for n in pairs:
            fill(n, k_all, key_cols, 2 * i + n)
        for head in range(heads):
            hs = slice(head * HD, (head + 1) * HD)
            vs = slice(cols + head * HD, cols + (head + 1) * HD)
            for n in pairs:
                b = 2 * i + n
                r = block_rows(b)
                scores = dot(q_v[r, hs], kvb[n, :, hs], NT) * scale
                shifted = jnp.exp(scores - jnp.max(scores, axis=-1, keepdims=True))
                prob = shifted * (1.0 / jnp.sum(shifted, axis=-1, keepdims=True))
                prob_v[head, r, :] = prob
                value_grad = dot(prob.astype(BF), gated[r, hs], TN).astype(BF)
                for j in range(PB):
                    reqg[j * blocks + b, :, vs] = value_grad[j * pass_len : (j + 1) * pass_len]

        @pl.when(i < n_some)
        def _():
            relay(1, 2, i)

        return c

    lax.fori_loop(0, blocks // 2, probs_step, 0)

    def half(ref, peer, part):
        return ref.at[peer, :, :, part]

    def back_copy(phase, part, peer):
        return z_copy(phase, half(ret, peer, part), half(arr, st, part), peer)

    def give_back(phase, part, span, order, first, last):
        def send(d, c):
            peer = order(d)
            for k in range(depth):
                ret[peer, k, :, span] = reqg[req_ref[peer, k]][:, span]
            back_copy(phase, part, peer).start()
            return c

        lax.fori_loop(first, last, send, 0)

    def keep_own(span):
        for k in range(depth):
            arr[st, k, :, span] = reqg[req_ref[st, k]][:, span]

    def near_peer(d):
        return far_peer(st_n - d)

    ks, vs_all = pl.ds(0, cols), pl.ds(cols, cols)
    def value_peer(d):
        return jnp.where(edge, near_peer(d % (st_n - 1) + 1), near_peer(d))

    give_back(
        1, vs_all, value_cols, value_peer, 1, jnp.where(edge, st_n, st_n - 1)
    )
    keep_own(value_cols)
    relay_rest(1, n_some + min(n_some, blocks // 2), relays)
    twin_wait(1)

    def block_step(i, c):
        for n in pairs:
            fill(n, k_all, key_cols, 2 * i + n)
            fill(n, v_all, value_cols, 2 * i + n)
        for head in range(heads):
            hs = slice(head * HD, (head + 1) * HD)
            vs = slice(cols + head * HD, cols + (head + 1) * HD)
            for n in pairs:
                b = 2 * i + n
                r = block_rows(b)
                value = kvb[n, :, vs]
                prob = prob_v[head, r, :]
                prob_grad = dot(gated[r, hs], value, NT)
                inner = jnp.sum(prob * prob_grad, axis=-1, keepdims=True)
                score_grad = (scale * prob * (prob_grad - inner)).astype(BF)
                key_grad = dot(score_grad, q_v[r, hs], TN).astype(BF)
                for j in range(PB):
                    reqg[j * blocks + b, :, hs] = key_grad[j * pass_len : (j + 1) * pass_len]
                gboth[r, hs] = dot(score_grad, kvb[n, :, hs]).astype(BF)
                attended = dot(prob.astype(BF), value)
                gboth[r, vs] = (attended * slope[r, hs]).astype(BF)
        return c

    lax.fori_loop(0, blocks // 2, block_step, 0)
    give_back(2, ks, key_cols, far_peer, 1, st_n)
    keep_own(key_cols)

    n_tile = tile_of(model, 512)

    def expand(h):
        a = gboth[pl.ds(pl.multiple_of(h * 2 * tok_pair, tok_pair), 2 * tok_pair), :]

        def step(i, c):
            n = pl.ds(pl.multiple_of(i * n_tile, n_tile), n_tile)
            part = dot(a, wqg[n, :], NT).astype(BF)
            tp_part[h * 2, :, n] = part[:tok_pair]
            tp_part[h * 2 + 1, :, n] = part[tok_pair:]
            return c

        lax.fori_loop(0, model // n_tile, step, 0)

    def pair_copy(h):
        return remote(tp_part.at[h * 2 + 1 - lo], tp_pair.at[h], ps.at[h], pr.at[h], mate)

    def cross(h):
        return remote(
            tp_part.at[h * 2 + lo], tp_recv.at[hi], xs.at[h], xr.at[hi], {"tp": h * 2 + lo}
        )

    for d in range(1, hi_n):
        w_wait(0, ((hi + d) % hi_n) * 2 + lo, w_mine)
        w_twin(d).start()
        w_onward(d, 0).start()

    tok_pair = tok_rows // tp_n
    for d in range(1, hi_n + 1):
        h = (hi + d) % hi_n
        expand(h)
        pair_copy(h).start()
    for d in range(1, hi_n):
        h = (hi + d) % hi_n
        pair_copy(h).wait_recv()
        tp_part[h * 2 + lo] = (tp_part[h * 2 + lo].astype(F32) + tp_pair[h].astype(F32)).astype(BF)
        cross(h).start()

    def ask_wait(d, c):
        peer = (st + d) % st_n
        z_wait(0, ask_v.at[peer], ask_in.at[peer], peer)
        return c

    lax.fori_loop(1, st_n, ask_wait, 0)
    hot_cols = depth * pass_len
    m_tile = tile_of(pass_rows, 256)

    def hot_step(o, c):
        target = ask_in[o][0:1, :hot_cols]
        for i in range(pass_rows // m_tile):
            line = lax.broadcasted_iota(jnp.int32, (m_tile, hot_cols), 0) + i * m_tile
            hot[o, i * m_tile : (i + 1) * m_tile, :] = jnp.where(line == target, 1.0, 0.0).astype(BF)
        return c

    lax.fori_loop(0, st_n, hot_step, 0)

    def gather_sums(kind, o, span, first):
        def step(i, c):
            r = pl.ds(pl.multiple_of(i * m_tile, m_tile), m_tile)
            part = dot(hot[o, r, :], arr[o, :, :, span].reshape(hot_cols, cols))
            acc[kind, r, :] = part if first else acc[kind, r, :] + part
            return c

        lax.fori_loop(0, pass_rows // m_tile, step, 0)

    sto_pair = pass_rows // tp_n

    def sums_copy(kind, part, d):
        t = (tp + d) % tp_n
        src = plow.at[pl.ds(pl.multiple_of(t * sto_pair, sto_pair), sto_pair), part]
        return remote(src, sums.at[tp, :, part], ss.at[kind, t], sr.at[kind, tp], {"tp": t})

    def sums_wait(kind, part, t):
        dst = sums.at[t, :, part]
        remote(dst, dst, ss.at[kind, t], sr.at[kind, t], mate).wait_recv()

    def grads_of(kind, peer):
        phase, part, span = (2, ks, key_cols) if kind == 0 else (1, vs_all, value_cols)
        z_wait(phase, half(ret, peer, part), half(arr, peer, part), peer)
        gather_sums(kind, peer, span, False)

    def sums_send(kind):
        part, span = (ks, key_cols) if kind == 0 else (vs_all, value_cols)
        plow[:, span] = acc[kind].astype(BF)
        for d in range(1, tp_n):
            sums_copy(kind, part, d).start()
        sums[tp, :, span] = plow[pl.ds(pl.multiple_of(tp * sto_pair, sto_pair), sto_pair), span]

    beyond = jnp.where(lower, st_n - 1, 0)
    middle = jnp.where(lower, st_n // 2, st_n // 2 - 1)
    beside_st = st + 1 - 2 * (st % 2)
    outer = edge
    inner = jnp.logical_not(outer)
    gather_sums(1, st, value_cols, True)
    gather_sums(0, st, key_cols, True)
    grads_of(1, beside_st)
    grads_of(1, jnp.where(outer, beyond, middle))

    grads_of(0, middle)

    @pl.when(inner)
    def _():
        give_back(1, vs_all, value_cols, near_peer, st_n - 1, st_n)

    grads_of(0, beyond)
    grads_of(0, beside_st)
    sums_send(0)

    share = model // st_n
    bits = 2
    bit = share // bits

    def dw_line(s, b):
        return pl.ds(pl.multiple_of(s * share + b * bit, bit), bit)

    def dw_copy(kind, b):
        line = pl.ds(b * bit, bit)
        if kind < 2:
            src, dst = dwp.at[dw_line(middle if kind else beyond, b)], dwc.at[kind, line]
            peer = beside_st
        elif kind == 2:
            src, dst, peer = dwp.at[dw_line(beside_st, b)], dwf.at[0, line], beside_st
        else:
            src, dst = dwc.at[kind - 3, line], dwf.at[1, line]
            peer = middle if kind == 4 else beyond
        return remote(src, dst, us.at[kind, b], ur.at[kind, b], {"st": peer})

    def dw_send(kind):
        for b in range(bits):
            dw_copy(kind, b).start()

    def dw_relay(q):
        for b in range(bits):
            line = slice(b * bit, (b + 1) * bit)
            dw_copy(q, b).wait_recv()
            own = dwp[dw_line(middle if q else beyond, b), :].astype(F32)
            dwc[q, line, :] = (dwc[q, line, :].astype(F32) + own).astype(BF)
            dw_copy(3 + q, b).start()

    def wkey_step(s):
        dwp[pl.ds(pl.multiple_of(s * chunk, chunk), chunk), :] = dot(
            rows[s], plow[:, key_cols], TN
        ).astype(BF)

    def wkey_turn(j, c):
        far = jnp.where(j == 0, beyond, middle)
        near = jnp.where(j == 2, beside_st, st)
        near_first = jnp.where(j == 0, beside_st, st)
        far_after = jnp.where(j == 1, beyond, middle)
        s = jnp.where(
            outer, jnp.where(j < 2, far, near), jnp.where((j == 0) | (j == 3), near_first, far_after)
        )
        wkey_step(s)
        for kind in range(3):
            @pl.when(outer & (j == kind))
            def _():
                dw_send(kind)

        @pl.when(inner & (j == 0))
        def _():
            dw_send(2)

        return c

    lax.fori_loop(0, st_n, wkey_turn, 0)

    @pl.when(inner)
    def _():
        dw_relay(0)

    for d in range(1, hi_n):
        t = ((hi + d) % hi_n) * 2 + lo
        w_wait(1, t, w_other)
        w_onward(d, 1).start()
    w_wait(4, mate_t, pl.ds(0, model))
    for d in range(1, hi_n):
        t = ((hi + d) % hi_n) * 2 + 1 - lo
        w_wait(2, t, w_mine)
        w_wait(3, t, w_other)

    def store_terms(span, done):
        def step(i, c):
            n = pl.ds(pl.multiple_of(i * n_tile, n_tile), n_tile)
            part = dot(sums[0, :, span], wall[0, n, span], NT)
            for t in range(1, tp_n):
                part = part + dot(sums[t, :, span], wall[t, n, span], NT)
            done(n, part)
            return c

        lax.fori_loop(0, model // n_tile, step, 0)

    def keep_terms(n, part):
        terms[:, n] = part

    def keep_store(n, part):
        store_out[:, n] = (terms[:, n] + part).astype(BF)

    grads_of(1, jnp.where(outer, middle, beyond))
    sums_send(1)

    for d in range(1, tp_n):
        sums_wait(0, ks, (tp + d) % tp_n)
    store_terms(key_cols, keep_terms)

    pair_copy(hi).wait_recv()
    for d in range(1, hi_n):
        h = (hi + d) % hi_n
        remote(
            tp_part.at[h * 2 + lo], tp_recv.at[h], xs.at[h], xr.at[h], {"tp": h * 2 + lo}
        ).wait_recv()
    total = tp_part[tp].astype(F32) + tp_pair[hi].astype(F32)
    for d in range(1, hi_n):
        total = total + tp_recv[(hi + d) % hi_n].astype(F32)
    tok_out[...] = total.astype(BF)

    @pl.when(inner)
    def _():
        dw_relay(1)

    for d in range(1, tp_n):
        sums_wait(1, vs_all, (tp + d) % tp_n)
    store_terms(value_cols, keep_store)

    for b in range(bits):
        line = slice(b * bit, (b + 1) * bit)
        dw_copy(2, b).wait_recv()
        wkey_out[line, :] = dwp[dw_line(st, b), :].astype(F32) + dwf[0, line, :].astype(F32)
    for b in range(bits):
        line = slice(b * bit, (b + 1) * bit)
        for kind, edge in ((3, outer), (4, inner)):
            @pl.when(edge)
            def _():
                dw_copy(kind, b).wait_recv()

        wkey_out[line, :] += dwf[1, line, :].astype(F32)

    def wait_send(copy):
        copy.wait_send()

    def rows_drain(i, c):
        for d in range(1, hi_n):
            across(d, i).wait_send()
            onward(d, i).wait_send()
        beside(i).wait_send()
        return c

    lax.fori_loop(0, 2 * n_some, rows_drain, 0)

    def all_drain(i, c):
        for kind in (0, 1):
            own_copies(kind, i, wait_send)
            for d in range(1, st_n):
                relay_copies(kind, d, i, wait_send, False)
        return c

    lax.fori_loop(0, n_some, all_drain, 0)
    for d in range(1, hi_n):
        w_across(d).wait_send()
        w_twin(d).wait_send()
        w_onward(d, 0).wait_send()
        w_onward(d, 1).wait_send()
    w_beside.wait_send()

    def drain(d, c):
        peer = (st + d) % st_n
        z_copy(0, ask_v.at[peer], ask_in.at[st], peer).wait_send()
        back_copy(1, vs_all, peer).wait_send()
        back_copy(2, ks, peer).wait_send()
        return c

    lax.fori_loop(1, st_n, drain, 0)
    for d in range(1, tp_n):
        sums_copy(0, ks, d).wait_send()
        sums_copy(1, vs_all, d).wait_send()
    for d in range(1, hi_n + 1):
        h = (hi + d) % hi_n
        pair_copy(h).wait_send()
        if d < hi_n:
            cross(h).wait_send()
    for b in range(bits):
        dw_copy(2, b).wait_send()
        for q in (0, 1):
            @pl.when(outer)
            def _():
                dw_copy(q, b).wait_send()

            @pl.when(inner)
            def _():
                dw_copy(3 + q, b).wait_send()


def local(pass_ids, store, queries, gate_pre, w_query, w_gate, w_key, w_value, d_mem):
    st_n = lax.axis_size("st")
    tp_n = lax.axis_size("tp")
    hi_n = tp_n // 2
    tok_rows, cols = queries.shape
    blocks = tok_rows // BLK
    passages, pass_len, chunk = store.shape
    model = w_key.shape[0]
    requests = blocks * PB
    depth = max(2, requests // st_n)
    pass_rows = passages * pass_len
    share = model // st_n

    vmem = pl.BlockSpec(memory_space=pltpu.VMEM)
    smem = pl.BlockSpec(memory_space=pltpu.SMEM)
    hbm = pl.BlockSpec(memory_space=pl.ANY)
    V = pltpu.VMEM
    DMA = pltpu.SemaphoreType.DMA
    pair = 2 * cols
    tok_pair = tok_rows // tp_n
    sto_pair = pass_rows // tp_n
    hot_cols = depth * pass_len
    width = -(-hot_cols // 128) * 128
    gathered_bytes = 2 * 2 * st_n * pass_rows * cols
    if lax.axis_size("grp") == 2 and hi_n == 2 and st_n == 4 and passages % 2 == 0 and gathered_bytes <= 8 << 20:
        half_pass = passages // 2
        n_some = half_pass // tile_of(half_pass, 2)
        d_tokens, d_store, d_wkey = pl.pallas_call(
            functools.partial(gathered_kernel, st_n, tp_n, depth, pass_len),
            out_shape=(
                jax.ShapeDtypeStruct((tok_pair, model), BF),
                jax.ShapeDtypeStruct((sto_pair, model), BF),
                jax.ShapeDtypeStruct((share, cols), F32),
            ),
            in_specs=[smem] + [hbm] * 8,
            out_specs=(vmem, vmem, vmem),
            scratch_shapes=[
                V((tp_n, pass_rows, chunk), BF),
                V((tp_n, model, pair), BF),
                V((model, pair), BF),
                V((tok_rows, cols), BF),
                V((tok_rows, cols), BF),
                V((tok_rows, cols), BF),
                V((2, pass_rows, cols), F32),
                V((sto_pair, model), F32),
                V((st_n * passages, pass_len, cols), BF),
                V((st_n * passages, pass_len, cols), BF),
                V((st_n, 8, width), jnp.int32),
                V((st_n, 8, width), jnp.int32),
                V((8, 128), jnp.int32),
                pltpu.SMEM((8, 128), jnp.int32),
                V((tok_rows, cols), BF),
                V((tok_rows, cols), F32),
                V((st_n, depth, pass_len, pair), BF),
                V((cols // HD, tok_rows, PB * pass_len), F32),
                V((2, PB * pass_len, pair), BF),
                V((requests, pass_len, pair), BF),
                V((tok_rows, pair), BF),
                V((st_n, depth, pass_len, pair), BF),
                V((st_n, pass_rows, hot_cols), BF),
                V((pass_rows, pair), BF),
                V((tp_n, sto_pair, pair), BF),
                V((model, cols), BF),
                V((2, share, cols), BF),
                V((2, share, cols), BF),
                V((tp_n, tok_pair, model), BF),
                V((hi_n, tok_pair, model), BF),
                V((hi_n, tok_pair, model), BF),
                DMA((9,)),
                DMA((3, hi_n, 2 * n_some)),
                DMA((tp_n, 2 * n_some)),
                DMA((2, st_n, n_some, 3)),
                DMA((2, st_n, n_some, 2)),
                DMA((3, st_n)),
                DMA((3, st_n)),
                DMA((hi_n,)),
                DMA((hi_n,)),
                DMA((hi_n,)),
                DMA((hi_n,)),
                DMA((5, hi_n)),
                DMA((5, tp_n)),
                DMA((2, tp_n)),
                DMA((2, tp_n)),
                DMA((5, 2)),
                DMA((5, 2)),
            ],
            compiler_params=pltpu.CompilerParams(
                collective_id=0, has_side_effects=True, vmem_limit_bytes=67043328
            ),
        )(
            pass_ids.T, store.reshape(pass_rows, chunk),
            queries, gate_pre, w_query, w_gate, w_key, w_value, d_mem,
        )
        return d_tokens, d_store.reshape(passages // tp_n, pass_len, model), d_wkey

    ids = pass_ids.reshape(-1)
    owners = ids // passages
    within = ids % passages
    order = jnp.arange(requests, dtype=jnp.int32)
    earlier = (owners[None, :] == owners[:, None]) & (order[None, :] < order[:, None])
    rank = jnp.sum(earlier.astype(jnp.int32), axis=1)
    slots = jnp.stack([owners, rank])
    o_i = jnp.arange(st_n, dtype=jnp.int32)[:, None, None]
    k_i = jnp.arange(depth, dtype=jnp.int32)[None, :, None]
    match = (owners[None, None, :] == o_i) & (rank[None, None, :] == k_i)
    asked = jnp.max(jnp.where(match, within[None, None, :], -1), axis=2)
    req_of = jnp.max(jnp.where(match, order[None, None, :], 0), axis=2)
    hot_cols = depth * pass_len
    width = -(-hot_cols // 128) * 128
    lane = jnp.arange(width, dtype=jnp.int32)
    spread = jnp.repeat(asked, pass_len, axis=1)
    spread = jnp.pad(spread, ((0, 0), (0, width - hot_cols)), constant_values=-1)
    target = jnp.where(spread < 0, -1, spread * pass_len + lane[None, :] % pass_len)
    flat = jnp.pad(jnp.maximum(asked, 0), ((0, 0), (0, width - depth)))
    ask = jnp.concatenate(
        [target[:, None], flat[:, None], jnp.zeros((st_n, 6, width), jnp.int32)], axis=1
    )

    d_tokens, d_store, d_wkey = pl.pallas_call(
        functools.partial(kernel, st_n, tp_n, depth, pass_len),
        out_shape=(
            jax.ShapeDtypeStruct((tok_pair, model), BF),
            jax.ShapeDtypeStruct((sto_pair, model), BF),
            jax.ShapeDtypeStruct((share, cols), F32),
        ),
        in_specs=[smem, smem, vmem] + [hbm] * 8,
        out_specs=(vmem, vmem, vmem),
        scratch_shapes=[
            V((tp_n, pass_rows, chunk), BF),
            V((model, pair), BF),
            V((model, pair), BF),
            V((tok_rows, cols), BF),
            V((tok_rows, cols), BF),
            V((tok_rows, cols), BF),
            V((pass_rows, pair), F32),
            V((passages, pass_len, pair), BF),
            V((st_n, 8, width), jnp.int32),
            pltpu.SMEM((st_n, 8, width), jnp.int32),
            V((st_n, depth, pass_len, pair), BF),
            V((st_n, depth, pass_len, cols), BF),
            V((st_n, depth, pass_len, cols), BF),
            V((st_n, depth, pass_len, pair), BF),
            V((cols // HD, tok_rows, PB * pass_len), F32),
            V((PB * pass_len, pair), BF),
            V((requests, pass_len, pair), BF),
            V((tok_rows, pair), BF),
            V((st_n, depth, pass_len, pair), BF),
            V((st_n, pass_rows, hot_cols), BF),
            V((pass_rows, pair), BF),
            V((model, cols), BF),
            V((st_n, share, cols), BF),
            V((tp_n, tok_pair, model), BF),
            V((hi_n, tok_pair, model), BF),
            V((hi_n, tok_pair, model), BF),
            V((tp_n, sto_pair, model), BF),
            V((hi_n, sto_pair, model), BF),
            V((hi_n, sto_pair, model), BF),
            DMA((9,)),
            DMA((3, hi_n)),
            DMA((tp_n,)),
            DMA((6, st_n)),
            DMA((6, st_n)),
            DMA((2, hi_n)),
            DMA((2, hi_n)),
            DMA((2, hi_n)),
            DMA((2, hi_n)),
        ],
        compiler_params=pltpu.CompilerParams(
            collective_id=0, has_side_effects=True, vmem_limit_bytes=67043328
        ),
    )(
        slots, req_of, ask, store.reshape(pass_rows, chunk),
        queries, gate_pre, w_query, w_gate, w_key, w_value, d_mem,
    )
    return d_tokens, d_store.reshape(passages // tp_n, pass_len, model), d_wkey


def solution(mesh):
    return jax.shard_map(
        local,
        mesh=mesh,
        in_specs=(
            P(("grp", "st"), None),
            P("st", None, "tp"),
            P(("grp", "st"), "tp"),
            P(("grp", "st"), "tp"),
            P(None, "tp"),
            P(None, "tp"),
            P(None, "tp"),
            P(None, "tp"),
            P(("grp", "st"), "tp"),
        ),
        out_specs=(
            P(("grp", "st", "tp"), None),
            P(("grp", "st", "tp"), None, None),
            P(("grp", "st"), "tp"),
        ),
        check_vma=False,
    )
```

```python
import functools

import jax
import jax.numpy as jnp
from jax import lax
from jax.experimental import pallas as pl
from jax.experimental.pallas import tpu as pltpu
from jax.sharding import PartitionSpec as P

HD = 256
BLK = 128
PB = 4
BF = jnp.bfloat16
F32 = jnp.float32
MESH = pl.DeviceIdType.MESH
NT = (((1,), (1,)), ((), ()))
TN = (((0,), (0,)), ((), ()))


def dot(a, b, dims=(((1,), (0,)), ((), ()))):
    return lax.dot_general(a, b, dims, preferred_element_type=F32)


def remote(src, dst, send, recv, device):
    return pltpu.make_async_remote_copy(
        src_ref=src,
        dst_ref=dst,
        send_sem=send,
        recv_sem=recv,
        device_id=device,
        device_id_type=MESH,
    )


def tile_of(size, most):
    while size % most:
        most //= 2
    return most


def kernel(
    st_n, tp_n, depth, pass_len,
    slot_ref, req_ref, ask_ref, store_ref, q_hbm, g_hbm, wq_hbm, wg_hbm, wk_hbm, wv_hbm, m_hbm,
    tok_out, store_out, wkey_out,
    rows, wkv, wqg, q_v, g_v, m_v, acc, kv, ask_in, ask_s, out, inc_k, inc_v, ret, prob_v, kvb, reqg, gboth, arr,
    hot, plow, dwp, dwr, tp_part, tp_pair, tp_recv, sp_part, sp_pair, sp_recv,
    lsem, gs, gr, zs, zr, ps, pr, xs, xr,
):
    st = lax.axis_index("st")
    tp = lax.axis_index("tp")
    hi_n = tp_n // 2
    hi, lo = tp // 2, tp % 2
    mate = {"tp": hi * 2 + 1 - lo}
    pass_rows, chunk = rows.shape[1], rows.shape[2]
    model = wqg.shape[0]
    cols = q_v.shape[1]
    heads = cols // HD
    tok_rows = q_v.shape[0]
    blocks = tok_rows // BLK
    blk_keys = PB * pass_len

    def local(i, src, dst):
        copy = pltpu.make_async_copy(src, dst, lsem.at[i])
        copy.start()
        return copy

    own_rows = local(0, store_ref, rows.at[tp])
    loads_kv = [
        local(1, wk_hbm, wkv.at[:, pl.ds(0, cols)]),
        local(2, wv_hbm, wkv.at[:, pl.ds(cols, cols)]),
    ]
    loads_q = [local(3, q_hbm, q_v), local(4, g_hbm, g_v), local(5, m_hbm, m_v)]
    loads_qg = [
        local(6, wq_hbm, wqg.at[:, pl.ds(0, cols)]),
        local(7, wg_hbm, wqg.at[:, pl.ds(cols, cols)]),
    ]

    barrier = pltpu.get_barrier_semaphore()

    def greet_st(d, c):
        pl.semaphore_signal(
            barrier, inc=1, device_id={"st": (st + d) % st_n}, device_id_type=MESH
        )
        return c

    lax.fori_loop(1, st_n, greet_st, 0)
    for d in range(1, tp_n):
        pl.semaphore_signal(
            barrier, inc=1, device_id={"tp": (tp + d) % tp_n}, device_id_type=MESH
        )
    pl.semaphore_wait(barrier, st_n - 1 + tp_n - 1)

    across = []
    for d in range(1, hi_n):
        h = (hi + d) % hi_n
        across.append(
            remote(store_ref, rows.at[tp], gs.at[0, h], gr.at[tp], {"tp": h * 2 + lo})
        )
        across[-1].start()
    beside = remote(store_ref, rows.at[tp], gs.at[1, hi], gr.at[tp], mate)
    beside.start()

    upper = st >= st_n // 2
    mark = jnp.where(upper, st, st_n - 1 - st)

    def far_peer(d):
        i = d - 1
        i = i + jnp.where(i >= mark, 1, 0)
        return jnp.where(upper, i, st_n - 1 - i)

    def z_copy(phase, src, dst, peer):
        return remote(src, dst, zs.at[phase, peer], zr.at[phase, st], {"st": peer})

    def z_wait(phase, src, dst, peer):
        remote(src, dst, zs.at[phase, peer], zr.at[phase, peer], {"st": peer}).wait_recv()

    def ask_send(d, c):
        peer = (st + d) % st_n
        z_copy(0, ask_ref.at[peer], ask_in.at[st], peer).start()
        return c

    lax.fori_loop(1, st_n, ask_send, 0)
    ask_in[st] = ask_ref[st]

    m_tile = tile_of(pass_rows, 256)

    def project(t, first):
        def step(i, c):
            r = pl.ds(pl.multiple_of(i * m_tile, m_tile), m_tile)
            part = dot(rows[t, r], wkv[pl.ds(pl.multiple_of(t * chunk, chunk), chunk), :])
            acc[r] = part if first else acc[r] + part
            return c

        lax.fori_loop(0, pass_rows // m_tile, step, 0)

    def g_wait(t):
        remote(store_ref, rows.at[t], gs.at[1, hi], gr.at[t], mate).wait_recv()

    own_rows.wait()
    for copy in loads_kv:
        copy.wait()
    project(tp, True)
    g_wait(hi * 2 + 1 - lo)
    project(hi * 2 + 1 - lo, False)

    def ask_wait(d, c):
        peer = (st + d) % st_n
        z_wait(0, ask_ref.at[peer], ask_in.at[peer], peer)
        return c

    lax.fori_loop(1, st_n, ask_wait, 0)
    ask_copy = local(8, ask_in, ask_s)
    ask_copy.wait()

    hot_cols = depth * pass_len

    def hot_step(o, c):
        target = ask_in[o][0:1, :hot_cols]
        for i in range(pass_rows // m_tile):
            line = lax.broadcasted_iota(jnp.int32, (m_tile, hot_cols), 0) + i * m_tile
            hot[o, i * m_tile : (i + 1) * m_tile, :] = jnp.where(line == target, 1.0, 0.0).astype(BF)
        return c

    lax.fori_loop(0, st_n, hot_step, 0)
    onward = []
    for d in range(1, hi_n):
        h = (hi + d) % hi_n
        t = h * 2 + lo
        g_wait(t)
        onward.append(remote(rows.at[t], rows.at[t], gs.at[2, h], gr.at[t], mate))
        onward[-1].start()
        project(t, False)
    for d in range(1, hi_n):
        t = ((hi + d) % hi_n) * 2 + 1 - lo
        g_wait(t)
        project(t, False)

    def low_step(i, c):
        kv[i] = acc[pl.ds(pl.multiple_of(i * pass_len, pass_len), pass_len), :].astype(BF)
        return c

    lax.fori_loop(0, pass_rows // pass_len, low_step, 0)

    ks, vs_all = pl.ds(0, cols), pl.ds(cols, cols)

    def half(ref, peer, part):
        return ref.at[peer, :, :, part]

    def key_copy(peer):
        return z_copy(1, half(out, peer, ks), inc_k.at[st], peer)

    def value_copy(peer):
        return z_copy(4, half(out, peer, vs_all), inc_v.at[st], peer)

    def kv_send(d, c):
        peer = far_peer(d)
        for k in range(depth):
            out[peer, k] = kv[ask_s[peer, 1, k]]
        key_copy(peer).start()
        return c

    def value_send(d, c):
        value_copy(far_peer(d)).start()
        return c

    lax.fori_loop(1, st_n, kv_send, 0)
    lax.fori_loop(1, st_n, value_send, 0)
    for k in range(depth):
        picked = kv[ask_s[st, 1, k]]
        inc_k[st, k] = picked[:, :cols]
        inc_v[st, k] = picked[:, cols:]
    for copy in loads_q + loads_qg:
        copy.wait()

    def key_wait(d, c):
        peer = (st + d) % st_n
        z_wait(1, half(out, peer, ks), inc_k.at[peer], peer)
        return c

    lax.fori_loop(1, st_n, key_wait, 0)
    scale = HD ** (-0.5)

    def probs_step(b, c):
        r = pl.ds(pl.multiple_of(b * BLK, BLK), BLK)
        for j in range(PB):
            kvb[j * pass_len : (j + 1) * pass_len, :cols] = inc_k[
                slot_ref[0, b * PB + j], slot_ref[1, b * PB + j]
            ]
        for head in range(heads):
            hs = slice(head * HD, (head + 1) * HD)
            vs = slice(cols + head * HD, cols + (head + 1) * HD)
            gate = g_v[r, hs].astype(F32)
            scores = dot(q_v[r, hs], kvb[:, hs], NT) * scale
            shifted = jnp.exp(scores - jnp.max(scores, axis=-1, keepdims=True))
            prob = shifted / jnp.sum(shifted, axis=-1, keepdims=True)
            prob_v[head, r, :] = prob
            sig = 1.0 / (1.0 + jnp.exp(-gate))
            att_grad = (gate * sig * m_v[r, hs].astype(F32)).astype(BF)
            value_grad = dot(prob.astype(BF), att_grad, TN).astype(BF)
            for j in range(PB):
                reqg[b * PB + j, :, vs] = value_grad[j * pass_len : (j + 1) * pass_len]
        return c

    lax.fori_loop(0, blocks, probs_step, 0)

    def back_copy(phase, part, peer):
        return z_copy(phase, half(ret, peer, part), half(arr, st, part), peer)

    def give_back(phase, part, span):
        def send(d, c):
            peer = far_peer(d)
            for k in range(depth):
                ret[peer, k, :, span] = reqg[req_ref[peer, k]][:, span]
            back_copy(phase, part, peer).start()
            return c

        lax.fori_loop(1, st_n, send, 0)
        for k in range(depth):
            arr[st, k, :, span] = reqg[req_ref[st, k]][:, span]

    give_back(2, vs_all, slice(cols, 2 * cols))

    def value_wait(d, c):
        peer = (st + d) % st_n
        z_wait(4, half(out, peer, vs_all), inc_v.at[peer], peer)
        return c

    lax.fori_loop(1, st_n, value_wait, 0)

    def block_step(b, c):
        r = pl.ds(pl.multiple_of(b * BLK, BLK), BLK)
        for j in range(PB):
            o, k = slot_ref[0, b * PB + j], slot_ref[1, b * PB + j]
            kvb[j * pass_len : (j + 1) * pass_len, :cols] = inc_k[o, k]
            kvb[j * pass_len : (j + 1) * pass_len, cols:] = inc_v[o, k]
        for head in range(heads):
            hs = slice(head * HD, (head + 1) * HD)
            vs = slice(cols + head * HD, cols + (head + 1) * HD)
            q = q_v[r, hs]
            key = kvb[:, hs]
            value = kvb[:, vs]
            gate = g_v[r, hs].astype(F32)
            grad = m_v[r, hs].astype(F32)
            prob = prob_v[head, r, :]
            attended = dot(prob.astype(BF), value)
            sig = 1.0 / (1.0 + jnp.exp(-gate))
            att_grad = (gate * sig * grad).astype(BF)
            gboth[r, vs] = (grad * attended * sig * (1.0 + gate * (1.0 - sig))).astype(BF)
            prob_grad = dot(att_grad, value, NT)
            inner = jnp.sum(prob * prob_grad, axis=-1, keepdims=True)
            score_grad = (scale * prob * (prob_grad - inner)).astype(BF)
            gboth[r, hs] = dot(score_grad, key).astype(BF)
            key_grad = dot(score_grad, q, TN).astype(BF)
            for j in range(PB):
                reqg[b * PB + j, :, hs] = key_grad[j * pass_len : (j + 1) * pass_len]
        return c

    lax.fori_loop(0, blocks, block_step, 0)
    give_back(5, ks, slice(0, cols))

    n_tile = tile_of(model, 512)

    def expand(src, weight, part, pair_rows, t):
        base = pl.multiple_of(t * pair_rows, pair_rows)
        a = src[pl.ds(base, pair_rows), :]

        def step(i, c):
            n = pl.ds(pl.multiple_of(i * n_tile, n_tile), n_tile)
            part[t, :, n] = dot(a, weight[n, :], NT).astype(BF)
            return c

        lax.fori_loop(0, model // n_tile, step, 0)

    def pair_copy(which, part, pair, h):
        return remote(part.at[h * 2 + 1 - lo], pair.at[h], ps.at[which, h], pr.at[which, h], mate)

    def scatter_first(which, src, weight, part, pair, pair_rows):
        for d in range(1, hi_n + 1):
            h = (hi + d) % hi_n
            expand(src, weight, part, pair_rows, h * 2 + 1 - lo)
            pair_copy(which, part, pair, h).start()

    def cross(which, send, recv, h):
        return remote(
            send.at[h * 2 + lo], recv.at[hi], xs.at[which, h], xr.at[which, hi], {"tp": h * 2 + lo}
        )

    def scatter_second(which, src, weight, part, pair, send, recv, pair_rows):
        for d in range(1, hi_n + 1):
            h = (hi + d) % hi_n
            expand(src, weight, part, pair_rows, h * 2 + lo)
            pair_copy(which, part, pair, h).wait_recv()
            if d < hi_n:
                part[h * 2 + lo] = (part[h * 2 + lo].astype(F32) + pair[h].astype(F32)).astype(BF)
                cross(which, part, recv, h).start()

    def scatter_last(which, part, pair, send, recv, result):
        for d in range(1, hi_n):
            h = (hi + d) % hi_n
            remote(
                send.at[h * 2 + lo], recv.at[h], xs.at[which, h], xr.at[which, h], {"tp": h * 2 + lo}
            ).wait_recv()
        total = part[tp].astype(F32) + pair[hi].astype(F32)
        for d in range(1, hi_n):
            total = total + recv[(hi + d) % hi_n].astype(F32)
        result[...] = total.astype(BF)

    tok_pair = tok_rows // tp_n
    sto_pair = pass_rows // tp_n
    scatter_first(0, gboth, wqg, tp_part, tp_pair, tok_pair)
    scatter_second(0, gboth, wqg, tp_part, tp_pair, tp_part, tp_recv, tok_pair)

    def gather_sums(o, span, first):
        def step(i, c):
            r = pl.ds(pl.multiple_of(i * m_tile, m_tile), m_tile)
            part = dot(hot[o, r, :], arr[o, :, :, span].reshape(hot_cols, cols))
            acc[r, span] = part if first else acc[r, span] + part
            return c

        lax.fori_loop(0, pass_rows // m_tile, step, 0)

    for phase, part, span in ((2, vs_all, slice(cols, 2 * cols)), (5, ks, slice(0, cols))):
        gather_sums(st, span, True)

        def grad_wait(d, c):
            peer = (st + d) % st_n
            z_wait(phase, half(ret, peer, part), half(arr, peer, part), peer)
            gather_sums(peer, span, False)
            return c

        lax.fori_loop(1, st_n, grad_wait, 0)
        plow[:, span] = acc[:, span].astype(BF)

    scatter_first(1, plow, wkv, sp_part, sp_pair, sto_pair)

    def wkey_step(t, c):
        dwp[pl.ds(pl.multiple_of(t * chunk, chunk), chunk), :] = dot(
            rows[t], plow[:, :cols], TN
        ).astype(BF)
        return c

    lax.fori_loop(0, tp_n, wkey_step, 0)
    share = model // st_n

    def part_of(s):
        return dwp.at[pl.ds(pl.multiple_of(s * share, share), share), :]

    def wkey_send(d, c):
        peer = far_peer(d)
        z_copy(3, part_of(peer), dwr.at[st], peer).start()
        return c

    lax.fori_loop(1, st_n, wkey_send, 0)
    scatter_second(1, plow, wkv, sp_part, sp_pair, sp_part, sp_recv, sto_pair)
    scatter_last(0, tp_part, tp_pair, tp_part, tp_recv, tok_out)
    wkey_out[...] = part_of(st)[...].astype(F32)

    def wkey_wait(d, c):
        peer = (st + d) % st_n
        z_wait(3, part_of(peer), dwr.at[peer], peer)
        wkey_out[...] += dwr[peer].astype(F32)
        return c

    lax.fori_loop(1, st_n, wkey_wait, 0)
    scatter_last(1, sp_part, sp_pair, sp_part, sp_recv, store_out)

    for copy in across + [beside] + onward:
        copy.wait_send()

    def drain(d, c):
        peer = (st + d) % st_n
        z_copy(0, ask_ref.at[peer], ask_in.at[st], peer).wait_send()
        key_copy(peer).wait_send()
        value_copy(peer).wait_send()
        back_copy(2, vs_all, peer).wait_send()
        back_copy(5, ks, peer).wait_send()
        z_copy(3, part_of(peer), dwr.at[st], peer).wait_send()
        return c

    lax.fori_loop(1, st_n, drain, 0)
    for d in range(1, hi_n + 1):
        h = (hi + d) % hi_n
        pair_copy(0, tp_part, tp_pair, h).wait_send()
        pair_copy(1, sp_part, sp_pair, h).wait_send()
        if d < hi_n:
            cross(0, tp_part, tp_recv, h).wait_send()
            cross(1, sp_part, sp_recv, h).wait_send()


def gathered_kernel(
    st_n, tp_n, depth, pass_len,
    ids_hbm, store_ref, q_hbm, g_hbm, wq_hbm, wg_hbm, wk_hbm, wv_hbm, m_hbm,
    tok_hbm, store_hbm, wkey_hbm,
    ids_ref, tok_out, store_out, wkey_out, rows, wall, wqg, q_v, g_v, m_v, acc, terms, k_all, v_all, ask_v, ask_in, order_v, req_ref, gated, slope, ret, prob_v, kvb, reqg, gboth, arr,
    hot, plow, sums, dwp, dwc, dwf, tp_part, tp_pair, tp_recv,
    lsem, gs, gr, fs, fr, zs, zr, ps, pr, xs, xr, ws, wr, ss, sr, us, ur,
):
    grp = lax.axis_index("grp")
    st = lax.axis_index("st")
    tp = lax.axis_index("tp")
    hi_n = tp_n // 2
    hi, lo = tp // 2, tp % 2
    mate_t = hi * 2 + 1 - lo
    mate = {"tp": mate_t}
    twin = {"grp": 1 - grp}
    pass_rows, chunk = rows.shape[1], rows.shape[2]
    passages = pass_rows // pass_len
    model = wqg.shape[0]
    cols = q_v.shape[1]
    heads = cols // HD
    tok_rows = q_v.shape[0]
    blocks = tok_rows // BLK
    half_pass = passages // 2
    some = tile_of(half_pass, 2)
    some_rows = some * pass_len
    n_some = half_pass // some
    key_cols, value_cols = slice(0, cols), slice(cols, 2 * cols)

    def local(i, src, dst):
        copy = pltpu.make_async_copy(src, dst, lsem.at[i])
        copy.start()
        return copy

    ids_copy = local(9, ids_hbm, ids_ref)
    own_rows = local(0, store_ref, rows.at[tp])
    loads_kv = [
        local(1, wk_hbm, wall.at[tp, :, pl.ds(0, cols)]),
        local(2, wv_hbm, wall.at[tp, :, pl.ds(cols, cols)]),
    ]
    loads_q = [
        local(3, q_hbm, q_v),
        local(4, g_hbm, g_v),
        local(5, m_hbm, m_v),
        local(6, wq_hbm, wqg.at[:, pl.ds(0, cols)]),
        local(7, wg_hbm, wqg.at[:, pl.ds(cols, cols)]),
    ]

    barrier = pltpu.get_barrier_semaphore()

    def greet_st(d, c):
        pl.semaphore_signal(
            barrier, inc=1, device_id={"st": (st + d) % st_n}, device_id_type=MESH
        )
        return c

    lax.fori_loop(1, st_n, greet_st, 0)
    for d in range(1, tp_n):
        pl.semaphore_signal(
            barrier, inc=1, device_id={"tp": (tp + d) % tp_n}, device_id_type=MESH
        )
    pl.semaphore_signal(barrier, inc=1, device_id=twin, device_id_type=MESH)

    ids_copy.wait()

    def plan(wide):
        line = lax.broadcasted_iota(jnp.int32, (8, wide), 0)
        return line, lax.broadcasted_iota(jnp.int32, (8, wide), 1)

    width = ask_v.shape[2]
    line, lane = plan(width)
    slot, place = lane // pass_len, lane % pass_len
    short_line, short_lane = plan(order_v.shape[1])
    target = jnp.full((8, width), -1, jnp.int32)
    order = jnp.zeros(order_v.shape, jnp.int32)
    taken = [jnp.int32(0)] * st_n
    for j in range(PB):
        for n in range(blocks):
            i = ids_ref[j, n]
            owner = lax.div(i, jnp.int32(passages))
            within = i - owner * passages
            rank = sum(jnp.where(owner == o, taken[o], 0) for o in range(st_n))
            taken = [taken[o] + jnp.where(owner == o, 1, 0) for o in range(st_n)]
            target = jnp.where(
                (line == owner) & (slot == rank), within * pass_len + place, target
            )
            order = jnp.where(
                (short_line == owner) & (short_lane == rank), j * blocks + n, order
            )
    order_v[...] = order
    for o in range(st_n):
        ask_v[o] = jnp.broadcast_to(target[o : o + 1], (8, width))
    pl.semaphore_wait(barrier, st_n + tp_n - 1)

    def first_row(i):
        part = (grp + i // n_some) % 2
        return pl.multiple_of((part * n_some + i % n_some) * some_rows, some_rows)

    def g_copy(way, i, t, source, peer, slot):
        r = pl.ds(first_row(i), some_rows)
        return remote(rows.at[source, r], rows.at[t, r], gs.at[way, slot, i], gr.at[t, i], peer)

    def across(d, i):
        h = (hi + d) % hi_n
        return g_copy(0, i, tp, tp, {"tp": h * 2 + lo}, h)

    def beside(i):
        return g_copy(1, i, tp, tp, mate, hi)

    def onward(d, i):
        h = (hi + d) % hi_n
        return g_copy(2, i, h * 2 + lo, h * 2 + lo, mate, h)

    def g_wait(t, i):
        g_copy(1, i, t, t, mate, hi).wait_recv()

    def rows_send(i, c):
        for d in range(1, hi_n):
            across(d, i).start()
        beside(i).start()
        return c

    own_rows.wait()
    lax.fori_loop(0, 2 * n_some, rows_send, 0)

    upper = st >= st_n // 2
    mark = jnp.where(upper, st, st_n - 1 - st)

    def far_peer(d):
        i = d - 1
        i = i + jnp.where(i >= mark, 1, 0)
        return jnp.where(upper, i, st_n - 1 - i)

    def z_copy(phase, src, dst, peer):
        return remote(src, dst, zs.at[phase, peer], zr.at[phase, st], {"st": peer})

    def z_wait(phase, src, dst, peer):
        remote(src, dst, zs.at[phase, peer], zr.at[phase, peer], {"st": peer}).wait_recv()

    def ask_send(d, c):
        peer = (st + d) % st_n
        z_copy(0, ask_v.at[peer], ask_in.at[st], peer).start()
        return c

    lax.fori_loop(1, st_n, ask_send, 0)
    ask_in[st] = ask_v[st]
    order_copy = local(8, order_v, req_ref)

    def project(i, count, send):
        r = pl.ds(first_row(i), count * some_rows)

        def term(t, span):
            return dot(rows[t, r], wall[tp, pl.ds(pl.multiple_of(t * chunk, chunk), chunk), span])

        for q in range(count):
            for d in range(1, hi_n):
                g_wait(((hi + d) % hi_n) * 2 + lo, i + q)
                onward(d, i + q).start()
            g_wait(mate_t, i + q)
        near = [tp, mate_t] + [((hi + d) % hi_n) * 2 + lo for d in range(1, hi_n)]
        late = [((hi + d) % hi_n) * 2 + 1 - lo for d in range(1, hi_n)]
        total = sum(term(t, key_cols) for t in near[1:]) + term(near[0], key_cols)
        for t in late:
            for q in range(count):
                g_wait(t, i + q)
            total = total + term(t, key_cols)
        first = st * passages + first_row(i) // pass_len

        def keep(ref, total):
            low = total.astype(BF)
            for p in range(count * some):
                ref[first + p] = low[p * pass_len : (p + 1) * pass_len]

        keep(k_all, total)
        send()
        keep(v_all, sum(term(t, value_cols) for t in near + late))

    def part_of_all(kind, o, c, side):
        ref = k_all if kind == 0 else v_all
        return ref.at[pl.ds(o * passages + side * half_pass + c * some, some)]

    def chain_copy(kind, o, c, way, peer):
        part = part_of_all(kind, o, c, grp)
        return remote(part, part, fs.at[kind, o, c, way], fr.at[kind, o, c, 0], {"st": peer})

    def twin_copy(kind, o, c):
        part = part_of_all(kind, o, c, grp)
        return remote(part, part, fs.at[kind, o, c, 2], fr.at[kind, o, c, 1], twin)

    lower = st < st_n // 2
    edge = (st == 0) | (st == st_n - 1)

    def own_copies(kind, c, act, inward=True, outward=True):
        ways = ((0, st + 1, lower), (1, st - 1, jnp.logical_not(lower)))
        for way, onto, toward in ways:
            there = (onto >= 0) & (onto < st_n)
            if not outward:
                there = there & toward
            if not inward:
                there = there & jnp.logical_not(toward)

            @pl.when(there)
            def _():
                act(chain_copy(kind, st, c, way, onto))

    def relay_copies(kind, d, c, act, ready):
        for way, sign in ((0, -1), (1, 1)):
            o = st + sign * d
            onto = st - sign

            @pl.when((o >= 0) & (o < st_n))
            def _():
                if ready:
                    chain_copy(kind, o, c, way, st).wait_recv()

                @pl.when((onto >= 0) & (onto < st_n))
                def _():
                    act(chain_copy(kind, o, c, way, onto))

                act(twin_copy(kind, o, c))

    def start(copy):
        copy.start()

    def own_send(kind, c, **which):
        own_copies(kind, c, start, **which)

    def relay(kind, d, c):
        relay_copies(kind, d, c, start, True)

    def twin_wait(kind):
        def step(i, c):
            o = (st + 1 + i // n_some) % st_n
            k = i % n_some
            part = part_of_all(kind, o, k, 1 - grp)
            remote(part, part, fs.at[kind, o, k, 2], fr.at[kind, o, k, 1], twin).wait_recv()
            return c

        lax.fori_loop(0, (st_n - 1) * n_some, step, 0)

    for copy in loads_kv + loads_q[:3]:
        copy.wait()

    gate_rows = tok_rows // n_some

    def gates(i):
        r = pl.ds(pl.multiple_of(i * gate_rows, gate_rows), gate_rows)
        gate = g_v[r, :].astype(F32)
        grad = m_v[r, :].astype(F32)
        sig = 1.0 / (1.0 + jnp.exp(-gate))
        gated[r, :] = (gate * sig * grad).astype(BF)
        slope[r, :] = grad * (sig * (1.0 + gate * (1.0 - sig)))

    def early_step(i, c):
        project(i, 1, lambda: own_send(0, i))

        @pl.when(i >= 1)
        def _():
            relay(0, 1, i - 1)

        @pl.when(edge | (i == 0))
        def _():
            own_send(1, i, outward=False)

        gates(i)
        return c

    lax.fori_loop(0, n_some, early_step, 0)
    for i in range(n_some - 1, n_some):
        relay(0, 1, i)

    def inward_send(i, c):
        own_send(1, i, outward=False)
        return c

    lax.fori_loop(jnp.where(edge, n_some, 1), n_some, inward_send, 0)

    def second_step(i, c):
        relay(0, 2, i)
        return c

    def outward_send(i, c):
        own_send(1, i, inward=False)
        return c

    lax.fori_loop(0, n_some, second_step, 0)
    lax.fori_loop(0, n_some, outward_send, 0)

    n_part = tile_of(n_some, 2)

    def late_step(i, c):
        project(n_some + i * n_part, n_part, lambda: None)
        for q in range(n_part):
            @pl.when(edge)
            def _():
                relay(0, 3, i * n_part + q)

            @pl.when(jnp.logical_not(edge))
            def _():
                relay(1, 1, i * n_part + q)

        return c

    w_part = model // 2
    w_mine = pl.ds(pl.multiple_of(grp * w_part, w_part), w_part)
    w_other = pl.ds(pl.multiple_of((1 - grp) * w_part, w_part), w_part)

    def w_across(d):
        h = (hi + d) % hi_n
        part = wall.at[tp, w_mine]
        return remote(part, part, ws.at[0, h], wr.at[0, tp], {"tp": h * 2 + lo})

    def w_twin(d):
        t = ((hi + d) % hi_n) * 2 + lo
        part = wall.at[t, w_mine]
        return remote(part, part, ws.at[1, (hi + d) % hi_n], wr.at[1, t], twin)

    def w_onward(d, k):
        t = ((hi + d) % hi_n) * 2 + lo
        part = wall.at[t, w_other if k else w_mine]
        return remote(part, part, ws.at[2 + k, (hi + d) % hi_n], wr.at[2 + k, t], mate)

    w_beside = remote(wall.at[tp], wall.at[tp], ws.at[4, 0], wr.at[4, tp], mate)

    def w_wait(kind, t, part):
        remote(wall.at[t, part], wall.at[t, part], ws.at[kind, 0], wr.at[kind, t], mate).wait_recv()

    for d in range(1, hi_n):
        w_across(d).start()

    def relay_rest(kind, first, last):
        def step(i, c):
            relay(kind, 1 + i // n_some, i % n_some)
            return c

        lax.fori_loop(first, last, step, 0)

    relays = (st_n - 1) * n_some
    lax.fori_loop(0, n_some // n_part, late_step, 0)
    w_beside.start()
    relay_rest(1, 0, jnp.where(edge, n_some, 0))
    for copy in loads_q[3:]:
        copy.wait()
    order_copy.wait()
    twin_wait(0)
    scale = HD ** (-0.5)

    def fill(n, ref, span, b):
        for j in range(PB):
            kvb[n, j * pass_len : (j + 1) * pass_len, span] = ref[ids_ref[j, b]]

    pairs = range(4)

    def block_rows(b):
        return pl.ds(pl.multiple_of(b * BLK, BLK), BLK)

    per_step = n_some // (blocks // 4)

    def probs_step(i, c):
        for n in pairs:
            fill(n, k_all, key_cols, 4 * i + n)
        for head in range(heads):
            hs = slice(head * HD, (head + 1) * HD)
            vs = slice(cols + head * HD, cols + (head + 1) * HD)
            for n in pairs:
                b = 4 * i + n
                r = block_rows(b)
                scores = dot(q_v[r, hs], kvb[n, :, hs], NT) * scale
                shifted = jnp.exp(scores - jnp.max(scores, axis=-1, keepdims=True))
                prob = shifted * (1.0 / jnp.sum(shifted, axis=-1, keepdims=True))
                prob_v[head, r, :] = prob
                value_grad = dot(prob.astype(BF), gated[r, hs], TN).astype(BF)
                for j in range(PB):
                    reqg[j * blocks + b, :, vs] = value_grad[j * pass_len : (j + 1) * pass_len]

        for q in range(per_step):
            relay(1, 2, i * per_step + q)

        return c

    lax.fori_loop(0, blocks // 4, probs_step, 0)

    def half(ref, peer, part):
        return ref.at[peer, :, :, part]

    def back_copy(phase, part, peer):
        return z_copy(phase, half(ret, peer, part), half(arr, st, part), peer)

    def give_back(phase, part, span, order, first, last):
        def send(d, c):
            peer = order(d)
            for k in range(depth):
                ret[peer, k, :, span] = reqg[req_ref[peer, k]][:, span]
            back_copy(phase, part, peer).start()
            return c

        lax.fori_loop(first, last, send, 0)

    def keep_own(span):
        for k in range(depth):
            arr[st, k, :, span] = reqg[req_ref[st, k]][:, span]

    def near_peer(d):
        return far_peer(st_n - d)

    ks, vs_all = pl.ds(0, cols), pl.ds(cols, cols)
    def value_peer(d):
        return jnp.where(edge, near_peer(d % (st_n - 1) + 1), near_peer(d))

    give_back(
        1, vs_all, value_cols, value_peer, 1, jnp.where(edge, st_n, st_n - 1)
    )
    keep_own(value_cols)
    relay_rest(1, n_some + per_step * (blocks // 4), relays)
    twin_wait(1)

    def block_step(i, c):
        for n in pairs:
            fill(n, k_all, key_cols, 4 * i + n)
            fill(n, v_all, value_cols, 4 * i + n)
        for head in range(heads):
            hs = slice(head * HD, (head + 1) * HD)
            vs = slice(cols + head * HD, cols + (head + 1) * HD)
            for n in pairs:
                b = 4 * i + n
                r = block_rows(b)
                value = kvb[n, :, vs]
                prob = prob_v[head, r, :]
                prob_grad = dot(gated[r, hs], value, NT)
                inner = jnp.sum(prob * prob_grad, axis=-1, keepdims=True)
                score_grad = (scale * prob * (prob_grad - inner)).astype(BF)
                key_grad = dot(score_grad, q_v[r, hs], TN).astype(BF)
                for j in range(PB):
                    reqg[j * blocks + b, :, hs] = key_grad[j * pass_len : (j + 1) * pass_len]
                gboth[r, hs] = dot(score_grad, kvb[n, :, hs]).astype(BF)
                attended = dot(prob.astype(BF), value)
                gboth[r, vs] = (attended * slope[r, hs]).astype(BF)
        return c

    lax.fori_loop(0, blocks // 4, block_step, 0)
    def key_peer(d):
        return jnp.where(edge, near_peer(jnp.where(d == 1, 1, st_n + 1 - d)), far_peer(d))

    give_back(2, ks, key_cols, key_peer, 1, st_n)
    keep_own(key_cols)

    n_tile = tile_of(model, 512)

    def expand(h):
        a = gboth[pl.ds(pl.multiple_of(h * 2 * tok_pair, tok_pair), 2 * tok_pair), :]

        def step(i, c):
            n = pl.ds(pl.multiple_of(i * n_tile, n_tile), n_tile)
            part = dot(a, wqg[n, :], NT).astype(BF)
            tp_part[h * 2, :, n] = part[:tok_pair]
            tp_part[h * 2 + 1, :, n] = part[tok_pair:]
            return c

        lax.fori_loop(0, model // n_tile, step, 0)

    def pair_copy(h):
        return remote(tp_part.at[h * 2 + 1 - lo], tp_pair.at[h], ps.at[h], pr.at[h], mate)

    def cross(h):
        return remote(
            tp_part.at[h * 2 + lo], tp_recv.at[hi], xs.at[h], xr.at[hi], {"tp": h * 2 + lo}
        )

    for d in range(1, hi_n):
        w_wait(0, ((hi + d) % hi_n) * 2 + lo, w_mine)
        w_twin(d).start()
        w_onward(d, 0).start()

    tok_pair = tok_rows // tp_n
    for d in range(1, hi_n + 1):
        h = (hi + d) % hi_n
        expand(h)
        pair_copy(h).start()
    for d in range(1, hi_n):
        h = (hi + d) % hi_n
        pair_copy(h).wait_recv()
        tp_part[h * 2 + lo] = (tp_part[h * 2 + lo].astype(F32) + tp_pair[h].astype(F32)).astype(BF)
        cross(h).start()

    def ask_wait(d, c):
        peer = (st + d) % st_n
        z_wait(0, ask_v.at[peer], ask_in.at[peer], peer)
        return c

    lax.fori_loop(1, st_n, ask_wait, 0)
    hot_cols = depth * pass_len
    m_tile = tile_of(pass_rows, 256)

    def hot_step(o, c):
        target = ask_in[o][0:1, :hot_cols]
        for i in range(pass_rows // m_tile):
            line = lax.broadcasted_iota(jnp.int32, (m_tile, hot_cols), 0) + i * m_tile
            hot[o, i * m_tile : (i + 1) * m_tile, :] = jnp.where(line == target, 1.0, 0.0).astype(BF)
        return c

    lax.fori_loop(0, st_n, hot_step, 0)

    def gather_sums(kind, o, span, first):
        def step(i, c):
            r = pl.ds(pl.multiple_of(i * m_tile, m_tile), m_tile)
            part = dot(hot[o, r, :], arr[o, :, :, span].reshape(hot_cols, cols))
            acc[kind, r, :] = part if first else acc[kind, r, :] + part
            return c

        lax.fori_loop(0, pass_rows // m_tile, step, 0)

    sto_pair = pass_rows // tp_n

    def sums_copy(kind, part, d):
        t = (tp + d) % tp_n
        src = plow.at[pl.ds(pl.multiple_of(t * sto_pair, sto_pair), sto_pair), part]
        return remote(src, sums.at[tp, :, part], ss.at[kind, t], sr.at[kind, tp], {"tp": t})

    def sums_wait(kind, part, t):
        dst = sums.at[t, :, part]
        remote(dst, dst, ss.at[kind, t], sr.at[kind, t], mate).wait_recv()

    def grads_of(kind, peer):
        phase, part, span = (2, ks, key_cols) if kind == 0 else (1, vs_all, value_cols)
        z_wait(phase, half(ret, peer, part), half(arr, peer, part), peer)
        gather_sums(kind, peer, span, False)

    def sums_send(kind):
        part, span = (ks, key_cols) if kind == 0 else (vs_all, value_cols)
        plow[:, span] = acc[kind].astype(BF)
        for d in range(1, tp_n):
            sums_copy(kind, part, d).start()
        sums[tp, :, span] = plow[pl.ds(pl.multiple_of(tp * sto_pair, sto_pair), sto_pair), span]

    beyond = jnp.where(lower, st_n - 1, 0)
    middle = jnp.where(lower, st_n // 2, st_n // 2 - 1)
    beside_st = st + 1 - 2 * (st % 2)
    outer = edge
    inner = jnp.logical_not(outer)
    gather_sums(1, st, value_cols, True)
    gather_sums(0, st, key_cols, True)
    grads_of(1, beside_st)
    grads_of(1, jnp.where(outer, beyond, middle))

    grads_of(0, middle)

    @pl.when(inner)
    def _():
        give_back(1, vs_all, value_cols, near_peer, st_n - 1, st_n)

    grads_of(0, beyond)
    grads_of(0, beside_st)
    sums_send(0)

    share = model // st_n
    bits = 2
    bit = share // bits

    def dw_line(s, b):
        return pl.ds(pl.multiple_of(s * share + b * bit, bit), bit)

    def dw_copy(kind, b):
        line = pl.ds(b * bit, bit)
        if kind < 2:
            src, dst = dwp.at[dw_line(middle if kind else beyond, b)], dwc.at[kind, line]
            peer = beside_st
        elif kind == 2:
            src, dst, peer = dwp.at[dw_line(beside_st, b)], dwf.at[0, line], beside_st
        else:
            src, dst = dwc.at[kind - 3, line], dwf.at[1, line]
            peer = middle if kind == 4 else beyond
        return remote(src, dst, us.at[kind, b], ur.at[kind, b], {"st": peer})

    def dw_send(kind):
        for b in range(bits):
            dw_copy(kind, b).start()

    def dw_relay(q):
        for b in range(bits):
            line = slice(b * bit, (b + 1) * bit)
            dw_copy(q, b).wait_recv()
            own = dwp[dw_line(middle if q else beyond, b), :].astype(F32)
            dwc[q, line, :] = (dwc[q, line, :].astype(F32) + own).astype(BF)
            dw_copy(3 + q, b).start()

    def wkey_step(s):
        dwp[pl.ds(pl.multiple_of(s * chunk, chunk), chunk), :] = dot(
            rows[s], plow[:, key_cols], TN
        ).astype(BF)

    def wkey_turn(j, c):
        far = jnp.where(j == 0, beyond, middle)
        near = jnp.where(j == 2, beside_st, st)
        near_first = jnp.where(j == 0, beside_st, st)
        far_after = jnp.where(j == 1, beyond, middle)
        s = jnp.where(
            outer, jnp.where(j < 2, far, near), jnp.where((j == 0) | (j == 3), near_first, far_after)
        )
        wkey_step(s)
        for kind in range(3):
            @pl.when(outer & (j == kind))
            def _():
                dw_send(kind)

        @pl.when(inner & (j == 0))
        def _():
            dw_send(2)

        return c

    lax.fori_loop(0, st_n, wkey_turn, 0)

    @pl.when(inner)
    def _():
        dw_relay(0)

    for d in range(1, hi_n):
        t = ((hi + d) % hi_n) * 2 + lo
        w_wait(1, t, w_other)
        w_onward(d, 1).start()
    w_wait(4, mate_t, pl.ds(0, model))
    for d in range(1, hi_n):
        t = ((hi + d) % hi_n) * 2 + 1 - lo
        w_wait(2, t, w_mine)
        w_wait(3, t, w_other)

    def store_terms(span, done):
        def step(i, c):
            n = pl.ds(pl.multiple_of(i * n_tile, n_tile), n_tile)
            part = dot(sums[0, :, span], wall[0, n, span], NT)
            for t in range(1, tp_n):
                part = part + dot(sums[t, :, span], wall[t, n, span], NT)
            done(n, part)
            return c

        lax.fori_loop(0, model // n_tile, step, 0)

    def keep_terms(n, part):
        terms[:, n] = part

    def keep_store(n, part):
        store_out[:, n] = (terms[:, n] + part).astype(BF)

    grads_of(1, jnp.where(outer, middle, beyond))
    sums_send(1)

    for d in range(1, tp_n):
        sums_wait(0, ks, (tp + d) % tp_n)
    store_terms(key_cols, keep_terms)

    pair_copy(hi).wait_recv()
    for d in range(1, hi_n):
        h = (hi + d) % hi_n
        remote(
            tp_part.at[h * 2 + lo], tp_recv.at[h], xs.at[h], xr.at[h], {"tp": h * 2 + lo}
        ).wait_recv()
    total = tp_part[tp].astype(F32) + tp_pair[hi].astype(F32)
    for d in range(1, hi_n):
        total = total + tp_recv[(hi + d) % hi_n].astype(F32)
    tok_out[...] = total.astype(BF)
    tok_done = local(10, tok_out, tok_hbm)

    @pl.when(inner)
    def _():
        dw_relay(1)

    for d in range(1, tp_n):
        sums_wait(1, vs_all, (tp + d) % tp_n)
    store_terms(value_cols, keep_store)
    store_done = local(11, store_out, store_hbm)

    for b in range(bits):
        line = slice(b * bit, (b + 1) * bit)
        dw_copy(2, b).wait_recv()
        wkey_out[line, :] = dwp[dw_line(st, b), :].astype(F32) + dwf[0, line, :].astype(F32)
    for b in range(bits):
        line = slice(b * bit, (b + 1) * bit)
        for kind, edge in ((3, outer), (4, inner)):
            @pl.when(edge)
            def _():
                dw_copy(kind, b).wait_recv()

        wkey_out[line, :] += dwf[1, line, :].astype(F32)

    wkey_done = local(12, wkey_out, wkey_hbm)

    def wait_send(copy):
        copy.wait_send()

    def rows_drain(i, c):
        for d in range(1, hi_n):
            across(d, i).wait_send()
            onward(d, i).wait_send()
        beside(i).wait_send()
        return c

    lax.fori_loop(0, 2 * n_some, rows_drain, 0)

    def all_drain(i, c):
        for kind in (0, 1):
            own_copies(kind, i, wait_send)
            for d in range(1, st_n):
                relay_copies(kind, d, i, wait_send, False)
        return c

    lax.fori_loop(0, n_some, all_drain, 0)
    for d in range(1, hi_n):
        w_across(d).wait_send()
        w_twin(d).wait_send()
        w_onward(d, 0).wait_send()
        w_onward(d, 1).wait_send()
    w_beside.wait_send()

    def drain(d, c):
        peer = (st + d) % st_n
        z_copy(0, ask_v.at[peer], ask_in.at[st], peer).wait_send()
        back_copy(1, vs_all, peer).wait_send()
        back_copy(2, ks, peer).wait_send()
        return c

    lax.fori_loop(1, st_n, drain, 0)
    for d in range(1, tp_n):
        sums_copy(0, ks, d).wait_send()
        sums_copy(1, vs_all, d).wait_send()
    for d in range(1, hi_n + 1):
        h = (hi + d) % hi_n
        pair_copy(h).wait_send()
        if d < hi_n:
            cross(h).wait_send()
    for b in range(bits):
        dw_copy(2, b).wait_send()
        for q in (0, 1):
            @pl.when(outer)
            def _():
                dw_copy(q, b).wait_send()

            @pl.when(inner)
            def _():
                dw_copy(3 + q, b).wait_send()
    for copy in (tok_done, store_done, wkey_done):
        copy.wait()


def settle_kernel(*refs):
    n = (len(refs) - 2) // 3
    sources, results, held = refs[:n], refs[n : 2 * n], refs[2 * n : 3 * n]
    ins, outs = refs[3 * n], refs[3 * n + 1]
    pieces = []
    for a, (source, result, here) in enumerate(zip(sources, results, held)):
        part = source.shape[0] // 2
        for i in range(2):
            r = pl.ds(i * part, part)
            pieces.append(
                (
                    pltpu.make_async_copy(source.at[r], here.at[r], ins.at[a, i]),
                    pltpu.make_async_copy(here.at[r], result.at[r], outs.at[a, i]),
                )
            )
    for fetch, _ in pieces:
        fetch.start()
    for fetch, put in pieces:
        fetch.wait()
        put.start()
    for _, put in pieces:
        put.wait()


def settle(*arrays):
    hbm = pl.BlockSpec(memory_space=pl.ANY)
    n = len(arrays)
    return pl.pallas_call(
        settle_kernel,
        out_shape=tuple(jax.ShapeDtypeStruct(a.shape, a.dtype) for a in arrays),
        in_specs=[hbm] * n,
        out_specs=(hbm,) * n,
        scratch_shapes=[pltpu.VMEM(a.shape, a.dtype) for a in arrays]
        + [pltpu.SemaphoreType.DMA((n, 2)), pltpu.SemaphoreType.DMA((n, 2))],
    )(*arrays)


def local(pass_ids, store, queries, gate_pre, w_query, w_gate, w_key, w_value, d_mem):
    st_n = lax.axis_size("st")
    tp_n = lax.axis_size("tp")
    hi_n = tp_n // 2
    tok_rows, cols = queries.shape
    blocks = tok_rows // BLK
    passages, pass_len, chunk = store.shape
    model = w_key.shape[0]
    requests = blocks * PB
    depth = max(2, requests // st_n)
    pass_rows = passages * pass_len
    share = model // st_n

    vmem = pl.BlockSpec(memory_space=pltpu.VMEM)
    smem = pl.BlockSpec(memory_space=pltpu.SMEM)
    hbm = pl.BlockSpec(memory_space=pl.ANY)
    V = pltpu.VMEM
    DMA = pltpu.SemaphoreType.DMA
    pair = 2 * cols
    tok_pair = tok_rows // tp_n
    sto_pair = pass_rows // tp_n
    hot_cols = depth * pass_len
    width = -(-hot_cols // 128) * 128
    gathered_bytes = 2 * 2 * st_n * pass_rows * cols
    steps = blocks // 4
    fits = lax.axis_size("grp") == 2 and hi_n == 2 and st_n == 4 and st_n == tp_n
    fits = fits and passages % 4 == 0 and blocks % 4 == 0 and passages // 4 % steps == 0
    if fits and gathered_bytes <= 8 << 20:
        half_pass = passages // 2
        n_some = half_pass // tile_of(half_pass, 2)
        d_tokens, d_store, d_wkey = pl.pallas_call(
            functools.partial(gathered_kernel, st_n, tp_n, depth, pass_len),
            out_shape=(
                jax.ShapeDtypeStruct((tok_pair, model), BF),
                jax.ShapeDtypeStruct((sto_pair, model), BF),
                jax.ShapeDtypeStruct((share, cols), F32),
            ),
            in_specs=[hbm] * 9,
            out_specs=(hbm, hbm, hbm),
            scratch_shapes=[
                pltpu.SMEM((PB, blocks), jnp.int32),
                V((tok_pair, model), BF),
                V((sto_pair, model), BF),
                V((share, cols), F32),
                V((tp_n, pass_rows, chunk), BF),
                V((tp_n, model, pair), BF),
                V((model, pair), BF),
                V((tok_rows, cols), BF),
                V((tok_rows, cols), BF),
                V((tok_rows, cols), BF),
                V((2, pass_rows, cols), F32),
                V((sto_pair, model), F32),
                V((st_n * passages, pass_len, cols), BF),
                V((st_n * passages, pass_len, cols), BF),
                V((st_n, 8, width), jnp.int32),
                V((st_n, 8, width), jnp.int32),
                V((8, 128), jnp.int32),
                pltpu.SMEM((8, 128), jnp.int32),
                V((tok_rows, cols), BF),
                V((tok_rows, cols), F32),
                V((st_n, depth, pass_len, pair), BF),
                V((cols // HD, tok_rows, PB * pass_len), F32),
                V((4, PB * pass_len, pair), BF),
                V((requests, pass_len, pair), BF),
                V((tok_rows, pair), BF),
                V((st_n, depth, pass_len, pair), BF),
                V((st_n, pass_rows, hot_cols), BF),
                V((pass_rows, pair), BF),
                V((tp_n, sto_pair, pair), BF),
                V((model, cols), BF),
                V((2, share, cols), BF),
                V((2, share, cols), BF),
                V((tp_n, tok_pair, model), BF),
                V((hi_n, tok_pair, model), BF),
                V((hi_n, tok_pair, model), BF),
                DMA((13,)),
                DMA((3, hi_n, 2 * n_some)),
                DMA((tp_n, 2 * n_some)),
                DMA((2, st_n, n_some, 3)),
                DMA((2, st_n, n_some, 2)),
                DMA((3, st_n)),
                DMA((3, st_n)),
                DMA((hi_n,)),
                DMA((hi_n,)),
                DMA((hi_n,)),
                DMA((hi_n,)),
                DMA((5, hi_n)),
                DMA((5, tp_n)),
                DMA((2, tp_n)),
                DMA((2, tp_n)),
                DMA((5, 2)),
                DMA((5, 2)),
            ],
            compiler_params=pltpu.CompilerParams(
                collective_id=0, has_side_effects=True, vmem_limit_bytes=67043328
            ),
        )(
            pass_ids.T, store.reshape(pass_rows, chunk),
            queries, gate_pre, w_query, w_gate, w_key, w_value, d_mem,
        )
        d_tokens, d_store, d_wkey = settle(d_tokens, d_store, d_wkey)
        return d_tokens, d_store.reshape(passages // tp_n, pass_len, model), d_wkey

    ids = pass_ids.reshape(-1)
    owners = ids // passages
    within = ids % passages
    order = jnp.arange(requests, dtype=jnp.int32)
    earlier = (owners[None, :] == owners[:, None]) & (order[None, :] < order[:, None])
    rank = jnp.sum(earlier.astype(jnp.int32), axis=1)
    slots = jnp.stack([owners, rank])
    o_i = jnp.arange(st_n, dtype=jnp.int32)[:, None, None]
    k_i = jnp.arange(depth, dtype=jnp.int32)[None, :, None]
    match = (owners[None, None, :] == o_i) & (rank[None, None, :] == k_i)
    asked = jnp.max(jnp.where(match, within[None, None, :], -1), axis=2)
    req_of = jnp.max(jnp.where(match, order[None, None, :], 0), axis=2)
    hot_cols = depth * pass_len
    width = -(-hot_cols // 128) * 128
    lane = jnp.arange(width, dtype=jnp.int32)
    spread = jnp.repeat(asked, pass_len, axis=1)
    spread = jnp.pad(spread, ((0, 0), (0, width - hot_cols)), constant_values=-1)
    target = jnp.where(spread < 0, -1, spread * pass_len + lane[None, :] % pass_len)
    flat = jnp.pad(jnp.maximum(asked, 0), ((0, 0), (0, width - depth)))
    ask = jnp.concatenate(
        [target[:, None], flat[:, None], jnp.zeros((st_n, 6, width), jnp.int32)], axis=1
    )

    d_tokens, d_store, d_wkey = pl.pallas_call(
        functools.partial(kernel, st_n, tp_n, depth, pass_len),
        out_shape=(
            jax.ShapeDtypeStruct((tok_pair, model), BF),
            jax.ShapeDtypeStruct((sto_pair, model), BF),
            jax.ShapeDtypeStruct((share, cols), F32),
        ),
        in_specs=[smem, smem, vmem] + [hbm] * 8,
        out_specs=(vmem, vmem, vmem),
        scratch_shapes=[
            V((tp_n, pass_rows, chunk), BF),
            V((model, pair), BF),
            V((model, pair), BF),
            V((tok_rows, cols), BF),
            V((tok_rows, cols), BF),
            V((tok_rows, cols), BF),
            V((pass_rows, pair), F32),
            V((passages, pass_len, pair), BF),
            V((st_n, 8, width), jnp.int32),
            pltpu.SMEM((st_n, 8, width), jnp.int32),
            V((st_n, depth, pass_len, pair), BF),
            V((st_n, depth, pass_len, cols), BF),
            V((st_n, depth, pass_len, cols), BF),
            V((st_n, depth, pass_len, pair), BF),
            V((cols // HD, tok_rows, PB * pass_len), F32),
            V((PB * pass_len, pair), BF),
            V((requests, pass_len, pair), BF),
            V((tok_rows, pair), BF),
            V((st_n, depth, pass_len, pair), BF),
            V((st_n, pass_rows, hot_cols), BF),
            V((pass_rows, pair), BF),
            V((model, cols), BF),
            V((st_n, share, cols), BF),
            V((tp_n, tok_pair, model), BF),
            V((hi_n, tok_pair, model), BF),
            V((hi_n, tok_pair, model), BF),
            V((tp_n, sto_pair, model), BF),
            V((hi_n, sto_pair, model), BF),
            V((hi_n, sto_pair, model), BF),
            DMA((9,)),
            DMA((3, hi_n)),
            DMA((tp_n,)),
            DMA((6, st_n)),
            DMA((6, st_n)),
            DMA((2, hi_n)),
            DMA((2, hi_n)),
            DMA((2, hi_n)),
            DMA((2, hi_n)),
        ],
        compiler_params=pltpu.CompilerParams(
            collective_id=0, has_side_effects=True, vmem_limit_bytes=67043328
        ),
    )(
        slots, req_of, ask, store.reshape(pass_rows, chunk),
        queries, gate_pre, w_query, w_gate, w_key, w_value, d_mem,
    )
    return d_tokens, d_store.reshape(passages // tp_n, pass_len, model), d_wkey


def solution(mesh):
    return jax.shard_map(
        local,
        mesh=mesh,
        in_specs=(
            P(("grp", "st"), None),
            P("st", None, "tp"),
            P(("grp", "st"), "tp"),
            P(("grp", "st"), "tp"),
            P(None, "tp"),
            P(None, "tp"),
            P(None, "tp"),
            P(None, "tp"),
            P(("grp", "st"), "tp"),
        ),
        out_specs=(
            P(("grp", "st", "tp"), None),
            P(("grp", "st", "tp"), None, None),
            P(("grp", "st"), "tp"),
        ),
        check_vma=False,
    )
```

```python
import functools

import jax
import jax.numpy as jnp
from jax import lax
from jax.experimental import pallas as pl
from jax.experimental.pallas import tpu as pltpu
from jax.sharding import PartitionSpec as P

HD = 256
BLK = 128
PB = 4
BF = jnp.bfloat16
F32 = jnp.float32
MESH = pl.DeviceIdType.MESH
NT = (((1,), (1,)), ((), ()))
TN = (((0,), (0,)), ((), ()))


def dot(a, b, dims=(((1,), (0,)), ((), ()))):
    return lax.dot_general(a, b, dims, preferred_element_type=F32)


def remote(src, dst, send, recv, device):
    return pltpu.make_async_remote_copy(
        src_ref=src,
        dst_ref=dst,
        send_sem=send,
        recv_sem=recv,
        device_id=device,
        device_id_type=MESH,
    )


def tile_of(size, most):
    while size % most:
        most //= 2
    return most


def kernel(
    st_n, tp_n, depth, pass_len,
    slot_ref, req_ref, ask_ref, store_ref, q_hbm, g_hbm, wq_hbm, wg_hbm, wk_hbm, wv_hbm, m_hbm,
    tok_out, store_out, wkey_out,
    rows, wkv, wqg, q_v, g_v, m_v, acc, kv, ask_in, ask_s, out, inc_k, inc_v, ret, prob_v, kvb, reqg, gboth, arr,
    hot, plow, dwp, dwr, tp_part, tp_pair, tp_recv, sp_part, sp_pair, sp_recv,
    lsem, gs, gr, zs, zr, ps, pr, xs, xr,
):
    st = lax.axis_index("st")
    tp = lax.axis_index("tp")
    hi_n = tp_n // 2
    hi, lo = tp // 2, tp % 2
    mate = {"tp": hi * 2 + 1 - lo}
    pass_rows, chunk = rows.shape[1], rows.shape[2]
    model = wqg.shape[0]
    cols = q_v.shape[1]
    heads = cols // HD
    tok_rows = q_v.shape[0]
    blocks = tok_rows // BLK
    blk_keys = PB * pass_len

    def local(i, src, dst):
        copy = pltpu.make_async_copy(src, dst, lsem.at[i])
        copy.start()
        return copy

    own_rows = local(0, store_ref, rows.at[tp])
    loads_kv = [
        local(1, wk_hbm, wkv.at[:, pl.ds(0, cols)]),
        local(2, wv_hbm, wkv.at[:, pl.ds(cols, cols)]),
    ]
    loads_q = [local(3, q_hbm, q_v), local(4, g_hbm, g_v), local(5, m_hbm, m_v)]
    loads_qg = [
        local(6, wq_hbm, wqg.at[:, pl.ds(0, cols)]),
        local(7, wg_hbm, wqg.at[:, pl.ds(cols, cols)]),
    ]

    barrier = pltpu.get_barrier_semaphore()

    def greet_st(d, c):
        pl.semaphore_signal(
            barrier, inc=1, device_id={"st": (st + d) % st_n}, device_id_type=MESH
        )
        return c

    lax.fori_loop(1, st_n, greet_st, 0)
    for d in range(1, tp_n):
        pl.semaphore_signal(
            barrier, inc=1, device_id={"tp": (tp + d) % tp_n}, device_id_type=MESH
        )
    pl.semaphore_wait(barrier, st_n - 1 + tp_n - 1)

    across = []
    for d in range(1, hi_n):
        h = (hi + d) % hi_n
        across.append(
            remote(store_ref, rows.at[tp], gs.at[0, h], gr.at[tp], {"tp": h * 2 + lo})
        )
        across[-1].start()
    beside = remote(store_ref, rows.at[tp], gs.at[1, hi], gr.at[tp], mate)
    beside.start()

    upper = st >= st_n // 2
    mark = jnp.where(upper, st, st_n - 1 - st)

    def far_peer(d):
        i = d - 1
        i = i + jnp.where(i >= mark, 1, 0)
        return jnp.where(upper, i, st_n - 1 - i)

    def z_copy(phase, src, dst, peer):
        return remote(src, dst, zs.at[phase, peer], zr.at[phase, st], {"st": peer})

    def z_wait(phase, src, dst, peer):
        remote(src, dst, zs.at[phase, peer], zr.at[phase, peer], {"st": peer}).wait_recv()

    def ask_send(d, c):
        peer = (st + d) % st_n
        z_copy(0, ask_ref.at[peer], ask_in.at[st], peer).start()
        return c

    lax.fori_loop(1, st_n, ask_send, 0)
    ask_in[st] = ask_ref[st]

    m_tile = tile_of(pass_rows, 256)

    def project(t, first):
        def step(i, c):
            r = pl.ds(pl.multiple_of(i * m_tile, m_tile), m_tile)
            part = dot(rows[t, r], wkv[pl.ds(pl.multiple_of(t * chunk, chunk), chunk), :])
            acc[r] = part if first else acc[r] + part
            return c

        lax.fori_loop(0, pass_rows // m_tile, step, 0)

    def g_wait(t):
        remote(store_ref, rows.at[t], gs.at[1, hi], gr.at[t], mate).wait_recv()

    own_rows.wait()
    for copy in loads_kv:
        copy.wait()
    project(tp, True)
    g_wait(hi * 2 + 1 - lo)
    project(hi * 2 + 1 - lo, False)

    def ask_wait(d, c):
        peer = (st + d) % st_n
        z_wait(0, ask_ref.at[peer], ask_in.at[peer], peer)
        return c

    lax.fori_loop(1, st_n, ask_wait, 0)
    ask_copy = local(8, ask_in, ask_s)
    ask_copy.wait()

    hot_cols = depth * pass_len

    def hot_step(o, c):
        target = ask_in[o][0:1, :hot_cols]
        for i in range(pass_rows // m_tile):
            line = lax.broadcasted_iota(jnp.int32, (m_tile, hot_cols), 0) + i * m_tile
            hot[o, i * m_tile : (i + 1) * m_tile, :] = jnp.where(line == target, 1.0, 0.0).astype(BF)
        return c

    lax.fori_loop(0, st_n, hot_step, 0)
    onward = []
    for d in range(1, hi_n):
        h = (hi + d) % hi_n
        t = h * 2 + lo
        g_wait(t)
        onward.append(remote(rows.at[t], rows.at[t], gs.at[2, h], gr.at[t], mate))
        onward[-1].start()
        project(t, False)
    for d in range(1, hi_n):
        t = ((hi + d) % hi_n) * 2 + 1 - lo
        g_wait(t)
        project(t, False)

    def low_step(i, c):
        kv[i] = acc[pl.ds(pl.multiple_of(i * pass_len, pass_len), pass_len), :].astype(BF)
        return c

    lax.fori_loop(0, pass_rows // pass_len, low_step, 0)

    ks, vs_all = pl.ds(0, cols), pl.ds(cols, cols)

    def half(ref, peer, part):
        return ref.at[peer, :, :, part]

    def key_copy(peer):
        return z_copy(1, half(out, peer, ks), inc_k.at[st], peer)

    def value_copy(peer):
        return z_copy(4, half(out, peer, vs_all), inc_v.at[st], peer)

    def kv_send(d, c):
        peer = far_peer(d)
        for k in range(depth):
            out[peer, k] = kv[ask_s[peer, 1, k]]
        key_copy(peer).start()
        return c

    def value_send(d, c):
        value_copy(far_peer(d)).start()
        return c

    lax.fori_loop(1, st_n, kv_send, 0)
    lax.fori_loop(1, st_n, value_send, 0)
    for k in range(depth):
        picked = kv[ask_s[st, 1, k]]
        inc_k[st, k] = picked[:, :cols]
        inc_v[st, k] = picked[:, cols:]
    for copy in loads_q + loads_qg:
        copy.wait()

    def key_wait(d, c):
        peer = (st + d) % st_n
        z_wait(1, half(out, peer, ks), inc_k.at[peer], peer)
        return c

    lax.fori_loop(1, st_n, key_wait, 0)
    scale = HD ** (-0.5)

    def probs_step(b, c):
        r = pl.ds(pl.multiple_of(b * BLK, BLK), BLK)
        for j in range(PB):
            kvb[j * pass_len : (j + 1) * pass_len, :cols] = inc_k[
                slot_ref[0, b * PB + j], slot_ref[1, b * PB + j]
            ]
        for head in range(heads):
            hs = slice(head * HD, (head + 1) * HD)
            vs = slice(cols + head * HD, cols + (head + 1) * HD)
            gate = g_v[r, hs].astype(F32)
            scores = dot(q_v[r, hs], kvb[:, hs], NT) * scale
            shifted = jnp.exp(scores - jnp.max(scores, axis=-1, keepdims=True))
            prob = shifted / jnp.sum(shifted, axis=-1, keepdims=True)
            prob_v[head, r, :] = prob
            sig = 1.0 / (1.0 + jnp.exp(-gate))
            att_grad = (gate * sig * m_v[r, hs].astype(F32)).astype(BF)
            value_grad = dot(prob.astype(BF), att_grad, TN).astype(BF)
            for j in range(PB):
                reqg[b * PB + j, :, vs] = value_grad[j * pass_len : (j + 1) * pass_len]
        return c

    lax.fori_loop(0, blocks, probs_step, 0)

    def back_copy(phase, part, peer):
        return z_copy(phase, half(ret, peer, part), half(arr, st, part), peer)

    def give_back(phase, part, span):
        def send(d, c):
            peer = far_peer(d)
            for k in range(depth):
                ret[peer, k, :, span] = reqg[req_ref[peer, k]][:, span]
            back_copy(phase, part, peer).start()
            return c

        lax.fori_loop(1, st_n, send, 0)
        for k in range(depth):
            arr[st, k, :, span] = reqg[req_ref[st, k]][:, span]

    give_back(2, vs_all, slice(cols, 2 * cols))

    def value_wait(d, c):
        peer = (st + d) % st_n
        z_wait(4, half(out, peer, vs_all), inc_v.at[peer], peer)
        return c

    lax.fori_loop(1, st_n, value_wait, 0)

    def block_step(b, c):
        r = pl.ds(pl.multiple_of(b * BLK, BLK), BLK)
        for j in range(PB):
            o, k = slot_ref[0, b * PB + j], slot_ref[1, b * PB + j]
            kvb[j * pass_len : (j + 1) * pass_len, :cols] = inc_k[o, k]
            kvb[j * pass_len : (j + 1) * pass_len, cols:] = inc_v[o, k]
        for head in range(heads):
            hs = slice(head * HD, (head + 1) * HD)
            vs = slice(cols + head * HD, cols + (head + 1) * HD)
            q = q_v[r, hs]
            key = kvb[:, hs]
            value = kvb[:, vs]
            gate = g_v[r, hs].astype(F32)
            grad = m_v[r, hs].astype(F32)
            prob = prob_v[head, r, :]
            attended = dot(prob.astype(BF), value)
            sig = 1.0 / (1.0 + jnp.exp(-gate))
            att_grad = (gate * sig * grad).astype(BF)
            gboth[r, vs] = (grad * attended * sig * (1.0 + gate * (1.0 - sig))).astype(BF)
            prob_grad = dot(att_grad, value, NT)
            inner = jnp.sum(prob * prob_grad, axis=-1, keepdims=True)
            score_grad = (scale * prob * (prob_grad - inner)).astype(BF)
            gboth[r, hs] = dot(score_grad, key).astype(BF)
            key_grad = dot(score_grad, q, TN).astype(BF)
            for j in range(PB):
                reqg[b * PB + j, :, hs] = key_grad[j * pass_len : (j + 1) * pass_len]
        return c

    lax.fori_loop(0, blocks, block_step, 0)
    give_back(5, ks, slice(0, cols))

    n_tile = tile_of(model, 512)

    def expand(src, weight, part, pair_rows, t):
        base = pl.multiple_of(t * pair_rows, pair_rows)
        a = src[pl.ds(base, pair_rows), :]

        def step(i, c):
            n = pl.ds(pl.multiple_of(i * n_tile, n_tile), n_tile)
            part[t, :, n] = dot(a, weight[n, :], NT).astype(BF)
            return c

        lax.fori_loop(0, model // n_tile, step, 0)

    def pair_copy(which, part, pair, h):
        return remote(part.at[h * 2 + 1 - lo], pair.at[h], ps.at[which, h], pr.at[which, h], mate)

    def scatter_first(which, src, weight, part, pair, pair_rows):
        for d in range(1, hi_n + 1):
            h = (hi + d) % hi_n
            expand(src, weight, part, pair_rows, h * 2 + 1 - lo)
            pair_copy(which, part, pair, h).start()

    def cross(which, send, recv, h):
        return remote(
            send.at[h * 2 + lo], recv.at[hi], xs.at[which, h], xr.at[which, hi], {"tp": h * 2 + lo}
        )

    def scatter_second(which, src, weight, part, pair, send, recv, pair_rows):
        for d in range(1, hi_n + 1):
            h = (hi + d) % hi_n
            expand(src, weight, part, pair_rows, h * 2 + lo)
            pair_copy(which, part, pair, h).wait_recv()
            if d < hi_n:
                part[h * 2 + lo] = (part[h * 2 + lo].astype(F32) + pair[h].astype(F32)).astype(BF)
                cross(which, part, recv, h).start()

    def scatter_last(which, part, pair, send, recv, result):
        for d in range(1, hi_n):
            h = (hi + d) % hi_n
            remote(
                send.at[h * 2 + lo], recv.at[h], xs.at[which, h], xr.at[which, h], {"tp": h * 2 + lo}
            ).wait_recv()
        total = part[tp].astype(F32) + pair[hi].astype(F32)
        for d in range(1, hi_n):
            total = total + recv[(hi + d) % hi_n].astype(F32)
        result[...] = total.astype(BF)

    tok_pair = tok_rows // tp_n
    sto_pair = pass_rows // tp_n
    scatter_first(0, gboth, wqg, tp_part, tp_pair, tok_pair)
    scatter_second(0, gboth, wqg, tp_part, tp_pair, tp_part, tp_recv, tok_pair)

    def gather_sums(o, span, first):
        def step(i, c):
            r = pl.ds(pl.multiple_of(i * m_tile, m_tile), m_tile)
            part = dot(hot[o, r, :], arr[o, :, :, span].reshape(hot_cols, cols))
            acc[r, span] = part if first else acc[r, span] + part
            return c

        lax.fori_loop(0, pass_rows // m_tile, step, 0)

    for phase, part, span in ((2, vs_all, slice(cols, 2 * cols)), (5, ks, slice(0, cols))):
        gather_sums(st, span, True)

        def grad_wait(d, c):
            peer = (st + d) % st_n
            z_wait(phase, half(ret, peer, part), half(arr, peer, part), peer)
            gather_sums(peer, span, False)
            return c

        lax.fori_loop(1, st_n, grad_wait, 0)
        plow[:, span] = acc[:, span].astype(BF)

    scatter_first(1, plow, wkv, sp_part, sp_pair, sto_pair)

    def wkey_step(t, c):
        dwp[pl.ds(pl.multiple_of(t * chunk, chunk), chunk), :] = dot(
            rows[t], plow[:, :cols], TN
        ).astype(BF)
        return c

    lax.fori_loop(0, tp_n, wkey_step, 0)
    share = model // st_n

    def part_of(s):
        return dwp.at[pl.ds(pl.multiple_of(s * share, share), share), :]

    def wkey_send(d, c):
        peer = far_peer(d)
        z_copy(3, part_of(peer), dwr.at[st], peer).start()
        return c

    lax.fori_loop(1, st_n, wkey_send, 0)
    scatter_second(1, plow, wkv, sp_part, sp_pair, sp_part, sp_recv, sto_pair)
    scatter_last(0, tp_part, tp_pair, tp_part, tp_recv, tok_out)
    wkey_out[...] = part_of(st)[...].astype(F32)

    def wkey_wait(d, c):
        peer = (st + d) % st_n
        z_wait(3, part_of(peer), dwr.at[peer], peer)
        wkey_out[...] += dwr[peer].astype(F32)
        return c

    lax.fori_loop(1, st_n, wkey_wait, 0)
    scatter_last(1, sp_part, sp_pair, sp_part, sp_recv, store_out)

    for copy in across + [beside] + onward:
        copy.wait_send()

    def drain(d, c):
        peer = (st + d) % st_n
        z_copy(0, ask_ref.at[peer], ask_in.at[st], peer).wait_send()
        key_copy(peer).wait_send()
        value_copy(peer).wait_send()
        back_copy(2, vs_all, peer).wait_send()
        back_copy(5, ks, peer).wait_send()
        z_copy(3, part_of(peer), dwr.at[st], peer).wait_send()
        return c

    lax.fori_loop(1, st_n, drain, 0)
    for d in range(1, hi_n + 1):
        h = (hi + d) % hi_n
        pair_copy(0, tp_part, tp_pair, h).wait_send()
        pair_copy(1, sp_part, sp_pair, h).wait_send()
        if d < hi_n:
            cross(0, tp_part, tp_recv, h).wait_send()
            cross(1, sp_part, sp_recv, h).wait_send()


def gathered_kernel(
    st_n, tp_n, depth, pass_len,
    ids_hbm, store_ref, q_hbm, g_hbm, wq_hbm, wg_hbm, wk_hbm, wv_hbm, m_hbm,
    tok_hbm, store_hbm, wkey_hbm,
    ids_ref, tok_out, store_out, wkey_out, rows, wall, wqg, q_v, g_v, m_v, acc, terms, k_all, v_all, ask_v, ask_in, order_v, req_ref, gated, slope, ret, prob_v, kvb, reqg, gboth, arr,
    hot, plow, sums, dwp, dwc, dwf, tp_part, tp_pair, tp_recv,
    lsem, gs, gr, fs, fr, fw, zs, zr, ps, pr, xs, xr, ws, wr, ss, sr, us, ur,
):
    grp = lax.axis_index("grp")
    st = lax.axis_index("st")
    tp = lax.axis_index("tp")
    hi_n = tp_n // 2
    hi, lo = tp // 2, tp % 2
    mate_t = hi * 2 + 1 - lo
    mate = {"tp": mate_t}
    twin = {"grp": 1 - grp}
    pass_rows, chunk = rows.shape[1], rows.shape[2]
    passages = pass_rows // pass_len
    model = wqg.shape[0]
    cols = q_v.shape[1]
    heads = cols // HD
    tok_rows = q_v.shape[0]
    blocks = tok_rows // BLK
    half_pass = passages // 2
    some = tile_of(half_pass, 2)
    some_rows = some * pass_len
    n_some = half_pass // some
    key_cols, value_cols = slice(0, cols), slice(cols, 2 * cols)

    def local(i, src, dst):
        copy = pltpu.make_async_copy(src, dst, lsem.at[i])
        copy.start()
        return copy

    def sent(ref, sem):
        remote(ref, ref, sem, pr.at[0], mate).wait_send()

    def landed(ref, sem):
        remote(ref, ref, ps.at[0], sem, mate).wait_recv()

    ids_copy = local(7, ids_hbm, ids_ref)
    own_rows = local(0, store_ref, rows.at[tp])
    local(1, wk_hbm, wall.at[tp, :, pl.ds(0, cols)])
    local(1, wv_hbm, wall.at[tp, :, pl.ds(cols, cols)])
    loads_q = [local(2, q_hbm, q_v), local(3, g_hbm, g_v), local(4, m_hbm, m_v)]
    local(5, wq_hbm, wqg.at[:, pl.ds(0, cols)])
    local(5, wg_hbm, wqg.at[:, pl.ds(cols, cols)])

    barrier = pltpu.get_barrier_semaphore()

    def greet_st(d, c):
        pl.semaphore_signal(
            barrier, inc=1, device_id={"st": (st + d) % st_n}, device_id_type=MESH
        )
        return c

    lax.fori_loop(1, st_n, greet_st, 0)
    for d in range(1, tp_n):
        pl.semaphore_signal(
            barrier, inc=1, device_id={"tp": (tp + d) % tp_n}, device_id_type=MESH
        )
    pl.semaphore_signal(barrier, inc=1, device_id=twin, device_id_type=MESH)

    ids_copy.wait()

    def plan(wide):
        line = lax.broadcasted_iota(jnp.int32, (8, wide), 0)
        return line, lax.broadcasted_iota(jnp.int32, (8, wide), 1)

    width = ask_v.shape[2]
    line, lane = plan(width)
    slot, place = lane // pass_len, lane % pass_len
    short_line, short_lane = plan(order_v.shape[1])
    target = jnp.full((8, width), -1, jnp.int32)
    order = jnp.zeros(order_v.shape, jnp.int32)
    taken = [jnp.int32(0)] * st_n
    for j in range(PB):
        for n in range(blocks):
            i = ids_ref[j, n]
            owner = lax.div(i, jnp.int32(passages))
            within = i - owner * passages
            rank = sum(jnp.where(owner == o, taken[o], 0) for o in range(st_n))
            taken = [taken[o] + jnp.where(owner == o, 1, 0) for o in range(st_n)]
            target = jnp.where(
                (line == owner) & (slot == rank), within * pass_len + place, target
            )
            order = jnp.where(
                (short_line == owner) & (short_lane == rank), j * blocks + n, order
            )
    order_v[...] = order
    for o in range(st_n):
        ask_v[o] = jnp.broadcast_to(target[o : o + 1], (8, width))
    pl.semaphore_wait(barrier, st_n + tp_n - 1)

    def first_row(i):
        part = (grp + i // n_some) % 2
        return pl.multiple_of((part * n_some + i % n_some) * some_rows, some_rows)

    n_part = tile_of(n_some, 2)

    def g_copy(way, lot, t, onto):
        i, count, slot = lot
        r = pl.ds(first_row(i), count * some_rows)
        away = (t - onto + tp_n) % tp_n - 1
        return remote(rows.at[t, r], rows.at[t, r], gs.at[way], gr.at[away, slot], {"tp": onto})

    def small(i):
        return i, 1, i

    def large(i):
        return n_some + i * n_part, n_part, n_some + i

    def onward(d, lot):
        return g_copy(2, lot, ((hi + d) % hi_n) * 2 + lo, mate_t)

    def g_wait(t, lot):
        g_copy(1, lot, t, tp).wait_recv()

    def rows_send(lot):
        for d in range(1, hi_n):
            g_copy(0, lot, tp, ((hi + d) % hi_n) * 2 + lo).start()
        g_copy(1, lot, tp, mate_t).start()

    def rows_small(i, c):
        rows_send(small(i))
        return c

    def rows_large(i, c):
        rows_send(large(i))
        return c

    own_rows.wait()
    lax.fori_loop(0, n_some, rows_small, 0)
    lax.fori_loop(0, n_some // n_part, rows_large, 0)

    upper = st >= st_n // 2
    mark = jnp.where(upper, st, st_n - 1 - st)

    def far_peer(d):
        i = d - 1
        i = i + jnp.where(i >= mark, 1, 0)
        return jnp.where(upper, i, st_n - 1 - i)

    def z_copy(phase, src, dst, peer):
        away = (st - peer + st_n) % st_n - 1
        return remote(src, dst, zs.at[phase], zr.at[phase, away], {"st": peer})

    def z_wait(phase, src, dst, peer):
        landed(dst, zr.at[phase, (peer - st + st_n) % st_n - 1])

    def ask_send(d, c):
        peer = (st + d) % st_n
        z_copy(0, ask_v.at[peer], ask_in.at[st], peer).start()
        return c

    lax.fori_loop(1, st_n, ask_send, 0)
    ask_in[st] = ask_v[st]
    order_copy = local(6, order_v, req_ref)

    def project(lot, send):
        i, count, _ = lot
        r = pl.ds(first_row(i), count * some_rows)

        def term(t, span):
            return dot(rows[t, r], wall[tp, pl.ds(pl.multiple_of(t * chunk, chunk), chunk), span])

        for d in range(1, hi_n):
            g_wait(((hi + d) % hi_n) * 2 + lo, lot)
            onward(d, lot).start()
        g_wait(mate_t, lot)
        near = [tp, mate_t] + [((hi + d) % hi_n) * 2 + lo for d in range(1, hi_n)]
        late = [((hi + d) % hi_n) * 2 + 1 - lo for d in range(1, hi_n)]
        total = sum(term(t, key_cols) for t in near[1:]) + term(near[0], key_cols)
        for t in late:
            g_wait(t, lot)
            total = total + term(t, key_cols)
        first = st * passages + first_row(i) // pass_len

        def keep(ref, total):
            low = total.astype(BF)
            for p in range(count * some):
                ref[first + p] = low[p * pass_len : (p + 1) * pass_len]

        keep(k_all, total)
        send()
        keep(v_all, sum(term(t, value_cols) for t in near + late))

    def part_of_all(kind, o, c, side):
        ref = k_all if kind == 0 else v_all
        return ref.at[pl.ds(o * passages + side * half_pass + c * some, some)]

    def chain_copy(kind, o, c, peer):
        part = part_of_all(kind, o, c, grp)
        away = (o - peer + st_n) % st_n - 1
        return remote(part, part, fs.at[kind, 0], fr.at[kind, away, c], {"st": peer})

    def twin_copy(kind, o, c):
        part = part_of_all(kind, o, c, grp)
        return remote(part, part, fs.at[kind, 1], fw.at[kind], twin)

    lower = st < st_n // 2
    edge = (st == 0) | (st == st_n - 1)

    def own_send(kind, c, inward=True, outward=True):
        for onto, toward in ((st + 1, lower), (st - 1, jnp.logical_not(lower))):
            there = (onto >= 0) & (onto < st_n)
            if not outward:
                there = there & toward
            if not inward:
                there = there & jnp.logical_not(toward)

            @pl.when(there)
            def _():
                chain_copy(kind, st, c, onto).start()

    def relay(kind, d, c):
        for sign in (-1, 1):
            o = st + sign * d
            onto = st - sign

            @pl.when((o >= 0) & (o < st_n))
            def _():
                chain_copy(kind, o, c, st).wait_recv()

                @pl.when((onto >= 0) & (onto < st_n))
                def _():
                    chain_copy(kind, o, c, onto).start()

                twin_copy(kind, o, c).start()

    relayed = (st_n - 1) * half_pass

    def twin_wait(kind):
        landed((k_all, v_all)[kind].at[pl.ds(0, relayed)], fw.at[kind])

    landed(wall.at[tp], lsem.at[1])
    for copy in loads_q:
        copy.wait()

    gate_rows = tok_rows // n_some

    def gates(i):
        r = pl.ds(pl.multiple_of(i * gate_rows, gate_rows), gate_rows)
        gate = g_v[r, :].astype(F32)
        grad = m_v[r, :].astype(F32)
        sig = 1.0 / (1.0 + jnp.exp(-gate))
        gated[r, :] = (gate * sig * grad).astype(BF)
        slope[r, :] = grad * (sig * (1.0 + gate * (1.0 - sig)))

    def early_step(i, c):
        project(small(i), lambda: own_send(0, i))

        @pl.when(i >= 1)
        def _():
            relay(0, 1, i - 1)

        @pl.when(edge | (i == 0))
        def _():
            own_send(1, i, outward=False)

        gates(i)
        return c

    lax.fori_loop(0, n_some, early_step, 0)
    for i in range(n_some - 1, n_some):
        relay(0, 1, i)

    def inward_send(i, c):
        own_send(1, i, outward=False)
        return c

    lax.fori_loop(jnp.where(edge, n_some, 1), n_some, inward_send, 0)

    def second_step(i, c):
        relay(0, 2, i)
        return c

    def outward_send(i, c):
        own_send(1, i, inward=False)
        return c

    lax.fori_loop(0, n_some, second_step, 0)
    lax.fori_loop(0, n_some, outward_send, 0)

    def late_step(i, c):
        project(large(i), lambda: None)
        for q in range(n_part):
            @pl.when(edge)
            def _():
                relay(0, 3, i * n_part + q)

            @pl.when(jnp.logical_not(edge))
            def _():
                relay(1, 1, i * n_part + q)

        return c

    w_part = model // 2
    w_mine = pl.ds(pl.multiple_of(grp * w_part, w_part), w_part)
    w_other = pl.ds(pl.multiple_of((1 - grp) * w_part, w_part), w_part)

    def w_across(d):
        h = (hi + d) % hi_n
        part = wall.at[tp, w_mine]
        return remote(part, part, ws.at[0], wr.at[0], {"tp": h * 2 + lo})

    def w_twin(d):
        t = ((hi + d) % hi_n) * 2 + lo
        part = wall.at[t, w_mine]
        return remote(part, part, ws.at[0], wr.at[1], twin)

    def w_onward(d, k):
        t = ((hi + d) % hi_n) * 2 + lo
        part = wall.at[t, w_other if k else w_mine]
        return remote(part, part, ws.at[0], wr.at[2], mate)

    w_beside = remote(wall.at[tp], wall.at[tp], ws.at[0], wr.at[2], mate)

    def w_wait(kind, t, part):
        landed(wall.at[t, part], wr.at[kind])

    for d in range(1, hi_n):
        w_across(d).start()

    def relay_rest(kind, first, last):
        def step(i, c):
            relay(kind, 1 + i // n_some, i % n_some)
            return c

        lax.fori_loop(first, last, step, 0)

    relays = (st_n - 1) * n_some
    lax.fori_loop(0, n_some // n_part, late_step, 0)
    w_beside.start()
    relay_rest(1, 0, jnp.where(edge, n_some, 0))
    landed(wqg, lsem.at[5])
    order_copy.wait()
    twin_wait(0)
    scale = HD ** (-0.5)

    def fill(n, ref, span, b):
        for j in range(PB):
            kvb[n, j * pass_len : (j + 1) * pass_len, span] = ref[ids_ref[j, b]]

    pairs = range(4)

    def block_rows(b):
        return pl.ds(pl.multiple_of(b * BLK, BLK), BLK)

    per_step = n_some // (blocks // 4)

    def probs_step(i, c):
        for n in pairs:
            fill(n, k_all, key_cols, 4 * i + n)
        for head in range(heads):
            hs = slice(head * HD, (head + 1) * HD)
            vs = slice(cols + head * HD, cols + (head + 1) * HD)
            for n in pairs:
                b = 4 * i + n
                r = block_rows(b)
                scores = dot(q_v[r, hs], kvb[n, :, hs], NT) * scale
                shifted = jnp.exp(scores - jnp.max(scores, axis=-1, keepdims=True))
                prob = shifted * (1.0 / jnp.sum(shifted, axis=-1, keepdims=True))
                prob_v[head, r, :] = prob
                value_grad = dot(prob.astype(BF), gated[r, hs], TN).astype(BF)
                for j in range(PB):
                    reqg[j * blocks + b, :, vs] = value_grad[j * pass_len : (j + 1) * pass_len]

        for q in range(per_step):
            relay(1, 2, i * per_step + q)

        return c

    lax.fori_loop(0, blocks // 4, probs_step, 0)

    def half(ref, peer, part):
        return ref.at[peer, :, :, part]

    def back_copy(phase, part, peer):
        return z_copy(phase, half(ret, peer, part), half(arr, st, part), peer)

    def give_back(phase, part, span, order, first, last):
        def send(d, c):
            peer = order(d)
            for k in range(depth):
                ret[peer, k, :, span] = reqg[req_ref[peer, k]][:, span]
            back_copy(phase, part, peer).start()
            return c

        lax.fori_loop(first, last, send, 0)

    def keep_own(span):
        for k in range(depth):
            arr[st, k, :, span] = reqg[req_ref[st, k]][:, span]

    def near_peer(d):
        return far_peer(st_n - d)

    ks, vs_all = pl.ds(0, cols), pl.ds(cols, cols)
    def value_peer(d):
        return jnp.where(edge, near_peer(d % (st_n - 1) + 1), near_peer(d))

    give_back(
        1, vs_all, value_cols, value_peer, 1, jnp.where(edge, st_n, st_n - 1)
    )
    keep_own(value_cols)
    relay_rest(1, n_some + per_step * (blocks // 4), relays)
    twin_wait(1)

    def block_step(i, c):
        for n in pairs:
            fill(n, k_all, key_cols, 4 * i + n)
            fill(n, v_all, value_cols, 4 * i + n)
        for head in range(heads):
            hs = slice(head * HD, (head + 1) * HD)
            vs = slice(cols + head * HD, cols + (head + 1) * HD)
            for n in pairs:
                b = 4 * i + n
                r = block_rows(b)
                value = kvb[n, :, vs]
                prob = prob_v[head, r, :]
                prob_grad = dot(gated[r, hs], value, NT)
                inner = jnp.sum(prob * prob_grad, axis=-1, keepdims=True)
                score_grad = (scale * prob * (prob_grad - inner)).astype(BF)
                key_grad = dot(score_grad, q_v[r, hs], TN).astype(BF)
                for j in range(PB):
                    reqg[j * blocks + b, :, hs] = key_grad[j * pass_len : (j + 1) * pass_len]
                gboth[r, hs] = dot(score_grad, kvb[n, :, hs]).astype(BF)
                attended = dot(prob.astype(BF), value)
                gboth[r, vs] = (attended * slope[r, hs]).astype(BF)
        return c

    lax.fori_loop(0, blocks // 4, block_step, 0)
    def key_peer(d):
        return jnp.where(edge, near_peer(jnp.where(d == 1, 1, st_n + 1 - d)), far_peer(d))

    give_back(2, ks, key_cols, key_peer, 1, st_n)
    keep_own(key_cols)

    n_tile = tile_of(model, 512)

    def expand(h):
        a = gboth[pl.ds(pl.multiple_of(h * 2 * tok_pair, tok_pair), 2 * tok_pair), :]

        def step(i, c):
            n = pl.ds(pl.multiple_of(i * n_tile, n_tile), n_tile)
            part = dot(a, wqg[n, :], NT).astype(BF)
            tp_part[h * 2, :, n] = part[:tok_pair]
            tp_part[h * 2 + 1, :, n] = part[tok_pair:]
            return c

        lax.fori_loop(0, model // n_tile, step, 0)

    def pair_copy(h):
        return remote(tp_part.at[h * 2 + 1 - lo], tp_pair.at[h], ps.at[0], pr.at[h], mate)

    def cross(h):
        return remote(
            tp_part.at[h * 2 + lo], tp_recv.at[hi], xs.at[0], xr.at[0], {"tp": h * 2 + lo}
        )

    for d in range(1, hi_n):
        w_wait(0, ((hi + d) % hi_n) * 2 + lo, w_mine)
        w_twin(d).start()
        w_onward(d, 0).start()

    tok_pair = tok_rows // tp_n
    for d in range(1, hi_n + 1):
        h = (hi + d) % hi_n
        expand(h)
        pair_copy(h).start()
    for d in range(1, hi_n):
        h = (hi + d) % hi_n
        pair_copy(h).wait_recv()
        tp_part[h * 2 + lo] = (tp_part[h * 2 + lo].astype(F32) + tp_pair[h].astype(F32)).astype(BF)
        cross(h).start()

    def ask_wait(d, c):
        peer = (st + d) % st_n
        z_wait(0, ask_v.at[peer], ask_in.at[peer], peer)
        return c

    lax.fori_loop(1, st_n, ask_wait, 0)
    hot_cols = depth * pass_len
    m_tile = tile_of(pass_rows, 256)

    def hot_step(o, c):
        target = ask_in[o][0:1, :hot_cols]
        for i in range(pass_rows // m_tile):
            line = lax.broadcasted_iota(jnp.int32, (m_tile, hot_cols), 0) + i * m_tile
            hot[o, i * m_tile : (i + 1) * m_tile, :] = jnp.where(line == target, 1.0, 0.0).astype(BF)
        return c

    lax.fori_loop(0, st_n, hot_step, 0)

    def gather_sums(kind, o, span, first):
        def step(i, c):
            r = pl.ds(pl.multiple_of(i * m_tile, m_tile), m_tile)
            part = dot(hot[o, r, :], arr[o, :, :, span].reshape(hot_cols, cols))
            acc[kind, r, :] = part if first else acc[kind, r, :] + part
            return c

        lax.fori_loop(0, pass_rows // m_tile, step, 0)

    sto_pair = pass_rows // tp_n

    def sums_copy(kind, part, d):
        t = (tp + d) % tp_n
        src = plow.at[pl.ds(pl.multiple_of(t * sto_pair, sto_pair), sto_pair), part]
        return remote(src, sums.at[tp, :, part], ss.at[kind], sr.at[kind], {"tp": t})

    def sums_of(part):
        return sums.at[pl.ds(0, tp_n - 1), :, part]

    def grads_of(kind, peer):
        phase, part, span = (2, ks, key_cols) if kind == 0 else (1, vs_all, value_cols)
        z_wait(phase, half(ret, peer, part), half(arr, peer, part), peer)
        gather_sums(kind, peer, span, False)

    def sums_send(kind):
        part, span = (ks, key_cols) if kind == 0 else (vs_all, value_cols)
        plow[:, span] = acc[kind].astype(BF)
        for d in range(1, tp_n):
            sums_copy(kind, part, d).start()
        sums[tp, :, span] = plow[pl.ds(pl.multiple_of(tp * sto_pair, sto_pair), sto_pair), span]

    beyond = jnp.where(lower, st_n - 1, 0)
    middle = jnp.where(lower, st_n // 2, st_n // 2 - 1)
    beside_st = st + 1 - 2 * (st % 2)
    outer = edge
    inner = jnp.logical_not(outer)
    gather_sums(1, st, value_cols, True)
    gather_sums(0, st, key_cols, True)
    grads_of(1, beside_st)
    grads_of(1, jnp.where(outer, beyond, middle))

    grads_of(0, middle)

    @pl.when(inner)
    def _():
        give_back(1, vs_all, value_cols, near_peer, st_n - 1, st_n)

    grads_of(0, beyond)
    grads_of(0, beside_st)
    sums_send(0)

    share = model // st_n
    bits = 2
    bit = share // bits

    def dw_line(s, b):
        return pl.ds(pl.multiple_of(s * share + b * bit, bit), bit)

    def dw_copy(kind, b):
        line = pl.ds(b * bit, bit)
        if kind < 2:
            src, dst = dwp.at[dw_line(middle if kind else beyond, b)], dwc.at[kind, line]
            peer = beside_st
        elif kind == 2:
            src, dst, peer = dwp.at[dw_line(beside_st, b)], dwf.at[0, line], beside_st
        else:
            src, dst = dwc.at[kind - 3, line], dwf.at[1, line]
            peer = middle if kind == 4 else beyond
        return remote(src, dst, us.at[0], ur.at[min(kind, 3), b], {"st": peer})

    def dw_send(kind):
        for b in range(bits):
            dw_copy(kind, b).start()

    def dw_relay(q):
        for b in range(bits):
            line = slice(b * bit, (b + 1) * bit)
            dw_copy(q, b).wait_recv()
            own = dwp[dw_line(middle if q else beyond, b), :].astype(F32)
            dwc[q, line, :] = (dwc[q, line, :].astype(F32) + own).astype(BF)
            dw_copy(3 + q, b).start()

    def wkey_step(s):
        dwp[pl.ds(pl.multiple_of(s * chunk, chunk), chunk), :] = dot(
            rows[s], plow[:, key_cols], TN
        ).astype(BF)

    def wkey_turn(j, c):
        far = jnp.where(j == 0, beyond, middle)
        near = jnp.where(j == 2, beside_st, st)
        near_first = jnp.where(j == 0, beside_st, st)
        far_after = jnp.where(j == 1, beyond, middle)
        s = jnp.where(
            outer, jnp.where(j < 2, far, near), jnp.where((j == 0) | (j == 3), near_first, far_after)
        )
        wkey_step(s)
        for kind in range(3):
            @pl.when(outer & (j == kind))
            def _():
                dw_send(kind)

        @pl.when(inner & (j == 0))
        def _():
            dw_send(2)

        return c

    lax.fori_loop(0, st_n, wkey_turn, 0)

    @pl.when(inner)
    def _():
        dw_relay(0)

    for d in range(1, hi_n):
        t = ((hi + d) % hi_n) * 2 + lo
        w_wait(1, t, w_other)
        w_onward(d, 1).start()
    landed(wall.at[pl.ds(0, hi_n)], wr.at[2])

    def store_terms(span, done):
        def step(i, c):
            n = pl.ds(pl.multiple_of(i * n_tile, n_tile), n_tile)
            part = dot(sums[0, :, span], wall[0, n, span], NT)
            for t in range(1, tp_n):
                part = part + dot(sums[t, :, span], wall[t, n, span], NT)
            done(n, part)
            return c

        lax.fori_loop(0, model // n_tile, step, 0)

    def keep_terms(n, part):
        terms[:, n] = part

    def keep_store(n, part):
        store_out[:, n] = (terms[:, n] + part).astype(BF)

    grads_of(1, jnp.where(outer, middle, beyond))
    sums_send(1)

    landed(sums_of(ks), sr.at[0])
    store_terms(key_cols, keep_terms)

    pair_copy(hi).wait_recv()
    for d in range(1, hi_n):
        h = (hi + d) % hi_n
        landed(tp_recv.at[h], xr.at[0])
    total = tp_part[tp].astype(F32) + tp_pair[hi].astype(F32)
    for d in range(1, hi_n):
        total = total + tp_recv[(hi + d) % hi_n].astype(F32)
    tok_out[...] = total.astype(BF)
    tok_done = local(2, tok_out, tok_hbm)

    @pl.when(inner)
    def _():
        dw_relay(1)

    landed(sums_of(vs_all), sr.at[1])
    store_terms(value_cols, keep_store)
    store_done = local(3, store_out, store_hbm)

    for b in range(bits):
        line = slice(b * bit, (b + 1) * bit)
        dw_copy(2, b).wait_recv()
        wkey_out[line, :] = dwp[dw_line(st, b), :].astype(F32) + dwf[0, line, :].astype(F32)
    for b in range(bits):
        line = slice(b * bit, (b + 1) * bit)
        for kind, edge in ((3, outer), (4, inner)):
            @pl.when(edge)
            def _():
                dw_copy(kind, b).wait_recv()

        wkey_out[line, :] += dwf[1, line, :].astype(F32)

    wkey_done = local(4, wkey_out, wkey_hbm)

    for way in range(3):
        sent(rows.at[tp], gs.at[way])
    for kind, ref in ((0, k_all), (1, v_all)):
        sent(ref.at[pl.ds(0, relayed)], fs.at[kind, 1])
        for s in range(st_n):
            up, down = (s + 1) * (s + 1 < st_n), (st_n - s) * (s > 0)

            @pl.when(st == s)
            def _():
                sent(ref.at[pl.ds(0, (up + down) * half_pass)], fs.at[kind, 0])

    sent(wall.at[pl.ds(0, hi_n + 1)], ws.at[0])
    sent(ask_in.at[pl.ds(0, st_n - 1)], zs.at[0])
    sent(ret.at[pl.ds(0, st_n - 1), :, :, vs_all], zs.at[1])
    sent(ret.at[pl.ds(0, st_n - 1), :, :, ks], zs.at[2])
    sent(sums_of(ks), ss.at[0])
    sent(sums_of(vs_all), ss.at[1])
    sent(tp_pair, ps.at[0])
    sent(tp_recv.at[0], xs.at[0])
    sent(dwp.at[pl.ds(0, 3 * share)], us.at[0])
    for copy in (tok_done, store_done, wkey_done):
        copy.wait()


def settle_kernel(*refs):
    n = (len(refs) - 2) // 3
    sources, results, held = refs[:n], refs[n : 2 * n], refs[2 * n : 3 * n]
    ins, outs = refs[3 * n], refs[3 * n + 1]
    pieces = []
    for a, (source, result, here) in enumerate(zip(sources, results, held)):
        part = source.shape[0] // 2
        for i in range(2):
            r = pl.ds(i * part, part)
            pieces.append(
                (
                    pltpu.make_async_copy(source.at[r], here.at[r], ins.at[a, i]),
                    pltpu.make_async_copy(here.at[r], result.at[r], outs.at[a, i]),
                )
            )
    for fetch, _ in pieces:
        fetch.start()
    for fetch, put in pieces:
        fetch.wait()
        put.start()
    for _, put in pieces:
        put.wait()


def settle(*arrays):
    hbm = pl.BlockSpec(memory_space=pl.ANY)
    n = len(arrays)
    return pl.pallas_call(
        settle_kernel,
        out_shape=tuple(jax.ShapeDtypeStruct(a.shape, a.dtype) for a in arrays),
        in_specs=[hbm] * n,
        out_specs=(hbm,) * n,
        scratch_shapes=[pltpu.VMEM(a.shape, a.dtype) for a in arrays]
        + [pltpu.SemaphoreType.DMA((n, 2)), pltpu.SemaphoreType.DMA((n, 2))],
    )(*arrays)


def local(pass_ids, store, queries, gate_pre, w_query, w_gate, w_key, w_value, d_mem):
    st_n = lax.axis_size("st")
    tp_n = lax.axis_size("tp")
    hi_n = tp_n // 2
    tok_rows, cols = queries.shape
    blocks = tok_rows // BLK
    passages, pass_len, chunk = store.shape
    model = w_key.shape[0]
    requests = blocks * PB
    depth = max(2, requests // st_n)
    pass_rows = passages * pass_len
    share = model // st_n

    vmem = pl.BlockSpec(memory_space=pltpu.VMEM)
    smem = pl.BlockSpec(memory_space=pltpu.SMEM)
    hbm = pl.BlockSpec(memory_space=pl.ANY)
    V = pltpu.VMEM
    DMA = pltpu.SemaphoreType.DMA
    pair = 2 * cols
    tok_pair = tok_rows // tp_n
    sto_pair = pass_rows // tp_n
    hot_cols = depth * pass_len
    width = -(-hot_cols // 128) * 128
    gathered_bytes = 2 * 2 * st_n * pass_rows * cols
    steps = blocks // 4
    fits = lax.axis_size("grp") == 2 and hi_n == 2 and st_n == 4 and st_n == tp_n
    fits = fits and passages % 4 == 0 and blocks % 4 == 0 and passages // 4 % steps == 0
    if fits and gathered_bytes <= 8 << 20:
        half_pass = passages // 2
        n_some = half_pass // tile_of(half_pass, 2)
        d_tokens, d_store, d_wkey = pl.pallas_call(
            functools.partial(gathered_kernel, st_n, tp_n, depth, pass_len),
            out_shape=(
                jax.ShapeDtypeStruct((tok_pair, model), BF),
                jax.ShapeDtypeStruct((sto_pair, model), BF),
                jax.ShapeDtypeStruct((share, cols), F32),
            ),
            in_specs=[hbm] * 9,
            out_specs=(hbm, hbm, hbm),
            scratch_shapes=[
                pltpu.SMEM((PB, blocks), jnp.int32),
                V((tok_pair, model), BF),
                V((sto_pair, model), BF),
                V((share, cols), F32),
                V((tp_n, pass_rows, chunk), BF),
                V((tp_n, model, pair), BF),
                V((model, pair), BF),
                V((tok_rows, cols), BF),
                V((tok_rows, cols), BF),
                V((tok_rows, cols), BF),
                V((2, pass_rows, cols), F32),
                V((sto_pair, model), F32),
                V((st_n * passages, pass_len, cols), BF),
                V((st_n * passages, pass_len, cols), BF),
                V((st_n, 8, width), jnp.int32),
                V((st_n, 8, width), jnp.int32),
                V((8, 128), jnp.int32),
                pltpu.SMEM((8, 128), jnp.int32),
                V((tok_rows, cols), BF),
                V((tok_rows, cols), F32),
                V((st_n, depth, pass_len, pair), BF),
                V((cols // HD, tok_rows, PB * pass_len), F32),
                V((4, PB * pass_len, pair), BF),
                V((requests, pass_len, pair), BF),
                V((tok_rows, pair), BF),
                V((st_n, depth, pass_len, pair), BF),
                V((st_n, pass_rows, hot_cols), BF),
                V((pass_rows, pair), BF),
                V((tp_n, sto_pair, pair), BF),
                V((model, cols), BF),
                V((2, share, cols), BF),
                V((2, share, cols), BF),
                V((tp_n, tok_pair, model), BF),
                V((hi_n, tok_pair, model), BF),
                V((hi_n, tok_pair, model), BF),
                DMA((8,)),
                DMA((3,)),
                DMA((tp_n - 1, n_some + n_some // tile_of(n_some, 2))),
                DMA((2, 2)),
                DMA((2, st_n - 1, n_some)),
                DMA((2,)),
                DMA((3,)),
                DMA((3, st_n - 1)),
                DMA((1,)),
                DMA((hi_n,)),
                DMA((1,)),
                DMA((1,)),
                DMA((1,)),
                DMA((3,)),
                DMA((2,)),
                DMA((2,)),
                DMA((1,)),
                DMA((4, 2)),
            ],
            compiler_params=pltpu.CompilerParams(
                collective_id=0, has_side_effects=True, vmem_limit_bytes=67043328
            ),
        )(
            pass_ids.T, store.reshape(pass_rows, chunk),
            queries, gate_pre, w_query, w_gate, w_key, w_value, d_mem,
        )
        d_tokens, d_store, d_wkey = settle(d_tokens, d_store, d_wkey)
        return d_tokens, d_store.reshape(passages // tp_n, pass_len, model), d_wkey

    ids = pass_ids.reshape(-1)
    owners = ids // passages
    within = ids % passages
    order = jnp.arange(requests, dtype=jnp.int32)
    earlier = (owners[None, :] == owners[:, None]) & (order[None, :] < order[:, None])
    rank = jnp.sum(earlier.astype(jnp.int32), axis=1)
    slots = jnp.stack([owners, rank])
    o_i = jnp.arange(st_n, dtype=jnp.int32)[:, None, None]
    k_i = jnp.arange(depth, dtype=jnp.int32)[None, :, None]
    match = (owners[None, None, :] == o_i) & (rank[None, None, :] == k_i)
    asked = jnp.max(jnp.where(match, within[None, None, :], -1), axis=2)
    req_of = jnp.max(jnp.where(match, order[None, None, :], 0), axis=2)
    hot_cols = depth * pass_len
    width = -(-hot_cols // 128) * 128
    lane = jnp.arange(width, dtype=jnp.int32)
    spread = jnp.repeat(asked, pass_len, axis=1)
    spread = jnp.pad(spread, ((0, 0), (0, width - hot_cols)), constant_values=-1)
    target = jnp.where(spread < 0, -1, spread * pass_len + lane[None, :] % pass_len)
    flat = jnp.pad(jnp.maximum(asked, 0), ((0, 0), (0, width - depth)))
    ask = jnp.concatenate(
        [target[:, None], flat[:, None], jnp.zeros((st_n, 6, width), jnp.int32)], axis=1
    )

    d_tokens, d_store, d_wkey = pl.pallas_call(
        functools.partial(kernel, st_n, tp_n, depth, pass_len),
        out_shape=(
            jax.ShapeDtypeStruct((tok_pair, model), BF),
            jax.ShapeDtypeStruct((sto_pair, model), BF),
            jax.ShapeDtypeStruct((share, cols), F32),
        ),
        in_specs=[smem, smem, vmem] + [hbm] * 8,
        out_specs=(vmem, vmem, vmem),
        scratch_shapes=[
            V((tp_n, pass_rows, chunk), BF),
            V((model, pair), BF),
            V((model, pair), BF),
            V((tok_rows, cols), BF),
            V((tok_rows, cols), BF),
            V((tok_rows, cols), BF),
            V((pass_rows, pair), F32),
            V((passages, pass_len, pair), BF),
            V((st_n, 8, width), jnp.int32),
            pltpu.SMEM((st_n, 8, width), jnp.int32),
            V((st_n, depth, pass_len, pair), BF),
            V((st_n, depth, pass_len, cols), BF),
            V((st_n, depth, pass_len, cols), BF),
            V((st_n, depth, pass_len, pair), BF),
            V((cols // HD, tok_rows, PB * pass_len), F32),
            V((PB * pass_len, pair), BF),
            V((requests, pass_len, pair), BF),
            V((tok_rows, pair), BF),
            V((st_n, depth, pass_len, pair), BF),
            V((st_n, pass_rows, hot_cols), BF),
            V((pass_rows, pair), BF),
            V((model, cols), BF),
            V((st_n, share, cols), BF),
            V((tp_n, tok_pair, model), BF),
            V((hi_n, tok_pair, model), BF),
            V((hi_n, tok_pair, model), BF),
            V((tp_n, sto_pair, model), BF),
            V((hi_n, sto_pair, model), BF),
            V((hi_n, sto_pair, model), BF),
            DMA((9,)),
            DMA((3, hi_n)),
            DMA((tp_n,)),
            DMA((6, st_n)),
            DMA((6, st_n)),
            DMA((2, hi_n)),
            DMA((2, hi_n)),
            DMA((2, hi_n)),
            DMA((2, hi_n)),
        ],
        compiler_params=pltpu.CompilerParams(
            collective_id=0, has_side_effects=True, vmem_limit_bytes=67043328
        ),
    )(
        slots, req_of, ask, store.reshape(pass_rows, chunk),
        queries, gate_pre, w_query, w_gate, w_key, w_value, d_mem,
    )
    return d_tokens, d_store.reshape(passages // tp_n, pass_len, model), d_wkey


def solution(mesh):
    return jax.shard_map(
        local,
        mesh=mesh,
        in_specs=(
            P(("grp", "st"), None),
            P("st", None, "tp"),
            P(("grp", "st"), "tp"),
            P(("grp", "st"), "tp"),
            P(None, "tp"),
            P(None, "tp"),
            P(None, "tp"),
            P(None, "tp"),
            P(("grp", "st"), "tp"),
        ),
        out_specs=(
            P(("grp", "st", "tp"), None),
            P(("grp", "st", "tp"), None, None),
            P(("grp", "st"), "tp"),
        ),
        check_vma=False,
    )
```

```python
import functools

import jax
import jax.numpy as jnp
from jax import lax
from jax.experimental import pallas as pl
from jax.experimental.pallas import tpu as pltpu
from jax.sharding import PartitionSpec as P

HD = 256
BLK = 128
PB = 4
BF = jnp.bfloat16
F32 = jnp.float32
MESH = pl.DeviceIdType.MESH
NT = (((1,), (1,)), ((), ()))
TN = (((0,), (0,)), ((), ()))


def dot(a, b, dims=(((1,), (0,)), ((), ()))):
    return lax.dot_general(a, b, dims, preferred_element_type=F32)


def remote(src, dst, send, recv, device):
    return pltpu.make_async_remote_copy(
        src_ref=src,
        dst_ref=dst,
        send_sem=send,
        recv_sem=recv,
        device_id=device,
        device_id_type=MESH,
    )


def tile_of(size, most):
    while size % most:
        most //= 2
    return most


def kernel(
    st_n, tp_n, depth, pass_len,
    slot_ref, req_ref, ask_ref, store_ref, q_hbm, g_hbm, wq_hbm, wg_hbm, wk_hbm, wv_hbm, m_hbm,
    tok_out, store_out, wkey_out,
    rows, wkv, wqg, q_v, g_v, m_v, acc, kv, ask_in, ask_s, out, inc_k, inc_v, ret, prob_v, kvb, reqg, gboth, arr,
    hot, plow, dwp, dwr, tp_part, tp_pair, tp_recv, sp_part, sp_pair, sp_recv,
    lsem, gs, gr, zs, zr, ps, pr, xs, xr,
):
    st = lax.axis_index("st")
    tp = lax.axis_index("tp")
    hi_n = tp_n // 2
    hi, lo = tp // 2, tp % 2
    mate = {"tp": hi * 2 + 1 - lo}
    pass_rows, chunk = rows.shape[1], rows.shape[2]
    model = wqg.shape[0]
    cols = q_v.shape[1]
    heads = cols // HD
    tok_rows = q_v.shape[0]
    blocks = tok_rows // BLK
    blk_keys = PB * pass_len

    def local(i, src, dst):
        copy = pltpu.make_async_copy(src, dst, lsem.at[i])
        copy.start()
        return copy

    own_rows = local(0, store_ref, rows.at[tp])
    loads_kv = [
        local(1, wk_hbm, wkv.at[:, pl.ds(0, cols)]),
        local(2, wv_hbm, wkv.at[:, pl.ds(cols, cols)]),
    ]
    loads_q = [local(3, q_hbm, q_v), local(4, g_hbm, g_v), local(5, m_hbm, m_v)]
    loads_qg = [
        local(6, wq_hbm, wqg.at[:, pl.ds(0, cols)]),
        local(7, wg_hbm, wqg.at[:, pl.ds(cols, cols)]),
    ]

    barrier = pltpu.get_barrier_semaphore()

    def greet_st(d, c):
        pl.semaphore_signal(
            barrier, inc=1, device_id={"st": (st + d) % st_n}, device_id_type=MESH
        )
        return c

    lax.fori_loop(1, st_n, greet_st, 0)
    for d in range(1, tp_n):
        pl.semaphore_signal(
            barrier, inc=1, device_id={"tp": (tp + d) % tp_n}, device_id_type=MESH
        )
    pl.semaphore_wait(barrier, st_n - 1 + tp_n - 1)

    across = []
    for d in range(1, hi_n):
        h = (hi + d) % hi_n
        across.append(
            remote(store_ref, rows.at[tp], gs.at[0, h], gr.at[tp], {"tp": h * 2 + lo})
        )
        across[-1].start()
    beside = remote(store_ref, rows.at[tp], gs.at[1, hi], gr.at[tp], mate)
    beside.start()

    upper = st >= st_n // 2
    mark = jnp.where(upper, st, st_n - 1 - st)

    def far_peer(d):
        i = d - 1
        i = i + jnp.where(i >= mark, 1, 0)
        return jnp.where(upper, i, st_n - 1 - i)

    def z_copy(phase, src, dst, peer):
        return remote(src, dst, zs.at[phase, peer], zr.at[phase, st], {"st": peer})

    def z_wait(phase, src, dst, peer):
        remote(src, dst, zs.at[phase, peer], zr.at[phase, peer], {"st": peer}).wait_recv()

    def ask_send(d, c):
        peer = (st + d) % st_n
        z_copy(0, ask_ref.at[peer], ask_in.at[st], peer).start()
        return c

    lax.fori_loop(1, st_n, ask_send, 0)
    ask_in[st] = ask_ref[st]

    m_tile = tile_of(pass_rows, 256)

    def project(t, first):
        def step(i, c):
            r = pl.ds(pl.multiple_of(i * m_tile, m_tile), m_tile)
            part = dot(rows[t, r], wkv[pl.ds(pl.multiple_of(t * chunk, chunk), chunk), :])
            acc[r] = part if first else acc[r] + part
            return c

        lax.fori_loop(0, pass_rows // m_tile, step, 0)

    def g_wait(t):
        remote(store_ref, rows.at[t], gs.at[1, hi], gr.at[t], mate).wait_recv()

    own_rows.wait()
    for copy in loads_kv:
        copy.wait()
    project(tp, True)
    g_wait(hi * 2 + 1 - lo)
    project(hi * 2 + 1 - lo, False)

    def ask_wait(d, c):
        peer = (st + d) % st_n
        z_wait(0, ask_ref.at[peer], ask_in.at[peer], peer)
        return c

    lax.fori_loop(1, st_n, ask_wait, 0)
    ask_copy = local(8, ask_in, ask_s)
    ask_copy.wait()

    hot_cols = depth * pass_len

    def hot_step(o, c):
        target = ask_in[o][0:1, :hot_cols]
        for i in range(pass_rows // m_tile):
            line = lax.broadcasted_iota(jnp.int32, (m_tile, hot_cols), 0) + i * m_tile
            hot[o, i * m_tile : (i + 1) * m_tile, :] = jnp.where(line == target, 1.0, 0.0).astype(BF)
        return c

    lax.fori_loop(0, st_n, hot_step, 0)
    onward = []
    for d in range(1, hi_n):
        h = (hi + d) % hi_n
        t = h * 2 + lo
        g_wait(t)
        onward.append(remote(rows.at[t], rows.at[t], gs.at[2, h], gr.at[t], mate))
        onward[-1].start()
        project(t, False)
    for d in range(1, hi_n):
        t = ((hi + d) % hi_n) * 2 + 1 - lo
        g_wait(t)
        project(t, False)

    def low_step(i, c):
        kv[i] = acc[pl.ds(pl.multiple_of(i * pass_len, pass_len), pass_len), :].astype(BF)
        return c

    lax.fori_loop(0, pass_rows // pass_len, low_step, 0)

    ks, vs_all = pl.ds(0, cols), pl.ds(cols, cols)

    def half(ref, peer, part):
        return ref.at[peer, :, :, part]

    def key_copy(peer):
        return z_copy(1, half(out, peer, ks), inc_k.at[st], peer)

    def value_copy(peer):
        return z_copy(4, half(out, peer, vs_all), inc_v.at[st], peer)

    def kv_send(d, c):
        peer = far_peer(d)
        for k in range(depth):
            out[peer, k] = kv[ask_s[peer, 1, k]]
        key_copy(peer).start()
        return c

    def value_send(d, c):
        value_copy(far_peer(d)).start()
        return c

    lax.fori_loop(1, st_n, kv_send, 0)
    lax.fori_loop(1, st_n, value_send, 0)
    for k in range(depth):
        picked = kv[ask_s[st, 1, k]]
        inc_k[st, k] = picked[:, :cols]
        inc_v[st, k] = picked[:, cols:]
    for copy in loads_q + loads_qg:
        copy.wait()

    def key_wait(d, c):
        peer = (st + d) % st_n
        z_wait(1, half(out, peer, ks), inc_k.at[peer], peer)
        return c

    lax.fori_loop(1, st_n, key_wait, 0)
    scale = HD ** (-0.5)

    def probs_step(b, c):
        r = pl.ds(pl.multiple_of(b * BLK, BLK), BLK)
        for j in range(PB):
            kvb[j * pass_len : (j + 1) * pass_len, :cols] = inc_k[
                slot_ref[0, b * PB + j], slot_ref[1, b * PB + j]
            ]
        for head in range(heads):
            hs = slice(head * HD, (head + 1) * HD)
            vs = slice(cols + head * HD, cols + (head + 1) * HD)
            gate = g_v[r, hs].astype(F32)
            scores = dot(q_v[r, hs], kvb[:, hs], NT) * scale
            shifted = jnp.exp(scores - jnp.max(scores, axis=-1, keepdims=True))
            prob = shifted / jnp.sum(shifted, axis=-1, keepdims=True)
            prob_v[head, r, :] = prob
            sig = 1.0 / (1.0 + jnp.exp(-gate))
            att_grad = (gate * sig * m_v[r, hs].astype(F32)).astype(BF)
            value_grad = dot(prob.astype(BF), att_grad, TN).astype(BF)
            for j in range(PB):
                reqg[b * PB + j, :, vs] = value_grad[j * pass_len : (j + 1) * pass_len]
        return c

    lax.fori_loop(0, blocks, probs_step, 0)

    def back_copy(phase, part, peer):
        return z_copy(phase, half(ret, peer, part), half(arr, st, part), peer)

    def give_back(phase, part, span):
        def send(d, c):
            peer = far_peer(d)
            for k in range(depth):
                ret[peer, k, :, span] = reqg[req_ref[peer, k]][:, span]
            back_copy(phase, part, peer).start()
            return c

        lax.fori_loop(1, st_n, send, 0)
        for k in range(depth):
            arr[st, k, :, span] = reqg[req_ref[st, k]][:, span]

    give_back(2, vs_all, slice(cols, 2 * cols))

    def value_wait(d, c):
        peer = (st + d) % st_n
        z_wait(4, half(out, peer, vs_all), inc_v.at[peer], peer)
        return c

    lax.fori_loop(1, st_n, value_wait, 0)

    def block_step(b, c):
        r = pl.ds(pl.multiple_of(b * BLK, BLK), BLK)
        for j in range(PB):
            o, k = slot_ref[0, b * PB + j], slot_ref[1, b * PB + j]
            kvb[j * pass_len : (j + 1) * pass_len, :cols] = inc_k[o, k]
            kvb[j * pass_len : (j + 1) * pass_len, cols:] = inc_v[o, k]
        for head in range(heads):
            hs = slice(head * HD, (head + 1) * HD)
            vs = slice(cols + head * HD, cols + (head + 1) * HD)
            q = q_v[r, hs]
            key = kvb[:, hs]
            value = kvb[:, vs]
            gate = g_v[r, hs].astype(F32)
            grad = m_v[r, hs].astype(F32)
            prob = prob_v[head, r, :]
            attended = dot(prob.astype(BF), value)
            sig = 1.0 / (1.0 + jnp.exp(-gate))
            att_grad = (gate * sig * grad).astype(BF)
            gboth[r, vs] = (grad * attended * sig * (1.0 + gate * (1.0 - sig))).astype(BF)
            prob_grad = dot(att_grad, value, NT)
            inner = jnp.sum(prob * prob_grad, axis=-1, keepdims=True)
            score_grad = (scale * prob * (prob_grad - inner)).astype(BF)
            gboth[r, hs] = dot(score_grad, key).astype(BF)
            key_grad = dot(score_grad, q, TN).astype(BF)
            for j in range(PB):
                reqg[b * PB + j, :, hs] = key_grad[j * pass_len : (j + 1) * pass_len]
        return c

    lax.fori_loop(0, blocks, block_step, 0)
    give_back(5, ks, slice(0, cols))

    n_tile = tile_of(model, 512)

    def expand(src, weight, part, pair_rows, t):
        base = pl.multiple_of(t * pair_rows, pair_rows)
        a = src[pl.ds(base, pair_rows), :]

        def step(i, c):
            n = pl.ds(pl.multiple_of(i * n_tile, n_tile), n_tile)
            part[t, :, n] = dot(a, weight[n, :], NT).astype(BF)
            return c

        lax.fori_loop(0, model // n_tile, step, 0)

    def pair_copy(which, part, pair, h):
        return remote(part.at[h * 2 + 1 - lo], pair.at[h], ps.at[which, h], pr.at[which, h], mate)

    def scatter_first(which, src, weight, part, pair, pair_rows):
        for d in range(1, hi_n + 1):
            h = (hi + d) % hi_n
            expand(src, weight, part, pair_rows, h * 2 + 1 - lo)
            pair_copy(which, part, pair, h).start()

    def cross(which, send, recv, h):
        return remote(
            send.at[h * 2 + lo], recv.at[hi], xs.at[which, h], xr.at[which, hi], {"tp": h * 2 + lo}
        )

    def scatter_second(which, src, weight, part, pair, send, recv, pair_rows):
        for d in range(1, hi_n + 1):
            h = (hi + d) % hi_n
            expand(src, weight, part, pair_rows, h * 2 + lo)
            pair_copy(which, part, pair, h).wait_recv()
            if d < hi_n:
                part[h * 2 + lo] = (part[h * 2 + lo].astype(F32) + pair[h].astype(F32)).astype(BF)
                cross(which, part, recv, h).start()

    def scatter_last(which, part, pair, send, recv, result):
        for d in range(1, hi_n):
            h = (hi + d) % hi_n
            remote(
                send.at[h * 2 + lo], recv.at[h], xs.at[which, h], xr.at[which, h], {"tp": h * 2 + lo}
            ).wait_recv()
        total = part[tp].astype(F32) + pair[hi].astype(F32)
        for d in range(1, hi_n):
            total = total + recv[(hi + d) % hi_n].astype(F32)
        result[...] = total.astype(BF)

    tok_pair = tok_rows // tp_n
    sto_pair = pass_rows // tp_n
    scatter_first(0, gboth, wqg, tp_part, tp_pair, tok_pair)
    scatter_second(0, gboth, wqg, tp_part, tp_pair, tp_part, tp_recv, tok_pair)

    def gather_sums(o, span, first):
        def step(i, c):
            r = pl.ds(pl.multiple_of(i * m_tile, m_tile), m_tile)
            part = dot(hot[o, r, :], arr[o, :, :, span].reshape(hot_cols, cols))
            acc[r, span] = part if first else acc[r, span] + part
            return c

        lax.fori_loop(0, pass_rows // m_tile, step, 0)

    for phase, part, span in ((2, vs_all, slice(cols, 2 * cols)), (5, ks, slice(0, cols))):
        gather_sums(st, span, True)

        def grad_wait(d, c):
            peer = (st + d) % st_n
            z_wait(phase, half(ret, peer, part), half(arr, peer, part), peer)
            gather_sums(peer, span, False)
            return c

        lax.fori_loop(1, st_n, grad_wait, 0)
        plow[:, span] = acc[:, span].astype(BF)

    scatter_first(1, plow, wkv, sp_part, sp_pair, sto_pair)

    def wkey_step(t, c):
        dwp[pl.ds(pl.multiple_of(t * chunk, chunk), chunk), :] = dot(
            rows[t], plow[:, :cols], TN
        ).astype(BF)
        return c

    lax.fori_loop(0, tp_n, wkey_step, 0)
    share = model // st_n

    def part_of(s):
        return dwp.at[pl.ds(pl.multiple_of(s * share, share), share), :]

    def wkey_send(d, c):
        peer = far_peer(d)
        z_copy(3, part_of(peer), dwr.at[st], peer).start()
        return c

    lax.fori_loop(1, st_n, wkey_send, 0)
    scatter_second(1, plow, wkv, sp_part, sp_pair, sp_part, sp_recv, sto_pair)
    scatter_last(0, tp_part, tp_pair, tp_part, tp_recv, tok_out)
    wkey_out[...] = part_of(st)[...].astype(F32)

    def wkey_wait(d, c):
        peer = (st + d) % st_n
        z_wait(3, part_of(peer), dwr.at[peer], peer)
        wkey_out[...] += dwr[peer].astype(F32)
        return c

    lax.fori_loop(1, st_n, wkey_wait, 0)
    scatter_last(1, sp_part, sp_pair, sp_part, sp_recv, store_out)

    for copy in across + [beside] + onward:
        copy.wait_send()

    def drain(d, c):
        peer = (st + d) % st_n
        z_copy(0, ask_ref.at[peer], ask_in.at[st], peer).wait_send()
        key_copy(peer).wait_send()
        value_copy(peer).wait_send()
        back_copy(2, vs_all, peer).wait_send()
        back_copy(5, ks, peer).wait_send()
        z_copy(3, part_of(peer), dwr.at[st], peer).wait_send()
        return c

    lax.fori_loop(1, st_n, drain, 0)
    for d in range(1, hi_n + 1):
        h = (hi + d) % hi_n
        pair_copy(0, tp_part, tp_pair, h).wait_send()
        pair_copy(1, sp_part, sp_pair, h).wait_send()
        if d < hi_n:
            cross(0, tp_part, tp_recv, h).wait_send()
            cross(1, sp_part, sp_recv, h).wait_send()


def gathered_kernel(
    st_n, tp_n, depth, pass_len,
    ids_hbm, store_ref, q_hbm, g_hbm, wq_hbm, wg_hbm, wk_hbm, wv_hbm, m_hbm,
    tok_hbm, store_hbm, wkey_hbm,
    ids_ref, tok_out, store_out, wkey_out, rows, wall, wqg, q_v, g_v, m_v, acc, terms, k_all, v_all, ask_v, ask_in, order_v, req_ref, gated, slope, ret, prob_v, kvb, reqg, gboth, arr,
    hot, plow, sums, dwp, dwc, dwf, tp_part, tp_pair, tp_recv,
    lsem, gs, gr, fs, fr, fw, zs, zr, ps, pr, xs, xr, ws, wr, ss, sr, us, ur,
):
    grp = lax.axis_index("grp")
    st = lax.axis_index("st")
    tp = lax.axis_index("tp")
    hi_n = tp_n // 2
    hi, lo = tp // 2, tp % 2
    mate_t = hi * 2 + 1 - lo
    mate = {"tp": mate_t}
    twin = {"grp": 1 - grp}
    pass_rows, chunk = rows.shape[1], rows.shape[2]
    passages = pass_rows // pass_len
    model = wqg.shape[0]
    cols = q_v.shape[1]
    heads = cols // HD
    tok_rows = q_v.shape[0]
    blocks = tok_rows // BLK
    half_pass = passages // 2
    some = tile_of(half_pass, 2)
    some_rows = some * pass_len
    n_some = half_pass // some
    key_cols, value_cols = slice(0, cols), slice(cols, 2 * cols)

    def local(i, src, dst):
        copy = pltpu.make_async_copy(src, dst, lsem.at[i])
        copy.start()
        return copy

    def sent(ref, sem):
        remote(ref, ref, sem, pr.at[0], mate).wait_send()

    def landed(ref, sem):
        remote(ref, ref, ps.at[0], sem, mate).wait_recv()

    ids_copy = local(7, ids_hbm, ids_ref)
    own_rows = local(0, store_ref, rows.at[tp])
    local(1, wk_hbm, wall.at[tp, :, pl.ds(0, cols)])
    local(1, wv_hbm, wall.at[tp, :, pl.ds(cols, cols)])
    loads_q = [local(2, q_hbm, q_v), local(3, g_hbm, g_v), local(4, m_hbm, m_v)]
    local(5, wq_hbm, wqg.at[:, pl.ds(0, cols)])
    local(5, wg_hbm, wqg.at[:, pl.ds(cols, cols)])

    barrier = pltpu.get_barrier_semaphore()

    def greet_st(d, c):
        pl.semaphore_signal(
            barrier, inc=1, device_id={"st": (st + d) % st_n}, device_id_type=MESH
        )
        return c

    lax.fori_loop(1, st_n, greet_st, 0)
    for d in range(1, tp_n):
        pl.semaphore_signal(
            barrier, inc=1, device_id={"tp": (tp + d) % tp_n}, device_id_type=MESH
        )
    pl.semaphore_signal(barrier, inc=1, device_id=twin, device_id_type=MESH)

    ids_copy.wait()

    def plan(wide):
        line = lax.broadcasted_iota(jnp.int32, (8, wide), 0)
        return line, lax.broadcasted_iota(jnp.int32, (8, wide), 1)

    width = ask_v.shape[2]
    line, lane = plan(width)
    slot, place = lane // pass_len, lane % pass_len
    short_line, short_lane = plan(order_v.shape[1])
    target = jnp.full((8, width), -1, jnp.int32)
    order = jnp.zeros(order_v.shape, jnp.int32)
    taken = [jnp.int32(0)] * st_n
    for j in range(PB):
        for n in range(blocks):
            i = ids_ref[j, n]
            owner = lax.div(i, jnp.int32(passages))
            within = i - owner * passages
            rank = sum(jnp.where(owner == o, taken[o], 0) for o in range(st_n))
            taken = [taken[o] + jnp.where(owner == o, 1, 0) for o in range(st_n)]
            target = jnp.where(
                (line == owner) & (slot == rank), within * pass_len + place, target
            )
            order = jnp.where(
                (short_line == owner) & (short_lane == rank), j * blocks + n, order
            )
    order_v[...] = order
    for o in range(st_n):
        ask_v[o] = jnp.broadcast_to(target[o : o + 1], (8, width))
    pl.semaphore_wait(barrier, st_n + tp_n - 1)

    def first_row(i):
        part = (grp + i // n_some) % 2
        return pl.multiple_of((part * n_some + i % n_some) * some_rows, some_rows)

    n_part = tile_of(n_some, 2)

    def g_copy(way, lot, t, onto):
        i, count, slot = lot
        r = pl.ds(first_row(i), count * some_rows)
        away = (t - onto + tp_n) % tp_n - 1
        return remote(rows.at[t, r], rows.at[t, r], gs.at[way], gr.at[away, slot], {"tp": onto})

    def small(i):
        return i, 1, i

    def large(i):
        return n_some + i * n_part, n_part, n_some + i

    def onward(d, lot):
        return g_copy(2, lot, ((hi + d) % hi_n) * 2 + lo, mate_t)

    def g_wait(t, lot):
        g_copy(1, lot, t, tp).wait_recv()

    def rows_send(lot):
        for d in range(1, hi_n):
            g_copy(0, lot, tp, ((hi + d) % hi_n) * 2 + lo).start()
        g_copy(1, lot, tp, mate_t).start()

    def rows_small(i, c):
        rows_send(small(i))
        return c

    def rows_large(i, c):
        rows_send(large(i))
        return c

    own_rows.wait()
    lax.fori_loop(0, n_some, rows_small, 0)
    lax.fori_loop(0, n_some // n_part, rows_large, 0)

    upper = st >= st_n // 2
    mark = jnp.where(upper, st, st_n - 1 - st)

    def far_peer(d):
        i = d - 1
        i = i + jnp.where(i >= mark, 1, 0)
        return jnp.where(upper, i, st_n - 1 - i)

    def z_copy(phase, src, dst, peer):
        away = (st - peer + st_n) % st_n - 1
        return remote(src, dst, zs.at[phase], zr.at[phase, away], {"st": peer})

    def z_wait(phase, src, dst, peer):
        landed(dst, zr.at[phase, (peer - st + st_n) % st_n - 1])

    def ask_send(d, c):
        peer = (st + d) % st_n
        z_copy(0, ask_v.at[peer], ask_in.at[st], peer).start()
        return c

    lax.fori_loop(1, st_n, ask_send, 0)
    ask_in[st] = ask_v[st]
    order_copy = local(6, order_v, req_ref)

    def project(lot, send):
        i, count, _ = lot
        r = pl.ds(first_row(i), count * some_rows)

        def term(t, span):
            return dot(rows[t, r], wall[tp, pl.ds(pl.multiple_of(t * chunk, chunk), chunk), span])

        for d in range(1, hi_n):
            g_wait(((hi + d) % hi_n) * 2 + lo, lot)
            onward(d, lot).start()
        g_wait(mate_t, lot)
        near = [tp, mate_t] + [((hi + d) % hi_n) * 2 + lo for d in range(1, hi_n)]
        late = [((hi + d) % hi_n) * 2 + 1 - lo for d in range(1, hi_n)]
        total = sum(term(t, key_cols) for t in near[1:]) + term(near[0], key_cols)
        for t in late:
            g_wait(t, lot)
            total = total + term(t, key_cols)
        first = st * passages + first_row(i) // pass_len

        def keep(ref, total):
            low = total.astype(BF)
            for p in range(count * some):
                ref[first + p] = low[p * pass_len : (p + 1) * pass_len]

        keep(k_all, total)
        send()
        keep(v_all, sum(term(t, value_cols) for t in near + late))

    def part_of_all(kind, o, c, side):
        ref = k_all if kind == 0 else v_all
        return ref.at[pl.ds(o * passages + side * half_pass + c * some, some)]

    def chain_copy(kind, o, c, peer):
        part = part_of_all(kind, o, c, grp)
        away = (o - peer + st_n) % st_n - 1
        return remote(part, part, fs.at[kind, 0], fr.at[kind, away, c], {"st": peer})

    def twin_copy(kind, o, c):
        part = part_of_all(kind, o, c, grp)
        return remote(part, part, fs.at[kind, 1], fw.at[kind], twin)

    lower = st < st_n // 2
    edge = (st == 0) | (st == st_n - 1)

    def own_send(kind, c, inward=True, outward=True):
        for onto, toward in ((st + 1, lower), (st - 1, jnp.logical_not(lower))):
            there = (onto >= 0) & (onto < st_n)
            if not outward:
                there = there & toward
            if not inward:
                there = there & jnp.logical_not(toward)

            @pl.when(there)
            def _():
                chain_copy(kind, st, c, onto).start()

    def relay(kind, d, c):
        for sign in (-1, 1):
            o = st + sign * d
            onto = st - sign

            @pl.when((o >= 0) & (o < st_n))
            def _():
                chain_copy(kind, o, c, st).wait_recv()

                @pl.when((onto >= 0) & (onto < st_n))
                def _():
                    chain_copy(kind, o, c, onto).start()

                twin_copy(kind, o, c).start()

    relayed = (st_n - 1) * half_pass

    def twin_wait(kind):
        landed((k_all, v_all)[kind].at[pl.ds(0, relayed)], fw.at[kind])

    landed(wall.at[tp], lsem.at[1])
    for copy in loads_q:
        copy.wait()

    gate_rows = tok_rows // n_some

    def gates(i):
        r = pl.ds(pl.multiple_of(i * gate_rows, gate_rows), gate_rows)
        gate = g_v[r, :].astype(F32)
        grad = m_v[r, :].astype(F32)
        sig = 1.0 / (1.0 + jnp.exp(-gate))
        gated[r, :] = (gate * sig * grad).astype(BF)
        slope[r, :] = grad * (sig * (1.0 + gate * (1.0 - sig)))

    def early_step(i, c):
        project(small(i), lambda: own_send(0, i))

        for d in range(1, st_n):
            @pl.when(i >= d)
            def _():
                relay(0, d, i - d)

        @pl.when(edge | (i == 0))
        def _():
            own_send(1, i)

        gates(i)
        return c

    lax.fori_loop(0, n_some, early_step, 0)
    for i in range(n_some - 1, n_some):
        relay(0, 1, i)

    def inward_send(i, c):
        own_send(1, i, outward=False)
        return c

    lax.fori_loop(jnp.where(edge, n_some, 1), n_some, inward_send, 0)

    def second_step(i, c):
        relay(0, 2, i)
        return c

    def outward_send(i, c):
        own_send(1, i, inward=False)
        return c

    lax.fori_loop(n_some - 2, n_some, second_step, 0)
    @pl.when(edge)
    def _():
        relay(1, 1, 0)

    lax.fori_loop(jnp.where(edge, n_some, 1), n_some, outward_send, 0)

    def late_step(i, c):
        project(large(i), lambda: None)
        for q in range(n_part):
            @pl.when(edge & (i * n_part + q >= n_some - 3))
            def _():
                relay(0, 3, i * n_part + q)

            @pl.when(jnp.logical_not(edge))
            def _():
                relay(1, 1, i * n_part + q)

        return c

    w_part = model // 2
    w_mine = pl.ds(pl.multiple_of(grp * w_part, w_part), w_part)
    w_other = pl.ds(pl.multiple_of((1 - grp) * w_part, w_part), w_part)

    def w_across(d):
        h = (hi + d) % hi_n
        part = wall.at[tp, w_mine]
        return remote(part, part, ws.at[0], wr.at[0], {"tp": h * 2 + lo})

    def w_twin(d):
        t = ((hi + d) % hi_n) * 2 + lo
        part = wall.at[t, w_mine]
        return remote(part, part, ws.at[0], wr.at[1], twin)

    def w_onward(d, k):
        t = ((hi + d) % hi_n) * 2 + lo
        part = wall.at[t, w_other if k else w_mine]
        return remote(part, part, ws.at[0], wr.at[2], mate)

    w_beside = remote(wall.at[tp], wall.at[tp], ws.at[0], wr.at[2], mate)

    def w_wait(kind, t, part):
        landed(wall.at[t, part], wr.at[kind])

    for d in range(1, hi_n):
        w_across(d).start()

    def relay_rest(kind, first, last):
        def step(i, c):
            relay(kind, 1 + i // n_some, i % n_some)
            return c

        lax.fori_loop(first, last, step, 0)

    relays = (st_n - 1) * n_some
    lax.fori_loop(0, n_some // n_part, late_step, 0)
    w_beside.start()
    relay_rest(1, 1, jnp.where(edge, n_some, 1))
    landed(wqg, lsem.at[5])
    order_copy.wait()
    twin_wait(0)
    scale = HD ** (-0.5)

    def fill(n, ref, span, b):
        for j in range(PB):
            kvb[n, j * pass_len : (j + 1) * pass_len, span] = ref[ids_ref[j, b]]

    pairs = range(4)

    def block_rows(b):
        return pl.ds(pl.multiple_of(b * BLK, BLK), BLK)

    per_step = n_some // (blocks // 4)

    def probs_step(i, c):
        for n in pairs:
            fill(n, k_all, key_cols, 4 * i + n)
        for head in range(heads):
            hs = slice(head * HD, (head + 1) * HD)
            vs = slice(cols + head * HD, cols + (head + 1) * HD)
            for n in pairs:
                b = 4 * i + n
                r = block_rows(b)
                scores = dot(q_v[r, hs], kvb[n, :, hs], NT) * scale
                shifted = jnp.exp(scores - jnp.max(scores, axis=-1, keepdims=True))
                prob = shifted * (1.0 / jnp.sum(shifted, axis=-1, keepdims=True))
                prob_v[head, r, :] = prob
                value_grad = dot(prob.astype(BF), gated[r, hs], TN).astype(BF)
                for j in range(PB):
                    reqg[j * blocks + b, :, vs] = value_grad[j * pass_len : (j + 1) * pass_len]

        for q in range(per_step):
            relay(1, 2, i * per_step + q)

        return c

    lax.fori_loop(0, blocks // 4, probs_step, 0)

    def half(ref, peer, part):
        return ref.at[peer, :, :, part]

    def back_copy(phase, part, peer):
        return z_copy(phase, half(ret, peer, part), half(arr, st, part), peer)

    def give_back(phase, part, span, order, first, last):
        def send(d, c):
            peer = order(d)
            for k in range(depth):
                ret[peer, k, :, span] = reqg[req_ref[peer, k]][:, span]
            back_copy(phase, part, peer).start()
            return c

        lax.fori_loop(first, last, send, 0)

    def keep_own(span):
        for k in range(depth):
            arr[st, k, :, span] = reqg[req_ref[st, k]][:, span]

    def near_peer(d):
        return far_peer(st_n - d)

    ks, vs_all = pl.ds(0, cols), pl.ds(cols, cols)
    def value_peer(d):
        return jnp.where(edge, near_peer(d % (st_n - 1) + 1), near_peer(d))

    give_back(
        1, vs_all, value_cols, value_peer, 1, jnp.where(edge, st_n, st_n - 1)
    )
    keep_own(value_cols)
    relay_rest(1, n_some + per_step * (blocks // 4), relays)
    twin_wait(1)

    def block_step(i, c):
        for n in pairs:
            fill(n, k_all, key_cols, 4 * i + n)
            fill(n, v_all, value_cols, 4 * i + n)
        for head in range(heads):
            hs = slice(head * HD, (head + 1) * HD)
            vs = slice(cols + head * HD, cols + (head + 1) * HD)
            for n in pairs:
                b = 4 * i + n
                r = block_rows(b)
                value = kvb[n, :, vs]
                prob = prob_v[head, r, :]
                prob_grad = dot(gated[r, hs], value, NT)
                inner = jnp.sum(prob * prob_grad, axis=-1, keepdims=True)
                score_grad = (scale * prob * (prob_grad - inner)).astype(BF)
                key_grad = dot(score_grad, q_v[r, hs], TN).astype(BF)
                for j in range(PB):
                    reqg[j * blocks + b, :, hs] = key_grad[j * pass_len : (j + 1) * pass_len]
                gboth[r, hs] = dot(score_grad, kvb[n, :, hs]).astype(BF)
                attended = dot(prob.astype(BF), value)
                gboth[r, vs] = (attended * slope[r, hs]).astype(BF)
        return c

    lax.fori_loop(0, blocks // 4, block_step, 0)
    def key_peer(d):
        return jnp.where(edge, near_peer(jnp.where(d == 1, 1, st_n + 1 - d)), far_peer(d))

    give_back(2, ks, key_cols, key_peer, 1, st_n)
    keep_own(key_cols)

    @pl.when(jnp.logical_not(edge))
    def _():
        give_back(1, vs_all, value_cols, near_peer, st_n - 1, st_n)

    n_tile = tile_of(model, 512)

    n_tiles = model // n_tile
    tok_pair = tok_rows // tp_n

    def tile(i):
        return pl.ds(pl.multiple_of(i * n_tile, n_tile), n_tile)

    def expand(h, i):
        a = gboth[pl.ds(pl.multiple_of(h * 2 * tok_pair, tok_pair), 2 * tok_pair), :]
        part = dot(a, wqg[tile(i), :], NT).astype(BF)
        tp_part[h * 2, :, tile(i)] = part[:tok_pair]
        tp_part[h * 2 + 1, :, tile(i)] = part[tok_pair:]

    def pair_copy(h, n, slot):
        src, dst = tp_part.at[h * 2 + 1 - lo, :, n], tp_pair.at[h, :, n]
        return remote(src, dst, ps.at[0], pr.at[slot], mate)

    def cross(h, n):
        src, dst = tp_part.at[h * 2 + lo, :, n], tp_recv.at[hi, :, n]
        return remote(src, dst, xs.at[0], xr.at[0], {"tp": h * 2 + lo})

    for d in range(1, hi_n):
        w_wait(0, ((hi + d) % hi_n) * 2 + lo, w_mine)
        w_twin(d).start()
        w_onward(d, 0).start()

    there = 1 - hi

    def far_tile(i, c):
        expand(there, i)
        pair_copy(there, tile(i), 1 + i).start()
        return c

    def cross_tile(i, c):
        n = tile(i)
        pair_copy(there, n, 1 + i).wait_recv()
        own = tp_part[there * 2 + lo, :, n].astype(F32)
        tp_part[there * 2 + lo, :, n] = (own + tp_pair[there, :, n].astype(F32)).astype(BF)
        cross(there, n).start()
        return c

    def own_tile(i, c):
        expand(hi, i)
        return c

    lax.fori_loop(0, n_tiles, far_tile, 0)
    lax.fori_loop(0, n_tiles, cross_tile, 0)
    lax.fori_loop(0, n_tiles, own_tile, 0)
    pair_copy(hi, pl.ds(0, model), 0).start()

    def ask_wait(d, c):
        peer = (st + d) % st_n
        z_wait(0, ask_v.at[peer], ask_in.at[peer], peer)
        return c

    lax.fori_loop(1, st_n, ask_wait, 0)
    hot_cols = depth * pass_len
    m_tile = tile_of(pass_rows, 256)

    def hot_step(o, c):
        target = ask_in[o][0:1, :hot_cols]
        for i in range(pass_rows // m_tile):
            line = lax.broadcasted_iota(jnp.int32, (m_tile, hot_cols), 0) + i * m_tile
            hot[o, i * m_tile : (i + 1) * m_tile, :] = jnp.where(line == target, 1.0, 0.0).astype(BF)
        return c

    lax.fori_loop(0, st_n, hot_step, 0)

    def gather_sums(kind, o, span, first=False, last=False):
        def step(i, c):
            r = pl.ds(pl.multiple_of(i * m_tile, m_tile), m_tile)
            part = dot(hot[o, r, :], arr[o, :, :, span].reshape(hot_cols, cols))
            part = part if first else acc[kind, r, :] + part
            if last:
                plow[r, span] = part.astype(BF)
            else:
                acc[kind, r, :] = part
            return c

        lax.fori_loop(0, pass_rows // m_tile, step, 0)

    sto_pair = pass_rows // tp_n

    def sums_copy(kind, part, d):
        t = (tp + d) % tp_n
        src = plow.at[pl.ds(pl.multiple_of(t * sto_pair, sto_pair), sto_pair), part]
        return remote(src, sums.at[tp, :, part], ss.at[kind], sr.at[kind], {"tp": t})

    def sums_of(part):
        return sums.at[pl.ds(0, tp_n - 1), :, part]

    def grads_of(kind, peer, last=False):
        phase, part, span = (2, ks, key_cols) if kind == 0 else (1, vs_all, value_cols)
        z_wait(phase, half(ret, peer, part), half(arr, peer, part), peer)
        gather_sums(kind, peer, span, last=last)

    def sums_send(kind):
        part, span = (ks, key_cols) if kind == 0 else (vs_all, value_cols)
        for d in range(1, tp_n):
            sums_copy(kind, part, d).start()
        sums[tp, :, span] = plow[pl.ds(pl.multiple_of(tp * sto_pair, sto_pair), sto_pair), span]

    beyond = jnp.where(lower, st_n - 1, 0)
    middle = jnp.where(lower, st_n // 2, st_n // 2 - 1)
    beside_st = st + 1 - 2 * (st % 2)
    outer = edge
    inner = jnp.logical_not(outer)
    gather_sums(1, st, value_cols, first=True)
    gather_sums(0, st, key_cols, first=True)
    grads_of(1, beside_st)
    grads_of(1, jnp.where(outer, beyond, middle))

    grads_of(0, middle)

    grads_of(0, beyond)
    grads_of(0, beside_st, last=True)
    sums_send(0)

    share = model // st_n
    bits = 2
    bit = share // bits

    def dw_line(s, b):
        return pl.ds(pl.multiple_of(s * share + b * bit, bit), bit)

    def dw_copy(kind, b):
        line = pl.ds(b * bit, bit)
        if kind < 2:
            src, dst = dwp.at[dw_line(middle if kind else beyond, b)], dwc.at[kind, line]
            peer = beside_st
        elif kind == 2:
            src, dst, peer = dwp.at[dw_line(beside_st, b)], dwf.at[0, line], beside_st
        else:
            src, dst = dwc.at[kind - 3, line], dwf.at[1, line]
            peer = middle if kind == 4 else beyond
        return remote(src, dst, us.at[0], ur.at[min(kind, 3), b], {"st": peer})

    def dw_send(kind):
        for b in range(bits):
            dw_copy(kind, b).start()

    def dw_relay(q):
        for b in range(bits):
            line = slice(b * bit, (b + 1) * bit)
            dw_copy(q, b).wait_recv()
            own = dwp[dw_line(middle if q else beyond, b), :].astype(F32)
            dwc[q, line, :] = (dwc[q, line, :].astype(F32) + own).astype(BF)
            dw_copy(3 + q, b).start()

    def wkey_step(s):
        dwp[pl.ds(pl.multiple_of(s * chunk, chunk), chunk), :] = dot(
            rows[s], plow[:, key_cols], TN
        ).astype(BF)

    def wkey_turn(j, c):
        far = jnp.where(j == 0, beyond, middle)
        near = jnp.where(j == 2, beside_st, st)
        near_first = jnp.where(j == 0, beside_st, st)
        far_after = jnp.where(j == 1, beyond, middle)
        s = jnp.where(
            outer, jnp.where(j < 2, far, near), jnp.where((j == 0) | (j == 3), near_first, far_after)
        )
        wkey_step(s)
        for kind in range(3):
            @pl.when(outer & (j == kind))
            def _():
                dw_send(kind)

        @pl.when(inner & (j == 0))
        def _():
            dw_send(2)

        return c

    lax.fori_loop(0, st_n, wkey_turn, 0)

    @pl.when(inner)
    def _():
        dw_relay(0)

    for d in range(1, hi_n):
        t = ((hi + d) % hi_n) * 2 + lo
        w_wait(1, t, w_other)
        w_onward(d, 1).start()
    landed(wall.at[pl.ds(0, hi_n)], wr.at[2])

    def store_terms(span, done):
        def step(i, c):
            n = pl.ds(pl.multiple_of(i * n_tile, n_tile), n_tile)
            part = dot(sums[0, :, span], wall[0, n, span], NT)
            for t in range(1, tp_n):
                part = part + dot(sums[t, :, span], wall[t, n, span], NT)
            done(n, part)
            return c

        lax.fori_loop(0, model // n_tile, step, 0)

    def keep_terms(n, part):
        terms[:, n] = part

    def keep_store(n, part):
        store_out[:, n] = (terms[:, n] + part).astype(BF)

    grads_of(1, jnp.where(outer, middle, beyond), last=True)
    sums_send(1)

    landed(sums_of(ks), sr.at[0])
    store_terms(key_cols, keep_terms)

    pair_copy(hi, pl.ds(0, model), 0).wait_recv()
    landed(tp_recv.at[there], xr.at[0])
    total = tp_part[tp].astype(F32) + tp_pair[hi].astype(F32) + tp_recv[there].astype(F32)
    tok_out[...] = total.astype(BF)
    tok_done = local(2, tok_out, tok_hbm)

    @pl.when(inner)
    def _():
        dw_relay(1)

    landed(sums_of(vs_all), sr.at[1])
    store_terms(value_cols, keep_store)
    store_done = local(3, store_out, store_hbm)

    for b in range(bits):
        line = slice(b * bit, (b + 1) * bit)
        dw_copy(2, b).wait_recv()
        wkey_out[line, :] = dwp[dw_line(st, b), :].astype(F32) + dwf[0, line, :].astype(F32)
    for b in range(bits):
        line = slice(b * bit, (b + 1) * bit)
        for kind, edge in ((3, outer), (4, inner)):
            @pl.when(edge)
            def _():
                dw_copy(kind, b).wait_recv()

        wkey_out[line, :] += dwf[1, line, :].astype(F32)

    wkey_done = local(4, wkey_out, wkey_hbm)

    for way in range(3):
        sent(rows.at[tp], gs.at[way])
    for kind, ref in ((0, k_all), (1, v_all)):
        sent(ref.at[pl.ds(0, relayed)], fs.at[kind, 1])
        for s in range(st_n):
            up, down = (s + 1) * (s + 1 < st_n), (st_n - s) * (s > 0)

            @pl.when(st == s)
            def _():
                sent(ref.at[pl.ds(0, (up + down) * half_pass)], fs.at[kind, 0])

    sent(wall.at[pl.ds(0, hi_n + 1)], ws.at[0])
    sent(ask_in.at[pl.ds(0, st_n - 1)], zs.at[0])
    sent(ret.at[pl.ds(0, st_n - 1), :, :, vs_all], zs.at[1])
    sent(ret.at[pl.ds(0, st_n - 1), :, :, ks], zs.at[2])
    sent(sums_of(ks), ss.at[0])
    sent(sums_of(vs_all), ss.at[1])
    sent(tp_pair, ps.at[0])
    sent(tp_recv.at[0], xs.at[0])
    sent(dwp.at[pl.ds(0, 3 * share)], us.at[0])
    for copy in (tok_done, store_done, wkey_done):
        copy.wait()


def settle_kernel(*refs):
    n = (len(refs) - 2) // 3
    sources, results, held = refs[:n], refs[n : 2 * n], refs[2 * n : 3 * n]
    ins, outs = refs[3 * n], refs[3 * n + 1]
    pieces = []
    for a, (source, result, here) in enumerate(zip(sources, results, held)):
        part = source.shape[0] // 2
        for i in range(2):
            r = pl.ds(i * part, part)
            pieces.append(
                (
                    pltpu.make_async_copy(source.at[r], here.at[r], ins.at[a, i]),
                    pltpu.make_async_copy(here.at[r], result.at[r], outs.at[a, i]),
                )
            )
    for fetch, _ in pieces:
        fetch.start()
    for fetch, put in pieces:
        fetch.wait()
        put.start()
    for _, put in pieces:
        put.wait()


def settle(*arrays):
    hbm = pl.BlockSpec(memory_space=pl.ANY)
    n = len(arrays)
    return pl.pallas_call(
        settle_kernel,
        out_shape=tuple(jax.ShapeDtypeStruct(a.shape, a.dtype) for a in arrays),
        in_specs=[hbm] * n,
        out_specs=(hbm,) * n,
        scratch_shapes=[pltpu.VMEM(a.shape, a.dtype) for a in arrays]
        + [pltpu.SemaphoreType.DMA((n, 2)), pltpu.SemaphoreType.DMA((n, 2))],
    )(*arrays)


def local(pass_ids, store, queries, gate_pre, w_query, w_gate, w_key, w_value, d_mem):
    st_n = lax.axis_size("st")
    tp_n = lax.axis_size("tp")
    hi_n = tp_n // 2
    tok_rows, cols = queries.shape
    blocks = tok_rows // BLK
    passages, pass_len, chunk = store.shape
    model = w_key.shape[0]
    requests = blocks * PB
    depth = max(2, requests // st_n)
    pass_rows = passages * pass_len
    share = model // st_n

    vmem = pl.BlockSpec(memory_space=pltpu.VMEM)
    smem = pl.BlockSpec(memory_space=pltpu.SMEM)
    hbm = pl.BlockSpec(memory_space=pl.ANY)
    V = pltpu.VMEM
    DMA = pltpu.SemaphoreType.DMA
    pair = 2 * cols
    tok_pair = tok_rows // tp_n
    sto_pair = pass_rows // tp_n
    hot_cols = depth * pass_len
    width = -(-hot_cols // 128) * 128
    gathered_bytes = 2 * 2 * st_n * pass_rows * cols
    steps = blocks // 4
    fits = lax.axis_size("grp") == 2 and hi_n == 2 and st_n == 4 and st_n == tp_n
    fits = fits and passages % 4 == 0 and blocks % 4 == 0 and passages // 4 % steps == 0
    if fits and gathered_bytes <= 8 << 20:
        half_pass = passages // 2
        n_some = half_pass // tile_of(half_pass, 2)
        d_tokens, d_store, d_wkey = pl.pallas_call(
            functools.partial(gathered_kernel, st_n, tp_n, depth, pass_len),
            out_shape=(
                jax.ShapeDtypeStruct((tok_pair, model), BF),
                jax.ShapeDtypeStruct((sto_pair, model), BF),
                jax.ShapeDtypeStruct((share, cols), F32),
            ),
            in_specs=[hbm] * 9,
            out_specs=(hbm, hbm, hbm),
            scratch_shapes=[
                pltpu.SMEM((PB, blocks), jnp.int32),
                V((tok_pair, model), BF),
                V((sto_pair, model), BF),
                V((share, cols), F32),
                V((tp_n, pass_rows, chunk), BF),
                V((tp_n, model, pair), BF),
                V((model, pair), BF),
                V((tok_rows, cols), BF),
                V((tok_rows, cols), BF),
                V((tok_rows, cols), BF),
                V((2, pass_rows, cols), F32),
                V((sto_pair, model), F32),
                V((st_n * passages, pass_len, cols), BF),
                V((st_n * passages, pass_len, cols), BF),
                V((st_n, 8, width), jnp.int32),
                V((st_n, 8, width), jnp.int32),
                V((8, 128), jnp.int32),
                pltpu.SMEM((8, 128), jnp.int32),
                V((tok_rows, cols), BF),
                V((tok_rows, cols), F32),
                V((st_n, depth, pass_len, pair), BF),
                V((cols // HD, tok_rows, PB * pass_len), F32),
                V((4, PB * pass_len, pair), BF),
                V((requests, pass_len, pair), BF),
                V((tok_rows, pair), BF),
                V((st_n, depth, pass_len, pair), BF),
                V((st_n, pass_rows, hot_cols), BF),
                V((pass_rows, pair), BF),
                V((tp_n, sto_pair, pair), BF),
                V((model, cols), BF),
                V((2, share, cols), BF),
                V((2, share, cols), BF),
                V((tp_n, tok_pair, model), BF),
                V((hi_n, tok_pair, model), BF),
                V((hi_n, tok_pair, model), BF),
                DMA((8,)),
                DMA((3,)),
                DMA((tp_n - 1, n_some + n_some // tile_of(n_some, 2))),
                DMA((2, 2)),
                DMA((2, st_n - 1, n_some)),
                DMA((2,)),
                DMA((3,)),
                DMA((3, st_n - 1)),
                DMA((1,)),
                DMA((1 + model // tile_of(model, 512),)),
                DMA((1,)),
                DMA((1,)),
                DMA((1,)),
                DMA((3,)),
                DMA((2,)),
                DMA((2,)),
                DMA((1,)),
                DMA((4, 2)),
            ],
            compiler_params=pltpu.CompilerParams(
                collective_id=0, has_side_effects=True, vmem_limit_bytes=67043328
            ),
        )(
            pass_ids.T, store.reshape(pass_rows, chunk),
            queries, gate_pre, w_query, w_gate, w_key, w_value, d_mem,
        )
        d_tokens, d_store, d_wkey = settle(d_tokens, d_store, d_wkey)
        return d_tokens, d_store.reshape(passages // tp_n, pass_len, model), d_wkey

    ids = pass_ids.reshape(-1)
    owners = ids // passages
    within = ids % passages
    order = jnp.arange(requests, dtype=jnp.int32)
    earlier = (owners[None, :] == owners[:, None]) & (order[None, :] < order[:, None])
    rank = jnp.sum(earlier.astype(jnp.int32), axis=1)
    slots = jnp.stack([owners, rank])
    o_i = jnp.arange(st_n, dtype=jnp.int32)[:, None, None]
    k_i = jnp.arange(depth, dtype=jnp.int32)[None, :, None]
    match = (owners[None, None, :] == o_i) & (rank[None, None, :] == k_i)
    asked = jnp.max(jnp.where(match, within[None, None, :], -1), axis=2)
    req_of = jnp.max(jnp.where(match, order[None, None, :], 0), axis=2)
    hot_cols = depth * pass_len
    width = -(-hot_cols // 128) * 128
    lane = jnp.arange(width, dtype=jnp.int32)
    spread = jnp.repeat(asked, pass_len, axis=1)
    spread = jnp.pad(spread, ((0, 0), (0, width - hot_cols)), constant_values=-1)
    target = jnp.where(spread < 0, -1, spread * pass_len + lane[None, :] % pass_len)
    flat = jnp.pad(jnp.maximum(asked, 0), ((0, 0), (0, width - depth)))
    ask = jnp.concatenate(
        [target[:, None], flat[:, None], jnp.zeros((st_n, 6, width), jnp.int32)], axis=1
    )

    d_tokens, d_store, d_wkey = pl.pallas_call(
        functools.partial(kernel, st_n, tp_n, depth, pass_len),
        out_shape=(
            jax.ShapeDtypeStruct((tok_pair, model), BF),
            jax.ShapeDtypeStruct((sto_pair, model), BF),
            jax.ShapeDtypeStruct((share, cols), F32),
        ),
        in_specs=[smem, smem, vmem] + [hbm] * 8,
        out_specs=(vmem, vmem, vmem),
        scratch_shapes=[
            V((tp_n, pass_rows, chunk), BF),
            V((model, pair), BF),
            V((model, pair), BF),
            V((tok_rows, cols), BF),
            V((tok_rows, cols), BF),
            V((tok_rows, cols), BF),
            V((pass_rows, pair), F32),
            V((passages, pass_len, pair), BF),
            V((st_n, 8, width), jnp.int32),
            pltpu.SMEM((st_n, 8, width), jnp.int32),
            V((st_n, depth, pass_len, pair), BF),
            V((st_n, depth, pass_len, cols), BF),
            V((st_n, depth, pass_len, cols), BF),
            V((st_n, depth, pass_len, pair), BF),
            V((cols // HD, tok_rows, PB * pass_len), F32),
            V((PB * pass_len, pair), BF),
            V((requests, pass_len, pair), BF),
            V((tok_rows, pair), BF),
            V((st_n, depth, pass_len, pair), BF),
            V((st_n, pass_rows, hot_cols), BF),
            V((pass_rows, pair), BF),
            V((model, cols), BF),
            V((st_n, share, cols), BF),
            V((tp_n, tok_pair, model), BF),
            V((hi_n, tok_pair, model), BF),
            V((hi_n, tok_pair, model), BF),
            V((tp_n, sto_pair, model), BF),
            V((hi_n, sto_pair, model), BF),
            V((hi_n, sto_pair, model), BF),
            DMA((9,)),
            DMA((3, hi_n)),
            DMA((tp_n,)),
            DMA((6, st_n)),
            DMA((6, st_n)),
            DMA((2, hi_n)),
            DMA((2, hi_n)),
            DMA((2, hi_n)),
            DMA((2, hi_n)),
        ],
        compiler_params=pltpu.CompilerParams(
            collective_id=0, has_side_effects=True, vmem_limit_bytes=67043328
        ),
    )(
        slots, req_of, ask, store.reshape(pass_rows, chunk),
        queries, gate_pre, w_query, w_gate, w_key, w_value, d_mem,
    )
    return d_tokens, d_store.reshape(passages // tp_n, pass_len, model), d_wkey


def solution(mesh):
    return jax.shard_map(
        local,
        mesh=mesh,
        in_specs=(
            P(("grp", "st"), None),
            P("st", None, "tp"),
            P(("grp", "st"), "tp"),
            P(("grp", "st"), "tp"),
            P(None, "tp"),
            P(None, "tp"),
            P(None, "tp"),
            P(None, "tp"),
            P(("grp", "st"), "tp"),
        ),
        out_specs=(
            P(("grp", "st", "tp"), None),
            P(("grp", "st", "tp"), None, None),
            P(("grp", "st"), "tp"),
        ),
        check_vma=False,
    )
```

```python
import functools

import jax
import jax.numpy as jnp
from jax import lax
from jax.experimental import pallas as pl
from jax.experimental.pallas import tpu as pltpu
from jax.sharding import PartitionSpec as P

HD = 256
BLK = 128
PB = 4
BF = jnp.bfloat16
F32 = jnp.float32
MESH = pl.DeviceIdType.MESH
NT = (((1,), (1,)), ((), ()))
TN = (((0,), (0,)), ((), ()))


def dot(a, b, dims=(((1,), (0,)), ((), ()))):
    return lax.dot_general(a, b, dims, preferred_element_type=F32)


def remote(src, dst, send, recv, device):
    return pltpu.make_async_remote_copy(
        src_ref=src,
        dst_ref=dst,
        send_sem=send,
        recv_sem=recv,
        device_id=device,
        device_id_type=MESH,
    )


def tile_of(size, most):
    while size % most:
        most //= 2
    return most


def kernel(
    st_n, tp_n, depth, pass_len,
    slot_ref, req_ref, ask_ref, store_ref, q_hbm, g_hbm, wq_hbm, wg_hbm, wk_hbm, wv_hbm, m_hbm,
    tok_out, store_out, wkey_out,
    rows, wkv, wqg, q_v, g_v, m_v, acc, kv, ask_in, ask_s, out, inc_k, inc_v, ret, prob_v, kvb, reqg, gboth, arr,
    hot, plow, dwp, dwr, tp_part, tp_pair, tp_recv, sp_part, sp_pair, sp_recv,
    lsem, gs, gr, zs, zr, ps, pr, xs, xr,
):
    st = lax.axis_index("st")
    tp = lax.axis_index("tp")
    hi_n = tp_n // 2
    hi, lo = tp // 2, tp % 2
    mate = {"tp": hi * 2 + 1 - lo}
    pass_rows, chunk = rows.shape[1], rows.shape[2]
    model = wqg.shape[0]
    cols = q_v.shape[1]
    heads = cols // HD
    tok_rows = q_v.shape[0]
    blocks = tok_rows // BLK
    blk_keys = PB * pass_len

    def local(i, src, dst):
        copy = pltpu.make_async_copy(src, dst, lsem.at[i])
        copy.start()
        return copy

    own_rows = local(0, store_ref, rows.at[tp])
    loads_kv = [
        local(1, wk_hbm, wkv.at[:, pl.ds(0, cols)]),
        local(2, wv_hbm, wkv.at[:, pl.ds(cols, cols)]),
    ]
    loads_q = [local(3, q_hbm, q_v), local(4, g_hbm, g_v), local(5, m_hbm, m_v)]
    loads_qg = [
        local(6, wq_hbm, wqg.at[:, pl.ds(0, cols)]),
        local(7, wg_hbm, wqg.at[:, pl.ds(cols, cols)]),
    ]

    barrier = pltpu.get_barrier_semaphore()

    def greet_st(d, c):
        pl.semaphore_signal(
            barrier, inc=1, device_id={"st": (st + d) % st_n}, device_id_type=MESH
        )
        return c

    lax.fori_loop(1, st_n, greet_st, 0)
    for d in range(1, tp_n):
        pl.semaphore_signal(
            barrier, inc=1, device_id={"tp": (tp + d) % tp_n}, device_id_type=MESH
        )
    pl.semaphore_wait(barrier, st_n - 1 + tp_n - 1)

    across = []
    for d in range(1, hi_n):
        h = (hi + d) % hi_n
        across.append(
            remote(store_ref, rows.at[tp], gs.at[0, h], gr.at[tp], {"tp": h * 2 + lo})
        )
        across[-1].start()
    beside = remote(store_ref, rows.at[tp], gs.at[1, hi], gr.at[tp], mate)
    beside.start()

    upper = st >= st_n // 2
    mark = jnp.where(upper, st, st_n - 1 - st)

    def far_peer(d):
        i = d - 1
        i = i + jnp.where(i >= mark, 1, 0)
        return jnp.where(upper, i, st_n - 1 - i)

    def z_copy(phase, src, dst, peer):
        return remote(src, dst, zs.at[phase, peer], zr.at[phase, st], {"st": peer})

    def z_wait(phase, src, dst, peer):
        remote(src, dst, zs.at[phase, peer], zr.at[phase, peer], {"st": peer}).wait_recv()

    def ask_send(d, c):
        peer = (st + d) % st_n
        z_copy(0, ask_ref.at[peer], ask_in.at[st], peer).start()
        return c

    lax.fori_loop(1, st_n, ask_send, 0)
    ask_in[st] = ask_ref[st]

    m_tile = tile_of(pass_rows, 256)

    def project(t, first):
        def step(i, c):
            r = pl.ds(pl.multiple_of(i * m_tile, m_tile), m_tile)
            part = dot(rows[t, r], wkv[pl.ds(pl.multiple_of(t * chunk, chunk), chunk), :])
            acc[r] = part if first else acc[r] + part
            return c

        lax.fori_loop(0, pass_rows // m_tile, step, 0)

    def g_wait(t):
        remote(store_ref, rows.at[t], gs.at[1, hi], gr.at[t], mate).wait_recv()

    own_rows.wait()
    for copy in loads_kv:
        copy.wait()
    project(tp, True)
    g_wait(hi * 2 + 1 - lo)
    project(hi * 2 + 1 - lo, False)

    def ask_wait(d, c):
        peer = (st + d) % st_n
        z_wait(0, ask_ref.at[peer], ask_in.at[peer], peer)
        return c

    lax.fori_loop(1, st_n, ask_wait, 0)
    ask_copy = local(8, ask_in, ask_s)
    ask_copy.wait()

    hot_cols = depth * pass_len

    def hot_step(o, c):
        target = ask_in[o][0:1, :hot_cols]
        for i in range(pass_rows // m_tile):
            line = lax.broadcasted_iota(jnp.int32, (m_tile, hot_cols), 0) + i * m_tile
            hot[o, i * m_tile : (i + 1) * m_tile, :] = jnp.where(line == target, 1.0, 0.0).astype(BF)
        return c

    lax.fori_loop(0, st_n, hot_step, 0)
    onward = []
    for d in range(1, hi_n):
        h = (hi + d) % hi_n
        t = h * 2 + lo
        g_wait(t)
        onward.append(remote(rows.at[t], rows.at[t], gs.at[2, h], gr.at[t], mate))
        onward[-1].start()
        project(t, False)
    for d in range(1, hi_n):
        t = ((hi + d) % hi_n) * 2 + 1 - lo
        g_wait(t)
        project(t, False)

    def low_step(i, c):
        kv[i] = acc[pl.ds(pl.multiple_of(i * pass_len, pass_len), pass_len), :].astype(BF)
        return c

    lax.fori_loop(0, pass_rows // pass_len, low_step, 0)

    ks, vs_all = pl.ds(0, cols), pl.ds(cols, cols)

    def half(ref, peer, part):
        return ref.at[peer, :, :, part]

    def key_copy(peer):
        return z_copy(1, half(out, peer, ks), inc_k.at[st], peer)

    def value_copy(peer):
        return z_copy(4, half(out, peer, vs_all), inc_v.at[st], peer)

    def kv_send(d, c):
        peer = far_peer(d)
        for k in range(depth):
            out[peer, k] = kv[ask_s[peer, 1, k]]
        key_copy(peer).start()
        return c

    def value_send(d, c):
        value_copy(far_peer(d)).start()
        return c

    lax.fori_loop(1, st_n, kv_send, 0)
    lax.fori_loop(1, st_n, value_send, 0)
    for k in range(depth):
        picked = kv[ask_s[st, 1, k]]
        inc_k[st, k] = picked[:, :cols]
        inc_v[st, k] = picked[:, cols:]
    for copy in loads_q + loads_qg:
        copy.wait()

    def key_wait(d, c):
        peer = (st + d) % st_n
        z_wait(1, half(out, peer, ks), inc_k.at[peer], peer)
        return c

    lax.fori_loop(1, st_n, key_wait, 0)
    scale = HD ** (-0.5)

    def probs_step(b, c):
        r = pl.ds(pl.multiple_of(b * BLK, BLK), BLK)
        for j in range(PB):
            kvb[j * pass_len : (j + 1) * pass_len, :cols] = inc_k[
                slot_ref[0, b * PB + j], slot_ref[1, b * PB + j]
            ]
        for head in range(heads):
            hs = slice(head * HD, (head + 1) * HD)
            vs = slice(cols + head * HD, cols + (head + 1) * HD)
            gate = g_v[r, hs].astype(F32)
            scores = dot(q_v[r, hs], kvb[:, hs], NT) * scale
            shifted = jnp.exp(scores - jnp.max(scores, axis=-1, keepdims=True))
            prob = shifted / jnp.sum(shifted, axis=-1, keepdims=True)
            prob_v[head, r, :] = prob
            sig = 1.0 / (1.0 + jnp.exp(-gate))
            att_grad = (gate * sig * m_v[r, hs].astype(F32)).astype(BF)
            value_grad = dot(prob.astype(BF), att_grad, TN).astype(BF)
            for j in range(PB):
                reqg[b * PB + j, :, vs] = value_grad[j * pass_len : (j + 1) * pass_len]
        return c

    lax.fori_loop(0, blocks, probs_step, 0)

    def back_copy(phase, part, peer):
        return z_copy(phase, half(ret, peer, part), half(arr, st, part), peer)

    def give_back(phase, part, span):
        def send(d, c):
            peer = far_peer(d)
            for k in range(depth):
                ret[peer, k, :, span] = reqg[req_ref[peer, k]][:, span]
            back_copy(phase, part, peer).start()
            return c

        lax.fori_loop(1, st_n, send, 0)
        for k in range(depth):
            arr[st, k, :, span] = reqg[req_ref[st, k]][:, span]

    give_back(2, vs_all, slice(cols, 2 * cols))

    def value_wait(d, c):
        peer = (st + d) % st_n
        z_wait(4, half(out, peer, vs_all), inc_v.at[peer], peer)
        return c

    lax.fori_loop(1, st_n, value_wait, 0)

    def block_step(b, c):
        r = pl.ds(pl.multiple_of(b * BLK, BLK), BLK)
        for j in range(PB):
            o, k = slot_ref[0, b * PB + j], slot_ref[1, b * PB + j]
            kvb[j * pass_len : (j + 1) * pass_len, :cols] = inc_k[o, k]
            kvb[j * pass_len : (j + 1) * pass_len, cols:] = inc_v[o, k]
        for head in range(heads):
            hs = slice(head * HD, (head + 1) * HD)
            vs = slice(cols + head * HD, cols + (head + 1) * HD)
            q = q_v[r, hs]
            key = kvb[:, hs]
            value = kvb[:, vs]
            gate = g_v[r, hs].astype(F32)
            grad = m_v[r, hs].astype(F32)
            prob = prob_v[head, r, :]
            attended = dot(prob.astype(BF), value)
            sig = 1.0 / (1.0 + jnp.exp(-gate))
            att_grad = (gate * sig * grad).astype(BF)
            gboth[r, vs] = (grad * attended * sig * (1.0 + gate * (1.0 - sig))).astype(BF)
            prob_grad = dot(att_grad, value, NT)
            inner = jnp.sum(prob * prob_grad, axis=-1, keepdims=True)
            score_grad = (scale * prob * (prob_grad - inner)).astype(BF)
            gboth[r, hs] = dot(score_grad, key).astype(BF)
            key_grad = dot(score_grad, q, TN).astype(BF)
            for j in range(PB):
                reqg[b * PB + j, :, hs] = key_grad[j * pass_len : (j + 1) * pass_len]
        return c

    lax.fori_loop(0, blocks, block_step, 0)
    give_back(5, ks, slice(0, cols))

    n_tile = tile_of(model, 512)

    def expand(src, weight, part, pair_rows, t):
        base = pl.multiple_of(t * pair_rows, pair_rows)
        a = src[pl.ds(base, pair_rows), :]

        def step(i, c):
            n = pl.ds(pl.multiple_of(i * n_tile, n_tile), n_tile)
            part[t, :, n] = dot(a, weight[n, :], NT).astype(BF)
            return c

        lax.fori_loop(0, model // n_tile, step, 0)

    def pair_copy(which, part, pair, h):
        return remote(part.at[h * 2 + 1 - lo], pair.at[h], ps.at[which, h], pr.at[which, h], mate)

    def scatter_first(which, src, weight, part, pair, pair_rows):
        for d in range(1, hi_n + 1):
            h = (hi + d) % hi_n
            expand(src, weight, part, pair_rows, h * 2 + 1 - lo)
            pair_copy(which, part, pair, h).start()

    def cross(which, send, recv, h):
        return remote(
            send.at[h * 2 + lo], recv.at[hi], xs.at[which, h], xr.at[which, hi], {"tp": h * 2 + lo}
        )

    def scatter_second(which, src, weight, part, pair, send, recv, pair_rows):
        for d in range(1, hi_n + 1):
            h = (hi + d) % hi_n
            expand(src, weight, part, pair_rows, h * 2 + lo)
            pair_copy(which, part, pair, h).wait_recv()
            if d < hi_n:
                part[h * 2 + lo] = (part[h * 2 + lo].astype(F32) + pair[h].astype(F32)).astype(BF)
                cross(which, part, recv, h).start()

    def scatter_last(which, part, pair, send, recv, result):
        for d in range(1, hi_n):
            h = (hi + d) % hi_n
            remote(
                send.at[h * 2 + lo], recv.at[h], xs.at[which, h], xr.at[which, h], {"tp": h * 2 + lo}
            ).wait_recv()
        total = part[tp].astype(F32) + pair[hi].astype(F32)
        for d in range(1, hi_n):
            total = total + recv[(hi + d) % hi_n].astype(F32)
        result[...] = total.astype(BF)

    tok_pair = tok_rows // tp_n
    sto_pair = pass_rows // tp_n
    scatter_first(0, gboth, wqg, tp_part, tp_pair, tok_pair)
    scatter_second(0, gboth, wqg, tp_part, tp_pair, tp_part, tp_recv, tok_pair)

    def gather_sums(o, span, first):
        def step(i, c):
            r = pl.ds(pl.multiple_of(i * m_tile, m_tile), m_tile)
            part = dot(hot[o, r, :], arr[o, :, :, span].reshape(hot_cols, cols))
            acc[r, span] = part if first else acc[r, span] + part
            return c

        lax.fori_loop(0, pass_rows // m_tile, step, 0)

    for phase, part, span in ((2, vs_all, slice(cols, 2 * cols)), (5, ks, slice(0, cols))):
        gather_sums(st, span, True)

        def grad_wait(d, c):
            peer = (st + d) % st_n
            z_wait(phase, half(ret, peer, part), half(arr, peer, part), peer)
            gather_sums(peer, span, False)
            return c

        lax.fori_loop(1, st_n, grad_wait, 0)
        plow[:, span] = acc[:, span].astype(BF)

    scatter_first(1, plow, wkv, sp_part, sp_pair, sto_pair)

    def wkey_step(t, c):
        dwp[pl.ds(pl.multiple_of(t * chunk, chunk), chunk), :] = dot(
            rows[t], plow[:, :cols], TN
        ).astype(BF)
        return c

    lax.fori_loop(0, tp_n, wkey_step, 0)
    share = model // st_n

    def part_of(s):
        return dwp.at[pl.ds(pl.multiple_of(s * share, share), share), :]

    def wkey_send(d, c):
        peer = far_peer(d)
        z_copy(3, part_of(peer), dwr.at[st], peer).start()
        return c

    lax.fori_loop(1, st_n, wkey_send, 0)
    scatter_second(1, plow, wkv, sp_part, sp_pair, sp_part, sp_recv, sto_pair)
    scatter_last(0, tp_part, tp_pair, tp_part, tp_recv, tok_out)
    wkey_out[...] = part_of(st)[...].astype(F32)

    def wkey_wait(d, c):
        peer = (st + d) % st_n
        z_wait(3, part_of(peer), dwr.at[peer], peer)
        wkey_out[...] += dwr[peer].astype(F32)
        return c

    lax.fori_loop(1, st_n, wkey_wait, 0)
    scatter_last(1, sp_part, sp_pair, sp_part, sp_recv, store_out)

    for copy in across + [beside] + onward:
        copy.wait_send()

    def drain(d, c):
        peer = (st + d) % st_n
        z_copy(0, ask_ref.at[peer], ask_in.at[st], peer).wait_send()
        key_copy(peer).wait_send()
        value_copy(peer).wait_send()
        back_copy(2, vs_all, peer).wait_send()
        back_copy(5, ks, peer).wait_send()
        z_copy(3, part_of(peer), dwr.at[st], peer).wait_send()
        return c

    lax.fori_loop(1, st_n, drain, 0)
    for d in range(1, hi_n + 1):
        h = (hi + d) % hi_n
        pair_copy(0, tp_part, tp_pair, h).wait_send()
        pair_copy(1, sp_part, sp_pair, h).wait_send()
        if d < hi_n:
            cross(0, tp_part, tp_recv, h).wait_send()
            cross(1, sp_part, sp_recv, h).wait_send()


def gathered_kernel(
    st_n, tp_n, depth, pass_len,
    ids_hbm, store_ref, q_hbm, g_hbm, wq_hbm, wg_hbm, wk_hbm, wv_hbm, m_hbm,
    tok_hbm, store_hbm, wkey_hbm,
    ids_ref, tok_out, store_out, wkey_out, rows, wall, wqg, q_v, g_v, m_v, acc, terms, k_all, v_all, ask_v, ask_in, order_v, req_ref, gated, slope, ret, prob_v, kvb, reqg, gboth, arr,
    hot, plow, sums, dwp, dwc, dwf, tp_part, tp_pair, tp_recv,
    lsem, gs, gr, fs, fr, fw, zs, zr, ps, pr, xs, xr, ws, wr, ss, sr, us, ur,
):
    grp = lax.axis_index("grp")
    st = lax.axis_index("st")
    tp = lax.axis_index("tp")
    hi_n = tp_n // 2
    hi, lo = tp // 2, tp % 2
    mate_t = hi * 2 + 1 - lo
    mate = {"tp": mate_t}
    twin = {"grp": 1 - grp}
    pass_rows, chunk = rows.shape[1], rows.shape[2]
    passages = pass_rows // pass_len
    model = wqg.shape[0]
    cols = q_v.shape[1]
    heads = cols // HD
    tok_rows = q_v.shape[0]
    blocks = tok_rows // BLK
    half_pass = passages // 2
    some = tile_of(half_pass, 2)
    some_rows = some * pass_len
    n_some = half_pass // some
    key_cols, value_cols = slice(0, cols), slice(cols, 2 * cols)

    def local(i, src, dst):
        copy = pltpu.make_async_copy(src, dst, lsem.at[i])
        copy.start()
        return copy

    def sent(ref, sem):
        remote(ref, ref, sem, pr.at[0], mate).wait_send()

    def landed(ref, sem):
        remote(ref, ref, ps.at[0], sem, mate).wait_recv()

    ids_copy = local(7, ids_hbm, ids_ref)
    own_rows = local(0, store_ref, rows.at[tp])
    local(1, wk_hbm, wall.at[tp, :, pl.ds(0, cols)])
    local(1, wv_hbm, wall.at[tp, :, pl.ds(cols, cols)])
    loads_q = [local(2, q_hbm, q_v), local(3, g_hbm, g_v), local(4, m_hbm, m_v)]
    local(5, wq_hbm, wqg.at[:, pl.ds(0, cols)])
    local(5, wg_hbm, wqg.at[:, pl.ds(cols, cols)])

    barrier = pltpu.get_barrier_semaphore()

    def greet_st(d, c):
        pl.semaphore_signal(
            barrier, inc=1, device_id={"st": (st + d) % st_n}, device_id_type=MESH
        )
        return c

    lax.fori_loop(1, st_n, greet_st, 0)
    for d in range(1, tp_n):
        pl.semaphore_signal(
            barrier, inc=1, device_id={"tp": (tp + d) % tp_n}, device_id_type=MESH
        )
    pl.semaphore_signal(barrier, inc=1, device_id=twin, device_id_type=MESH)

    ids_copy.wait()

    def plan(wide):
        line = lax.broadcasted_iota(jnp.int32, (8, wide), 0)
        return line, lax.broadcasted_iota(jnp.int32, (8, wide), 1)

    width = ask_v.shape[2]
    line, lane = plan(width)
    slot, place = lane // pass_len, lane % pass_len
    short_line, short_lane = plan(order_v.shape[1])
    target = jnp.full((8, width), -1, jnp.int32)
    order = jnp.zeros(order_v.shape, jnp.int32)
    taken = [jnp.int32(0)] * st_n
    for j in range(PB):
        for n in range(blocks):
            i = ids_ref[j, n]
            owner = lax.div(i, jnp.int32(passages))
            within = i - owner * passages
            rank = sum(jnp.where(owner == o, taken[o], 0) for o in range(st_n))
            taken = [taken[o] + jnp.where(owner == o, 1, 0) for o in range(st_n)]
            target = jnp.where(
                (line == owner) & (slot == rank), within * pass_len + place, target
            )
            order = jnp.where(
                (short_line == owner) & (short_lane == rank), j * blocks + n, order
            )
    order_v[...] = order
    for o in range(st_n):
        ask_v[o] = jnp.broadcast_to(target[o : o + 1], (8, width))
    pl.semaphore_wait(barrier, st_n + tp_n - 1)

    def first_row(i):
        part = (grp + i // n_some) % 2
        return pl.multiple_of((part * n_some + i % n_some) * some_rows, some_rows)

    n_part = tile_of(n_some, 2)

    def g_copy(way, lot, t, onto):
        i, count, slot = lot
        r = pl.ds(first_row(i), count * some_rows)
        away = (t - onto + tp_n) % tp_n - 1
        return remote(rows.at[t, r], rows.at[t, r], gs.at[way], gr.at[away, slot], {"tp": onto})

    def small(i):
        return i, 1, i

    def large(i):
        return n_some + i * n_part, n_part, n_some + i

    def onward(d, lot):
        return g_copy(2, lot, ((hi + d) % hi_n) * 2 + lo, mate_t)

    def g_wait(t, lot):
        g_copy(1, lot, t, tp).wait_recv()

    def rows_send(lot):
        for d in range(1, hi_n):
            g_copy(0, lot, tp, ((hi + d) % hi_n) * 2 + lo).start()
        g_copy(1, lot, tp, mate_t).start()

    def rows_small(i, c):
        rows_send(small(i))
        return c

    def rows_large(i, c):
        rows_send(large(i))
        return c

    own_rows.wait()
    lax.fori_loop(0, n_some, rows_small, 0)
    lax.fori_loop(0, n_some // n_part, rows_large, 0)

    upper = st >= st_n // 2
    mark = jnp.where(upper, st, st_n - 1 - st)

    def far_peer(d):
        i = d - 1
        i = i + jnp.where(i >= mark, 1, 0)
        return jnp.where(upper, i, st_n - 1 - i)

    def z_copy(phase, src, dst, peer):
        away = (st - peer + st_n) % st_n - 1
        return remote(src, dst, zs.at[phase], zr.at[phase, away], {"st": peer})

    def z_wait(phase, src, dst, peer):
        landed(dst, zr.at[phase, (peer - st + st_n) % st_n - 1])

    def ask_send(d, c):
        peer = (st + d) % st_n
        z_copy(0, ask_v.at[peer], ask_in.at[st], peer).start()
        return c

    lax.fori_loop(1, st_n, ask_send, 0)
    ask_in[st] = ask_v[st]
    order_copy = local(6, order_v, req_ref)

    def project(lot, send):
        i, count, _ = lot
        r = pl.ds(first_row(i), count * some_rows)

        def term(t, span):
            return dot(rows[t, r], wall[tp, pl.ds(pl.multiple_of(t * chunk, chunk), chunk), span])

        for d in range(1, hi_n):
            g_wait(((hi + d) % hi_n) * 2 + lo, lot)
            onward(d, lot).start()
        g_wait(mate_t, lot)
        near = [tp, mate_t] + [((hi + d) % hi_n) * 2 + lo for d in range(1, hi_n)]
        late = [((hi + d) % hi_n) * 2 + 1 - lo for d in range(1, hi_n)]
        total = sum(term(t, key_cols) for t in near[1:]) + term(near[0], key_cols)
        for t in late:
            g_wait(t, lot)
            total = total + term(t, key_cols)
        first = st * passages + first_row(i) // pass_len

        def keep(ref, total):
            low = total.astype(BF)
            for p in range(count * some):
                ref[first + p] = low[p * pass_len : (p + 1) * pass_len]

        keep(k_all, total)
        send()
        keep(v_all, sum(term(t, value_cols) for t in near + late))

    def part_of_all(kind, o, c, side):
        ref = k_all if kind == 0 else v_all
        return ref.at[pl.ds(o * passages + side * half_pass + c * some, some)]

    def chain_copy(kind, o, c, peer):
        part = part_of_all(kind, o, c, grp)
        away = (o - peer + st_n) % st_n - 1
        return remote(part, part, fs.at[kind, 0], fr.at[kind, away, c], {"st": peer})

    def twin_copy(kind, o, c):
        part = part_of_all(kind, o, c, grp)
        return remote(part, part, fs.at[kind, 1], fw.at[kind], twin)

    lower = st < st_n // 2
    edge = (st == 0) | (st == st_n - 1)

    def own_send(kind, c, inward=True, outward=True):
        for onto, toward in ((st + 1, lower), (st - 1, jnp.logical_not(lower))):
            there = (onto >= 0) & (onto < st_n)
            if not outward:
                there = there & toward
            if not inward:
                there = there & jnp.logical_not(toward)

            @pl.when(there)
            def _():
                chain_copy(kind, st, c, onto).start()

    def relay(kind, d, c):
        for sign in (-1, 1):
            o = st + sign * d
            onto = st - sign

            @pl.when((o >= 0) & (o < st_n))
            def _():
                chain_copy(kind, o, c, st).wait_recv()

                @pl.when((onto >= 0) & (onto < st_n))
                def _():
                    chain_copy(kind, o, c, onto).start()

                twin_copy(kind, o, c).start()

    relayed = (st_n - 1) * half_pass

    def twin_wait(kind):
        landed((k_all, v_all)[kind].at[pl.ds(0, relayed)], fw.at[kind])

    landed(wall.at[tp], lsem.at[1])
    for copy in loads_q:
        copy.wait()

    gate_rows = tok_rows // n_some

    def gates(i):
        r = pl.ds(pl.multiple_of(i * gate_rows, gate_rows), gate_rows)
        gate = g_v[r, :].astype(F32)
        grad = m_v[r, :].astype(F32)
        sig = 1.0 / (1.0 + jnp.exp(-gate))
        gated[r, :] = (gate * sig * grad).astype(BF)
        slope[r, :] = grad * (sig * (1.0 + gate * (1.0 - sig)))

    def early_step(i, c):
        project(small(i), lambda: own_send(0, i))

        for d in range(1, st_n):
            @pl.when(i >= d)
            def _():
                relay(0, d, i - d)

        @pl.when(edge | (i == 0))
        def _():
            own_send(1, i)

        gates(i)
        return c

    lax.fori_loop(0, n_some, early_step, 0)
    for i in range(n_some - 1, n_some):
        relay(0, 1, i)

    def inward_send(i, c):
        own_send(1, i, outward=False)
        return c

    lax.fori_loop(jnp.where(edge, n_some, 1), n_some, inward_send, 0)

    def second_step(i, c):
        relay(0, 2, i)
        return c

    def outward_send(i, c):
        own_send(1, i, inward=False)
        return c

    lax.fori_loop(n_some - 2, n_some, second_step, 0)
    @pl.when(edge)
    def _():
        relay(1, 1, 0)

    lax.fori_loop(jnp.where(edge, n_some, 1), n_some, outward_send, 0)

    def late_step(i, c):
        project(large(i), lambda: None)
        for q in range(n_part):
            @pl.when(jnp.logical_not(edge))
            def _():
                relay(1, 1, i * n_part + q)

        return c

    w_part = model // 2
    w_mine = pl.ds(pl.multiple_of(grp * w_part, w_part), w_part)
    w_other = pl.ds(pl.multiple_of((1 - grp) * w_part, w_part), w_part)

    def w_across(d):
        h = (hi + d) % hi_n
        part = wall.at[tp, w_mine]
        return remote(part, part, ws.at[0], wr.at[0], {"tp": h * 2 + lo})

    def w_twin(d):
        t = ((hi + d) % hi_n) * 2 + lo
        part = wall.at[t, w_mine]
        return remote(part, part, ws.at[0], wr.at[1], twin)

    def w_onward(d, k):
        t = ((hi + d) % hi_n) * 2 + lo
        part = wall.at[t, w_other if k else w_mine]
        return remote(part, part, ws.at[0], wr.at[2], mate)

    w_beside = remote(wall.at[tp], wall.at[tp], ws.at[0], wr.at[2], mate)

    def w_wait(kind, t, part):
        landed(wall.at[t, part], wr.at[kind])

    for d in range(1, hi_n):
        w_across(d).start()

    def relay_rest(kind, first, last):
        def step(i, c):
            relay(kind, 1 + i // n_some, i % n_some)
            return c

        lax.fori_loop(first, last, step, 0)

    relays = (st_n - 1) * n_some
    relay_rest(0, 3 * n_some - 3, jnp.where(edge, 3 * n_some, 0))
    lax.fori_loop(0, n_some // n_part, late_step, 0)
    w_beside.start()
    relay_rest(1, 1, jnp.where(edge, n_some, 1))
    landed(wqg, lsem.at[5])
    order_copy.wait()
    twin_wait(0)
    scale = HD ** (-0.5)

    def fill(n, ref, span, b):
        for j in range(PB):
            kvb[n, j * pass_len : (j + 1) * pass_len, span] = ref[ids_ref[j, b]]

    pairs = range(4)

    def block_rows(b):
        return pl.ds(pl.multiple_of(b * BLK, BLK), BLK)

    per_step = n_some // (blocks // 4)

    def probs_step(i, c):
        for n in pairs:
            fill(n, k_all, key_cols, 4 * i + n)
        for head in range(heads):
            hs = slice(head * HD, (head + 1) * HD)
            vs = slice(cols + head * HD, cols + (head + 1) * HD)
            for n in pairs:
                b = 4 * i + n
                r = block_rows(b)
                scores = dot(q_v[r, hs], kvb[n, :, hs], NT) * scale
                shifted = jnp.exp(scores - jnp.max(scores, axis=-1, keepdims=True))
                prob = shifted * (1.0 / jnp.sum(shifted, axis=-1, keepdims=True))
                prob_v[head, r, :] = prob
                value_grad = dot(prob.astype(BF), gated[r, hs], TN).astype(BF)
                for j in range(PB):
                    reqg[j * blocks + b, :, vs] = value_grad[j * pass_len : (j + 1) * pass_len]

        for q in range(per_step):
            relay(1, 2, i * per_step + q)

        return c

    lax.fori_loop(0, blocks // 4, probs_step, 0)

    def half(ref, peer, part):
        return ref.at[peer, :, :, part]

    def back_copy(phase, part, peer):
        return z_copy(phase, half(ret, peer, part), half(arr, st, part), peer)

    def give_back(phase, part, span, order, first, last):
        def send(d, c):
            peer = order(d)
            for k in range(depth):
                ret[peer, k, :, span] = reqg[req_ref[peer, k]][:, span]
            back_copy(phase, part, peer).start()
            return c

        lax.fori_loop(first, last, send, 0)

    def keep_own(span):
        for k in range(depth):
            arr[st, k, :, span] = reqg[req_ref[st, k]][:, span]

    def near_peer(d):
        return far_peer(st_n - d)

    ks, vs_all = pl.ds(0, cols), pl.ds(cols, cols)
    def value_peer(d):
        return jnp.where(edge, near_peer(d % (st_n - 1) + 1), near_peer(d))

    give_back(
        1, vs_all, value_cols, value_peer, 1, jnp.where(edge, st_n, st_n - 1)
    )
    keep_own(value_cols)
    relay_rest(1, n_some + per_step * (blocks // 4), relays)
    twin_wait(1)

    def block_step(i, c):
        for n in pairs:
            fill(n, k_all, key_cols, 4 * i + n)
            fill(n, v_all, value_cols, 4 * i + n)
        for head in range(heads):
            hs = slice(head * HD, (head + 1) * HD)
            vs = slice(cols + head * HD, cols + (head + 1) * HD)
            for n in pairs:
                b = 4 * i + n
                r = block_rows(b)
                value = kvb[n, :, vs]
                prob = prob_v[head, r, :]
                prob_grad = dot(gated[r, hs], value, NT)
                inner = jnp.sum(prob * prob_grad, axis=-1, keepdims=True)
                score_grad = (scale * prob * (prob_grad - inner)).astype(BF)
                key_grad = dot(score_grad, q_v[r, hs], TN).astype(BF)
                for j in range(PB):
                    reqg[j * blocks + b, :, hs] = key_grad[j * pass_len : (j + 1) * pass_len]
                gboth[r, hs] = dot(score_grad, kvb[n, :, hs]).astype(BF)
                attended = dot(prob.astype(BF), value)
                gboth[r, vs] = (attended * slope[r, hs]).astype(BF)
        return c

    lax.fori_loop(0, blocks // 4, block_step, 0)
    def key_peer(d):
        return jnp.where(edge, near_peer(jnp.where(d == 1, 1, st_n + 1 - d)), far_peer(d))

    give_back(2, ks, key_cols, key_peer, 1, st_n)
    keep_own(key_cols)

    @pl.when(jnp.logical_not(edge))
    def _():
        give_back(1, vs_all, value_cols, near_peer, st_n - 1, st_n)

    n_tile = tile_of(model, 512)

    n_tiles = model // n_tile
    tok_pair = tok_rows // tp_n

    def tile(i):
        return pl.ds(pl.multiple_of(i * n_tile, n_tile), n_tile)

    def expand(h, i):
        a = gboth[pl.ds(pl.multiple_of(h * 2 * tok_pair, tok_pair), 2 * tok_pair), :]
        part = dot(a, wqg[tile(i), :], NT).astype(BF)
        tp_part[h * 2, :, tile(i)] = part[:tok_pair]
        tp_part[h * 2 + 1, :, tile(i)] = part[tok_pair:]

    def pair_copy(h, n, slot):
        src, dst = tp_part.at[h * 2 + 1 - lo, :, n], tp_pair.at[h, :, n]
        return remote(src, dst, ps.at[0], pr.at[slot], mate)

    def cross(h, n):
        src, dst = tp_part.at[h * 2 + lo, :, n], tp_recv.at[hi, :, n]
        return remote(src, dst, xs.at[0], xr.at[0], {"tp": h * 2 + lo})

    for d in range(1, hi_n):
        w_wait(0, ((hi + d) % hi_n) * 2 + lo, w_mine)
        w_twin(d).start()
        w_onward(d, 0).start()

    there = 1 - hi

    def far_tile(i, c):
        expand(there, i)
        pair_copy(there, tile(i), 1 + i).start()
        return c

    def cross_tile(i, c):
        n = tile(i)
        pair_copy(there, n, 1 + i).wait_recv()
        own = tp_part[there * 2 + lo, :, n].astype(F32)
        tp_part[there * 2 + lo, :, n] = (own + tp_pair[there, :, n].astype(F32)).astype(BF)
        cross(there, n).start()
        return c

    def own_tile(i, c):
        expand(hi, i)
        return c

    lax.fori_loop(0, n_tiles, far_tile, 0)
    lax.fori_loop(0, n_tiles, cross_tile, 0)
    lax.fori_loop(0, n_tiles, own_tile, 0)
    pair_copy(hi, pl.ds(0, model), 0).start()

    def ask_wait(d, c):
        peer = (st + d) % st_n
        z_wait(0, ask_v.at[peer], ask_in.at[peer], peer)
        return c

    lax.fori_loop(1, st_n, ask_wait, 0)
    hot_cols = depth * pass_len
    m_tile = tile_of(pass_rows, 256)
    s_tile = tile_of(pass_rows, 1024)

    def hot_step(o, c):
        target = ask_in[o][0:1, :hot_cols]
        for i in range(pass_rows // m_tile):
            line = lax.broadcasted_iota(jnp.int32, (m_tile, hot_cols), 0) + i * m_tile
            hot[o, i * m_tile : (i + 1) * m_tile, :] = jnp.where(line == target, 1.0, 0.0).astype(BF)
        return c

    lax.fori_loop(0, st_n, hot_step, 0)

    def gather_sums(kind, o, span, first=False, last=False):
        def step(i, c):
            r = pl.ds(pl.multiple_of(i * s_tile, s_tile), s_tile)
            part = dot(hot[o, r, :], arr[o, :, :, span].reshape(hot_cols, cols))
            part = part if first else acc[kind, r, :] + part
            if last:
                plow[r, span] = part.astype(BF)
            else:
                acc[kind, r, :] = part
            return c

        lax.fori_loop(0, pass_rows // s_tile, step, 0)

    sto_pair = pass_rows // tp_n

    far_tps = (there * 2, there * 2 + 1)

    def sums_copy(kind, part, t, far):
        src = plow.at[pl.ds(pl.multiple_of(t * sto_pair, sto_pair), sto_pair), part]
        return remote(src, sums.at[tp, :, part], ss.at[kind], sr.at[kind, far], {"tp": t})

    def sums_of(part, count):
        return sums.at[pl.ds(0, count), :, part]

    def grads_of(kind, peer, last=False):
        phase, part, span = (2, ks, key_cols) if kind == 0 else (1, vs_all, value_cols)
        z_wait(phase, half(ret, peer, part), half(arr, peer, part), peer)
        gather_sums(kind, peer, span, last=last)

    def sums_send(kind):
        part, span = (ks, key_cols) if kind == 0 else (vs_all, value_cols)
        for t in far_tps:
            sums_copy(kind, part, t, 1).start()
        sums_copy(kind, part, mate_t, 0).start()
        sums[tp, :, span] = plow[pl.ds(pl.multiple_of(tp * sto_pair, sto_pair), sto_pair), span]

    beyond = jnp.where(lower, st_n - 1, 0)
    middle = jnp.where(lower, st_n // 2, st_n // 2 - 1)
    beside_st = st + 1 - 2 * (st % 2)
    outer = edge
    inner = jnp.logical_not(outer)
    gather_sums(1, st, value_cols, first=True)
    gather_sums(0, st, key_cols, first=True)
    grads_of(1, beside_st)
    grads_of(1, jnp.where(outer, beyond, middle))

    grads_of(0, middle)

    grads_of(0, beyond)
    grads_of(0, beside_st, last=True)
    sums_send(0)

    share = model // st_n
    bits = 2
    bit = share // bits

    def dw_line(s, b):
        return pl.ds(pl.multiple_of(s * share + b * bit, bit), bit)

    def dw_copy(kind, b):
        line = pl.ds(b * bit, bit)
        if kind < 2:
            src, dst = dwp.at[dw_line(middle if kind else beyond, b)], dwc.at[kind, line]
            peer = beside_st
        elif kind == 2:
            src, dst, peer = dwp.at[dw_line(beside_st, b)], dwf.at[0, line], beside_st
        else:
            src, dst = dwc.at[kind - 3, line], dwf.at[1, line]
            peer = middle if kind == 4 else beyond
        return remote(src, dst, us.at[0], ur.at[min(kind, 3), b], {"st": peer})

    def dw_send(kind):
        for b in range(bits):
            dw_copy(kind, b).start()

    def dw_relay(q):
        for b in range(bits):
            line = slice(b * bit, (b + 1) * bit)
            dw_copy(q, b).wait_recv()
            own = dwp[dw_line(middle if q else beyond, b), :].astype(F32)
            dwc[q, line, :] = (dwc[q, line, :].astype(F32) + own).astype(BF)
            dw_copy(3 + q, b).start()

    def wkey_step(s):
        dwp[pl.ds(pl.multiple_of(s * chunk, chunk), chunk), :] = dot(
            rows[s], plow[:, key_cols], TN
        ).astype(BF)

    def wkey_turn(j, c):
        far = jnp.where(j == 0, beyond, middle)
        near = jnp.where(j == 2, beside_st, st)
        near_first = jnp.where(j == 0, beside_st, st)
        far_after = jnp.where(j == 1, beyond, middle)
        s = jnp.where(
            outer, jnp.where(j < 2, far, near), jnp.where((j == 0) | (j == 3), near_first, far_after)
        )
        wkey_step(s)
        for kind in range(3):
            @pl.when(outer & (j == kind))
            def _():
                dw_send(kind)

        @pl.when(inner & (j == 0))
        def _():
            dw_send(2)

        return c

    lax.fori_loop(0, st_n, wkey_turn, 0)

    @pl.when(inner)
    def _():
        dw_relay(0)

    for d in range(1, hi_n):
        t = ((hi + d) % hi_n) * 2 + lo
        w_wait(1, t, w_other)
        w_onward(d, 1).start()
    landed(wall.at[pl.ds(0, hi_n)], wr.at[2])

    def store_terms(sources, span, done):
        def step(i, c):
            n = tile(i)
            parts = [dot(sums[t, :, span], wall[t, n, span], NT) for t in sources]
            done(n, sum(parts[1:], parts[0]))
            return c

        lax.fori_loop(0, n_tiles, step, 0)

    def set_terms(n, part):
        terms[:, n] = part

    def add_terms(n, part):
        terms[:, n] += part

    def store_tile(n):
        return pltpu.make_async_copy(store_out.at[:, n], store_hbm.at[:, n], lsem.at[3])

    def keep_store(n, part):
        store_out[:, n] = (terms[:, n] + part).astype(BF)
        store_tile(n).start()

    grads_of(1, jnp.where(outer, middle, beyond), last=True)
    sums_send(1)

    landed(sums_of(ks, 1), sr.at[0, 0])
    landed(sums_of(ks, 2), sr.at[0, 1])
    store_terms((tp, mate_t) + far_tps, key_cols, set_terms)

    pair_copy(hi, pl.ds(0, model), 0).wait_recv()
    landed(tp_recv.at[there], xr.at[0])
    total = tp_part[tp].astype(F32) + tp_pair[hi].astype(F32) + tp_recv[there].astype(F32)
    tok_out[...] = total.astype(BF)
    tok_done = local(2, tok_out, tok_hbm)

    @pl.when(inner)
    def _():
        dw_relay(1)

    landed(sums_of(vs_all, 1), sr.at[1, 0])
    store_terms((tp, mate_t), value_cols, add_terms)
    landed(sums_of(vs_all, 2), sr.at[1, 1])
    store_terms(far_tps, value_cols, keep_store)

    for b in range(bits):
        line = slice(b * bit, (b + 1) * bit)
        dw_copy(2, b).wait_recv()
        wkey_out[line, :] = dwp[dw_line(st, b), :].astype(F32) + dwf[0, line, :].astype(F32)
    for b in range(bits):
        line = slice(b * bit, (b + 1) * bit)
        for kind, edge in ((3, outer), (4, inner)):
            @pl.when(edge)
            def _():
                dw_copy(kind, b).wait_recv()

        wkey_out[line, :] += dwf[1, line, :].astype(F32)

    wkey_done = local(4, wkey_out, wkey_hbm)

    for way in range(3):
        sent(rows.at[tp], gs.at[way])
    for kind, ref in ((0, k_all), (1, v_all)):
        sent(ref.at[pl.ds(0, relayed)], fs.at[kind, 1])
        for s in range(st_n):
            up, down = (s + 1) * (s + 1 < st_n), (st_n - s) * (s > 0)

            @pl.when(st == s)
            def _():
                sent(ref.at[pl.ds(0, (up + down) * half_pass)], fs.at[kind, 0])

    sent(wall.at[pl.ds(0, hi_n + 1)], ws.at[0])
    sent(ask_in.at[pl.ds(0, st_n - 1)], zs.at[0])
    sent(ret.at[pl.ds(0, st_n - 1), :, :, vs_all], zs.at[1])
    sent(ret.at[pl.ds(0, st_n - 1), :, :, ks], zs.at[2])
    sent(sums_of(ks, tp_n - 1), ss.at[0])
    sent(sums_of(vs_all, tp_n - 1), ss.at[1])
    sent(tp_pair, ps.at[0])
    sent(tp_recv.at[0], xs.at[0])
    sent(dwp.at[pl.ds(0, 3 * share)], us.at[0])
    for copy in (tok_done, store_tile(pl.ds(0, model)), wkey_done):
        copy.wait()


def settle_kernel(*refs):
    n = (len(refs) - 2) // 3
    sources, results, held = refs[:n], refs[n : 2 * n], refs[2 * n : 3 * n]
    ins, outs = refs[3 * n], refs[3 * n + 1]
    pieces = []
    for a, (source, result, here) in enumerate(zip(sources, results, held)):
        part = source.shape[0] // 2
        for i in range(2):
            r = pl.ds(i * part, part)
            pieces.append(
                (
                    pltpu.make_async_copy(source.at[r], here.at[r], ins.at[a, i]),
                    pltpu.make_async_copy(here.at[r], result.at[r], outs.at[a, i]),
                )
            )
    for fetch, _ in pieces:
        fetch.start()
    for fetch, put in pieces:
        fetch.wait()
        put.start()
    for _, put in pieces:
        put.wait()


def settle(*arrays):
    hbm = pl.BlockSpec(memory_space=pl.ANY)
    n = len(arrays)
    return pl.pallas_call(
        settle_kernel,
        out_shape=tuple(jax.ShapeDtypeStruct(a.shape, a.dtype) for a in arrays),
        in_specs=[hbm] * n,
        out_specs=(hbm,) * n,
        scratch_shapes=[pltpu.VMEM(a.shape, a.dtype) for a in arrays]
        + [pltpu.SemaphoreType.DMA((n, 2)), pltpu.SemaphoreType.DMA((n, 2))],
    )(*arrays)


def local(pass_ids, store, queries, gate_pre, w_query, w_gate, w_key, w_value, d_mem):
    st_n = lax.axis_size("st")
    tp_n = lax.axis_size("tp")
    hi_n = tp_n // 2
    tok_rows, cols = queries.shape
    blocks = tok_rows // BLK
    passages, pass_len, chunk = store.shape
    model = w_key.shape[0]
    requests = blocks * PB
    depth = max(2, requests // st_n)
    pass_rows = passages * pass_len
    share = model // st_n

    vmem = pl.BlockSpec(memory_space=pltpu.VMEM)
    smem = pl.BlockSpec(memory_space=pltpu.SMEM)
    hbm = pl.BlockSpec(memory_space=pl.ANY)
    V = pltpu.VMEM
    DMA = pltpu.SemaphoreType.DMA
    pair = 2 * cols
    tok_pair = tok_rows // tp_n
    sto_pair = pass_rows // tp_n
    hot_cols = depth * pass_len
    width = -(-hot_cols // 128) * 128
    gathered_bytes = 2 * 2 * st_n * pass_rows * cols
    steps = blocks // 4
    fits = lax.axis_size("grp") == 2 and hi_n == 2 and st_n == 4 and st_n == tp_n
    fits = fits and passages % 4 == 0 and blocks % 4 == 0 and passages // 4 % steps == 0
    if fits and gathered_bytes <= 8 << 20:
        half_pass = passages // 2
        n_some = half_pass // tile_of(half_pass, 2)
        d_tokens, d_store, d_wkey = pl.pallas_call(
            functools.partial(gathered_kernel, st_n, tp_n, depth, pass_len),
            out_shape=(
                jax.ShapeDtypeStruct((tok_pair, model), BF),
                jax.ShapeDtypeStruct((sto_pair, model), BF),
                jax.ShapeDtypeStruct((share, cols), F32),
            ),
            in_specs=[hbm] * 9,
            out_specs=(hbm, hbm, hbm),
            scratch_shapes=[
                pltpu.SMEM((PB, blocks), jnp.int32),
                V((tok_pair, model), BF),
                V((sto_pair, model), BF),
                V((share, cols), F32),
                V((tp_n, pass_rows, chunk), BF),
                V((tp_n, model, pair), BF),
                V((model, pair), BF),
                V((tok_rows, cols), BF),
                V((tok_rows, cols), BF),
                V((tok_rows, cols), BF),
                V((2, pass_rows, cols), F32),
                V((sto_pair, model), F32),
                V((st_n * passages, pass_len, cols), BF),
                V((st_n * passages, pass_len, cols), BF),
                V((st_n, 8, width), jnp.int32),
                V((st_n, 8, width), jnp.int32),
                V((8, 128), jnp.int32),
                pltpu.SMEM((8, 128), jnp.int32),
                V((tok_rows, cols), BF),
                V((tok_rows, cols), F32),
                V((st_n, depth, pass_len, pair), BF),
                V((cols // HD, tok_rows, PB * pass_len), F32),
                V((4, PB * pass_len, pair), BF),
                V((requests, pass_len, pair), BF),
                V((tok_rows, pair), BF),
                V((st_n, depth, pass_len, pair), BF),
                V((st_n, pass_rows, hot_cols), BF),
                V((pass_rows, pair), BF),
                V((tp_n, sto_pair, pair), BF),
                V((model, cols), BF),
                V((2, share, cols), BF),
                V((2, share, cols), BF),
                V((tp_n, tok_pair, model), BF),
                V((hi_n, tok_pair, model), BF),
                V((hi_n, tok_pair, model), BF),
                DMA((8,)),
                DMA((3,)),
                DMA((tp_n - 1, n_some + n_some // tile_of(n_some, 2))),
                DMA((2, 2)),
                DMA((2, st_n - 1, n_some)),
                DMA((2,)),
                DMA((3,)),
                DMA((3, st_n - 1)),
                DMA((1,)),
                DMA((1 + model // tile_of(model, 512),)),
                DMA((1,)),
                DMA((1,)),
                DMA((1,)),
                DMA((3,)),
                DMA((2,)),
                DMA((2, 2)),
                DMA((1,)),
                DMA((4, 2)),
            ],
            compiler_params=pltpu.CompilerParams(
                collective_id=0, has_side_effects=True, vmem_limit_bytes=67043328
            ),
        )(
            pass_ids.T, store.reshape(pass_rows, chunk),
            queries, gate_pre, w_query, w_gate, w_key, w_value, d_mem,
        )
        d_tokens, d_store, d_wkey = settle(d_tokens, d_store, d_wkey)
        return d_tokens, d_store.reshape(passages // tp_n, pass_len, model), d_wkey

    ids = pass_ids.reshape(-1)
    owners = ids // passages
    within = ids % passages
    order = jnp.arange(requests, dtype=jnp.int32)
    earlier = (owners[None, :] == owners[:, None]) & (order[None, :] < order[:, None])
    rank = jnp.sum(earlier.astype(jnp.int32), axis=1)
    slots = jnp.stack([owners, rank])
    o_i = jnp.arange(st_n, dtype=jnp.int32)[:, None, None]
    k_i = jnp.arange(depth, dtype=jnp.int32)[None, :, None]
    match = (owners[None, None, :] == o_i) & (rank[None, None, :] == k_i)
    asked = jnp.max(jnp.where(match, within[None, None, :], -1), axis=2)
    req_of = jnp.max(jnp.where(match, order[None, None, :], 0), axis=2)
    hot_cols = depth * pass_len
    width = -(-hot_cols // 128) * 128
    lane = jnp.arange(width, dtype=jnp.int32)
    spread = jnp.repeat(asked, pass_len, axis=1)
    spread = jnp.pad(spread, ((0, 0), (0, width - hot_cols)), constant_values=-1)
    target = jnp.where(spread < 0, -1, spread * pass_len + lane[None, :] % pass_len)
    flat = jnp.pad(jnp.maximum(asked, 0), ((0, 0), (0, width - depth)))
    ask = jnp.concatenate(
        [target[:, None], flat[:, None], jnp.zeros((st_n, 6, width), jnp.int32)], axis=1
    )

    d_tokens, d_store, d_wkey = pl.pallas_call(
        functools.partial(kernel, st_n, tp_n, depth, pass_len),
        out_shape=(
            jax.ShapeDtypeStruct((tok_pair, model), BF),
            jax.ShapeDtypeStruct((sto_pair, model), BF),
            jax.ShapeDtypeStruct((share, cols), F32),
        ),
        in_specs=[smem, smem, vmem] + [hbm] * 8,
        out_specs=(vmem, vmem, vmem),
        scratch_shapes=[
            V((tp_n, pass_rows, chunk), BF),
            V((model, pair), BF),
            V((model, pair), BF),
            V((tok_rows, cols), BF),
            V((tok_rows, cols), BF),
            V((tok_rows, cols), BF),
            V((pass_rows, pair), F32),
            V((passages, pass_len, pair), BF),
            V((st_n, 8, width), jnp.int32),
            pltpu.SMEM((st_n, 8, width), jnp.int32),
            V((st_n, depth, pass_len, pair), BF),
            V((st_n, depth, pass_len, cols), BF),
            V((st_n, depth, pass_len, cols), BF),
            V((st_n, depth, pass_len, pair), BF),
            V((cols // HD, tok_rows, PB * pass_len), F32),
            V((PB * pass_len, pair), BF),
            V((requests, pass_len, pair), BF),
            V((tok_rows, pair), BF),
            V((st_n, depth, pass_len, pair), BF),
            V((st_n, pass_rows, hot_cols), BF),
            V((pass_rows, pair), BF),
            V((model, cols), BF),
            V((st_n, share, cols), BF),
            V((tp_n, tok_pair, model), BF),
            V((hi_n, tok_pair, model), BF),
            V((hi_n, tok_pair, model), BF),
            V((tp_n, sto_pair, model), BF),
            V((hi_n, sto_pair, model), BF),
            V((hi_n, sto_pair, model), BF),
            DMA((9,)),
            DMA((3, hi_n)),
            DMA((tp_n,)),
            DMA((6, st_n)),
            DMA((6, st_n)),
            DMA((2, hi_n)),
            DMA((2, hi_n)),
            DMA((2, hi_n)),
            DMA((2, hi_n)),
        ],
        compiler_params=pltpu.CompilerParams(
            collective_id=0, has_side_effects=True, vmem_limit_bytes=67043328
        ),
    )(
        slots, req_of, ask, store.reshape(pass_rows, chunk),
        queries, gate_pre, w_query, w_gate, w_key, w_value, d_mem,
    )
    return d_tokens, d_store.reshape(passages // tp_n, pass_len, model), d_wkey


def solution(mesh):
    return jax.shard_map(
        local,
        mesh=mesh,
        in_specs=(
            P(("grp", "st"), None),
            P("st", None, "tp"),
            P(("grp", "st"), "tp"),
            P(("grp", "st"), "tp"),
            P(None, "tp"),
            P(None, "tp"),
            P(None, "tp"),
            P(None, "tp"),
            P(("grp", "st"), "tp"),
        ),
        out_specs=(
            P(("grp", "st", "tp"), None),
            P(("grp", "st", "tp"), None, None),
            P(("grp", "st"), "tp"),
        ),
        check_vma=False,
    )
```

```python
import functools

import jax
import jax.numpy as jnp
from jax import lax
from jax.experimental import pallas as pl
from jax.experimental.pallas import tpu as pltpu
from jax.sharding import PartitionSpec as P

HD = 256
BLK = 128
PB = 4
BF = jnp.bfloat16
F32 = jnp.float32
MESH = pl.DeviceIdType.MESH
NT = (((1,), (1,)), ((), ()))
TN = (((0,), (0,)), ((), ()))


def dot(a, b, dims=(((1,), (0,)), ((), ()))):
    return lax.dot_general(a, b, dims, preferred_element_type=F32)


def remote(src, dst, send, recv, device):
    return pltpu.make_async_remote_copy(
        src_ref=src,
        dst_ref=dst,
        send_sem=send,
        recv_sem=recv,
        device_id=device,
        device_id_type=MESH,
    )


def tile_of(size, most):
    while size % most:
        most //= 2
    return most


def kernel(
    st_n, tp_n, depth, pass_len,
    slot_ref, req_ref, ask_ref, store_ref, q_hbm, g_hbm, wq_hbm, wg_hbm, wk_hbm, wv_hbm, m_hbm,
    tok_out, store_out, wkey_out,
    rows, wkv, wqg, q_v, g_v, m_v, acc, kv, ask_in, ask_s, out, inc_k, inc_v, ret, prob_v, kvb, reqg, gboth, arr,
    hot, plow, dwp, dwr, tp_part, tp_pair, tp_recv, sp_part, sp_pair, sp_recv,
    lsem, gs, gr, zs, zr, ps, pr, xs, xr,
):
    st = lax.axis_index("st")
    tp = lax.axis_index("tp")
    hi_n = tp_n // 2
    hi, lo = tp // 2, tp % 2
    mate = {"tp": hi * 2 + 1 - lo}
    pass_rows, chunk = rows.shape[1], rows.shape[2]
    model = wqg.shape[0]
    cols = q_v.shape[1]
    heads = cols // HD
    tok_rows = q_v.shape[0]
    blocks = tok_rows // BLK
    blk_keys = PB * pass_len

    def local(i, src, dst):
        copy = pltpu.make_async_copy(src, dst, lsem.at[i])
        copy.start()
        return copy

    own_rows = local(0, store_ref, rows.at[tp])
    loads_kv = [
        local(1, wk_hbm, wkv.at[:, pl.ds(0, cols)]),
        local(2, wv_hbm, wkv.at[:, pl.ds(cols, cols)]),
    ]
    loads_q = [local(3, q_hbm, q_v), local(4, g_hbm, g_v), local(5, m_hbm, m_v)]
    loads_qg = [
        local(6, wq_hbm, wqg.at[:, pl.ds(0, cols)]),
        local(7, wg_hbm, wqg.at[:, pl.ds(cols, cols)]),
    ]

    barrier = pltpu.get_barrier_semaphore()

    def greet_st(d, c):
        pl.semaphore_signal(
            barrier, inc=1, device_id={"st": (st + d) % st_n}, device_id_type=MESH
        )
        return c

    lax.fori_loop(1, st_n, greet_st, 0)
    for d in range(1, tp_n):
        pl.semaphore_signal(
            barrier, inc=1, device_id={"tp": (tp + d) % tp_n}, device_id_type=MESH
        )
    pl.semaphore_wait(barrier, st_n - 1 + tp_n - 1)

    across = []
    for d in range(1, hi_n):
        h = (hi + d) % hi_n
        across.append(
            remote(store_ref, rows.at[tp], gs.at[0, h], gr.at[tp], {"tp": h * 2 + lo})
        )
        across[-1].start()
    beside = remote(store_ref, rows.at[tp], gs.at[1, hi], gr.at[tp], mate)
    beside.start()

    upper = st >= st_n // 2
    mark = jnp.where(upper, st, st_n - 1 - st)

    def far_peer(d):
        i = d - 1
        i = i + jnp.where(i >= mark, 1, 0)
        return jnp.where(upper, i, st_n - 1 - i)

    def z_copy(phase, src, dst, peer):
        return remote(src, dst, zs.at[phase, peer], zr.at[phase, st], {"st": peer})

    def z_wait(phase, src, dst, peer):
        remote(src, dst, zs.at[phase, peer], zr.at[phase, peer], {"st": peer}).wait_recv()

    def ask_send(d, c):
        peer = (st + d) % st_n
        z_copy(0, ask_ref.at[peer], ask_in.at[st], peer).start()
        return c

    lax.fori_loop(1, st_n, ask_send, 0)
    ask_in[st] = ask_ref[st]

    m_tile = tile_of(pass_rows, 256)

    def project(t, first):
        def step(i, c):
            r = pl.ds(pl.multiple_of(i * m_tile, m_tile), m_tile)
            part = dot(rows[t, r], wkv[pl.ds(pl.multiple_of(t * chunk, chunk), chunk), :])
            acc[r] = part if first else acc[r] + part
            return c

        lax.fori_loop(0, pass_rows // m_tile, step, 0)

    def g_wait(t):
        remote(store_ref, rows.at[t], gs.at[1, hi], gr.at[t], mate).wait_recv()

    own_rows.wait()
    for copy in loads_kv:
        copy.wait()
    project(tp, True)
    g_wait(hi * 2 + 1 - lo)
    project(hi * 2 + 1 - lo, False)

    def ask_wait(d, c):
        peer = (st + d) % st_n
        z_wait(0, ask_ref.at[peer], ask_in.at[peer], peer)
        return c

    lax.fori_loop(1, st_n, ask_wait, 0)
    ask_copy = local(8, ask_in, ask_s)
    ask_copy.wait()

    hot_cols = depth * pass_len

    def hot_step(o, c):
        target = ask_in[o][0:1, :hot_cols]
        for i in range(pass_rows // m_tile):
            line = lax.broadcasted_iota(jnp.int32, (m_tile, hot_cols), 0) + i * m_tile
            hot[o, i * m_tile : (i + 1) * m_tile, :] = jnp.where(line == target, 1.0, 0.0).astype(BF)
        return c

    lax.fori_loop(0, st_n, hot_step, 0)
    onward = []
    for d in range(1, hi_n):
        h = (hi + d) % hi_n
        t = h * 2 + lo
        g_wait(t)
        onward.append(remote(rows.at[t], rows.at[t], gs.at[2, h], gr.at[t], mate))
        onward[-1].start()
        project(t, False)
    for d in range(1, hi_n):
        t = ((hi + d) % hi_n) * 2 + 1 - lo
        g_wait(t)
        project(t, False)

    def low_step(i, c):
        kv[i] = acc[pl.ds(pl.multiple_of(i * pass_len, pass_len), pass_len), :].astype(BF)
        return c

    lax.fori_loop(0, pass_rows // pass_len, low_step, 0)

    ks, vs_all = pl.ds(0, cols), pl.ds(cols, cols)

    def half(ref, peer, part):
        return ref.at[peer, :, :, part]

    def key_copy(peer):
        return z_copy(1, half(out, peer, ks), inc_k.at[st], peer)

    def value_copy(peer):
        return z_copy(4, half(out, peer, vs_all), inc_v.at[st], peer)

    def kv_send(d, c):
        peer = far_peer(d)
        for k in range(depth):
            out[peer, k] = kv[ask_s[peer, 1, k]]
        key_copy(peer).start()
        return c

    def value_send(d, c):
        value_copy(far_peer(d)).start()
        return c

    lax.fori_loop(1, st_n, kv_send, 0)
    lax.fori_loop(1, st_n, value_send, 0)
    for k in range(depth):
        picked = kv[ask_s[st, 1, k]]
        inc_k[st, k] = picked[:, :cols]
        inc_v[st, k] = picked[:, cols:]
    for copy in loads_q + loads_qg:
        copy.wait()

    def key_wait(d, c):
        peer = (st + d) % st_n
        z_wait(1, half(out, peer, ks), inc_k.at[peer], peer)
        return c

    lax.fori_loop(1, st_n, key_wait, 0)
    scale = HD ** (-0.5)

    def probs_step(b, c):
        r = pl.ds(pl.multiple_of(b * BLK, BLK), BLK)
        for j in range(PB):
            kvb[j * pass_len : (j + 1) * pass_len, :cols] = inc_k[
                slot_ref[0, b * PB + j], slot_ref[1, b * PB + j]
            ]
        for head in range(heads):
            hs = slice(head * HD, (head + 1) * HD)
            vs = slice(cols + head * HD, cols + (head + 1) * HD)
            gate = g_v[r, hs].astype(F32)
            scores = dot(q_v[r, hs], kvb[:, hs], NT) * scale
            shifted = jnp.exp(scores - jnp.max(scores, axis=-1, keepdims=True))
            prob = shifted / jnp.sum(shifted, axis=-1, keepdims=True)
            prob_v[head, r, :] = prob
            sig = 1.0 / (1.0 + jnp.exp(-gate))
            att_grad = (gate * sig * m_v[r, hs].astype(F32)).astype(BF)
            value_grad = dot(prob.astype(BF), att_grad, TN).astype(BF)
            for j in range(PB):
                reqg[b * PB + j, :, vs] = value_grad[j * pass_len : (j + 1) * pass_len]
        return c

    lax.fori_loop(0, blocks, probs_step, 0)

    def back_copy(phase, part, peer):
        return z_copy(phase, half(ret, peer, part), half(arr, st, part), peer)

    def give_back(phase, part, span):
        def send(d, c):
            peer = far_peer(d)
            for k in range(depth):
                ret[peer, k, :, span] = reqg[req_ref[peer, k]][:, span]
            back_copy(phase, part, peer).start()
            return c

        lax.fori_loop(1, st_n, send, 0)
        for k in range(depth):
            arr[st, k, :, span] = reqg[req_ref[st, k]][:, span]

    give_back(2, vs_all, slice(cols, 2 * cols))

    def value_wait(d, c):
        peer = (st + d) % st_n
        z_wait(4, half(out, peer, vs_all), inc_v.at[peer], peer)
        return c

    lax.fori_loop(1, st_n, value_wait, 0)

    def block_step(b, c):
        r = pl.ds(pl.multiple_of(b * BLK, BLK), BLK)
        for j in range(PB):
            o, k = slot_ref[0, b * PB + j], slot_ref[1, b * PB + j]
            kvb[j * pass_len : (j + 1) * pass_len, :cols] = inc_k[o, k]
            kvb[j * pass_len : (j + 1) * pass_len, cols:] = inc_v[o, k]
        for head in range(heads):
            hs = slice(head * HD, (head + 1) * HD)
            vs = slice(cols + head * HD, cols + (head + 1) * HD)
            q = q_v[r, hs]
            key = kvb[:, hs]
            value = kvb[:, vs]
            gate = g_v[r, hs].astype(F32)
            grad = m_v[r, hs].astype(F32)
            prob = prob_v[head, r, :]
            attended = dot(prob.astype(BF), value)
            sig = 1.0 / (1.0 + jnp.exp(-gate))
            att_grad = (gate * sig * grad).astype(BF)
            gboth[r, vs] = (grad * attended * sig * (1.0 + gate * (1.0 - sig))).astype(BF)
            prob_grad = dot(att_grad, value, NT)
            inner = jnp.sum(prob * prob_grad, axis=-1, keepdims=True)
            score_grad = (scale * prob * (prob_grad - inner)).astype(BF)
            gboth[r, hs] = dot(score_grad, key).astype(BF)
            key_grad = dot(score_grad, q, TN).astype(BF)
            for j in range(PB):
                reqg[b * PB + j, :, hs] = key_grad[j * pass_len : (j + 1) * pass_len]
        return c

    lax.fori_loop(0, blocks, block_step, 0)
    give_back(5, ks, slice(0, cols))

    n_tile = tile_of(model, 512)

    def expand(src, weight, part, pair_rows, t):
        base = pl.multiple_of(t * pair_rows, pair_rows)
        a = src[pl.ds(base, pair_rows), :]

        def step(i, c):
            n = pl.ds(pl.multiple_of(i * n_tile, n_tile), n_tile)
            part[t, :, n] = dot(a, weight[n, :], NT).astype(BF)
            return c

        lax.fori_loop(0, model // n_tile, step, 0)

    def pair_copy(which, part, pair, h):
        return remote(part.at[h * 2 + 1 - lo], pair.at[h], ps.at[which, h], pr.at[which, h], mate)

    def scatter_first(which, src, weight, part, pair, pair_rows):
        for d in range(1, hi_n + 1):
            h = (hi + d) % hi_n
            expand(src, weight, part, pair_rows, h * 2 + 1 - lo)
            pair_copy(which, part, pair, h).start()

    def cross(which, send, recv, h):
        return remote(
            send.at[h * 2 + lo], recv.at[hi], xs.at[which, h], xr.at[which, hi], {"tp": h * 2 + lo}
        )

    def scatter_second(which, src, weight, part, pair, send, recv, pair_rows):
        for d in range(1, hi_n + 1):
            h = (hi + d) % hi_n
            expand(src, weight, part, pair_rows, h * 2 + lo)
            pair_copy(which, part, pair, h).wait_recv()
            if d < hi_n:
                part[h * 2 + lo] = (part[h * 2 + lo].astype(F32) + pair[h].astype(F32)).astype(BF)
                cross(which, part, recv, h).start()

    def scatter_last(which, part, pair, send, recv, result):
        for d in range(1, hi_n):
            h = (hi + d) % hi_n
            remote(
                send.at[h * 2 + lo], recv.at[h], xs.at[which, h], xr.at[which, h], {"tp": h * 2 + lo}
            ).wait_recv()
        total = part[tp].astype(F32) + pair[hi].astype(F32)
        for d in range(1, hi_n):
            total = total + recv[(hi + d) % hi_n].astype(F32)
        result[...] = total.astype(BF)

    tok_pair = tok_rows // tp_n
    sto_pair = pass_rows // tp_n
    scatter_first(0, gboth, wqg, tp_part, tp_pair, tok_pair)
    scatter_second(0, gboth, wqg, tp_part, tp_pair, tp_part, tp_recv, tok_pair)

    def gather_sums(o, span, first):
        def step(i, c):
            r = pl.ds(pl.multiple_of(i * m_tile, m_tile), m_tile)
            part = dot(hot[o, r, :], arr[o, :, :, span].reshape(hot_cols, cols))
            acc[r, span] = part if first else acc[r, span] + part
            return c

        lax.fori_loop(0, pass_rows // m_tile, step, 0)

    for phase, part, span in ((2, vs_all, slice(cols, 2 * cols)), (5, ks, slice(0, cols))):
        gather_sums(st, span, True)

        def grad_wait(d, c):
            peer = (st + d) % st_n
            z_wait(phase, half(ret, peer, part), half(arr, peer, part), peer)
            gather_sums(peer, span, False)
            return c

        lax.fori_loop(1, st_n, grad_wait, 0)
        plow[:, span] = acc[:, span].astype(BF)

    scatter_first(1, plow, wkv, sp_part, sp_pair, sto_pair)

    def wkey_step(t, c):
        dwp[pl.ds(pl.multiple_of(t * chunk, chunk), chunk), :] = dot(
            rows[t], plow[:, :cols], TN
        ).astype(BF)
        return c

    lax.fori_loop(0, tp_n, wkey_step, 0)
    share = model // st_n

    def part_of(s):
        return dwp.at[pl.ds(pl.multiple_of(s * share, share), share), :]

    def wkey_send(d, c):
        peer = far_peer(d)
        z_copy(3, part_of(peer), dwr.at[st], peer).start()
        return c

    lax.fori_loop(1, st_n, wkey_send, 0)
    scatter_second(1, plow, wkv, sp_part, sp_pair, sp_part, sp_recv, sto_pair)
    scatter_last(0, tp_part, tp_pair, tp_part, tp_recv, tok_out)
    wkey_out[...] = part_of(st)[...].astype(F32)

    def wkey_wait(d, c):
        peer = (st + d) % st_n
        z_wait(3, part_of(peer), dwr.at[peer], peer)
        wkey_out[...] += dwr[peer].astype(F32)
        return c

    lax.fori_loop(1, st_n, wkey_wait, 0)
    scatter_last(1, sp_part, sp_pair, sp_part, sp_recv, store_out)

    for copy in across + [beside] + onward:
        copy.wait_send()

    def drain(d, c):
        peer = (st + d) % st_n
        z_copy(0, ask_ref.at[peer], ask_in.at[st], peer).wait_send()
        key_copy(peer).wait_send()
        value_copy(peer).wait_send()
        back_copy(2, vs_all, peer).wait_send()
        back_copy(5, ks, peer).wait_send()
        z_copy(3, part_of(peer), dwr.at[st], peer).wait_send()
        return c

    lax.fori_loop(1, st_n, drain, 0)
    for d in range(1, hi_n + 1):
        h = (hi + d) % hi_n
        pair_copy(0, tp_part, tp_pair, h).wait_send()
        pair_copy(1, sp_part, sp_pair, h).wait_send()
        if d < hi_n:
            cross(0, tp_part, tp_recv, h).wait_send()
            cross(1, sp_part, sp_recv, h).wait_send()


def gathered_kernel(
    st_n, tp_n, depth, pass_len,
    ids_hbm, store_ref, q_hbm, g_hbm, wq_hbm, wg_hbm, wk_hbm, wv_hbm, m_hbm,
    tok_hbm, store_hbm, wkey_hbm,
    ids_ref, tok_out, store_out, wkey_out, rows, wall, wqg, q_v, g_v, m_v, acc, terms, k_all, v_all, ask_v, ask_in, order_v, req_ref, gated, slope, ret, prob_v, score_v, kvb, reqg, gboth, arr,
    hot, plow, sums, dwp, dwc, dwf, tp_part, tp_pair, tp_recv,
    lsem, gs, gr, fs, fr, fw, zs, zr, ps, pr, xs, xr, ws, wr, ss, sr, us, ur,
):
    grp = lax.axis_index("grp")
    st = lax.axis_index("st")
    tp = lax.axis_index("tp")
    hi_n = tp_n // 2
    hi, lo = tp // 2, tp % 2
    mate_t = hi * 2 + 1 - lo
    mate = {"tp": mate_t}
    twin = {"grp": 1 - grp}
    pass_rows, chunk = rows.shape[1], rows.shape[2]
    passages = pass_rows // pass_len
    model = wqg.shape[0]
    cols = q_v.shape[1]
    heads = cols // HD
    tok_rows = q_v.shape[0]
    blocks = tok_rows // BLK
    half_pass = passages // 2
    some = tile_of(half_pass, 2)
    some_rows = some * pass_len
    n_some = half_pass // some
    key_cols, value_cols = slice(0, cols), slice(cols, 2 * cols)

    def local(i, src, dst):
        copy = pltpu.make_async_copy(src, dst, lsem.at[i])
        copy.start()
        return copy

    def sent(ref, sem):
        remote(ref, ref, sem, pr.at[0], mate).wait_send()

    def landed(ref, sem):
        remote(ref, ref, ps.at[0], sem, mate).wait_recv()

    ids_copy = local(7, ids_hbm, ids_ref)
    own_rows = local(0, store_ref, rows.at[tp])
    local(1, wk_hbm, wall.at[tp, :, pl.ds(0, cols)])
    local(1, wv_hbm, wall.at[tp, :, pl.ds(cols, cols)])
    loads_q = [local(2, q_hbm, q_v), local(3, g_hbm, g_v), local(4, m_hbm, m_v)]
    local(5, wq_hbm, wqg.at[:, pl.ds(0, cols)])
    local(5, wg_hbm, wqg.at[:, pl.ds(cols, cols)])

    barrier = pltpu.get_barrier_semaphore()

    def greet_st(d, c):
        pl.semaphore_signal(
            barrier, inc=1, device_id={"st": (st + d) % st_n}, device_id_type=MESH
        )
        return c

    lax.fori_loop(1, st_n, greet_st, 0)
    for d in range(1, tp_n):
        pl.semaphore_signal(
            barrier, inc=1, device_id={"tp": (tp + d) % tp_n}, device_id_type=MESH
        )
    pl.semaphore_signal(barrier, inc=1, device_id=twin, device_id_type=MESH)

    ids_copy.wait()

    def plan(wide):
        line = lax.broadcasted_iota(jnp.int32, (8, wide), 0)
        return line, lax.broadcasted_iota(jnp.int32, (8, wide), 1)

    width = ask_v.shape[2]
    line, lane = plan(width)
    slot, place = lane // pass_len, lane % pass_len
    short_line, short_lane = plan(order_v.shape[1])
    target = jnp.full((8, width), -1, jnp.int32)
    order = jnp.zeros(order_v.shape, jnp.int32)
    taken = [jnp.int32(0)] * st_n
    for j in range(PB):
        for n in range(blocks):
            i = ids_ref[j, n]
            owner = lax.div(i, jnp.int32(passages))
            within = i - owner * passages
            rank = sum(jnp.where(owner == o, taken[o], 0) for o in range(st_n))
            taken = [taken[o] + jnp.where(owner == o, 1, 0) for o in range(st_n)]
            target = jnp.where(
                (line == owner) & (slot == rank), within * pass_len + place, target
            )
            order = jnp.where(
                (short_line == owner) & (short_lane == rank), j * blocks + n, order
            )
    order_v[...] = order
    for o in range(st_n):
        ask_v[o] = jnp.broadcast_to(target[o : o + 1], (8, width))
    pl.semaphore_wait(barrier, st_n + tp_n - 1)

    def first_row(i):
        part = (grp + i // n_some) % 2
        return pl.multiple_of((part * n_some + i % n_some) * some_rows, some_rows)

    n_part = tile_of(n_some, 2)

    def g_copy(way, lot, t, onto):
        i, count, slot = lot
        r = pl.ds(first_row(i), count * some_rows)
        away = (t - onto + tp_n) % tp_n - 1
        return remote(rows.at[t, r], rows.at[t, r], gs.at[way], gr.at[away, slot], {"tp": onto})

    def small(i):
        return i, 1, i

    def large(i):
        return n_some + i * n_part, n_part, n_some + i

    def onward(d, lot):
        return g_copy(2, lot, ((hi + d) % hi_n) * 2 + lo, mate_t)

    def g_wait(t, lot):
        g_copy(1, lot, t, tp).wait_recv()

    def rows_send(lot):
        for d in range(1, hi_n):
            g_copy(0, lot, tp, ((hi + d) % hi_n) * 2 + lo).start()
        g_copy(1, lot, tp, mate_t).start()

    def rows_small(i, c):
        rows_send(small(i))
        return c

    def rows_large(i, c):
        rows_send(large(i))
        return c

    own_rows.wait()
    lax.fori_loop(0, n_some, rows_small, 0)
    lax.fori_loop(0, n_some // n_part, rows_large, 0)

    upper = st >= st_n // 2
    mark = jnp.where(upper, st, st_n - 1 - st)

    def far_peer(d):
        i = d - 1
        i = i + jnp.where(i >= mark, 1, 0)
        return jnp.where(upper, i, st_n - 1 - i)

    def z_copy(phase, src, dst, peer):
        away = (st - peer + st_n) % st_n - 1
        return remote(src, dst, zs.at[phase], zr.at[phase, away], {"st": peer})

    def z_wait(phase, src, dst, peer):
        landed(dst, zr.at[phase, (peer - st + st_n) % st_n - 1])

    def ask_send(d, c):
        peer = (st + d) % st_n
        z_copy(0, ask_v.at[peer], ask_in.at[st], peer).start()
        return c

    lax.fori_loop(1, st_n, ask_send, 0)
    ask_in[st] = ask_v[st]
    order_copy = local(6, order_v, req_ref)

    def project(lot, send):
        i, count, _ = lot
        r = pl.ds(first_row(i), count * some_rows)

        def term(t, span):
            return dot(rows[t, r], wall[tp, pl.ds(pl.multiple_of(t * chunk, chunk), chunk), span])

        for d in range(1, hi_n):
            g_wait(((hi + d) % hi_n) * 2 + lo, lot)
            onward(d, lot).start()
        g_wait(mate_t, lot)
        near = [tp, mate_t] + [((hi + d) % hi_n) * 2 + lo for d in range(1, hi_n)]
        late = [((hi + d) % hi_n) * 2 + 1 - lo for d in range(1, hi_n)]
        total = sum(term(t, key_cols) for t in near[1:]) + term(near[0], key_cols)
        for t in late:
            g_wait(t, lot)
            total = total + term(t, key_cols)
        first = st * passages + first_row(i) // pass_len

        def keep(ref, total):
            low = total.astype(BF)
            for p in range(count * some):
                ref[first + p] = low[p * pass_len : (p + 1) * pass_len]

        keep(k_all, total)
        send()
        keep(v_all, sum(term(t, value_cols) for t in near + late))

    def part_of_all(kind, o, c, side):
        ref = k_all if kind == 0 else v_all
        return ref.at[pl.ds(o * passages + side * half_pass + c * some, some)]

    def chain_copy(kind, o, c, peer):
        part = part_of_all(kind, o, c, grp)
        away = (o - peer + st_n) % st_n - 1
        return remote(part, part, fs.at[kind, 0], fr.at[kind, away, c], {"st": peer})

    def twin_copy(kind, o, c):
        part = part_of_all(kind, o, c, grp)
        return remote(part, part, fs.at[kind, 1], fw.at[kind], twin)

    lower = st < st_n // 2
    edge = (st == 0) | (st == st_n - 1)

    def own_send(kind, c, inward=True, outward=True):
        for onto, toward in ((st + 1, lower), (st - 1, jnp.logical_not(lower))):
            there = (onto >= 0) & (onto < st_n)
            if not outward:
                there = there & toward
            if not inward:
                there = there & jnp.logical_not(toward)

            @pl.when(there)
            def _():
                chain_copy(kind, st, c, onto).start()

    def relay(kind, d, c):
        for sign in (-1, 1):
            o = st + sign * d
            onto = st - sign

            @pl.when((o >= 0) & (o < st_n))
            def _():
                chain_copy(kind, o, c, st).wait_recv()

                @pl.when((onto >= 0) & (onto < st_n))
                def _():
                    chain_copy(kind, o, c, onto).start()

                twin_copy(kind, o, c).start()

    relayed = (st_n - 1) * half_pass

    def twin_wait(kind):
        landed((k_all, v_all)[kind].at[pl.ds(0, relayed)], fw.at[kind])

    landed(wall.at[tp], lsem.at[1])
    for copy in loads_q:
        copy.wait()

    gate_rows = tok_rows // n_some

    def gates(i):
        r = pl.ds(pl.multiple_of(i * gate_rows, gate_rows), gate_rows)
        gate = g_v[r, :].astype(F32)
        grad = m_v[r, :].astype(F32)
        sig = 1.0 / (1.0 + jnp.exp(-gate))
        gated[r, :] = (gate * sig * grad).astype(BF)
        slope[r, :] = grad * (sig * (1.0 + gate * (1.0 - sig)))

    def early_step(i, c):
        project(small(i), lambda: own_send(0, i))

        for d in range(1, st_n):
            @pl.when(i >= d)
            def _():
                relay(0, d, i - d)

        @pl.when(edge | (i == 0))
        def _():
            own_send(1, i)

        gates(i)
        return c

    lax.fori_loop(0, n_some, early_step, 0)
    for i in range(n_some - 1, n_some):
        relay(0, 1, i)

    def inward_send(i, c):
        own_send(1, i, outward=False)
        return c

    lax.fori_loop(jnp.where(edge, n_some, 1), n_some, inward_send, 0)

    def second_step(i, c):
        relay(0, 2, i)
        return c

    def outward_send(i, c):
        own_send(1, i, inward=False)
        return c

    lax.fori_loop(n_some - 2, n_some, second_step, 0)
    @pl.when(edge)
    def _():
        relay(1, 1, 0)

    lax.fori_loop(jnp.where(edge, n_some, 1), n_some, outward_send, 0)

    def late_step(i, c):
        project(large(i), lambda: None)
        for q in range(n_part):
            @pl.when(jnp.logical_not(edge))
            def _():
                relay(1, 1, i * n_part + q)

        return c

    w_part = model // 2
    w_mine = pl.ds(pl.multiple_of(grp * w_part, w_part), w_part)
    w_other = pl.ds(pl.multiple_of((1 - grp) * w_part, w_part), w_part)

    def w_across(d):
        h = (hi + d) % hi_n
        part = wall.at[tp, w_mine]
        return remote(part, part, ws.at[0], wr.at[0], {"tp": h * 2 + lo})

    def w_twin(d):
        t = ((hi + d) % hi_n) * 2 + lo
        part = wall.at[t, w_mine]
        return remote(part, part, ws.at[0], wr.at[1], twin)

    def w_onward(d, k):
        t = ((hi + d) % hi_n) * 2 + lo
        part = wall.at[t, w_other if k else w_mine]
        return remote(part, part, ws.at[0], wr.at[2], mate)

    w_beside = remote(wall.at[tp], wall.at[tp], ws.at[0], wr.at[2], mate)

    def w_wait(kind, t, part):
        landed(wall.at[t, part], wr.at[kind])

    for d in range(1, hi_n):
        w_across(d).start()

    def relay_rest(kind, first, last):
        def step(i, c):
            relay(kind, 1 + i // n_some, i % n_some)
            return c

        lax.fori_loop(first, last, step, 0)

    relays = (st_n - 1) * n_some
    relay_rest(0, 3 * n_some - 3, jnp.where(edge, 3 * n_some, 0))
    lax.fori_loop(0, n_some // n_part, late_step, 0)
    w_beside.start()
    relay_rest(1, 1, jnp.where(edge, n_some, 1))
    landed(wqg, lsem.at[5])
    order_copy.wait()
    twin_wait(0)
    scale = HD ** (-0.5)

    def fill(n, ref, span, b):
        for j in range(PB):
            kvb[n, j * pass_len : (j + 1) * pass_len, span] = ref[ids_ref[j, b]]

    pairs = range(4)

    def block_rows(b):
        return pl.ds(pl.multiple_of(b * BLK, BLK), BLK)

    per_step = n_some // (blocks // 4)

    def probs_step(i, c):
        for n in pairs:
            fill(n, k_all, key_cols, 4 * i + n)
        for head in range(heads):
            hs = slice(head * HD, (head + 1) * HD)
            vs = slice(cols + head * HD, cols + (head + 1) * HD)
            for n in pairs:
                b = 4 * i + n
                r = block_rows(b)
                scores = dot(q_v[r, hs], kvb[n, :, hs], NT) * scale
                shifted = jnp.exp(scores - jnp.max(scores, axis=-1, keepdims=True))
                prob = shifted * (1.0 / jnp.sum(shifted, axis=-1, keepdims=True))
                prob_v[head, r, :] = prob
                value_grad = dot(prob.astype(BF), gated[r, hs], TN).astype(BF)
                for j in range(PB):
                    reqg[j * blocks + b, :, vs] = value_grad[j * pass_len : (j + 1) * pass_len]

        for q in range(per_step):
            relay(1, 2, i * per_step + q)

        return c

    lax.fori_loop(0, blocks // 4, probs_step, 0)

    def half(ref, peer, part):
        return ref.at[peer, :, :, part]

    def back_copy(phase, part, peer):
        return z_copy(phase, half(ret, peer, part), half(arr, st, part), peer)

    def give_back(phase, part, span, order, first, last):
        def send(d, c):
            peer = order(d)
            for k in range(depth):
                ret[peer, k, :, span] = reqg[req_ref[peer, k]][:, span]
            back_copy(phase, part, peer).start()
            return c

        lax.fori_loop(first, last, send, 0)

    def keep_own(span):
        for k in range(depth):
            arr[st, k, :, span] = reqg[req_ref[st, k]][:, span]

    def near_peer(d):
        return far_peer(st_n - d)

    ks, vs_all = pl.ds(0, cols), pl.ds(cols, cols)
    def value_peer(d):
        return jnp.where(edge, near_peer(d % (st_n - 1) + 1), near_peer(d))

    give_back(
        1, vs_all, value_cols, value_peer, 1, jnp.where(edge, st_n, st_n - 1)
    )
    keep_own(value_cols)
    relay_rest(1, n_some + per_step * (blocks // 4), relays)
    twin_wait(1)

    def block_step(i, c):
        for n in pairs:
            fill(n, v_all, value_cols, 4 * i + n)
        for head in range(heads):
            hs = slice(head * HD, (head + 1) * HD)
            vs = slice(cols + head * HD, cols + (head + 1) * HD)
            for n in pairs:
                b = 4 * i + n
                r = block_rows(b)
                prob = prob_v[head, r, :]
                prob_grad = dot(gated[r, hs], kvb[n, :, vs], NT)
                inner = jnp.sum(prob * prob_grad, axis=-1, keepdims=True)
                score_grad = (scale * prob * (prob_grad - inner)).astype(BF)
                score_v[head, r, :] = score_grad
                key_grad = dot(score_grad, q_v[r, hs], TN).astype(BF)
                for j in range(PB):
                    reqg[j * blocks + b, :, hs] = key_grad[j * pass_len : (j + 1) * pass_len]
        return c

    def token_step(i, c):
        for n in pairs:
            fill(n, k_all, key_cols, 4 * i + n)
            fill(n, v_all, value_cols, 4 * i + n)
        for head in range(heads):
            hs = slice(head * HD, (head + 1) * HD)
            vs = slice(cols + head * HD, cols + (head + 1) * HD)
            for n in pairs:
                r = block_rows(4 * i + n)
                gboth[r, hs] = dot(score_v[head, r, :], kvb[n, :, hs]).astype(BF)
                attended = dot(prob_v[head, r, :].astype(BF), kvb[n, :, vs])
                gboth[r, vs] = (attended * slope[r, hs]).astype(BF)
        return c

    lax.fori_loop(0, blocks // 4, block_step, 0)
    def key_peer(d):
        return jnp.where(edge, near_peer(jnp.where(d == 1, 1, st_n + 1 - d)), far_peer(d))

    give_back(2, ks, key_cols, key_peer, 1, st_n)
    keep_own(key_cols)

    @pl.when(jnp.logical_not(edge))
    def _():
        give_back(1, vs_all, value_cols, near_peer, st_n - 1, st_n)

    n_tile = tile_of(model, 512)

    n_tiles = model // n_tile
    tok_pair = tok_rows // tp_n

    def tile(i):
        return pl.ds(pl.multiple_of(i * n_tile, n_tile), n_tile)

    def expand(h, i):
        a = gboth[pl.ds(pl.multiple_of(h * 2 * tok_pair, tok_pair), 2 * tok_pair), :]
        part = dot(a, wqg[tile(i), :], NT).astype(BF)
        tp_part[h * 2, :, tile(i)] = part[:tok_pair]
        tp_part[h * 2 + 1, :, tile(i)] = part[tok_pair:]

    def pair_copy(h, n, slot):
        src, dst = tp_part.at[h * 2 + 1 - lo, :, n], tp_pair.at[h, :, n]
        return remote(src, dst, ps.at[0], pr.at[slot], mate)

    def cross(h, n):
        src, dst = tp_part.at[h * 2 + lo, :, n], tp_recv.at[hi, :, n]
        return remote(src, dst, xs.at[0], xr.at[0], {"tp": h * 2 + lo})

    there = 1 - hi

    def far_tile(i, c):
        expand(there, i)
        pair_copy(there, tile(i), 1 + i).start()
        return c

    for d in range(1, hi_n):
        w_wait(0, ((hi + d) % hi_n) * 2 + lo, w_mine)
        w_twin(d).start()
        w_onward(d, 0).start()

    def cross_tile(i, c):
        n = tile(i)
        pair_copy(there, n, 1 + i).wait_recv()
        own = tp_part[there * 2 + lo, :, n].astype(F32)
        tp_part[there * 2 + lo, :, n] = (own + tp_pair[there, :, n].astype(F32)).astype(BF)
        cross(there, n).start()
        return c

    def own_tile(i, c):
        expand(hi, i)
        return c

    token_step(there, 0)
    lax.fori_loop(0, n_tiles, far_tile, 0)
    token_step(hi, 0)
    lax.fori_loop(0, n_tiles, cross_tile, 0)
    lax.fori_loop(0, n_tiles, own_tile, 0)
    pair_copy(hi, pl.ds(0, model), 0).start()

    def ask_wait(d, c):
        peer = (st + d) % st_n
        z_wait(0, ask_v.at[peer], ask_in.at[peer], peer)
        return c

    lax.fori_loop(1, st_n, ask_wait, 0)
    hot_cols = depth * pass_len
    m_tile = tile_of(pass_rows, 256)
    s_tile = tile_of(pass_rows, 1024)

    def hot_step(o, c):
        target = ask_in[o][0:1, :hot_cols]
        for i in range(pass_rows // m_tile):
            line = lax.broadcasted_iota(jnp.int32, (m_tile, hot_cols), 0) + i * m_tile
            hot[o, i * m_tile : (i + 1) * m_tile, :] = jnp.where(line == target, 1.0, 0.0).astype(BF)
        return c

    lax.fori_loop(0, st_n, hot_step, 0)

    def gather_sums(kind, o, span, first=False, last=False):
        def step(i, c):
            r = pl.ds(pl.multiple_of(i * s_tile, s_tile), s_tile)
            part = dot(hot[o, r, :], arr[o, :, :, span].reshape(hot_cols, cols))
            part = part if first else acc[kind, r, :] + part
            if last:
                plow[r, span] = part.astype(BF)
            else:
                acc[kind, r, :] = part
            return c

        lax.fori_loop(0, pass_rows // s_tile, step, 0)

    sto_pair = pass_rows // tp_n

    far_tps = (there * 2, there * 2 + 1)

    def sums_copy(kind, part, t, far):
        src = plow.at[pl.ds(pl.multiple_of(t * sto_pair, sto_pair), sto_pair), part]
        return remote(src, sums.at[tp, :, part], ss.at[kind], sr.at[kind, far], {"tp": t})

    def sums_of(part, count):
        return sums.at[pl.ds(0, count), :, part]

    def grads_of(kind, peer, last=False):
        phase, part, span = (2, ks, key_cols) if kind == 0 else (1, vs_all, value_cols)
        z_wait(phase, half(ret, peer, part), half(arr, peer, part), peer)
        gather_sums(kind, peer, span, last=last)

    def sums_send(kind):
        part, span = (ks, key_cols) if kind == 0 else (vs_all, value_cols)
        for t in far_tps:
            sums_copy(kind, part, t, 1).start()
        sums_copy(kind, part, mate_t, 0).start()
        sums[tp, :, span] = plow[pl.ds(pl.multiple_of(tp * sto_pair, sto_pair), sto_pair), span]

    beyond = jnp.where(lower, st_n - 1, 0)
    middle = jnp.where(lower, st_n // 2, st_n // 2 - 1)
    beside_st = st + 1 - 2 * (st % 2)
    outer = edge
    inner = jnp.logical_not(outer)
    gather_sums(1, st, value_cols, first=True)
    gather_sums(0, st, key_cols, first=True)
    grads_of(1, beside_st)
    grads_of(1, jnp.where(outer, beyond, middle))

    grads_of(0, middle)

    grads_of(0, beyond)
    grads_of(0, beside_st, last=True)
    sums_send(0)

    share = model // st_n
    bits = 2
    bit = share // bits

    def dw_line(s, b):
        return pl.ds(pl.multiple_of(s * share + b * bit, bit), bit)

    def dw_copy(kind, b):
        line = pl.ds(b * bit, bit)
        if kind < 2:
            src, dst = dwp.at[dw_line(middle if kind else beyond, b)], dwc.at[kind, line]
            peer = beside_st
        elif kind == 2:
            src, dst, peer = dwp.at[dw_line(beside_st, b)], dwf.at[0, line], beside_st
        else:
            src, dst = dwc.at[kind - 3, line], dwf.at[1, line]
            peer = middle if kind == 4 else beyond
        return remote(src, dst, us.at[0], ur.at[min(kind, 3), b], {"st": peer})

    def dw_send(kind):
        for b in range(bits):
            dw_copy(kind, b).start()

    def dw_relay(q):
        for b in range(bits):
            line = slice(b * bit, (b + 1) * bit)
            dw_copy(q, b).wait_recv()
            own = dwp[dw_line(middle if q else beyond, b), :].astype(F32)
            dwc[q, line, :] = (dwc[q, line, :].astype(F32) + own).astype(BF)
            dw_copy(3 + q, b).start()

    def wkey_step(s):
        dwp[pl.ds(pl.multiple_of(s * chunk, chunk), chunk), :] = dot(
            rows[s], plow[:, key_cols], TN
        ).astype(BF)

    def wkey_turn(j, c):
        far = jnp.where(j == 0, beyond, middle)
        near = jnp.where(j == 2, beside_st, st)
        near_first = jnp.where(j == 0, beside_st, st)
        far_after = jnp.where(j == 1, beyond, middle)
        s = jnp.where(
            outer, jnp.where(j < 2, far, near), jnp.where((j == 0) | (j == 3), near_first, far_after)
        )
        wkey_step(s)
        for kind in range(3):
            @pl.when(outer & (j == kind))
            def _():
                dw_send(kind)

        @pl.when(inner & (j == 0))
        def _():
            dw_send(2)

        return c

    lax.fori_loop(0, st_n, wkey_turn, 0)

    @pl.when(inner)
    def _():
        dw_relay(0)

    for d in range(1, hi_n):
        t = ((hi + d) % hi_n) * 2 + lo
        w_wait(1, t, w_other)
        w_onward(d, 1).start()
    landed(wall.at[pl.ds(0, hi_n)], wr.at[2])

    def store_terms(sources, span, done):
        def step(i, c):
            n = tile(i)
            parts = [dot(sums[t, :, span], wall[t, n, span], NT) for t in sources]
            done(n, sum(parts[1:], parts[0]))
            return c

        lax.fori_loop(0, n_tiles, step, 0)

    def set_terms(n, part):
        terms[:, n] = part

    def add_terms(n, part):
        terms[:, n] += part

    def store_tile(n):
        return pltpu.make_async_copy(store_out.at[:, n], store_hbm.at[:, n], lsem.at[3])

    def keep_store(n, part):
        store_out[:, n] = (terms[:, n] + part).astype(BF)
        store_tile(n).start()

    grads_of(1, jnp.where(outer, middle, beyond), last=True)
    sums_send(1)

    landed(sums_of(ks, 1), sr.at[0, 0])
    landed(sums_of(ks, 2), sr.at[0, 1])
    store_terms((tp, mate_t) + far_tps, key_cols, set_terms)

    pair_copy(hi, pl.ds(0, model), 0).wait_recv()
    landed(tp_recv.at[there], xr.at[0])
    total = tp_part[tp].astype(F32) + tp_pair[hi].astype(F32) + tp_recv[there].astype(F32)
    tok_out[...] = total.astype(BF)
    tok_done = local(2, tok_out, tok_hbm)

    @pl.when(inner)
    def _():
        dw_relay(1)

    landed(sums_of(vs_all, 1), sr.at[1, 0])
    store_terms((tp, mate_t), value_cols, add_terms)
    landed(sums_of(vs_all, 2), sr.at[1, 1])
    store_terms(far_tps, value_cols, keep_store)

    for b in range(bits):
        line = slice(b * bit, (b + 1) * bit)
        dw_copy(2, b).wait_recv()
        wkey_out[line, :] = dwp[dw_line(st, b), :].astype(F32) + dwf[0, line, :].astype(F32)
    for b in range(bits):
        line = slice(b * bit, (b + 1) * bit)
        for kind, edge in ((3, outer), (4, inner)):
            @pl.when(edge)
            def _():
                dw_copy(kind, b).wait_recv()

        wkey_out[line, :] += dwf[1, line, :].astype(F32)

    wkey_done = local(4, wkey_out, wkey_hbm)

    for way in range(3):
        sent(rows.at[tp], gs.at[way])
    for kind, ref in ((0, k_all), (1, v_all)):
        sent(ref.at[pl.ds(0, relayed)], fs.at[kind, 1])
        for s in range(st_n):
            up, down = (s + 1) * (s + 1 < st_n), (st_n - s) * (s > 0)

            @pl.when(st == s)
            def _():
                sent(ref.at[pl.ds(0, (up + down) * half_pass)], fs.at[kind, 0])

    sent(wall.at[pl.ds(0, hi_n + 1)], ws.at[0])
    sent(ask_in.at[pl.ds(0, st_n - 1)], zs.at[0])
    sent(ret.at[pl.ds(0, st_n - 1), :, :, vs_all], zs.at[1])
    sent(ret.at[pl.ds(0, st_n - 1), :, :, ks], zs.at[2])
    sent(sums_of(ks, tp_n - 1), ss.at[0])
    sent(sums_of(vs_all, tp_n - 1), ss.at[1])
    sent(tp_pair, ps.at[0])
    sent(tp_recv.at[0], xs.at[0])
    sent(dwp.at[pl.ds(0, 3 * share)], us.at[0])
    for copy in (tok_done, store_tile(pl.ds(0, model)), wkey_done):
        copy.wait()


def settle_kernel(*refs):
    n = (len(refs) - 2) // 3
    sources, results, held = refs[:n], refs[n : 2 * n], refs[2 * n : 3 * n]
    ins, outs = refs[3 * n], refs[3 * n + 1]
    pieces = []
    for a, (source, result, here) in enumerate(zip(sources, results, held)):
        part = source.shape[0] // 2
        for i in range(2):
            r = pl.ds(i * part, part)
            pieces.append(
                (
                    pltpu.make_async_copy(source.at[r], here.at[r], ins.at[a, i]),
                    pltpu.make_async_copy(here.at[r], result.at[r], outs.at[a, i]),
                )
            )
    for fetch, _ in pieces:
        fetch.start()
    for fetch, put in pieces:
        fetch.wait()
        put.start()
    for _, put in pieces:
        put.wait()


def settle(*arrays):
    hbm = pl.BlockSpec(memory_space=pl.ANY)
    n = len(arrays)
    return pl.pallas_call(
        settle_kernel,
        out_shape=tuple(jax.ShapeDtypeStruct(a.shape, a.dtype) for a in arrays),
        in_specs=[hbm] * n,
        out_specs=(hbm,) * n,
        scratch_shapes=[pltpu.VMEM(a.shape, a.dtype) for a in arrays]
        + [pltpu.SemaphoreType.DMA((n, 2)), pltpu.SemaphoreType.DMA((n, 2))],
    )(*arrays)


def local(pass_ids, store, queries, gate_pre, w_query, w_gate, w_key, w_value, d_mem):
    st_n = lax.axis_size("st")
    tp_n = lax.axis_size("tp")
    hi_n = tp_n // 2
    tok_rows, cols = queries.shape
    blocks = tok_rows // BLK
    passages, pass_len, chunk = store.shape
    model = w_key.shape[0]
    requests = blocks * PB
    depth = max(2, requests // st_n)
    pass_rows = passages * pass_len
    share = model // st_n

    vmem = pl.BlockSpec(memory_space=pltpu.VMEM)
    smem = pl.BlockSpec(memory_space=pltpu.SMEM)
    hbm = pl.BlockSpec(memory_space=pl.ANY)
    V = pltpu.VMEM
    DMA = pltpu.SemaphoreType.DMA
    pair = 2 * cols
    tok_pair = tok_rows // tp_n
    sto_pair = pass_rows // tp_n
    hot_cols = depth * pass_len
    width = -(-hot_cols // 128) * 128
    gathered_bytes = 2 * 2 * st_n * pass_rows * cols
    steps = blocks // 4
    fits = lax.axis_size("grp") == 2 and hi_n == 2 and st_n == 4 and st_n == tp_n
    fits = fits and passages % 4 == 0 and blocks % 4 == 0 and steps == hi_n and passages // 4 % steps == 0
    if fits and gathered_bytes <= 8 << 20:
        half_pass = passages // 2
        n_some = half_pass // tile_of(half_pass, 2)
        d_tokens, d_store, d_wkey = pl.pallas_call(
            functools.partial(gathered_kernel, st_n, tp_n, depth, pass_len),
            out_shape=(
                jax.ShapeDtypeStruct((tok_pair, model), BF),
                jax.ShapeDtypeStruct((sto_pair, model), BF),
                jax.ShapeDtypeStruct((share, cols), F32),
            ),
            in_specs=[hbm] * 9,
            out_specs=(hbm, hbm, hbm),
            scratch_shapes=[
                pltpu.SMEM((PB, blocks), jnp.int32),
                V((tok_pair, model), BF),
                V((sto_pair, model), BF),
                V((share, cols), F32),
                V((tp_n, pass_rows, chunk), BF),
                V((tp_n, model, pair), BF),
                V((model, pair), BF),
                V((tok_rows, cols), BF),
                V((tok_rows, cols), BF),
                V((tok_rows, cols), BF),
                V((2, pass_rows, cols), F32),
                V((sto_pair, model), F32),
                V((st_n * passages, pass_len, cols), BF),
                V((st_n * passages, pass_len, cols), BF),
                V((st_n, 8, width), jnp.int32),
                V((st_n, 8, width), jnp.int32),
                V((8, 128), jnp.int32),
                pltpu.SMEM((8, 128), jnp.int32),
                V((tok_rows, cols), BF),
                V((tok_rows, cols), F32),
                V((st_n, depth, pass_len, pair), BF),
                V((cols // HD, tok_rows, PB * pass_len), F32),
                V((cols // HD, tok_rows, PB * pass_len), BF),
                V((4, PB * pass_len, pair), BF),
                V((requests, pass_len, pair), BF),
                V((tok_rows, pair), BF),
                V((st_n, depth, pass_len, pair), BF),
                V((st_n, pass_rows, hot_cols), BF),
                V((pass_rows, pair), BF),
                V((tp_n, sto_pair, pair), BF),
                V((model, cols), BF),
                V((2, share, cols), BF),
                V((2, share, cols), BF),
                V((tp_n, tok_pair, model), BF),
                V((hi_n, tok_pair, model), BF),
                V((hi_n, tok_pair, model), BF),
                DMA((8,)),
                DMA((3,)),
                DMA((tp_n - 1, n_some + n_some // tile_of(n_some, 2))),
                DMA((2, 2)),
                DMA((2, st_n - 1, n_some)),
                DMA((2,)),
                DMA((3,)),
                DMA((3, st_n - 1)),
                DMA((1,)),
                DMA((1 + model // tile_of(model, 512),)),
                DMA((1,)),
                DMA((1,)),
                DMA((1,)),
                DMA((3,)),
                DMA((2,)),
                DMA((2, 2)),
                DMA((1,)),
                DMA((4, 2)),
            ],
            compiler_params=pltpu.CompilerParams(
                collective_id=0, has_side_effects=True, vmem_limit_bytes=67043328
            ),
        )(
            pass_ids.T, store.reshape(pass_rows, chunk),
            queries, gate_pre, w_query, w_gate, w_key, w_value, d_mem,
        )
        d_tokens, d_store, d_wkey = settle(d_tokens, d_store, d_wkey)
        return d_tokens, d_store.reshape(passages // tp_n, pass_len, model), d_wkey

    ids = pass_ids.reshape(-1)
    owners = ids // passages
    within = ids % passages
    order = jnp.arange(requests, dtype=jnp.int32)
    earlier = (owners[None, :] == owners[:, None]) & (order[None, :] < order[:, None])
    rank = jnp.sum(earlier.astype(jnp.int32), axis=1)
    slots = jnp.stack([owners, rank])
    o_i = jnp.arange(st_n, dtype=jnp.int32)[:, None, None]
    k_i = jnp.arange(depth, dtype=jnp.int32)[None, :, None]
    match = (owners[None, None, :] == o_i) & (rank[None, None, :] == k_i)
    asked = jnp.max(jnp.where(match, within[None, None, :], -1), axis=2)
    req_of = jnp.max(jnp.where(match, order[None, None, :], 0), axis=2)
    hot_cols = depth * pass_len
    width = -(-hot_cols // 128) * 128
    lane = jnp.arange(width, dtype=jnp.int32)
    spread = jnp.repeat(asked, pass_len, axis=1)
    spread = jnp.pad(spread, ((0, 0), (0, width - hot_cols)), constant_values=-1)
    target = jnp.where(spread < 0, -1, spread * pass_len + lane[None, :] % pass_len)
    flat = jnp.pad(jnp.maximum(asked, 0), ((0, 0), (0, width - depth)))
    ask = jnp.concatenate(
        [target[:, None], flat[:, None], jnp.zeros((st_n, 6, width), jnp.int32)], axis=1
    )

    d_tokens, d_store, d_wkey = pl.pallas_call(
        functools.partial(kernel, st_n, tp_n, depth, pass_len),
        out_shape=(
            jax.ShapeDtypeStruct((tok_pair, model), BF),
            jax.ShapeDtypeStruct((sto_pair, model), BF),
            jax.ShapeDtypeStruct((share, cols), F32),
        ),
        in_specs=[smem, smem, vmem] + [hbm] * 8,
        out_specs=(vmem, vmem, vmem),
        scratch_shapes=[
            V((tp_n, pass_rows, chunk), BF),
            V((model, pair), BF),
            V((model, pair), BF),
            V((tok_rows, cols), BF),
            V((tok_rows, cols), BF),
            V((tok_rows, cols), BF),
            V((pass_rows, pair), F32),
            V((passages, pass_len, pair), BF),
            V((st_n, 8, width), jnp.int32),
            pltpu.SMEM((st_n, 8, width), jnp.int32),
            V((st_n, depth, pass_len, pair), BF),
            V((st_n, depth, pass_len, cols), BF),
            V((st_n, depth, pass_len, cols), BF),
            V((st_n, depth, pass_len, pair), BF),
            V((cols // HD, tok_rows, PB * pass_len), F32),
            V((PB * pass_len, pair), BF),
            V((requests, pass_len, pair), BF),
            V((tok_rows, pair), BF),
            V((st_n, depth, pass_len, pair), BF),
            V((st_n, pass_rows, hot_cols), BF),
            V((pass_rows, pair), BF),
            V((model, cols), BF),
            V((st_n, share, cols), BF),
            V((tp_n, tok_pair, model), BF),
            V((hi_n, tok_pair, model), BF),
            V((hi_n, tok_pair, model), BF),
            V((tp_n, sto_pair, model), BF),
            V((hi_n, sto_pair, model), BF),
            V((hi_n, sto_pair, model), BF),
            DMA((9,)),
            DMA((3, hi_n)),
            DMA((tp_n,)),
            DMA((6, st_n)),
            DMA((6, st_n)),
            DMA((2, hi_n)),
            DMA((2, hi_n)),
            DMA((2, hi_n)),
            DMA((2, hi_n)),
        ],
        compiler_params=pltpu.CompilerParams(
            collective_id=0, has_side_effects=True, vmem_limit_bytes=67043328
        ),
    )(
        slots, req_of, ask, store.reshape(pass_rows, chunk),
        queries, gate_pre, w_query, w_gate, w_key, w_value, d_mem,
    )
    return d_tokens, d_store.reshape(passages // tp_n, pass_len, model), d_wkey


def solution(mesh):
    return jax.shard_map(
        local,
        mesh=mesh,
        in_specs=(
            P(("grp", "st"), None),
            P("st", None, "tp"),
            P(("grp", "st"), "tp"),
            P(("grp", "st"), "tp"),
            P(None, "tp"),
            P(None, "tp"),
            P(None, "tp"),
            P(None, "tp"),
            P(("grp", "st"), "tp"),
        ),
        out_specs=(
            P(("grp", "st", "tp"), None),
            P(("grp", "st", "tp"), None, None),
            P(("grp", "st"), "tp"),
        ),
        check_vma=False,
    )
```

```python
import functools

import jax
import jax.numpy as jnp
from jax import lax
from jax.experimental import pallas as pl
from jax.experimental.pallas import tpu as pltpu
from jax.sharding import PartitionSpec as P

HD = 256
BLK = 128
PB = 4
BF = jnp.bfloat16
F32 = jnp.float32
MESH = pl.DeviceIdType.MESH
NT = (((1,), (1,)), ((), ()))
TN = (((0,), (0,)), ((), ()))


def dot(a, b, dims=(((1,), (0,)), ((), ()))):
    return lax.dot_general(a, b, dims, preferred_element_type=F32)


def remote(src, dst, send, recv, device):
    return pltpu.make_async_remote_copy(
        src_ref=src,
        dst_ref=dst,
        send_sem=send,
        recv_sem=recv,
        device_id=device,
        device_id_type=MESH,
    )


def tile_of(size, most):
    while size % most:
        most //= 2
    return most


def kernel(
    st_n, tp_n, depth, pass_len,
    slot_ref, req_ref, ask_ref, store_ref, q_hbm, g_hbm, wq_hbm, wg_hbm, wk_hbm, wv_hbm, m_hbm,
    tok_out, store_out, wkey_out,
    rows, wkv, wqg, q_v, g_v, m_v, acc, kv, ask_in, ask_s, out, inc_k, inc_v, ret, prob_v, kvb, reqg, gboth, arr,
    hot, plow, dwp, dwr, tp_part, tp_pair, tp_recv, sp_part, sp_pair, sp_recv,
    lsem, gs, gr, zs, zr, ps, pr, xs, xr,
):
    st = lax.axis_index("st")
    tp = lax.axis_index("tp")
    hi_n = tp_n // 2
    hi, lo = tp // 2, tp % 2
    mate = {"tp": hi * 2 + 1 - lo}
    pass_rows, chunk = rows.shape[1], rows.shape[2]
    model = wqg.shape[0]
    cols = q_v.shape[1]
    heads = cols // HD
    tok_rows = q_v.shape[0]
    blocks = tok_rows // BLK
    blk_keys = PB * pass_len

    def local(i, src, dst):
        copy = pltpu.make_async_copy(src, dst, lsem.at[i])
        copy.start()
        return copy

    own_rows = local(0, store_ref, rows.at[tp])
    loads_kv = [
        local(1, wk_hbm, wkv.at[:, pl.ds(0, cols)]),
        local(2, wv_hbm, wkv.at[:, pl.ds(cols, cols)]),
    ]
    loads_q = [local(3, q_hbm, q_v), local(4, g_hbm, g_v), local(5, m_hbm, m_v)]
    loads_qg = [
        local(6, wq_hbm, wqg.at[:, pl.ds(0, cols)]),
        local(7, wg_hbm, wqg.at[:, pl.ds(cols, cols)]),
    ]

    barrier = pltpu.get_barrier_semaphore()

    def greet_st(d, c):
        pl.semaphore_signal(
            barrier, inc=1, device_id={"st": (st + d) % st_n}, device_id_type=MESH
        )
        return c

    lax.fori_loop(1, st_n, greet_st, 0)
    for d in range(1, tp_n):
        pl.semaphore_signal(
            barrier, inc=1, device_id={"tp": (tp + d) % tp_n}, device_id_type=MESH
        )
    pl.semaphore_wait(barrier, st_n - 1 + tp_n - 1)

    across = []
    for d in range(1, hi_n):
        h = (hi + d) % hi_n
        across.append(
            remote(store_ref, rows.at[tp], gs.at[0, h], gr.at[tp], {"tp": h * 2 + lo})
        )
        across[-1].start()
    beside = remote(store_ref, rows.at[tp], gs.at[1, hi], gr.at[tp], mate)
    beside.start()

    upper = st >= st_n // 2
    mark = jnp.where(upper, st, st_n - 1 - st)

    def far_peer(d):
        i = d - 1
        i = i + jnp.where(i >= mark, 1, 0)
        return jnp.where(upper, i, st_n - 1 - i)

    def z_copy(phase, src, dst, peer):
        return remote(src, dst, zs.at[phase, peer], zr.at[phase, st], {"st": peer})

    def z_wait(phase, src, dst, peer):
        remote(src, dst, zs.at[phase, peer], zr.at[phase, peer], {"st": peer}).wait_recv()

    def ask_send(d, c):
        peer = (st + d) % st_n
        z_copy(0, ask_ref.at[peer], ask_in.at[st], peer).start()
        return c

    lax.fori_loop(1, st_n, ask_send, 0)
    ask_in[st] = ask_ref[st]

    m_tile = tile_of(pass_rows, 256)

    def project(t, first):
        def step(i, c):
            r = pl.ds(pl.multiple_of(i * m_tile, m_tile), m_tile)
            part = dot(rows[t, r], wkv[pl.ds(pl.multiple_of(t * chunk, chunk), chunk), :])
            acc[r] = part if first else acc[r] + part
            return c

        lax.fori_loop(0, pass_rows // m_tile, step, 0)

    def g_wait(t):
        remote(store_ref, rows.at[t], gs.at[1, hi], gr.at[t], mate).wait_recv()

    own_rows.wait()
    for copy in loads_kv:
        copy.wait()
    project(tp, True)
    g_wait(hi * 2 + 1 - lo)
    project(hi * 2 + 1 - lo, False)

    def ask_wait(d, c):
        peer = (st + d) % st_n
        z_wait(0, ask_ref.at[peer], ask_in.at[peer], peer)
        return c

    lax.fori_loop(1, st_n, ask_wait, 0)
    ask_copy = local(8, ask_in, ask_s)
    ask_copy.wait()

    hot_cols = depth * pass_len

    def hot_step(o, c):
        target = ask_in[o][0:1, :hot_cols]
        for i in range(pass_rows // m_tile):
            line = lax.broadcasted_iota(jnp.int32, (m_tile, hot_cols), 0) + i * m_tile
            hot[o, i * m_tile : (i + 1) * m_tile, :] = jnp.where(line == target, 1.0, 0.0).astype(BF)
        return c

    lax.fori_loop(0, st_n, hot_step, 0)
    onward = []
    for d in range(1, hi_n):
        h = (hi + d) % hi_n
        t = h * 2 + lo
        g_wait(t)
        onward.append(remote(rows.at[t], rows.at[t], gs.at[2, h], gr.at[t], mate))
        onward[-1].start()
        project(t, False)
    for d in range(1, hi_n):
        t = ((hi + d) % hi_n) * 2 + 1 - lo
        g_wait(t)
        project(t, False)

    def low_step(i, c):
        kv[i] = acc[pl.ds(pl.multiple_of(i * pass_len, pass_len), pass_len), :].astype(BF)
        return c

    lax.fori_loop(0, pass_rows // pass_len, low_step, 0)

    ks, vs_all = pl.ds(0, cols), pl.ds(cols, cols)

    def half(ref, peer, part):
        return ref.at[peer, :, :, part]

    def key_copy(peer):
        return z_copy(1, half(out, peer, ks), inc_k.at[st], peer)

    def value_copy(peer):
        return z_copy(4, half(out, peer, vs_all), inc_v.at[st], peer)

    def kv_send(d, c):
        peer = far_peer(d)
        for k in range(depth):
            out[peer, k] = kv[ask_s[peer, 1, k]]
        key_copy(peer).start()
        return c

    def value_send(d, c):
        value_copy(far_peer(d)).start()
        return c

    lax.fori_loop(1, st_n, kv_send, 0)
    lax.fori_loop(1, st_n, value_send, 0)
    for k in range(depth):
        picked = kv[ask_s[st, 1, k]]
        inc_k[st, k] = picked[:, :cols]
        inc_v[st, k] = picked[:, cols:]
    for copy in loads_q + loads_qg:
        copy.wait()

    def key_wait(d, c):
        peer = (st + d) % st_n
        z_wait(1, half(out, peer, ks), inc_k.at[peer], peer)
        return c

    lax.fori_loop(1, st_n, key_wait, 0)
    scale = HD ** (-0.5)

    def probs_step(b, c):
        r = pl.ds(pl.multiple_of(b * BLK, BLK), BLK)
        for j in range(PB):
            kvb[j * pass_len : (j + 1) * pass_len, :cols] = inc_k[
                slot_ref[0, b * PB + j], slot_ref[1, b * PB + j]
            ]
        for head in range(heads):
            hs = slice(head * HD, (head + 1) * HD)
            vs = slice(cols + head * HD, cols + (head + 1) * HD)
            gate = g_v[r, hs].astype(F32)
            scores = dot(q_v[r, hs], kvb[:, hs], NT) * scale
            shifted = jnp.exp(scores - jnp.max(scores, axis=-1, keepdims=True))
            prob = shifted / jnp.sum(shifted, axis=-1, keepdims=True)
            prob_v[head, r, :] = prob
            sig = 1.0 / (1.0 + jnp.exp(-gate))
            att_grad = (gate * sig * m_v[r, hs].astype(F32)).astype(BF)
            value_grad = dot(prob.astype(BF), att_grad, TN).astype(BF)
            for j in range(PB):
                reqg[b * PB + j, :, vs] = value_grad[j * pass_len : (j + 1) * pass_len]
        return c

    lax.fori_loop(0, blocks, probs_step, 0)

    def back_copy(phase, part, peer):
        return z_copy(phase, half(ret, peer, part), half(arr, st, part), peer)

    def give_back(phase, part, span):
        def send(d, c):
            peer = far_peer(d)
            for k in range(depth):
                ret[peer, k, :, span] = reqg[req_ref[peer, k]][:, span]
            back_copy(phase, part, peer).start()
            return c

        lax.fori_loop(1, st_n, send, 0)
        for k in range(depth):
            arr[st, k, :, span] = reqg[req_ref[st, k]][:, span]

    give_back(2, vs_all, slice(cols, 2 * cols))

    def value_wait(d, c):
        peer = (st + d) % st_n
        z_wait(4, half(out, peer, vs_all), inc_v.at[peer], peer)
        return c

    lax.fori_loop(1, st_n, value_wait, 0)

    def block_step(b, c):
        r = pl.ds(pl.multiple_of(b * BLK, BLK), BLK)
        for j in range(PB):
            o, k = slot_ref[0, b * PB + j], slot_ref[1, b * PB + j]
            kvb[j * pass_len : (j + 1) * pass_len, :cols] = inc_k[o, k]
            kvb[j * pass_len : (j + 1) * pass_len, cols:] = inc_v[o, k]
        for head in range(heads):
            hs = slice(head * HD, (head + 1) * HD)
            vs = slice(cols + head * HD, cols + (head + 1) * HD)
            q = q_v[r, hs]
            key = kvb[:, hs]
            value = kvb[:, vs]
            gate = g_v[r, hs].astype(F32)
            grad = m_v[r, hs].astype(F32)
            prob = prob_v[head, r, :]
            attended = dot(prob.astype(BF), value)
            sig = 1.0 / (1.0 + jnp.exp(-gate))
            att_grad = (gate * sig * grad).astype(BF)
            gboth[r, vs] = (grad * attended * sig * (1.0 + gate * (1.0 - sig))).astype(BF)
            prob_grad = dot(att_grad, value, NT)
            inner = jnp.sum(prob * prob_grad, axis=-1, keepdims=True)
            score_grad = (scale * prob * (prob_grad - inner)).astype(BF)
            gboth[r, hs] = dot(score_grad, key).astype(BF)
            key_grad = dot(score_grad, q, TN).astype(BF)
            for j in range(PB):
                reqg[b * PB + j, :, hs] = key_grad[j * pass_len : (j + 1) * pass_len]
        return c

    lax.fori_loop(0, blocks, block_step, 0)
    give_back(5, ks, slice(0, cols))

    n_tile = tile_of(model, 512)

    def expand(src, weight, part, pair_rows, t):
        base = pl.multiple_of(t * pair_rows, pair_rows)
        a = src[pl.ds(base, pair_rows), :]

        def step(i, c):
            n = pl.ds(pl.multiple_of(i * n_tile, n_tile), n_tile)
            part[t, :, n] = dot(a, weight[n, :], NT).astype(BF)
            return c

        lax.fori_loop(0, model // n_tile, step, 0)

    def pair_copy(which, part, pair, h):
        return remote(part.at[h * 2 + 1 - lo], pair.at[h], ps.at[which, h], pr.at[which, h], mate)

    def scatter_first(which, src, weight, part, pair, pair_rows):
        for d in range(1, hi_n + 1):
            h = (hi + d) % hi_n
            expand(src, weight, part, pair_rows, h * 2 + 1 - lo)
            pair_copy(which, part, pair, h).start()

    def cross(which, send, recv, h):
        return remote(
            send.at[h * 2 + lo], recv.at[hi], xs.at[which, h], xr.at[which, hi], {"tp": h * 2 + lo}
        )

    def scatter_second(which, src, weight, part, pair, send, recv, pair_rows):
        for d in range(1, hi_n + 1):
            h = (hi + d) % hi_n
            expand(src, weight, part, pair_rows, h * 2 + lo)
            pair_copy(which, part, pair, h).wait_recv()
            if d < hi_n:
                part[h * 2 + lo] = (part[h * 2 + lo].astype(F32) + pair[h].astype(F32)).astype(BF)
                cross(which, part, recv, h).start()

    def scatter_last(which, part, pair, send, recv, result):
        for d in range(1, hi_n):
            h = (hi + d) % hi_n
            remote(
                send.at[h * 2 + lo], recv.at[h], xs.at[which, h], xr.at[which, h], {"tp": h * 2 + lo}
            ).wait_recv()
        total = part[tp].astype(F32) + pair[hi].astype(F32)
        for d in range(1, hi_n):
            total = total + recv[(hi + d) % hi_n].astype(F32)
        result[...] = total.astype(BF)

    tok_pair = tok_rows // tp_n
    sto_pair = pass_rows // tp_n
    scatter_first(0, gboth, wqg, tp_part, tp_pair, tok_pair)
    scatter_second(0, gboth, wqg, tp_part, tp_pair, tp_part, tp_recv, tok_pair)

    def gather_sums(o, span, first):
        def step(i, c):
            r = pl.ds(pl.multiple_of(i * m_tile, m_tile), m_tile)
            part = dot(hot[o, r, :], arr[o, :, :, span].reshape(hot_cols, cols))
            acc[r, span] = part if first else acc[r, span] + part
            return c

        lax.fori_loop(0, pass_rows // m_tile, step, 0)

    for phase, part, span in ((2, vs_all, slice(cols, 2 * cols)), (5, ks, slice(0, cols))):
        gather_sums(st, span, True)

        def grad_wait(d, c):
            peer = (st + d) % st_n
            z_wait(phase, half(ret, peer, part), half(arr, peer, part), peer)
            gather_sums(peer, span, False)
            return c

        lax.fori_loop(1, st_n, grad_wait, 0)
        plow[:, span] = acc[:, span].astype(BF)

    scatter_first(1, plow, wkv, sp_part, sp_pair, sto_pair)

    def wkey_step(t, c):
        dwp[pl.ds(pl.multiple_of(t * chunk, chunk), chunk), :] = dot(
            rows[t], plow[:, :cols], TN
        ).astype(BF)
        return c

    lax.fori_loop(0, tp_n, wkey_step, 0)
    share = model // st_n

    def part_of(s):
        return dwp.at[pl.ds(pl.multiple_of(s * share, share), share), :]

    def wkey_send(d, c):
        peer = far_peer(d)
        z_copy(3, part_of(peer), dwr.at[st], peer).start()
        return c

    lax.fori_loop(1, st_n, wkey_send, 0)
    scatter_second(1, plow, wkv, sp_part, sp_pair, sp_part, sp_recv, sto_pair)
    scatter_last(0, tp_part, tp_pair, tp_part, tp_recv, tok_out)
    wkey_out[...] = part_of(st)[...].astype(F32)

    def wkey_wait(d, c):
        peer = (st + d) % st_n
        z_wait(3, part_of(peer), dwr.at[peer], peer)
        wkey_out[...] += dwr[peer].astype(F32)
        return c

    lax.fori_loop(1, st_n, wkey_wait, 0)
    scatter_last(1, sp_part, sp_pair, sp_part, sp_recv, store_out)

    for copy in across + [beside] + onward:
        copy.wait_send()

    def drain(d, c):
        peer = (st + d) % st_n
        z_copy(0, ask_ref.at[peer], ask_in.at[st], peer).wait_send()
        key_copy(peer).wait_send()
        value_copy(peer).wait_send()
        back_copy(2, vs_all, peer).wait_send()
        back_copy(5, ks, peer).wait_send()
        z_copy(3, part_of(peer), dwr.at[st], peer).wait_send()
        return c

    lax.fori_loop(1, st_n, drain, 0)
    for d in range(1, hi_n + 1):
        h = (hi + d) % hi_n
        pair_copy(0, tp_part, tp_pair, h).wait_send()
        pair_copy(1, sp_part, sp_pair, h).wait_send()
        if d < hi_n:
            cross(0, tp_part, tp_recv, h).wait_send()
            cross(1, sp_part, sp_recv, h).wait_send()


def gathered_kernel(
    st_n, tp_n, depth, pass_len,
    ids_hbm, store_ref, q_hbm, g_hbm, wq_hbm, wg_hbm, wk_hbm, wv_hbm, m_hbm,
    tok_hbm, store_hbm, wkey_hbm,
    ids_ref, tok_out, store_out, wkey_out, rows, wall, wqg, q_v, g_v, m_v, acc, terms, k_all, v_all, ask_v, ask_in, order_v, req_ref, gated, slope, ret, prob_v, score_v, kvb, reqg, gboth, arr,
    hot, plow, sums, dwp, dwc, dwf, tp_part, tp_pair, tp_recv,
    lsem, gs, gr, fs, fr, fw, zs, zr, ps, pr, xs, xr, ws, wr, ss, sr, us, ur,
):
    grp = lax.axis_index("grp")
    st = lax.axis_index("st")
    tp = lax.axis_index("tp")
    hi_n = tp_n // 2
    hi, lo = tp // 2, tp % 2
    mate_t = hi * 2 + 1 - lo
    mate = {"tp": mate_t}
    twin = {"grp": 1 - grp}
    pass_rows, chunk = rows.shape[1], rows.shape[2]
    passages = pass_rows // pass_len
    model = wqg.shape[0]
    cols = q_v.shape[1]
    heads = cols // HD
    tok_rows = q_v.shape[0]
    blocks = tok_rows // BLK
    half_pass = passages // 2
    some = tile_of(half_pass, 2)
    some_rows = some * pass_len
    n_some = half_pass // some
    key_cols, value_cols = slice(0, cols), slice(cols, 2 * cols)

    def local(i, src, dst):
        copy = pltpu.make_async_copy(src, dst, lsem.at[i])
        copy.start()
        return copy

    def sent(ref, sem):
        remote(ref, ref, sem, pr.at[0], mate).wait_send()

    def landed(ref, sem):
        remote(ref, ref, ps.at[0], sem, mate).wait_recv()

    ids_copy = local(7, ids_hbm, ids_ref)
    own_rows = local(0, store_ref, rows.at[tp])
    local(1, wk_hbm, wall.at[tp, :, pl.ds(0, cols)])
    local(1, wv_hbm, wall.at[tp, :, pl.ds(cols, cols)])
    loads_q = [local(2, q_hbm, q_v), local(3, g_hbm, g_v), local(4, m_hbm, m_v)]
    local(5, wq_hbm, wqg.at[:, pl.ds(0, cols)])
    local(5, wg_hbm, wqg.at[:, pl.ds(cols, cols)])

    barrier = pltpu.get_barrier_semaphore()

    def greet_st(d, c):
        pl.semaphore_signal(
            barrier, inc=1, device_id={"st": (st + d) % st_n}, device_id_type=MESH
        )
        return c

    lax.fori_loop(1, st_n, greet_st, 0)
    for d in range(1, tp_n):
        pl.semaphore_signal(
            barrier, inc=1, device_id={"tp": (tp + d) % tp_n}, device_id_type=MESH
        )
    pl.semaphore_signal(barrier, inc=1, device_id=twin, device_id_type=MESH)

    ids_copy.wait()

    def plan(wide):
        line = lax.broadcasted_iota(jnp.int32, (8, wide), 0)
        return line, lax.broadcasted_iota(jnp.int32, (8, wide), 1)

    width = ask_v.shape[2]
    line, lane = plan(width)
    slot, place = lane // pass_len, lane % pass_len
    short_line, short_lane = plan(order_v.shape[1])
    target = jnp.full((8, width), -1, jnp.int32)
    order = jnp.zeros(order_v.shape, jnp.int32)
    taken = [jnp.int32(0)] * st_n
    for j in range(PB):
        for n in range(blocks):
            i = ids_ref[j, n]
            owner = lax.div(i, jnp.int32(passages))
            within = i - owner * passages
            rank = sum(jnp.where(owner == o, taken[o], 0) for o in range(st_n))
            taken = [taken[o] + jnp.where(owner == o, 1, 0) for o in range(st_n)]
            target = jnp.where(
                (line == owner) & (slot == rank), within * pass_len + place, target
            )
            order = jnp.where(
                (short_line == owner) & (short_lane == rank), j * blocks + n, order
            )
    order_v[...] = order
    for o in range(st_n):
        ask_v[o] = jnp.broadcast_to(target[o : o + 1], (8, width))
    pl.semaphore_wait(barrier, st_n + tp_n - 1)

    def first_row(i):
        part = (grp + i // n_some) % 2
        return pl.multiple_of((part * n_some + i % n_some) * some_rows, some_rows)

    n_part = tile_of(n_some, 2)

    def g_copy(way, lot, t, onto):
        i, count, slot = lot
        r = pl.ds(first_row(i), count * some_rows)
        away = (t - onto + tp_n) % tp_n - 1
        return remote(rows.at[t, r], rows.at[t, r], gs.at[way], gr.at[away, slot], {"tp": onto})

    def small(i):
        return i, 1, i

    def large(i):
        return n_some + i * n_part, n_part, n_some + i

    def onward(d, lot):
        return g_copy(2, lot, ((hi + d) % hi_n) * 2 + lo, mate_t)

    def g_wait(t, lot):
        g_copy(1, lot, t, tp).wait_recv()

    def rows_send(lot):
        for d in range(1, hi_n):
            g_copy(0, lot, tp, ((hi + d) % hi_n) * 2 + lo).start()
        g_copy(1, lot, tp, mate_t).start()

    def rows_small(i, c):
        rows_send(small(i))
        return c

    def rows_large(i, c):
        rows_send(large(i))
        return c

    own_rows.wait()
    lax.fori_loop(0, n_some, rows_small, 0)
    lax.fori_loop(0, n_some // n_part, rows_large, 0)

    upper = st >= st_n // 2
    mark = jnp.where(upper, st, st_n - 1 - st)

    def far_peer(d):
        i = d - 1
        i = i + jnp.where(i >= mark, 1, 0)
        return jnp.where(upper, i, st_n - 1 - i)

    def z_copy(phase, src, dst, peer):
        away = (st - peer + st_n) % st_n - 1
        return remote(src, dst, zs.at[phase], zr.at[phase, away], {"st": peer})

    def z_wait(phase, src, dst, peer):
        landed(dst, zr.at[phase, (peer - st + st_n) % st_n - 1])

    def ask_send(d, c):
        peer = (st + d) % st_n
        z_copy(0, ask_v.at[peer], ask_in.at[st], peer).start()
        return c

    lax.fori_loop(1, st_n, ask_send, 0)
    ask_in[st] = ask_v[st]
    order_copy = local(6, order_v, req_ref)

    def project(lot, send):
        i, count, _ = lot
        r = pl.ds(first_row(i), count * some_rows)

        def term(t, span):
            return dot(rows[t, r], wall[tp, pl.ds(pl.multiple_of(t * chunk, chunk), chunk), span])

        for d in range(1, hi_n):
            g_wait(((hi + d) % hi_n) * 2 + lo, lot)
            onward(d, lot).start()
        g_wait(mate_t, lot)
        near = [tp, mate_t] + [((hi + d) % hi_n) * 2 + lo for d in range(1, hi_n)]
        late = [((hi + d) % hi_n) * 2 + 1 - lo for d in range(1, hi_n)]
        total = sum(term(t, key_cols) for t in near[1:]) + term(near[0], key_cols)
        for t in late:
            g_wait(t, lot)
            total = total + term(t, key_cols)
        first = st * passages + first_row(i) // pass_len

        def keep(ref, total):
            low = total.astype(BF)
            for p in range(count * some):
                ref[first + p] = low[p * pass_len : (p + 1) * pass_len]

        keep(k_all, total)
        send()
        keep(v_all, sum(term(t, value_cols) for t in near + late))

    def part_of_all(kind, o, c, side):
        ref = k_all if kind == 0 else v_all
        return ref.at[pl.ds(o * passages + side * half_pass + c * some, some)]

    def chain_copy(kind, o, c, peer):
        part = part_of_all(kind, o, c, grp)
        away = (o - peer + st_n) % st_n - 1
        return remote(part, part, fs.at[kind, 0], fr.at[kind, away, c], {"st": peer})

    def twin_copy(kind, o, c):
        part = part_of_all(kind, o, c, grp)
        return remote(part, part, fs.at[kind, 1], fw.at[kind], twin)

    lower = st < st_n // 2
    edge = (st == 0) | (st == st_n - 1)

    def own_send(kind, c, inward=True, outward=True):
        for onto, toward in ((st + 1, lower), (st - 1, jnp.logical_not(lower))):
            there = (onto >= 0) & (onto < st_n)
            if not outward:
                there = there & toward
            if not inward:
                there = there & jnp.logical_not(toward)

            @pl.when(there)
            def _():
                chain_copy(kind, st, c, onto).start()

    def relay(kind, d, c):
        for sign in (-1, 1):
            o = st + sign * d
            onto = st - sign

            @pl.when((o >= 0) & (o < st_n))
            def _():
                chain_copy(kind, o, c, st).wait_recv()

                @pl.when((onto >= 0) & (onto < st_n))
                def _():
                    chain_copy(kind, o, c, onto).start()

                twin_copy(kind, o, c).start()

    relayed = (st_n - 1) * half_pass

    def twin_wait(kind):
        landed((k_all, v_all)[kind].at[pl.ds(0, relayed)], fw.at[kind])

    landed(wall.at[tp], lsem.at[1])
    for copy in loads_q:
        copy.wait()

    gate_rows = tok_rows // n_some

    def gates(i):
        r = pl.ds(pl.multiple_of(i * gate_rows, gate_rows), gate_rows)
        gate = g_v[r, :].astype(F32)
        grad = m_v[r, :].astype(F32)
        sig = 1.0 / (1.0 + jnp.exp(-gate))
        gated[r, :] = (gate * sig * grad).astype(BF)
        slope[r, :] = grad * (sig * (1.0 + gate * (1.0 - sig)))

    def early_step(i, c):
        project(small(i), lambda: own_send(0, i))

        for d in range(1, st_n):
            @pl.when(i >= d)
            def _():
                relay(0, d, i - d)

        @pl.when(edge | (i == 0))
        def _():
            own_send(1, i)

        gates(i)
        return c

    lax.fori_loop(0, n_some, early_step, 0)
    for i in range(n_some - 1, n_some):
        relay(0, 1, i)

    def inward_send(i, c):
        own_send(1, i, outward=False)
        return c

    lax.fori_loop(jnp.where(edge, n_some, 1), n_some, inward_send, 0)

    def second_step(i, c):
        relay(0, 2, i)
        return c

    def outward_send(i, c):
        own_send(1, i, inward=False)
        return c

    lax.fori_loop(n_some - 2, n_some, second_step, 0)
    @pl.when(edge)
    def _():
        relay(1, 1, 0)

    lax.fori_loop(jnp.where(edge, n_some, 1), n_some, outward_send, 0)

    def late_step(i, c):
        project(large(i), lambda: None)
        for q in range(n_part):
            @pl.when(jnp.logical_not(edge))
            def _():
                relay(1, 1, i * n_part + q)

        return c

    w_part = model // 2
    w_mine = pl.ds(pl.multiple_of(grp * w_part, w_part), w_part)
    w_other = pl.ds(pl.multiple_of((1 - grp) * w_part, w_part), w_part)

    def w_across(d):
        h = (hi + d) % hi_n
        part = wall.at[tp, w_mine]
        return remote(part, part, ws.at[0], wr.at[0], {"tp": h * 2 + lo})

    def w_twin(d):
        t = ((hi + d) % hi_n) * 2 + lo
        part = wall.at[t, w_mine]
        return remote(part, part, ws.at[0], wr.at[1], twin)

    def w_onward(d, k):
        t = ((hi + d) % hi_n) * 2 + lo
        part = wall.at[t, w_other if k else w_mine]
        return remote(part, part, ws.at[0], wr.at[2], mate)

    w_beside = remote(wall.at[tp], wall.at[tp], ws.at[0], wr.at[2], mate)

    def w_wait(kind, t, part):
        landed(wall.at[t, part], wr.at[kind])

    for d in range(1, hi_n):
        w_across(d).start()

    def relay_rest(kind, first, last):
        def step(i, c):
            relay(kind, 1 + i // n_some, i % n_some)
            return c

        lax.fori_loop(first, last, step, 0)

    relays = (st_n - 1) * n_some
    relay_rest(0, 3 * n_some - 3, jnp.where(edge, 3 * n_some, 0))
    lax.fori_loop(0, n_some // n_part, late_step, 0)
    w_beside.start()
    relay_rest(1, 1, jnp.where(edge, n_some, 1))
    landed(wqg, lsem.at[5])
    order_copy.wait()
    twin_wait(0)
    scale = HD ** (-0.5)

    def fill(n, ref, span, b):
        for j in range(PB):
            kvb[n, j * pass_len : (j + 1) * pass_len, span] = ref[ids_ref[j, b]]

    pairs = range(4)

    def block_rows(b):
        return pl.ds(pl.multiple_of(b * BLK, BLK), BLK)

    per_step = n_some // (blocks // 4)

    def probs_step(i, c):
        for n in pairs:
            fill(n, k_all, key_cols, 4 * i + n)
        for head in range(heads):
            hs = slice(head * HD, (head + 1) * HD)
            vs = slice(cols + head * HD, cols + (head + 1) * HD)
            for n in pairs:
                b = 4 * i + n
                r = block_rows(b)
                scores = dot(q_v[r, hs], kvb[n, :, hs], NT) * scale
                shifted = jnp.exp(scores - jnp.max(scores, axis=-1, keepdims=True))
                prob = shifted * (1.0 / jnp.sum(shifted, axis=-1, keepdims=True))
                prob_v[head, r, :] = prob
                value_grad = dot(prob.astype(BF), gated[r, hs], TN).astype(BF)
                for j in range(PB):
                    reqg[j * blocks + b, :, vs] = value_grad[j * pass_len : (j + 1) * pass_len]

        for q in range(per_step):
            relay(1, 2, i * per_step + q)

        return c

    lax.fori_loop(0, blocks // 4, probs_step, 0)

    def half(ref, peer, part):
        return ref.at[peer, :, :, part]

    def back_copy(phase, part, peer):
        return z_copy(phase, half(ret, peer, part), half(arr, st, part), peer)

    def give_back(phase, part, span, order, first, last):
        def send(d, c):
            peer = order(d)
            for k in range(depth):
                ret[peer, k, :, span] = reqg[req_ref[peer, k]][:, span]
            back_copy(phase, part, peer).start()
            return c

        lax.fori_loop(first, last, send, 0)

    def keep_own(span):
        for k in range(depth):
            arr[st, k, :, span] = reqg[req_ref[st, k]][:, span]

    def near_peer(d):
        return far_peer(st_n - d)

    ks, vs_all = pl.ds(0, cols), pl.ds(cols, cols)
    def value_peer(d):
        return jnp.where(edge, near_peer(d % (st_n - 1) + 1), near_peer(d))

    give_back(
        1, vs_all, value_cols, value_peer, 1, jnp.where(edge, st_n, st_n - 1)
    )
    keep_own(value_cols)
    relay_rest(1, n_some + per_step * (blocks // 4), relays)
    twin_wait(1)

    def block_step(i, c):
        for n in pairs:
            fill(n, v_all, value_cols, 4 * i + n)
        for head in range(heads):
            hs = slice(head * HD, (head + 1) * HD)
            vs = slice(cols + head * HD, cols + (head + 1) * HD)
            for n in pairs:
                b = 4 * i + n
                r = block_rows(b)
                prob = prob_v[head, r, :]
                prob_grad = dot(gated[r, hs], kvb[n, :, vs], NT)
                inner = jnp.sum(prob * prob_grad, axis=-1, keepdims=True)
                score_grad = (scale * prob * (prob_grad - inner)).astype(BF)
                score_v[head, r, :] = score_grad
                key_grad = dot(score_grad, q_v[r, hs], TN).astype(BF)
                for j in range(PB):
                    reqg[j * blocks + b, :, hs] = key_grad[j * pass_len : (j + 1) * pass_len]
        return c

    def token_step(i, c):
        for n in pairs:
            fill(n, k_all, key_cols, 4 * i + n)
            fill(n, v_all, value_cols, 4 * i + n)
        for head in range(heads):
            hs = slice(head * HD, (head + 1) * HD)
            vs = slice(cols + head * HD, cols + (head + 1) * HD)
            for n in pairs:
                r = block_rows(4 * i + n)
                gboth[r, hs] = dot(score_v[head, r, :], kvb[n, :, hs]).astype(BF)
                attended = dot(prob_v[head, r, :].astype(BF), kvb[n, :, vs])
                gboth[r, vs] = (attended * slope[r, hs]).astype(BF)
        return c

    lax.fori_loop(0, blocks // 4, block_step, 0)
    def key_peer(d):
        return jnp.where(edge, near_peer(jnp.where(d == 1, 1, st_n + 1 - d)), far_peer(d))

    give_back(2, ks, key_cols, key_peer, 1, st_n)
    keep_own(key_cols)

    @pl.when(jnp.logical_not(edge))
    def _():
        give_back(1, vs_all, value_cols, near_peer, st_n - 1, st_n)

    n_tile = tile_of(model, 512)

    n_tiles = model // n_tile
    tok_pair = tok_rows // tp_n

    def tile(i):
        return pl.ds(pl.multiple_of(i * n_tile, n_tile), n_tile)

    def expand(h, i):
        a = gboth[pl.ds(pl.multiple_of(h * 2 * tok_pair, tok_pair), 2 * tok_pair), :]
        part = dot(a, wqg[tile(i), :], NT).astype(BF)
        tp_part[h * 2, :, tile(i)] = part[:tok_pair]
        tp_part[h * 2 + 1, :, tile(i)] = part[tok_pair:]

    def pair_copy(h, n, slot):
        src, dst = tp_part.at[h * 2 + 1 - lo, :, n], tp_pair.at[h, :, n]
        return remote(src, dst, ps.at[0], pr.at[slot], mate)

    def cross(h, n):
        src, dst = tp_part.at[h * 2 + lo, :, n], tp_recv.at[hi, :, n]
        return remote(src, dst, xs.at[0], xr.at[0], {"tp": h * 2 + lo})

    there = 1 - hi

    def far_tile(i, c):
        expand(there, i)
        pair_copy(there, tile(i), 1 + i).start()
        return c

    for d in range(1, hi_n):
        w_wait(0, ((hi + d) % hi_n) * 2 + lo, w_mine)
        w_twin(d).start()
        w_onward(d, 0).start()

    def cross_tile(i, c):
        n = tile(i)
        pair_copy(there, n, 1 + i).wait_recv()
        own = tp_part[there * 2 + lo, :, n].astype(F32)
        tp_part[there * 2 + lo, :, n] = (own + tp_pair[there, :, n].astype(F32)).astype(BF)
        cross(there, n).start()
        return c

    def own_tile(i, c):
        expand(hi, i)
        return c

    token_step(there, 0)
    lax.fori_loop(0, n_tiles, far_tile, 0)
    lax.fori_loop(0, n_tiles, cross_tile, 0)
    token_step(hi, 0)
    lax.fori_loop(0, n_tiles, own_tile, 0)
    pair_copy(hi, pl.ds(0, model), 0).start()

    def ask_wait(d, c):
        peer = (st + d) % st_n
        z_wait(0, ask_v.at[peer], ask_in.at[peer], peer)
        return c

    lax.fori_loop(1, st_n, ask_wait, 0)
    hot_cols = depth * pass_len
    m_tile = tile_of(pass_rows, 256)
    s_tile = tile_of(pass_rows, 1024)

    def hot_step(o, c):
        target = ask_in[o][0:1, :hot_cols]
        for i in range(pass_rows // m_tile):
            line = lax.broadcasted_iota(jnp.int32, (m_tile, hot_cols), 0) + i * m_tile
            hot[o, i * m_tile : (i + 1) * m_tile, :] = jnp.where(line == target, 1.0, 0.0).astype(BF)
        return c

    lax.fori_loop(0, st_n, hot_step, 0)

    def gather_sums(kind, o, span, first=False, last=False):
        def step(i, c):
            r = pl.ds(pl.multiple_of(i * s_tile, s_tile), s_tile)
            part = dot(hot[o, r, :], arr[o, :, :, span].reshape(hot_cols, cols))
            part = part if first else acc[kind, r, :] + part
            if last:
                plow[r, span] = part.astype(BF)
            else:
                acc[kind, r, :] = part
            return c

        lax.fori_loop(0, pass_rows // s_tile, step, 0)

    sto_pair = pass_rows // tp_n

    far_tps = (there * 2, there * 2 + 1)

    def sums_copy(kind, part, t, far):
        src = plow.at[pl.ds(pl.multiple_of(t * sto_pair, sto_pair), sto_pair), part]
        return remote(src, sums.at[tp, :, part], ss.at[kind], sr.at[kind, far], {"tp": t})

    def sums_of(part, count):
        return sums.at[pl.ds(0, count), :, part]

    def grads_of(kind, peer, last=False):
        phase, part, span = (2, ks, key_cols) if kind == 0 else (1, vs_all, value_cols)
        z_wait(phase, half(ret, peer, part), half(arr, peer, part), peer)
        gather_sums(kind, peer, span, last=last)

    def sums_send(kind):
        part, span = (ks, key_cols) if kind == 0 else (vs_all, value_cols)
        for t in far_tps:
            sums_copy(kind, part, t, 1).start()
        sums_copy(kind, part, mate_t, 0).start()
        sums[tp, :, span] = plow[pl.ds(pl.multiple_of(tp * sto_pair, sto_pair), sto_pair), span]

    beyond = jnp.where(lower, st_n - 1, 0)
    middle = jnp.where(lower, st_n // 2, st_n // 2 - 1)
    beside_st = st + 1 - 2 * (st % 2)
    outer = edge
    inner = jnp.logical_not(outer)
    gather_sums(1, st, value_cols, first=True)
    gather_sums(0, st, key_cols, first=True)
    grads_of(1, beside_st)
    grads_of(1, jnp.where(outer, beyond, middle))

    grads_of(0, middle)

    grads_of(0, beyond)
    grads_of(0, beside_st, last=True)
    sums_send(0)

    share = model // st_n
    bits = 2
    bit = share // bits

    def dw_line(s, b):
        return pl.ds(pl.multiple_of(s * share + b * bit, bit), bit)

    def dw_copy(kind, b):
        line = pl.ds(b * bit, bit)
        if kind < 2:
            src, dst = dwp.at[dw_line(middle if kind else beyond, b)], dwc.at[kind, line]
            peer = beside_st
        elif kind == 2:
            src, dst, peer = dwp.at[dw_line(beside_st, b)], dwf.at[0, line], beside_st
        else:
            src, dst = dwc.at[kind - 3, line], dwf.at[1, line]
            peer = middle if kind == 4 else beyond
        return remote(src, dst, us.at[0], ur.at[min(kind, 3), b], {"st": peer})

    def dw_send(kind):
        for b in range(bits):
            dw_copy(kind, b).start()

    def dw_relay(q):
        for b in range(bits):
            line = slice(b * bit, (b + 1) * bit)
            dw_copy(q, b).wait_recv()
            own = dwp[dw_line(middle if q else beyond, b), :].astype(F32)
            dwc[q, line, :] = (dwc[q, line, :].astype(F32) + own).astype(BF)
            dw_copy(3 + q, b).start()

    def wkey_step(s):
        dwp[pl.ds(pl.multiple_of(s * chunk, chunk), chunk), :] = dot(
            rows[s], plow[:, key_cols], TN
        ).astype(BF)

    def wkey_turn(j, c):
        far = jnp.where(j == 0, beyond, middle)
        near = jnp.where(j == 2, beside_st, st)
        near_first = jnp.where(j == 0, beside_st, st)
        far_after = jnp.where(j == 1, beyond, middle)
        s = jnp.where(
            outer, jnp.where(j < 2, far, near), jnp.where((j == 0) | (j == 3), near_first, far_after)
        )
        wkey_step(s)
        for kind in range(3):
            @pl.when(outer & (j == kind))
            def _():
                dw_send(kind)

        @pl.when(inner & (j == 0))
        def _():
            dw_send(2)

        return c

    lax.fori_loop(0, st_n, wkey_turn, 0)

    @pl.when(inner)
    def _():
        dw_relay(0)

    for d in range(1, hi_n):
        t = ((hi + d) % hi_n) * 2 + lo
        w_wait(1, t, w_other)
        w_onward(d, 1).start()
    landed(wall.at[pl.ds(0, hi_n)], wr.at[2])

    def store_terms(sources, span, done):
        def step(i, c):
            n = tile(i)
            parts = [dot(sums[t, :, span], wall[t, n, span], NT) for t in sources]
            done(n, sum(parts[1:], parts[0]))
            return c

        lax.fori_loop(0, n_tiles, step, 0)

    def set_terms(n, part):
        terms[:, n] = part

    def add_terms(n, part):
        terms[:, n] += part

    def store_tile(n):
        return pltpu.make_async_copy(store_out.at[:, n], store_hbm.at[:, n], lsem.at[3])

    def keep_store(n, part):
        store_out[:, n] = (terms[:, n] + part).astype(BF)
        store_tile(n).start()

    grads_of(1, jnp.where(outer, middle, beyond), last=True)
    sums_send(1)

    landed(sums_of(ks, 1), sr.at[0, 0])
    landed(sums_of(ks, 2), sr.at[0, 1])
    store_terms((tp, mate_t) + far_tps, key_cols, set_terms)

    pair_copy(hi, pl.ds(0, model), 0).wait_recv()
    landed(tp_recv.at[there], xr.at[0])
    total = tp_part[tp].astype(F32) + tp_pair[hi].astype(F32) + tp_recv[there].astype(F32)
    tok_out[...] = total.astype(BF)
    tok_done = local(2, tok_out, tok_hbm)

    @pl.when(inner)
    def _():
        dw_relay(1)

    landed(sums_of(vs_all, 1), sr.at[1, 0])
    store_terms((tp, mate_t), value_cols, add_terms)
    landed(sums_of(vs_all, 2), sr.at[1, 1])
    store_terms(far_tps, value_cols, keep_store)

    for b in range(bits):
        line = slice(b * bit, (b + 1) * bit)
        dw_copy(2, b).wait_recv()
        wkey_out[line, :] = dwp[dw_line(st, b), :].astype(F32) + dwf[0, line, :].astype(F32)
    for b in range(bits):
        line = slice(b * bit, (b + 1) * bit)
        for kind, edge in ((3, outer), (4, inner)):
            @pl.when(edge)
            def _():
                dw_copy(kind, b).wait_recv()

        wkey_out[line, :] += dwf[1, line, :].astype(F32)

    wkey_done = local(4, wkey_out, wkey_hbm)

    for way in range(3):
        sent(rows.at[tp], gs.at[way])
    for kind, ref in ((0, k_all), (1, v_all)):
        sent(ref.at[pl.ds(0, relayed)], fs.at[kind, 1])
        for s in range(st_n):
            up, down = (s + 1) * (s + 1 < st_n), (st_n - s) * (s > 0)

            @pl.when(st == s)
            def _():
                sent(ref.at[pl.ds(0, (up + down) * half_pass)], fs.at[kind, 0])

    sent(wall.at[pl.ds(0, hi_n + 1)], ws.at[0])
    sent(ask_in.at[pl.ds(0, st_n - 1)], zs.at[0])
    sent(ret.at[pl.ds(0, st_n - 1), :, :, vs_all], zs.at[1])
    sent(ret.at[pl.ds(0, st_n - 1), :, :, ks], zs.at[2])
    sent(sums_of(ks, tp_n - 1), ss.at[0])
    sent(sums_of(vs_all, tp_n - 1), ss.at[1])
    sent(tp_pair, ps.at[0])
    sent(tp_recv.at[0], xs.at[0])
    sent(dwp.at[pl.ds(0, 3 * share)], us.at[0])
    for copy in (tok_done, store_tile(pl.ds(0, model)), wkey_done):
        copy.wait()


def settle_kernel(*refs):
    n = (len(refs) - 2) // 3
    sources, results, held = refs[:n], refs[n : 2 * n], refs[2 * n : 3 * n]
    ins, outs = refs[3 * n], refs[3 * n + 1]
    pieces = []
    for a, (source, result, here) in enumerate(zip(sources, results, held)):
        part = source.shape[0] // 2
        for i in range(2):
            r = pl.ds(i * part, part)
            pieces.append(
                (
                    pltpu.make_async_copy(source.at[r], here.at[r], ins.at[a, i]),
                    pltpu.make_async_copy(here.at[r], result.at[r], outs.at[a, i]),
                )
            )
    for fetch, _ in pieces:
        fetch.start()
    for fetch, put in pieces:
        fetch.wait()
        put.start()
    for _, put in pieces:
        put.wait()


def settle(*arrays):
    hbm = pl.BlockSpec(memory_space=pl.ANY)
    n = len(arrays)
    return pl.pallas_call(
        settle_kernel,
        out_shape=tuple(jax.ShapeDtypeStruct(a.shape, a.dtype) for a in arrays),
        in_specs=[hbm] * n,
        out_specs=(hbm,) * n,
        scratch_shapes=[pltpu.VMEM(a.shape, a.dtype) for a in arrays]
        + [pltpu.SemaphoreType.DMA((n, 2)), pltpu.SemaphoreType.DMA((n, 2))],
    )(*arrays)


def local(pass_ids, store, queries, gate_pre, w_query, w_gate, w_key, w_value, d_mem):
    st_n = lax.axis_size("st")
    tp_n = lax.axis_size("tp")
    hi_n = tp_n // 2
    tok_rows, cols = queries.shape
    blocks = tok_rows // BLK
    passages, pass_len, chunk = store.shape
    model = w_key.shape[0]
    requests = blocks * PB
    depth = max(2, requests // st_n)
    pass_rows = passages * pass_len
    share = model // st_n

    vmem = pl.BlockSpec(memory_space=pltpu.VMEM)
    smem = pl.BlockSpec(memory_space=pltpu.SMEM)
    hbm = pl.BlockSpec(memory_space=pl.ANY)
    V = pltpu.VMEM
    DMA = pltpu.SemaphoreType.DMA
    pair = 2 * cols
    tok_pair = tok_rows // tp_n
    sto_pair = pass_rows // tp_n
    hot_cols = depth * pass_len
    width = -(-hot_cols // 128) * 128
    gathered_bytes = 2 * 2 * st_n * pass_rows * cols
    steps = blocks // 4
    fits = lax.axis_size("grp") == 2 and hi_n == 2 and st_n == 4 and st_n == tp_n
    fits = fits and passages % 4 == 0 and blocks % 4 == 0 and steps == hi_n and passages // 4 % steps == 0
    if fits and gathered_bytes <= 8 << 20:
        half_pass = passages // 2
        n_some = half_pass // tile_of(half_pass, 2)
        d_tokens, d_store, d_wkey = pl.pallas_call(
            functools.partial(gathered_kernel, st_n, tp_n, depth, pass_len),
            out_shape=(
                jax.ShapeDtypeStruct((tok_pair, model), BF),
                jax.ShapeDtypeStruct((sto_pair, model), BF),
                jax.ShapeDtypeStruct((share, cols), F32),
            ),
            in_specs=[hbm] * 9,
            out_specs=(hbm, hbm, hbm),
            scratch_shapes=[
                pltpu.SMEM((PB, blocks), jnp.int32),
                V((tok_pair, model), BF),
                V((sto_pair, model), BF),
                V((share, cols), F32),
                V((tp_n, pass_rows, chunk), BF),
                V((tp_n, model, pair), BF),
                V((model, pair), BF),
                V((tok_rows, cols), BF),
                V((tok_rows, cols), BF),
                V((tok_rows, cols), BF),
                V((2, pass_rows, cols), F32),
                V((sto_pair, model), F32),
                V((st_n * passages, pass_len, cols), BF),
                V((st_n * passages, pass_len, cols), BF),
                V((st_n, 8, width), jnp.int32),
                V((st_n, 8, width), jnp.int32),
                V((8, 128), jnp.int32),
                pltpu.SMEM((8, 128), jnp.int32),
                V((tok_rows, cols), BF),
                V((tok_rows, cols), F32),
                V((st_n, depth, pass_len, pair), BF),
                V((cols // HD, tok_rows, PB * pass_len), F32),
                V((cols // HD, tok_rows, PB * pass_len), BF),
                V((4, PB * pass_len, pair), BF),
                V((requests, pass_len, pair), BF),
                V((tok_rows, pair), BF),
                V((st_n, depth, pass_len, pair), BF),
                V((st_n, pass_rows, hot_cols), BF),
                V((pass_rows, pair), BF),
                V((tp_n, sto_pair, pair), BF),
                V((model, cols), BF),
                V((2, share, cols), BF),
                V((2, share, cols), BF),
                V((tp_n, tok_pair, model), BF),
                V((hi_n, tok_pair, model), BF),
                V((hi_n, tok_pair, model), BF),
                DMA((8,)),
                DMA((3,)),
                DMA((tp_n - 1, n_some + n_some // tile_of(n_some, 2))),
                DMA((2, 2)),
                DMA((2, st_n - 1, n_some)),
                DMA((2,)),
                DMA((3,)),
                DMA((3, st_n - 1)),
                DMA((1,)),
                DMA((1 + model // tile_of(model, 512),)),
                DMA((1,)),
                DMA((1,)),
                DMA((1,)),
                DMA((3,)),
                DMA((2,)),
                DMA((2, 2)),
                DMA((1,)),
                DMA((4, 2)),
            ],
            compiler_params=pltpu.CompilerParams(
                collective_id=0, has_side_effects=True, vmem_limit_bytes=67043328
            ),
        )(
            pass_ids.T, store.reshape(pass_rows, chunk),
            queries, gate_pre, w_query, w_gate, w_key, w_value, d_mem,
        )
        d_tokens, d_store, d_wkey = settle(d_tokens, d_store, d_wkey)
        return d_tokens, d_store.reshape(passages // tp_n, pass_len, model), d_wkey

    ids = pass_ids.reshape(-1)
    owners = ids // passages
    within = ids % passages
    order = jnp.arange(requests, dtype=jnp.int32)
    earlier = (owners[None, :] == owners[:, None]) & (order[None, :] < order[:, None])
    rank = jnp.sum(earlier.astype(jnp.int32), axis=1)
    slots = jnp.stack([owners, rank])
    o_i = jnp.arange(st_n, dtype=jnp.int32)[:, None, None]
    k_i = jnp.arange(depth, dtype=jnp.int32)[None, :, None]
    match = (owners[None, None, :] == o_i) & (rank[None, None, :] == k_i)
    asked = jnp.max(jnp.where(match, within[None, None, :], -1), axis=2)
    req_of = jnp.max(jnp.where(match, order[None, None, :], 0), axis=2)
    hot_cols = depth * pass_len
    width = -(-hot_cols // 128) * 128
    lane = jnp.arange(width, dtype=jnp.int32)
    spread = jnp.repeat(asked, pass_len, axis=1)
    spread = jnp.pad(spread, ((0, 0), (0, width - hot_cols)), constant_values=-1)
    target = jnp.where(spread < 0, -1, spread * pass_len + lane[None, :] % pass_len)
    flat = jnp.pad(jnp.maximum(asked, 0), ((0, 0), (0, width - depth)))
    ask = jnp.concatenate(
        [target[:, None], flat[:, None], jnp.zeros((st_n, 6, width), jnp.int32)], axis=1
    )

    d_tokens, d_store, d_wkey = pl.pallas_call(
        functools.partial(kernel, st_n, tp_n, depth, pass_len),
        out_shape=(
            jax.ShapeDtypeStruct((tok_pair, model), BF),
            jax.ShapeDtypeStruct((sto_pair, model), BF),
            jax.ShapeDtypeStruct((share, cols), F32),
        ),
        in_specs=[smem, smem, vmem] + [hbm] * 8,
        out_specs=(vmem, vmem, vmem),
        scratch_shapes=[
            V((tp_n, pass_rows, chunk), BF),
            V((model, pair), BF),
            V((model, pair), BF),
            V((tok_rows, cols), BF),
            V((tok_rows, cols), BF),
            V((tok_rows, cols), BF),
            V((pass_rows, pair), F32),
            V((passages, pass_len, pair), BF),
            V((st_n, 8, width), jnp.int32),
            pltpu.SMEM((st_n, 8, width), jnp.int32),
            V((st_n, depth, pass_len, pair), BF),
            V((st_n, depth, pass_len, cols), BF),
            V((st_n, depth, pass_len, cols), BF),
            V((st_n, depth, pass_len, pair), BF),
            V((cols // HD, tok_rows, PB * pass_len), F32),
            V((PB * pass_len, pair), BF),
            V((requests, pass_len, pair), BF),
            V((tok_rows, pair), BF),
            V((st_n, depth, pass_len, pair), BF),
            V((st_n, pass_rows, hot_cols), BF),
            V((pass_rows, pair), BF),
            V((model, cols), BF),
            V((st_n, share, cols), BF),
            V((tp_n, tok_pair, model), BF),
            V((hi_n, tok_pair, model), BF),
            V((hi_n, tok_pair, model), BF),
            V((tp_n, sto_pair, model), BF),
            V((hi_n, sto_pair, model), BF),
            V((hi_n, sto_pair, model), BF),
            DMA((9,)),
            DMA((3, hi_n)),
            DMA((tp_n,)),
            DMA((6, st_n)),
            DMA((6, st_n)),
            DMA((2, hi_n)),
            DMA((2, hi_n)),
            DMA((2, hi_n)),
            DMA((2, hi_n)),
        ],
        compiler_params=pltpu.CompilerParams(
            collective_id=0, has_side_effects=True, vmem_limit_bytes=67043328
        ),
    )(
        slots, req_of, ask, store.reshape(pass_rows, chunk),
        queries, gate_pre, w_query, w_gate, w_key, w_value, d_mem,
    )
    return d_tokens, d_store.reshape(passages // tp_n, pass_len, model), d_wkey


def solution(mesh):
    return jax.shard_map(
        local,
        mesh=mesh,
        in_specs=(
            P(("grp", "st"), None),
            P("st", None, "tp"),
            P(("grp", "st"), "tp"),
            P(("grp", "st"), "tp"),
            P(None, "tp"),
            P(None, "tp"),
            P(None, "tp"),
            P(None, "tp"),
            P(("grp", "st"), "tp"),
        ),
        out_specs=(
            P(("grp", "st", "tp"), None),
            P(("grp", "st", "tp"), None, None),
            P(("grp", "st"), "tp"),
        ),
        check_vma=False,
    )
```
